32 devices in a mesh: sp: 8 (over z, x), tp: 4 (over y, core).
Axes of the slice: x: 2, y: 2, z: 4, core: 2. Of those that a mesh axis runs over, the one named last changes fastest.
Arguments:
- tokens: bfloat16 [6144, 4096], P('sp', 'tp'), may hold values from -6 to 6
- norm_gain: float32 [4096], replicated, may hold values from 0.1 to 1.9
- w_query: bfloat16 [4096, 2048], P('sp', 'tp'), may hold values from -0.09375 to 0.09375
- w_key: bfloat16 [4096, 1024], P('sp', 'tp'), may hold values from -0.09375 to 0.09375
- w_value: bfloat16 [4096, 1024], P('sp', 'tp'), may hold values from -0.09375 to 0.09375
- w_pool: bfloat16 [4096, 1024], P('sp', 'tp'), may hold values from -0.09375 to 0.09375
- query_gain: float32 [64], replicated, may hold values from 0.5 to 8
- key_gain: float32 [64], replicated, may hold values from 0.5 to 8
- sink_logit: float32 [32], P('tp'), may hold values from 1 to 5
- w_out_pool: bfloat16 [1024, 4096], P('tp', 'sp'), may hold values from -0.75 to 0.75
- w_out_attn: bfloat16 [2048, 4096], P('tp', 'sp'), may hold values from -1.5 to 1.5
Outputs:
- mixed: bfloat16 [6144, 4096], P(('sp', 'tp'))
The draws below stay inside these ranges and needn't reach their ends.
All inputs are finite; a program needn't handle non-finite values.
Results may differ from the reference program's by a relative error of at most 0.014.
The reference program's roundings to bfloat16 on the way count: a program that leaves them out, or rounds other values in their place, can miss the bound.
Values may be sent and summed in bfloat16 or wider, within the bound.
A program may use at most 128 MiB of HBM per device.

```python
import jax
import jax.numpy as jnp
from jax import lax

D = 4096
HEADS = 32
KV_HEADS = 16
HEAD = 64
POOL = 1024
WINDOW = 128
GRID_W = 64
SEQ = 6144
N_TP = 4


def draw_query_gain(key, part):
    return jax.random.uniform(jax.random.fold_in(key, 11), (HEAD,), jnp.float32, 0.5, 1.5)


def draw_key_gain(key, part):
    return jax.random.uniform(jax.random.fold_in(key, 23), (HEAD,), jnp.float32, 0.5, 1.5)


def shard_levels(key, extent, cuts, smallest, high):
    level = 1.0
    for dim, blocks in cuts:
        steps = jax.random.uniform(jax.random.fold_in(jax.random.fold_in(key, 6), dim), (blocks,), jnp.float32, smallest / len(cuts), high / len(cuts))
        level = level * jnp.repeat(jnp.exp(steps), extent[dim] // blocks).reshape((-1,) + (1,) * (len(extent) - 1 - dim))
    return level


def scatter_about(key, shape, spread, most, shards=(), kind=jnp.bfloat16):
    array = spread * jax.random.normal(key, shape, jnp.float32)
    if shards:
        array = array * shard_levels(key, shape, shards, -0.22, 0.18)
    return jnp.clip(array, -most, most).astype(kind)


def setup_inputs(seed: int = 0) -> dict:
    keys = jax.random.split(jax.random.key(seed), 12)
    return {
        "tokens": scatter_about(keys[0], (SEQ, D), 1.0, 6.0, ((0, 8), (1, 4))),
        "norm_gain": jnp.clip(1.0 + 0.18 * jax.random.normal(keys[1], (D,), jnp.float32), 0.1, 1.9),
        "w_query": scatter_about(keys[2], (D, HEADS * HEAD), D ** -0.5, 0.09375, ((0, 8), (1, 4))),
        "w_key": scatter_about(keys[3], (D, KV_HEADS * HEAD), D ** -0.5, 0.09375, ((0, 8), (1, 4))),
        "w_value": scatter_about(keys[4], (D, KV_HEADS * HEAD), D ** -0.5, 0.09375, ((0, 8), (1, 4))),
        "w_pool": scatter_about(keys[5], (D, POOL), D ** -0.5, 0.09375, ((0, 8), (1, 4))),
        "query_gain": draw_query_gain(jax.random.fold_in(keys[11], 71), 0),
        "key_gain": draw_key_gain(jax.random.fold_in(keys[11], 71), 0),
        "sink_logit": jnp.clip(1.0 + 4.0 * jax.random.uniform(keys[8], (HEADS,), jnp.float32) ** shard_levels(keys[8], (HEADS,), ((0, 4),), -0.2, 0.2), 1.0, 5.0),
        "w_out_pool": scatter_about(keys[9], (POOL, D), (POOL // 16) ** -0.5, 0.75, ((0, 4), (1, 8))),
        "w_out_attn": scatter_about(keys[10], (HEADS * HEAD, D), (HEADS * HEAD // 128) ** -0.5, 1.5, ((0, 4), (1, 8))),
    }


eps = 1e-06
rope_base = 10000.0
neg_big = -1e+30

def rope_tables(positions, head_size):
    quarter = head_size // 4
    freqs = 1.0 / rope_base ** (jnp.arange(quarter, dtype=jnp.float32) * 2.0 / (head_size // 2))
    row_angle = (positions // GRID_W).astype(jnp.float32)[:, None] * freqs
    col_angle = (positions % GRID_W).astype(jnp.float32)[:, None] * freqs
    angles = jnp.concatenate([row_angle, row_angle, col_angle, col_angle], axis=-1)
    return (jnp.cos(angles), jnp.sin(angles))

def rotate(heads_in, cosine, sine):
    part_one, part_two, part_three, part_four = jnp.split(heads_in, 4, axis=-1)
    turned = jnp.concatenate([-part_two, part_one, -part_four, part_three], axis=-1)
    return heads_in * cosine[:, None, :] + turned * sine[:, None, :]

def prepare(projected, gain, cosine, sine):
    rows_count = projected.shape[0]
    shaped = projected.reshape(rows_count, -1, HEAD)
    scaled = shaped * lax.rsqrt(lax.optimization_barrier(jnp.mean(shaped * shaped, axis=-1, keepdims=True)) + eps) * gain
    return rotate(scaled, cosine, sine).reshape(rows_count, -1).astype(jnp.bfloat16)

def reference(tokens, norm_gain, w_query, w_key, w_value, w_pool, query_gain, key_gain, sink_logit, w_out_pool, w_out_attn):
    seq = tokens.shape[0]
    widened = tokens.astype(jnp.float32)
    normed = (widened * lax.rsqrt(lax.optimization_barrier(jnp.mean(widened * widened, axis=1, keepdims=True)) + eps) * norm_gain).astype(jnp.bfloat16)
    query_raw = jnp.dot(normed, w_query, preferred_element_type=jnp.float32)
    key_raw = jnp.dot(normed, w_key, preferred_element_type=jnp.float32)
    values_all = jnp.dot(normed, w_value, preferred_element_type=jnp.float32).astype(jnp.bfloat16)
    pool_in = jnp.dot(normed, w_pool, preferred_element_type=jnp.float32).astype(jnp.bfloat16)
    positions = jnp.arange(seq, dtype=jnp.int32)
    cosine, sine = rope_tables(positions, HEAD)
    queries = prepare(query_raw, query_gain, cosine, sine)
    keys_all = prepare(key_raw, key_gain, cosine, sine)
    group = HEADS // KV_HEADS
    blocks = seq // WINDOW
    padded_keys = jnp.pad(keys_all, ((WINDOW, WINDOW), (0, 0)))
    padded_values = jnp.pad(values_all, ((WINDOW, WINDOW), (0, 0)))
    sink = sink_logit.astype(jnp.float32).reshape(KV_HEADS, group, 1, 1)

    def one_block(index):
        first_row = index * WINDOW
        block_q = lax.dynamic_slice_in_dim(queries, first_row, WINDOW, 0).reshape(WINDOW, KV_HEADS, group, HEAD).astype(jnp.float32)
        block_k = lax.dynamic_slice_in_dim(padded_keys, first_row, 3 * WINDOW, 0).reshape(3 * WINDOW, KV_HEADS, HEAD).astype(jnp.float32)
        block_v = lax.dynamic_slice_in_dim(padded_values, first_row, 3 * WINDOW, 0).reshape(3 * WINDOW, KV_HEADS, HEAD).astype(jnp.float32)
        scores = jnp.einsum('qhgd,khd->hgqk', block_q, block_k) * HEAD ** (-0.5)
        query_pos = first_row + jnp.arange(WINDOW, dtype=jnp.int32)[:, None]
        key_pos = first_row - WINDOW + jnp.arange(3 * WINDOW, dtype=jnp.int32)[None, :]
        inside = (jnp.abs(query_pos - key_pos) <= WINDOW) & (key_pos >= 0) & (key_pos < seq)
        scores = jnp.where(inside, scores, neg_big)
        top = jnp.maximum(lax.optimization_barrier(jnp.max(scores, axis=-1, keepdims=True)), sink)
        raised = jnp.exp(scores - top)
        totals = lax.optimization_barrier(jnp.sum(raised, axis=-1, keepdims=True)) + jnp.exp(sink - top)
        weights = (raised / totals).astype(jnp.bfloat16)
        result = jnp.einsum('hgqk,khd->qhgd', weights.astype(jnp.float32), block_v)
        return result.reshape(WINDOW, HEADS * HEAD).astype(jnp.bfloat16)
    attended = lax.map(one_block, jnp.arange(blocks, dtype=jnp.int32)).reshape(seq, HEADS * HEAD)
    pool_wide = pool_in.astype(jnp.float32)
    prefix = jnp.concatenate([jnp.zeros((1, POOL), jnp.float32), jnp.cumsum(pool_wide, axis=0)], axis=0)
    group_ch = POOL // 4
    levels = []
    for level in range(4):
        reach = 2 ** level
        low = jnp.clip(positions - reach, 0, seq - 1)
        high = jnp.clip(positions + reach - 1, 0, seq - 1)
        counted = (high - low + 1).astype(jnp.float32)
        columns = prefix[:, level * group_ch:(level + 1) * group_ch]
        summed = columns[high + 1] - columns[low]
        levels.append(summed / counted[:, None])
    pooled = jnp.concatenate(levels, axis=1).astype(jnp.bfloat16)
    pool_cols = POOL // N_TP
    attn_cols = HEADS * HEAD // N_TP
    outcome = jnp.zeros((seq, D), jnp.float32)
    for block_index in range(N_TP):
        term = jnp.dot(pooled[:, block_index * pool_cols:(block_index + 1) * pool_cols], w_out_pool[block_index * pool_cols:(block_index + 1) * pool_cols], preferred_element_type=jnp.float32)
        term = term + jnp.dot(attended[:, block_index * attn_cols:(block_index + 1) * attn_cols], w_out_attn[block_index * attn_cols:(block_index + 1) * attn_cols], preferred_element_type=jnp.float32)
        outcome = outcome + lax.optimization_barrier(term.astype(jnp.bfloat16)).astype(jnp.float32)
    return outcome.astype(jnp.bfloat16)
```

```python
import functools

import jax
import jax.numpy as jnp
import numpy as np
from jax import lax
from jax.experimental import pallas as pl
from jax.experimental.pallas import tpu as pltpu
from jax.sharding import PartitionSpec as P

HEAD = 64
POOL = 1024
WINDOW = 128
GRID_W = 64

eps = 1e-06
rope_base = 10000.0
neg_big = -1e30
pool_pad = 16
chunks = 4
token_chunks = 8
MESH = pl.DeviceIdType.MESH
f32, bf16 = jnp.float32, jnp.bfloat16


def rope_parts(rows_total):
    quarter = HEAD // 4
    steps = np.arange(quarter, dtype=np.float32) * np.float32(2.0) / np.float32(HEAD // 2)
    freqs = (np.float32(1.0) / np.float32(rope_base) ** steps).astype(np.float32)

    def table(count, first):
        angle = np.arange(count, dtype=np.float32)[:, None] * freqs
        twice = np.concatenate([angle, angle], axis=1).astype(np.float64)
        none = np.zeros_like(twice)
        made = []
        for part in (np.cos(twice), np.sin(twice)):
            head = [part, none] if first else [none, part]
            made.append(np.concatenate(head + head, axis=1).astype(np.float32))
        return made

    return table(rows_total // GRID_W, True) + table(GRID_W, False)


def ring_place(index, count, across):
    deep = count // across
    if across == 1 or deep % 2:
        return index
    z, x = index // across, index % across
    turn = deep - 1 - z
    inner = jnp.where(turn % 2 == 0, x - 1, across - 1 - x)
    return jnp.where(x == 0, z, deep + turn * (across - 1) + inner)


def ring_index(place, count, across):
    deep = count // across
    if across == 1 or deep % 2:
        return place
    rest = jnp.maximum(place - deep, 0)
    turn, inner = rest // (across - 1), rest % (across - 1)
    x = jnp.where(turn % 2 == 0, inner + 1, across - 1 - inner)
    return jnp.where(place < deep, place * across, (deep - 1 - turn) * across + x)


def norm_rope(raw, gain, cosine, sine, low_half, lead):
    squares = raw * raw
    low_sum = jnp.sum(jnp.where(low_half, squares, 0.0), axis=1, keepdims=True)
    high_sum = jnp.sum(jnp.where(low_half, 0.0, squares), axis=1, keepdims=True)
    mean = jnp.where(low_half, low_sum, high_sum) * (1.0 / HEAD)
    scaled = raw * lax.rsqrt(mean + eps) * gain
    turned = jnp.where(
        lead,
        -pltpu.roll(scaled, 2 * HEAD - HEAD // 4, 1),
        pltpu.roll(scaled, HEAD // 4, 1),
    )
    return scaled * cosine + turned * sine


def layer_kernel(
    count,
    members,
    tokens,
    wq,
    wk,
    wv,
    wp,
    wop,
    woa,
    norm_gain,
    query_gain,
    key_gain,
    row_cos,
    row_sin,
    col_cos,
    col_sin,
    sink,
    out,
    tok,
    normed,
    w_side,
    w_query,
    w_out,
    side,
    query,
    band,
    pool_band,
    cosines,
    sines,
    mixer,
    away,
    met,
    kept,
    y_send,
    y_recv,
    done,
    load_sem,
    side_send,
    side_recv,
    query_send,
    query_recv,
    out_send,
    out_recv,
    ty_send,
    ty_recv,
    td_send,
    td_recv,
    halo_send,
    halo_recv,
    met_send,
    met_recv,
    yy_send,
    yy_recv,
    done_sem,
):
    rows, features = tokens.shape
    depth, kw = wk.shape
    qw, pw, width = wq.shape[1], wp.shape[1], wop.shape[1]
    chips = members // 2
    share = rows // members
    half = (count - 1) // 2
    heads_k = kw // HEAD
    seq = count * rows
    across = chips

    me, tp = lax.axis_index("sp"), lax.axis_index("tp")
    chip, core = tp // 2, tp % 2
    partner = chip * 2 + 1 - core
    place = ring_place(me, count, across)
    owner_of = lambda spot: ring_index(spot, count, across)
    at = lambda offset: (place + offset + count) % count
    following, previous = owner_of(at(1)), owner_of(at(-1))

    loads = [
        pltpu.make_async_copy(wk, w_side.at[place, :, pl.ds(0, kw)], load_sem.at[0]),
        pltpu.make_async_copy(wv, w_side.at[place, :, pl.ds(kw, kw)], load_sem.at[1]),
        pltpu.make_async_copy(wp, w_side.at[place, :, pl.ds(2 * kw, pw)], load_sem.at[2]),
        pltpu.make_async_copy(tokens, tok.at[tp], load_sem.at[3]),
        pltpu.make_async_copy(wq, w_query.at[place], load_sem.at[4]),
        pltpu.make_async_copy(wop, w_out.at[place, pl.ds(0, pw), :], load_sem.at[5]),
        pltpu.make_async_copy(woa, w_out.at[place, pl.ds(pw, qw), :], load_sem.at[6]),
    ]
    for load in loads:
        load.start()

    barrier = pltpu.get_barrier_semaphore()
    greeted = [
        (following, tp),
        (previous, tp),
        (me, partner),
        ((me + 1) % count, tp),
        ((me + count - 1) % count, tp),
    ]
    greeted += [(me, (chip + hop) % chips * 2 + core) for hop in range(1, chips)]
    for device in greeted:
        pl.semaphore_signal(barrier, inc=1, device_id=device, device_id_type=MESH)
    pl.semaphore_wait(barrier, len(greeted))

    def remote(source, target, send_sem, recv_sem, device):
        return pltpu.make_async_remote_copy(
            src_ref=source,
            dst_ref=target,
            send_sem=send_sem,
            recv_sem=recv_sem,
            device_id=device,
            device_id_type=MESH,
        )

    def hop_copy(ring, way, spot, c):
        buffer, send_sem, recv_sem = ring
        size = buffer.shape[1] // chunks
        part = buffer.at[spot, pl.ds(pl.multiple_of(c * size, 16), size), :]
        device = (following if way == 0 else previous, tp)
        return remote(part, part, send_sem.at[way, spot, c], recv_sem.at[spot, c], device)

    def send_own(ring):
        for c in range(chunks):
            hop_copy(ring, 0, place, c).start()
            hop_copy(ring, 1, place, c).start()

    def event(ring, step, c):
        low, high = at(-step), at(step)
        hop_copy(ring, 0, low, c).wait_recv()

        @pl.when((step < half) | (c < chunks // 2))
        def _():
            hop_copy(ring, 0, low, c).start()

        hop_copy(ring, 1, high, c).wait_recv()

        @pl.when((step < half) | (c >= chunks // 2))
        def _():
            hop_copy(ring, 1, high, c).start()

    def events(ring, step):
        def body(c, carry):
            event(ring, step, c)
            return carry

        lax.fori_loop(0, chunks, body, 0)

    def opposite(ring):
        def body(c, carry):
            hop_copy(ring, 0, at(count // 2), c).wait_recv()
            return carry

        lax.fori_loop(0, chunks, body, 0)

    def sends_done(ring):
        def each(c, carry):
            hop_copy(ring, 0, place, c).wait_send()
            hop_copy(ring, 1, place, c).wait_send()

            def steps(step, inner):
                @pl.when((step < half) | (c < chunks // 2))
                def _():
                    hop_copy(ring, 0, at(-step), c).wait_send()

                @pl.when((step < half) | (c >= chunks // 2))
                def _():
                    hop_copy(ring, 1, at(step), c).wait_send()

                return inner

            return lax.fori_loop(1, half + 1, steps, carry)

        lax.fori_loop(0, chunks, each, 0)

    side_ring = (w_side, side_send, side_recv)
    query_ring = (w_query, query_send, query_recv)
    out_ring = (w_out, out_send, out_recv)

    for load in loads[:3]:
        load.wait()
    send_own(side_ring)
    loads[3].wait()

    token_rows = rows // token_chunks

    def token_part(owner, j):
        return tok.at[owner, pl.ds(pl.multiple_of(j * token_rows, 16), token_rows), :]

    def token_far(hop, owner, j):
        part = token_part(owner, j)
        target = (chip + hop) % chips * 2 + core
        return remote(
            part, part, ty_send.at[hop - 1, j], ty_recv.at[hop - 1, j], (me, target)
        )

    def token_near(slot, owner, j):
        part = token_part(owner, j)
        return remote(part, part, td_send.at[slot, j], td_recv.at[slot, j], (me, partner))

    def start_tokens(j, carry):
        for hop in range(1, chips):
            token_far(hop, tp, j).start()
        token_near(0, tp, j).start()
        return carry

    lax.fori_loop(0, token_chunks, start_tokens, 0)

    for g in range(rows // GRID_W):
        spot = pl.ds(me * (rows // GRID_W) + g, 1)
        grid_rows = pl.ds(g * GRID_W, GRID_W)
        cosines[grid_rows, :] = col_cos[...] + row_cos[spot, :]
        sines[grid_rows, :] = col_sin[...] + row_sin[spot, :]

    pieces = features // depth
    norm_rows = 32 if token_rows % 32 == 0 else 16

    def normalise(j):
        token_near(0, partner, j).wait_recv()
        for hop in range(1, chips):
            token_near(hop, (chip - hop + chips) % chips * 2 + 1 - core, j).wait_recv()

        def tile(i, carry):
            at_rows = pl.ds(pl.multiple_of(j * token_rows + i * norm_rows, 16), norm_rows)
            squares = jnp.zeros((norm_rows, 1), f32)
            for t in range(members):
                block = tok[t, at_rows, :].astype(f32)
                squares = squares + jnp.sum(block * block, axis=1, keepdims=True)
            scale = lax.rsqrt(squares / (members * features) + eps)
            for t in range(members):
                for piece in range(pieces):
                    first = piece * depth
                    gain = norm_gain[:, t * features + first : t * features + first + depth]
                    block = tok[t, at_rows, first : first + depth].astype(f32)
                    normed[t * pieces + piece, at_rows, :] = (block * scale * gain).astype(bf16)
            return carry

        lax.fori_loop(0, token_rows // norm_rows, tile, 0)

    def token_step(j, carry):
        for hop in range(1, chips):
            source = (chip - hop + chips) % chips * 2 + core
            token_far(hop, source, j).wait_recv()
            token_near(hop, source, j).start()

        @pl.when(j < half * chunks)
        def _():
            event(side_ring, j // chunks + 1, j % chunks)

        @pl.when(j >= 1)
        def _():
            normalise(j - 1)

        return carry

    lax.fori_loop(0, token_chunks, token_step, 0)
    normalise(token_chunks - 1)

    tile_rows = 256 if rows % 256 == 0 else 128

    def project(total, weights, spots, first=False):
        def body(i, carry):
            part = pl.ds(pl.multiple_of(i * tile_rows, tile_rows), tile_rows)
            terms = [
                jnp.dot(
                    normed[owner_of(spot), part, :], weights[spot], preferred_element_type=f32
                )
                for spot in spots
            ]
            value = functools.reduce(lambda a, b: a + b, terms)
            total[part, :] = value if first else total[part, :] + value
            return carry

        lax.fori_loop(0, rows // tile_rows, body, 0)

    project(side, w_side, [place], first=True)
    early = token_chunks // chunks

    def side_step(step, carry):
        @pl.when(step > early)
        def _():
            events(side_ring, step)

        project(side, w_side, [at(-step), at(step)])
        return carry

    lax.fori_loop(1, half + 1, side_step, 0)
    loads[4].wait()
    send_own(query_ring)
    opposite(side_ring)
    project(side, w_side, [at(count // 2)])

    lane = lax.broadcasted_iota(jnp.int32, (WINDOW, 2 * HEAD), 1)
    low_half = lane < HEAD
    lead = lane % (HEAD // 2) < HEAD // 4

    def prepare(i, carry):
        part = pl.ds(pl.multiple_of(i * WINDOW, WINDOW), WINDOW)
        shifted = pl.ds(pl.multiple_of((i + 1) * WINDOW, WINDOW), WINDOW)
        for h in range(kw // (2 * HEAD)):
            lanes = slice(h * 2 * HEAD, (h + 1) * 2 * HEAD)
            key = norm_rope(
                side[part, lanes], key_gain[...], cosines[part, :], sines[part, :], low_half, lead
            )
            band[shifted, lanes] = key.astype(bf16)
        band[shifted, kw : 2 * kw] = side[part, kw : 2 * kw].astype(bf16)
        pooled_rows = pl.ds(pl.multiple_of(i * WINDOW + pool_pad, pool_pad), WINDOW)
        pool_band[pooled_rows, :] = side[part, 2 * kw :].astype(bf16)
        return carry

    lax.fori_loop(0, rows // WINDOW, prepare, 0)

    before, behind = (me + count - 1) % count, (me + 1) % count

    def halo(index, buffer, size, upwards):
        if upwards:
            source, target, device = rows, 0, (behind, tp)
        else:
            source, target, device = size, rows + size, (before, tp)
        return remote(
            buffer.at[pl.ds(source, size), :],
            buffer.at[pl.ds(target, size), :],
            halo_send.at[index],
            halo_recv.at[index],
            device,
        )

    lower = [halo(0, band, WINDOW, False), halo(1, pool_band, pool_pad, False)]
    upper = [halo(2, band, WINDOW, True), halo(3, pool_band, pool_pad, True)]
    has_lower, has_upper = me > 0, me < count - 1

    @pl.when(has_lower)
    def _():
        for copy in lower:
            copy.start()

    @pl.when(has_upper)
    def _():
        for copy in upper:
            copy.start()

    @pl.when(jnp.logical_not(has_lower))
    def _():
        band[0:WINDOW, :] = jnp.zeros((WINDOW, 2 * kw), bf16)
        pool_band[0:pool_pad, :] = jnp.zeros((pool_pad, pw), bf16)

    @pl.when(jnp.logical_not(has_upper))
    def _():
        band[rows + WINDOW :, :] = jnp.zeros((WINDOW, 2 * kw), bf16)
        pool_band[rows + pool_pad :, :] = jnp.zeros((pool_pad, pw), bf16)

    project(query, w_query, [place], first=True)

    def query_step(step, carry):
        events(query_ring, step)
        project(query, w_query, [at(-step), at(step)])
        return carry

    lax.fori_loop(1, half + 1, query_step, 0)
    loads[5].wait()
    loads[6].wait()
    send_own(out_ring)

    @pl.when(has_lower)
    def _():
        for copy in upper:
            copy.wait_recv()

    @pl.when(has_upper)
    def _():
        for copy in lower:
            copy.wait_recv()

    level = tp * pw // (POOL // 4)
    reach = jnp.where(level == 0, 1, jnp.where(level == 1, 2, jnp.where(level == 2, 4, 8)))

    def pool(i, carry):
        wide = WINDOW + 2 * pool_pad
        part = pl.ds(pl.multiple_of(i * WINDOW, WINDOW), WINDOW)
        values = pool_band[pl.ds(pl.multiple_of(i * WINDOW, pool_pad), wide), :].astype(f32)
        total, chosen = values, None
        for step in range(4):
            size = 2**step
            total = total + pltpu.roll(total, wide - size, 0)
            shifted = pltpu.roll(total, size, 0)[pool_pad : pool_pad + WINDOW]
            chosen = shifted if chosen is None else jnp.where(level == step, shifted, chosen)
        spot = me * rows + i * WINDOW + lax.broadcasted_iota(jnp.int32, (WINDOW, 1), 0)
        low = jnp.maximum(spot - reach, 0)
        high = jnp.minimum(spot + reach - 1, seq - 1)
        mixer[part, 0:pw] = (chosen / (high - low + 1).astype(f32)).astype(bf16)
        return carry

    lax.fori_loop(0, rows // WINDOW, pool, 0)

    opposite(query_ring)
    project(query, w_query, [at(count // 2)])

    blocks = rows // WINDOW
    row = lax.broadcasted_iota(jnp.int32, (2 * WINDOW, 3 * WINDOW), 0) % WINDOW
    column = lax.broadcasted_iota(jnp.int32, (2 * WINDOW, 3 * WINDOW), 1)
    top_row = lax.broadcasted_iota(jnp.int32, (2 * WINDOW, 1), 0) < WINDOW

    def attend(i, carry):
        part = pl.ds(pl.multiple_of(i * WINDOW, WINDOW), WINDOW)
        key_rows = pl.ds(pl.multiple_of(i * WINDOW, WINDOW), 3 * WINDOW)
        key_pos = me * rows + i * WINDOW - WINDOW + column
        inside = (column >= row) & (column - row <= 2 * WINDOW) & (key_pos >= 0) & (key_pos < seq)
        for head in range(heads_k):
            lanes = slice(head * 2 * HEAD, (head + 1) * 2 * HEAD)
            rotated = norm_rope(
                query[part, lanes],
                query_gain[...],
                cosines[part, :],
                sines[part, :],
                low_half,
                lead,
            ) * HEAD ** (-0.5)
            other = pltpu.roll(rotated, HEAD, 1)
            if head % 2 == 0:
                pair = (jnp.where(low_half, rotated, 0.0), jnp.where(low_half, other, 0.0))
            else:
                pair = (jnp.where(low_half, 0.0, other), jnp.where(low_half, 0.0, rotated))
            stacked = jnp.concatenate(pair, axis=0).astype(bf16)
            tile = head // 2 * 2 * HEAD
            keys = band[key_rows, tile : tile + 2 * HEAD]
            values = band[key_rows, kw + tile : kw + tile + 2 * HEAD]
            scores = lax.dot_general(
                stacked, keys, (((1,), (1,)), ((), ())), preferred_element_type=f32
            )
            scores = jnp.where(inside, scores, neg_big)
            limit = jnp.where(top_row, sink[2 * head], sink[2 * head + 1])
            top = jnp.maximum(jnp.max(scores, axis=1, keepdims=True), limit)
            raised = jnp.exp(scores - top)
            totals = jnp.sum(raised, axis=1, keepdims=True) + jnp.exp(limit - top)
            weights = (raised * (1.0 / totals)).astype(bf16)
            result = jnp.dot(weights, values, preferred_element_type=f32)
            one, two = result[:WINDOW], result[WINDOW:]
            if head % 2 == 0:
                joined = jnp.where(low_half, one, pltpu.roll(two, HEAD, 1))
            else:
                joined = jnp.where(low_half, pltpu.roll(one, HEAD, 1), two)
            mixer[part, pw + head * 2 * HEAD : pw + (head + 1) * 2 * HEAD] = joined.astype(bf16)

        for c in range(chunks):

            @pl.when(i == ((c + 1) * blocks + chunks - 1) // chunks - 1)
            def _(c=c):
                event(out_ring, 1, c)

        return carry

    lax.fori_loop(0, blocks, attend, 0)

    def product(spot, which):
        left = jnp.concatenate(
            [
                mixer[pl.ds(pl.multiple_of((y * 2 + which) * share, 16), share), :]
                for y in range(chips)
            ],
            axis=0,
        )
        return jnp.dot(left, w_out[spot], preferred_element_type=f32).astype(bf16)

    def met_copy(spot):
        return remote(
            away.at[spot], met.at[spot], met_send.at[spot], met_recv.at[spot], (me, partner)
        )

    def y_copy(spot, hop):
        target = (chip + hop) % chips * 2 + core
        return remote(
            y_send.at[spot, hop - 1],
            y_recv.at[spot, hop - 1],
            yy_send.at[spot, hop - 1],
            yy_recv.at[spot, hop - 1],
            (me, target),
        )

    def done_copy(spot):
        columns = pl.ds(pl.multiple_of(owner_of(spot) * width, width), width)
        return pltpu.make_async_copy(done.at[spot], out.at[:, columns], done_sem.at[spot])

    def both_rows(spot, y):
        part = pl.ds(pl.multiple_of(y * share, 16), share)
        return kept[spot, part, :].astype(f32) + met[spot, part, :].astype(f32)

    def group(spots):
        def first(spot):
            away[spot] = product(spot, 1 - core)
            met_copy(spot).start()

        def second(spot):
            kept[spot] = product(spot, core)

        def third(spot):
            met_copy(spot).wait_recv()
            for hop in range(1, chips):
                y_send[spot, hop - 1] = both_rows(spot, (chip + hop) % chips).astype(bf16)
                y_copy(spot, hop).start()

        for part in (first, second, third):
            for spot in spots:
                part(spot)

    def finish(spot):
        total = both_rows(spot, chip)
        for hop in range(1, chips):
            y_copy(spot, hop).wait_recv()
            total = total + y_recv[spot, hop - 1].astype(f32)
        done[spot] = total.astype(bf16)
        done_copy(spot).start()

    group([place])

    def out_step(step, carry):
        @pl.when(step > 1)
        def _():
            events(out_ring, step)

        group([at(-step), at(step)])

        @pl.when(step == 1)
        def _():
            finish(place)

        @pl.when(step > 1)
        def _():
            finish(at(1 - step))
            finish(at(step - 1))

        return carry

    lax.fori_loop(1, half + 1, out_step, 0)
    opposite(out_ring)
    group([at(count // 2)])
    finish(at(-half))
    finish(at(half))
    finish(at(count // 2))

    for ring in (side_ring, query_ring, out_ring):
        sends_done(ring)

    def tokens_sent(j, carry):
        token_near(0, tp, j).wait_send()
        for hop in range(1, chips):
            token_far(hop, tp, j).wait_send()
            token_near(hop, (chip - hop + chips) % chips * 2 + core, j).wait_send()
        return carry

    lax.fori_loop(0, token_chunks, tokens_sent, 0)

    @pl.when(has_lower)
    def _():
        for copy in lower:
            copy.wait_send()

    @pl.when(has_upper)
    def _():
        for copy in upper:
            copy.wait_send()

    def blocks_sent(spot, carry):
        met_copy(spot).wait_send()
        for hop in range(1, chips):
            y_copy(spot, hop).wait_send()
        done_copy(spot).wait()
        return carry

    lax.fori_loop(0, count, blocks_sent, 0)


def shards(
    tokens,
    norm_gain,
    w_query,
    w_key,
    w_value,
    w_pool,
    query_gain,
    key_gain,
    sink_logit,
    w_out_pool,
    w_out_attn,
):
    count, members = lax.axis_size("sp"), lax.axis_size("tp")
    rows, features = tokens.shape
    depth, kw = w_key.shape
    qw, pw, width = w_query.shape[1], w_pool.shape[1], w_out_pool.shape[1]
    chips, share = members // 2, rows // members
    tables = [jnp.asarray(table) for table in rope_parts(count * rows)]
    twice = lambda gain: jnp.concatenate([gain, gain]).reshape(1, 2 * HEAD)
    anywhere = pl.BlockSpec(memory_space=pl.ANY)
    in_vmem = pl.BlockSpec(memory_space=pltpu.VMEM)
    dma = pltpu.SemaphoreType.DMA
    far = max(chips - 1, 1)
    return pl.pallas_call(
        functools.partial(layer_kernel, count, members),
        out_shape=jax.ShapeDtypeStruct((share, count * width), bf16),
        in_specs=[anywhere] * 7 + [in_vmem] * 7 + [pl.BlockSpec(memory_space=pltpu.SMEM)],
        out_specs=anywhere,
        scratch_shapes=[
            pltpu.VMEM((members, rows, features), bf16),
            pltpu.VMEM((count, rows, depth), bf16),
            pltpu.VMEM((count, depth, 2 * kw + pw), bf16),
            pltpu.VMEM((count, depth, qw), bf16),
            pltpu.VMEM((count, pw + qw, width), bf16),
            pltpu.VMEM((rows, 2 * kw + pw), f32),
            pltpu.VMEM((rows, qw), f32),
            pltpu.VMEM((rows + 2 * WINDOW, 2 * kw), bf16),
            pltpu.VMEM((rows + 2 * pool_pad, pw), bf16),
            pltpu.VMEM((rows, 2 * HEAD), f32),
            pltpu.VMEM((rows, 2 * HEAD), f32),
            pltpu.VMEM((rows, pw + qw), bf16),
            pltpu.VMEM((count, chips * share, width), bf16),
            pltpu.VMEM((count, chips * share, width), bf16),
            pltpu.VMEM((count, chips * share, width), bf16),
            pltpu.VMEM((count, far, share, width), bf16),
            pltpu.VMEM((count, far, share, width), bf16),
            pltpu.VMEM((count, share, width), bf16),
            dma((7,)),
            dma((2, count, chunks)),
            dma((count, chunks)),
            dma((2, count, chunks)),
            dma((count, chunks)),
            dma((2, count, chunks)),
            dma((count, chunks)),
            dma((far, token_chunks)),
            dma((far, token_chunks)),
            dma((chips, token_chunks)),
            dma((chips, token_chunks)),
            dma((4,)),
            dma((4,)),
            dma((count,)),
            dma((count,)),
            dma((count, far)),
            dma((count, far)),
            dma((count,)),
        ],
        compiler_params=pltpu.CompilerParams(
            collective_id=0, has_side_effects=True, vmem_limit_bytes=60 * 1024 * 1024
        ),
    )(
        tokens,
        w_query,
        w_key,
        w_value,
        w_pool,
        w_out_pool,
        w_out_attn,
        norm_gain.reshape(1, -1),
        twice(query_gain),
        twice(key_gain),
        *tables,
        sink_logit,
    )


def solution(mesh):
    placed = (
        P("sp", "tp"),
        P(),
        P("sp", "tp"),
        P("sp", "tp"),
        P("sp", "tp"),
        P("sp", "tp"),
        P(),
        P(),
        P("tp"),
        P("tp", "sp"),
        P("tp", "sp"),
    )
    return jax.shard_map(
        shards, mesh=mesh, in_specs=placed, out_specs=P(("sp", "tp"), None), check_vma=False
    )
```

```python
import functools

import jax
import jax.numpy as jnp
import numpy as np
from jax import lax
from jax.experimental import pallas as pl
from jax.experimental.pallas import tpu as pltpu
from jax.sharding import PartitionSpec as P

HEAD = 64
POOL = 1024
WINDOW = 128
GRID_W = 64

eps = 1e-06
rope_base = 10000.0
neg_big = -1e30
pool_pad = 16
chunks = 4
token_chunks = 8
in_parts = 4
out_parts = 2
MESH = pl.DeviceIdType.MESH
f32, bf16 = jnp.float32, jnp.bfloat16


def rope_parts(rows_total):
    quarter = HEAD // 4
    steps = np.arange(quarter, dtype=np.float32) * np.float32(2.0) / np.float32(HEAD // 2)
    freqs = (np.float32(1.0) / np.float32(rope_base) ** steps).astype(np.float32)

    def table(count, first):
        angle = np.arange(count, dtype=np.float32)[:, None] * freqs
        twice = np.concatenate([angle, angle], axis=1).astype(np.float64)
        none = np.zeros_like(twice)
        made = []
        for part in (np.cos(twice), np.sin(twice)):
            head = [part, none] if first else [none, part]
            made.append(np.concatenate(head + head, axis=1).astype(np.float32))
        return made

    return table(rows_total // GRID_W, True) + table(GRID_W, False)


def ring_place(index, count, across):
    deep = count // across
    if across == 1 or deep % 2:
        return index
    z, x = index // across, index % across
    turn = deep - 1 - z
    inner = jnp.where(turn % 2 == 0, x - 1, across - 1 - x)
    return jnp.where(x == 0, z, deep + turn * (across - 1) + inner)


def ring_index(place, count, across):
    deep = count // across
    if across == 1 or deep % 2:
        return place
    rest = jnp.maximum(place - deep, 0)
    turn, inner = rest // (across - 1), rest % (across - 1)
    x = jnp.where(turn % 2 == 0, inner + 1, across - 1 - inner)
    return jnp.where(place < deep, place * across, (deep - 1 - turn) * across + x)


def norm_rope(raw, gain, cosine, sine, low_half, lead):
    squares = raw * raw
    low_sum = jnp.sum(jnp.where(low_half, squares, 0.0), axis=1, keepdims=True)
    high_sum = jnp.sum(jnp.where(low_half, 0.0, squares), axis=1, keepdims=True)
    mean = jnp.where(low_half, low_sum, high_sum) * (1.0 / HEAD)
    scaled = raw * lax.rsqrt(mean + eps) * gain
    turned = jnp.where(
        lead,
        -pltpu.roll(scaled, 2 * HEAD - HEAD // 4, 1),
        pltpu.roll(scaled, HEAD // 4, 1),
    )
    return scaled * cosine + turned * sine


def layer_kernel(
    count,
    members,
    tokens,
    wq,
    wk,
    wv,
    wp,
    wop,
    woa,
    norm_gain,
    query_gain,
    key_gain,
    row_cos,
    row_sin,
    col_cos,
    col_sin,
    sink,
    out,
    tok,
    normed,
    w_side,
    w_query,
    w_out,
    side,
    query,
    band,
    pool_band,
    cosines,
    sines,
    mixer,
    away,
    met,
    kept,
    y_send,
    y_recv,
    done,
    load_sem,
    side_send,
    side_recv,
    query_send,
    query_recv,
    out_send,
    out_recv,
    ty_send,
    ty_recv,
    td_send,
    td_recv,
    halo_send,
    halo_recv,
    met_send,
    met_recv,
    yy_send,
    yy_recv,
    done_sem,
):
    rows, features = tokens.shape
    depth, kw = wk.shape
    qw, pw, width = wq.shape[1], wp.shape[1], wop.shape[1]
    chips = members // 2
    share = rows // members
    half = (count - 1) // 2
    heads_k = kw // HEAD
    seq = count * rows
    across = chips

    me, tp = lax.axis_index("sp"), lax.axis_index("tp")
    chip, core = tp // 2, tp % 2
    partner = chip * 2 + 1 - core
    place = ring_place(me, count, across)
    owner_of = lambda spot: ring_index(spot, count, across)
    at = lambda offset: (place + offset + count) % count
    following, previous = owner_of(at(1)), owner_of(at(-1))

    loads = [
        pltpu.make_async_copy(wk, w_side.at[place, :, pl.ds(0, kw)], load_sem.at[0]),
        pltpu.make_async_copy(wv, w_side.at[place, :, pl.ds(kw, kw)], load_sem.at[1]),
        pltpu.make_async_copy(wp, w_side.at[place, :, pl.ds(2 * kw, pw)], load_sem.at[2]),
        pltpu.make_async_copy(tokens, tok.at[tp], load_sem.at[3]),
        pltpu.make_async_copy(wq, w_query.at[place], load_sem.at[4]),
        pltpu.make_async_copy(wop, w_out.at[place, pl.ds(0, pw), :], load_sem.at[5]),
        pltpu.make_async_copy(woa, w_out.at[place, pl.ds(pw, qw), :], load_sem.at[6]),
    ]
    for load in loads:
        load.start()

    barrier = pltpu.get_barrier_semaphore()
    greeted = [
        (following, tp),
        (previous, tp),
        (me, partner),
        ((me + 1) % count, tp),
        ((me + count - 1) % count, tp),
    ]
    greeted += [(me, (chip + hop) % chips * 2 + core) for hop in range(1, chips)]
    for device in greeted:
        pl.semaphore_signal(barrier, inc=1, device_id=device, device_id_type=MESH)
    pl.semaphore_wait(barrier, len(greeted))

    def remote(source, target, send_sem, recv_sem, device):
        return pltpu.make_async_remote_copy(
            src_ref=source,
            dst_ref=target,
            send_sem=send_sem,
            recv_sem=recv_sem,
            device_id=device,
            device_id_type=MESH,
        )

    def hop_copy(ring, way, spot, c):
        buffer, send_sem, recv_sem = ring
        size = buffer.shape[1] // chunks
        part = buffer.at[spot, pl.ds(pl.multiple_of(c * size, 16), size), :]
        device = (following if way == 0 else previous, tp)
        return remote(part, part, send_sem.at[way, spot, c], recv_sem.at[spot, c], device)

    def send_own(ring):
        for c in range(chunks):
            hop_copy(ring, 0, place, c).start()
            hop_copy(ring, 1, place, c).start()

    def event(ring, step, c):
        low, high = at(-step), at(step)
        hop_copy(ring, 0, low, c).wait_recv()

        @pl.when((step < half) | (c < chunks // 2))
        def _():
            hop_copy(ring, 0, low, c).start()

        hop_copy(ring, 1, high, c).wait_recv()

        @pl.when((step < half) | (c >= chunks // 2))
        def _():
            hop_copy(ring, 1, high, c).start()

    def events(ring, step):
        def body(c, carry):
            event(ring, step, c)
            return carry

        lax.fori_loop(0, chunks, body, 0)

    def opposite(ring):
        def body(c, carry):
            hop_copy(ring, 0, at(count // 2), c).wait_recv()
            return carry

        lax.fori_loop(0, chunks, body, 0)

    def sends_done(ring):
        def each(c, carry):
            hop_copy(ring, 0, place, c).wait_send()
            hop_copy(ring, 1, place, c).wait_send()

            def steps(step, inner):
                @pl.when((step < half) | (c < chunks // 2))
                def _():
                    hop_copy(ring, 0, at(-step), c).wait_send()

                @pl.when((step < half) | (c >= chunks // 2))
                def _():
                    hop_copy(ring, 1, at(step), c).wait_send()

                return inner

            return lax.fori_loop(1, half + 1, steps, carry)

        lax.fori_loop(0, chunks, each, 0)

    side_ring = (w_side, side_send, side_recv)
    query_ring = (w_query, query_send, query_recv)
    out_ring = (w_out, out_send, out_recv)

    for load in loads[:3]:
        load.wait()
    send_own(side_ring)
    loads[3].wait()

    token_rows = rows // token_chunks

    def token_part(owner, j):
        return tok.at[owner, pl.ds(pl.multiple_of(j * token_rows, 16), token_rows), :]

    def token_far(hop, owner, j):
        part = token_part(owner, j)
        target = (chip + hop) % chips * 2 + core
        return remote(
            part, part, ty_send.at[hop - 1, j], ty_recv.at[hop - 1, j], (me, target)
        )

    def token_near(slot, owner, j):
        part = token_part(owner, j)
        return remote(part, part, td_send.at[slot, j], td_recv.at[slot, j], (me, partner))

    def start_tokens(j, carry):
        for hop in range(1, chips):
            token_far(hop, tp, j).start()
        token_near(0, tp, j).start()
        return carry

    lax.fori_loop(0, token_chunks, start_tokens, 0)

    for g in range(rows // GRID_W):
        spot = pl.ds(me * (rows // GRID_W) + g, 1)
        grid_rows = pl.ds(g * GRID_W, GRID_W)
        cosines[grid_rows, :] = col_cos[...] + row_cos[spot, :]
        sines[grid_rows, :] = col_sin[...] + row_sin[spot, :]

    pieces = features // depth
    norm_rows = 32 if token_rows % 32 == 0 else 16

    def normalise(j):
        token_near(0, partner, j).wait_recv()
        for hop in range(1, chips):
            token_near(hop, (chip - hop + chips) % chips * 2 + 1 - core, j).wait_recv()

        def tile(i, carry):
            at_rows = pl.ds(pl.multiple_of(j * token_rows + i * norm_rows, 16), norm_rows)
            squares = jnp.zeros((norm_rows, 1), f32)
            for t in range(members):
                block = tok[t, at_rows, :].astype(f32)
                squares = squares + jnp.sum(block * block, axis=1, keepdims=True)
            scale = lax.rsqrt(squares / (members * features) + eps)
            for t in range(members):
                for piece in range(pieces):
                    first = piece * depth
                    gain = norm_gain[:, t * features + first : t * features + first + depth]
                    block = tok[t, at_rows, first : first + depth].astype(f32)
                    normed[t * pieces + piece, at_rows, :] = (block * scale * gain).astype(bf16)
            return carry

        lax.fori_loop(0, token_rows // norm_rows, tile, 0)

    def token_step(j, carry):
        for hop in range(1, chips):
            source = (chip - hop + chips) % chips * 2 + core
            token_far(hop, source, j).wait_recv()
            token_near(hop, source, j).start()

        @pl.when(j < half * chunks)
        def _():
            event(side_ring, j // chunks + 1, j % chunks)

        @pl.when(j >= 1)
        def _():
            normalise(j - 1)

        return carry

    lax.fori_loop(0, token_chunks, token_step, 0)
    normalise(token_chunks - 1)

    tile_rows = 256 if rows % 256 == 0 else 128

    def project(total, weights, spots, first=False):
        def body(i, carry):
            part = pl.ds(pl.multiple_of(i * tile_rows, tile_rows), tile_rows)
            terms = [
                jnp.dot(
                    normed[owner_of(spot), part, :], weights[spot], preferred_element_type=f32
                )
                for spot in spots
            ]
            value = functools.reduce(lambda a, b: a + b, terms)
            total[part, :] = value if first else total[part, :] + value
            return carry

        lax.fori_loop(0, rows // tile_rows, body, 0)

    project(side, w_side, [place], first=True)
    early = token_chunks // chunks

    def side_step(step, carry):
        @pl.when(step > early)
        def _():
            events(side_ring, step)

        project(side, w_side, [at(-step), at(step)])
        return carry

    lax.fori_loop(1, half + 1, side_step, 0)
    loads[4].wait()
    send_own(query_ring)
    opposite(side_ring)
    project(side, w_side, [at(count // 2)])

    lane = lax.broadcasted_iota(jnp.int32, (WINDOW, 2 * HEAD), 1)
    low_half = lane < HEAD
    lead = lane % (HEAD // 2) < HEAD // 4

    def prepare(i, carry):
        part = pl.ds(pl.multiple_of(i * WINDOW, WINDOW), WINDOW)
        shifted = pl.ds(pl.multiple_of((i + 1) * WINDOW, WINDOW), WINDOW)
        for h in range(kw // (2 * HEAD)):
            lanes = slice(h * 2 * HEAD, (h + 1) * 2 * HEAD)
            key = norm_rope(
                side[part, lanes], key_gain[...], cosines[part, :], sines[part, :], low_half, lead
            )
            band[shifted, lanes] = key.astype(bf16)
        band[shifted, kw : 2 * kw] = side[part, kw : 2 * kw].astype(bf16)
        pooled_rows = pl.ds(pl.multiple_of(i * WINDOW + pool_pad, pool_pad), WINDOW)
        pool_band[pooled_rows, :] = side[part, 2 * kw :].astype(bf16)
        return carry

    lax.fori_loop(0, rows // WINDOW, prepare, 0)

    before, behind = (me + count - 1) % count, (me + 1) % count

    def halo(index, buffer, size, upwards):
        if upwards:
            source, target, device = rows, 0, (behind, tp)
        else:
            source, target, device = size, rows + size, (before, tp)
        return remote(
            buffer.at[pl.ds(source, size), :],
            buffer.at[pl.ds(target, size), :],
            halo_send.at[index],
            halo_recv.at[index],
            device,
        )

    lower = [halo(0, band, WINDOW, False), halo(1, pool_band, pool_pad, False)]
    upper = [halo(2, band, WINDOW, True), halo(3, pool_band, pool_pad, True)]
    has_lower, has_upper = me > 0, me < count - 1

    @pl.when(has_lower)
    def _():
        for copy in lower:
            copy.start()

    @pl.when(has_upper)
    def _():
        for copy in upper:
            copy.start()

    @pl.when(jnp.logical_not(has_lower))
    def _():
        band[0:WINDOW, :] = jnp.zeros((WINDOW, 2 * kw), bf16)
        pool_band[0:pool_pad, :] = jnp.zeros((pool_pad, pw), bf16)

    @pl.when(jnp.logical_not(has_upper))
    def _():
        band[rows + WINDOW :, :] = jnp.zeros((WINDOW, 2 * kw), bf16)
        pool_band[rows + pool_pad :, :] = jnp.zeros((pool_pad, pw), bf16)

    project(query, w_query, [place], first=True)

    def query_step(step, carry):
        events(query_ring, step)
        project(query, w_query, [at(-step), at(step)])
        return carry

    lax.fori_loop(1, half + 1, query_step, 0)
    loads[5].wait()
    loads[6].wait()
    send_own(out_ring)

    @pl.when(has_lower)
    def _():
        for copy in upper:
            copy.wait_recv()

    @pl.when(has_upper)
    def _():
        for copy in lower:
            copy.wait_recv()

    level = tp * pw // (POOL // 4)
    reach = jnp.where(level == 0, 1, jnp.where(level == 1, 2, jnp.where(level == 2, 4, 8)))

    def pool(i, carry):
        wide = WINDOW + 2 * pool_pad
        part = pl.ds(pl.multiple_of(i * WINDOW, WINDOW), WINDOW)
        values = pool_band[pl.ds(pl.multiple_of(i * WINDOW, pool_pad), wide), :].astype(f32)
        total, chosen = values, None
        for step in range(4):
            size = 2**step
            total = total + pltpu.roll(total, wide - size, 0)
            shifted = pltpu.roll(total, size, 0)[pool_pad : pool_pad + WINDOW]
            chosen = shifted if chosen is None else jnp.where(level == step, shifted, chosen)
        spot = me * rows + i * WINDOW + lax.broadcasted_iota(jnp.int32, (WINDOW, 1), 0)
        low = jnp.maximum(spot - reach, 0)
        high = jnp.minimum(spot + reach - 1, seq - 1)
        mixer[part, 0:pw] = (chosen / (high - low + 1).astype(f32)).astype(bf16)
        return carry

    lax.fori_loop(0, rows // WINDOW, pool, 0)

    opposite(query_ring)
    project(query, w_query, [at(count // 2)])

    blocks = rows // WINDOW
    row = lax.broadcasted_iota(jnp.int32, (2 * WINDOW, 3 * WINDOW), 0) % WINDOW
    column = lax.broadcasted_iota(jnp.int32, (2 * WINDOW, 3 * WINDOW), 1)
    top_row = lax.broadcasted_iota(jnp.int32, (2 * WINDOW, 1), 0) < WINDOW

    def attend(i, carry):
        part = pl.ds(pl.multiple_of(i * WINDOW, WINDOW), WINDOW)
        key_rows = pl.ds(pl.multiple_of(i * WINDOW, WINDOW), 3 * WINDOW)
        key_pos = me * rows + i * WINDOW - WINDOW + column
        inside = (column >= row) & (column - row <= 2 * WINDOW) & (key_pos >= 0) & (key_pos < seq)
        for head in range(heads_k):
            lanes = slice(head * 2 * HEAD, (head + 1) * 2 * HEAD)
            rotated = norm_rope(
                query[part, lanes],
                query_gain[...],
                cosines[part, :],
                sines[part, :],
                low_half,
                lead,
            ) * HEAD ** (-0.5)
            other = pltpu.roll(rotated, HEAD, 1)
            if head % 2 == 0:
                pair = (jnp.where(low_half, rotated, 0.0), jnp.where(low_half, other, 0.0))
            else:
                pair = (jnp.where(low_half, 0.0, other), jnp.where(low_half, 0.0, rotated))
            stacked = jnp.concatenate(pair, axis=0).astype(bf16)
            tile = head // 2 * 2 * HEAD
            keys = band[key_rows, tile : tile + 2 * HEAD]
            values = band[key_rows, kw + tile : kw + tile + 2 * HEAD]
            scores = lax.dot_general(
                stacked, keys, (((1,), (1,)), ((), ())), preferred_element_type=f32
            )
            scores = jnp.where(inside, scores, neg_big)
            limit = jnp.where(top_row, sink[2 * head], sink[2 * head + 1])
            top = jnp.maximum(jnp.max(scores, axis=1, keepdims=True), limit)
            raised = jnp.exp(scores - top)
            totals = jnp.sum(raised, axis=1, keepdims=True) + jnp.exp(limit - top)
            weights = (raised * (1.0 / totals)).astype(bf16)
            result = jnp.dot(weights, values, preferred_element_type=f32)
            one, two = result[:WINDOW], result[WINDOW:]
            if head % 2 == 0:
                joined = jnp.where(low_half, one, pltpu.roll(two, HEAD, 1))
            else:
                joined = jnp.where(low_half, pltpu.roll(one, HEAD, 1), two)
            mixer[part, pw + head * 2 * HEAD : pw + (head + 1) * 2 * HEAD] = joined.astype(bf16)

        for c in range(chunks):

            @pl.when(i == ((c + 1) * blocks + chunks - 1) // chunks - 1)
            def _(c=c):
                event(out_ring, 1, c)

        return carry

    lax.fori_loop(0, blocks, attend, 0)

    def product(spot, which):
        left = jnp.concatenate(
            [
                mixer[pl.ds(pl.multiple_of((y * 2 + which) * share, 16), share), :]
                for y in range(chips)
            ],
            axis=0,
        )
        return jnp.dot(left, w_out[spot], preferred_element_type=f32).astype(bf16)

    def met_copy(spot):
        return remote(
            away.at[spot], met.at[spot], met_send.at[spot], met_recv.at[spot], (me, partner)
        )

    def y_copy(spot, hop):
        target = (chip + hop) % chips * 2 + core
        return remote(
            y_send.at[spot, hop - 1],
            y_recv.at[spot, hop - 1],
            yy_send.at[spot, hop - 1],
            yy_recv.at[spot, hop - 1],
            (me, target),
        )

    def done_copy(spot):
        columns = pl.ds(pl.multiple_of(owner_of(spot) * width, width), width)
        return pltpu.make_async_copy(done.at[spot], out.at[:, columns], done_sem.at[spot])

    def both_rows(spot, y):
        part = pl.ds(pl.multiple_of(y * share, 16), share)
        return kept[spot, part, :].astype(f32) + met[spot, part, :].astype(f32)

    def group(spots):
        def first(spot):
            away[spot] = product(spot, 1 - core)
            met_copy(spot).start()

        def second(spot):
            kept[spot] = product(spot, core)

        def third(spot):
            met_copy(spot).wait_recv()
            for hop in range(1, chips):
                y_send[spot, hop - 1] = both_rows(spot, (chip + hop) % chips).astype(bf16)
                y_copy(spot, hop).start()

        for part in (first, second, third):
            for spot in spots:
                part(spot)

    def finish(spot):
        total = both_rows(spot, chip)
        for hop in range(1, chips):
            y_copy(spot, hop).wait_recv()
            total = total + y_recv[spot, hop - 1].astype(f32)
        done[spot] = total.astype(bf16)
        done_copy(spot).start()

    group([place])

    def out_step(step, carry):
        @pl.when(step > 1)
        def _():
            events(out_ring, step)

        group([at(-step), at(step)])

        @pl.when(step == 1)
        def _():
            finish(place)

        @pl.when(step > 1)
        def _():
            finish(at(1 - step))
            finish(at(step - 1))

        return carry

    lax.fori_loop(1, half + 1, out_step, 0)
    opposite(out_ring)
    group([at(count // 2)])
    finish(at(-half))
    finish(at(half))
    finish(at(count // 2))

    for ring in (side_ring, query_ring, out_ring):
        sends_done(ring)

    def tokens_sent(j, carry):
        token_near(0, tp, j).wait_send()
        for hop in range(1, chips):
            token_far(hop, tp, j).wait_send()
            token_near(hop, (chip - hop + chips) % chips * 2 + core, j).wait_send()
        return carry

    lax.fori_loop(0, token_chunks, tokens_sent, 0)

    @pl.when(has_lower)
    def _():
        for copy in lower:
            copy.wait_send()

    @pl.when(has_upper)
    def _():
        for copy in upper:
            copy.wait_send()

    def blocks_sent(spot, carry):
        met_copy(spot).wait_send()
        for hop in range(1, chips):
            y_copy(spot, hop).wait_send()
        done_copy(spot).wait()
        return carry

    lax.fori_loop(0, count, blocks_sent, 0)


def plane_kernel(
    count,
    members,
    tokens,
    wq,
    wk,
    wv,
    wp,
    wop,
    woa,
    norm_gain,
    query_gain,
    key_gain,
    row_cos,
    row_sin,
    col_cos,
    col_sin,
    sink,
    out,
    raw,
    sums,
    normed,
    w_in,
    w_pool,
    w_out,
    in_spare,
    pool_spare,
    out_spare,
    total,
    pool_total,
    band,
    pool_band,
    cosines,
    sines,
    mixer,
    away,
    met,
    kept,
    one_send,
    one_recv,
    two_send,
    two_recv,
    done,
    load_sem,
    sum_send,
    sum_recv,
    in_sems,
    pool_sems,
    out_sems,
    x_sems,
    tx_send,
    tx_recv,
    ty_send,
    ty_recv,
    td_send,
    td_recv,
    halo_send,
    halo_recv,
    met_send,
    met_recv,
    hop_send,
    hop_recv,
    done_sem,
):
    rows, features = tokens.shape
    depth = wk.shape[0]
    hk, hq, hp = wk.shape[1] // 2, wq.shape[1] // 2, wp.shape[1] // 2
    width = wop.shape[1]
    narrow = width // out_parts
    share = rows // members
    plane = 2 * rows
    heads_k = hk // HEAD
    seq = count * rows
    deep = count // 2
    pieces = features // depth
    tiles = rows // WINDOW

    me, tp = lax.axis_index("sp"), lax.axis_index("tp")
    z, x = me // 2, me % 2
    y, core = tp // 2, tp % 2
    me_x, tp_y, tp_c = me + 1 - 2 * x, (1 - y) * 2 + core, y * 2 + 1 - core
    tp_yc = (1 - y) * 2 + 1 - core
    up, down = (me + 2) % count, (me + count - 2) % count
    has_up, has_down = z < deep - 1, z > 0
    inner = has_up & has_down

    mine = lambda size: pl.ds(pl.multiple_of(x * size, 128), size)
    other = lambda size: pl.ds(pl.multiple_of((1 - x) * size, 128), size)
    loads = []

    def load(source, target):
        loads.append(pltpu.make_async_copy(source, target, load_sem.at[len(loads)]))
        loads[-1].start()

    for target, pick in ((w_in.at[me], mine), (in_spare, other)):
        load(wk.at[:, pick(hk)], target.at[:, pl.ds(0, hk)])
        load(wv.at[:, pick(hk)], target.at[:, pl.ds(hk, hk)])
        load(wq.at[:, pick(hq)], target.at[:, pl.ds(2 * hk, hq)])
    load(tokens, raw)
    for target, pick in ((w_pool.at[me], mine), (pool_spare, other)):
        load(wp.at[:, pick(hp)], target)
    for target, pick in ((w_out.at[me], mine), (out_spare, other)):
        for part in range(out_parts):
            columns = pl.ds(part * narrow, narrow)
            load(wop.at[pick(hp), columns], target.at[part, pl.ds(0, hp), :])
            load(woa.at[pick(hq), columns], target.at[part, pl.ds(hp, hq), :])

    barrier = pltpu.get_barrier_semaphore()
    greeted = [(up, tp), (down, tp), (me_x, tp), (me, tp_y), (me, tp_c), (me, tp_yc)]
    for device in greeted:
        pl.semaphore_signal(barrier, inc=1, device_id=device, device_id_type=MESH)
    pl.semaphore_wait(barrier, len(greeted))

    def remote(source, target, send_sem, recv_sem, device):
        return pltpu.make_async_remote_copy(
            src_ref=source,
            dst_ref=target,
            send_sem=send_sem,
            recv_sem=recv_sem,
            device_id=device,
            device_id_type=MESH,
        )

    def by_rows(parts):
        def view(buffer, c):
            size = buffer.shape[0] // parts
            return buffer.at[pl.ds(pl.multiple_of(c * size, 16), size), :]

        return view

    in_ring = (w_in, in_spare, in_sems, 0, in_parts, by_rows(in_parts), True)
    pool_ring = (w_pool, pool_spare, pool_sems, in_parts, 1, by_rows(1), False)
    out_ring = (
        w_out,
        out_spare,
        out_sems,
        in_parts + 1,
        out_parts,
        lambda buffer, c: buffer.at[c],
        False,
    )

    def z_copy(ring, way, source, c):
        buffer, _, sems, _, _, view, _ = ring
        part = view(buffer.at[source], c)
        return remote(
            part, part, sems.at[way, source, c], sems.at[2, source, c], ((up, down)[way], tp)
        )

    def x_copy(ring, source, c):
        buffer, spare, sems, first, _, view, _ = ring
        return remote(
            view(spare, c),
            view(buffer.at[source], c),
            x_sems.at[first + c],
            sems.at[2, source, c],
            (me_x, tp),
        )

    def both_ways(ring, source, c, act):
        @pl.when(has_up)
        def _():
            act(z_copy(ring, 0, source, c))

        @pl.when(has_down)
        def _():
            act(z_copy(ring, 1, source, c))

    start = lambda copy: copy.start()
    sent = lambda copy: copy.wait_send()

    def own_out(ring):
        for c in range(ring[4]):
            both_ways(ring, me, c, start)

    def side_out(ring):
        for c in range(ring[4]):
            x_copy(ring, me, c).start()

    def side_in(ring):
        for c in range(ring[4]):
            x_copy(ring, me_x, c).wait_recv()
            both_ways(ring, me_x, c, start)

    def passing(ring, n):
        parts = ring[4]
        step, j, c = n // (2 * parts) + 1, n // parts % 2, n % parts
        column = (x + j) % 2 if ring[6] else j
        low, high = z - step, z + step
        return (low >= 0, low * 2 + column), (high < deep, high * 2 + column), c

    def event(ring, n):
        (is_low, low), (is_high, high), c = passing(ring, n)

        @pl.when(is_low)
        def _():
            z_copy(ring, 0, low, c).wait_recv()

            @pl.when(has_up)
            def _():
                z_copy(ring, 0, low, c).start()

        @pl.when(is_high)
        def _():
            z_copy(ring, 1, high, c).wait_recv()

            @pl.when(has_down)
            def _():
                z_copy(ring, 1, high, c).start()

    def events(ring, first, last):
        def body(n, carry):
            event(ring, n)
            return carry

        lax.fori_loop(first, last, body, 0)

    def all_events(ring):
        return (deep - 1) * 2 * ring[4]

    def sends_done(ring):
        for c in range(ring[4]):
            both_ways(ring, me, c, sent)
            both_ways(ring, me_x, c, sent)
            x_copy(ring, me, c).wait_send()

        def body(n, carry):
            (is_low, low), (is_high, high), c = passing(ring, n)

            @pl.when(is_low & has_up)
            def _():
                z_copy(ring, 0, low, c).wait_send()

            @pl.when(is_high & has_down)
            def _():
                z_copy(ring, 1, high, c).wait_send()

            return carry

        lax.fori_loop(0, all_events(ring), body, 0)

    for copy in loads[:6]:
        copy.wait()
    for c in range(in_parts):
        x_copy(in_ring, me, c).start()
        both_ways(in_ring, me, c, start)

    loads[6].wait()
    sums[tp] = jnp.zeros_like(sums[tp])
    for i in range(tiles):
        block = raw[i * WINDOW : (i + 1) * WINDOW, :].astype(f32)
        square = jnp.sum(block * block, axis=1, keepdims=True)
        turned = jnp.transpose(jnp.broadcast_to(square, (WINDOW, WINDOW)))
        sums[tp, i : i + 1, :] = turned[0:1, :]

    def sum_copy(owner, hop):
        target = (tp + hop) % members
        return remote(
            sums.at[owner],
            sums.at[owner],
            sum_send.at[hop - 1],
            sum_recv.at[hop - 1],
            (me, target),
        )

    for hop in range(1, members):
        sum_copy(tp, hop).start()
    for g in range(plane // GRID_W):
        spot = pl.ds(z * (plane // GRID_W) + g, 1)
        grid_rows = pl.ds(g * GRID_W, GRID_W)
        cosines[grid_rows, :] = col_cos[...] + row_cos[spot, :]
        sines[grid_rows, :] = col_sin[...] + row_sin[spot, :]
    for hop in range(1, members):
        sum_copy((tp - hop + members) % members, hop).wait_recv()
    squares = sums[0]
    for t in range(1, members):
        squares = squares + sums[t]
    scales = lax.rsqrt(squares / (members * features) + eps)

    def token_part(side, owner, j):
        return normed.at[
            side,
            pl.ds(owner * pieces, pieces),
            pl.ds(pl.multiple_of(j * WINDOW, WINDOW), WINDOW),
            :,
        ]

    def over_x(slot, side, owner, j):
        part = token_part(side, owner, j)
        return remote(part, part, tx_send.at[slot, j], tx_recv.at[slot, j], (me_x, tp))

    def over_y(slot, side, owner, j):
        part = token_part(side, owner, j)
        return remote(part, part, ty_send.at[slot, j], ty_recv.at[slot, j], (me, tp_y))

    def over_core(slot, side, owner, j):
        part = token_part(side, owner, j)
        return remote(part, part, td_send.at[slot, j], td_recv.at[slot, j], (me, tp_c))

    gains = norm_gain[pl.ds(tp, 1), :]
    for i in range(tiles):
        here = slice(i * WINDOW, (i + 1) * WINDOW)
        scale = jnp.transpose(jnp.broadcast_to(scales[i : i + 1, :], (WINDOW, WINDOW)))
        for first in range(0, features, WINDOW):
            block = raw[here, first : first + WINDOW].astype(f32)
            value = (block * scale * gains[:, first : first + WINDOW]).astype(bf16)
            inside = first % depth
            normed[x, tp * pieces + first // depth, here, inside : inside + WINDOW] = value
        over_y(0, x, tp, i).start()
        over_x(0, x, tp, i).start()
        over_core(0, x, tp, i).start()

    side_in(in_ring)
    whole = all_events(in_ring)
    reached = lambda part: whole * part // 24
    events(in_ring, 0, reached(4))

    def by_x(j):
        return j % 3 == 0

    def direct(j, carry):
        over_y(0, x, tp_y, j).wait_recv()
        over_core(2, x, tp_y, j).start()

        @pl.when(by_x(j))
        def _():
            over_x(1, x, tp_y, j).start()

        over_x(0, 1 - x, tp, j).wait_recv()
        over_core(1, 1 - x, tp, j).start()

        @pl.when(jnp.logical_not(by_x(j)))
        def _():
            over_y(1, 1 - x, tp, j).start()

        events(in_ring, reached(4 + 12 * j // tiles), reached(4 + 12 * (j + 1) // tiles))
        return carry

    lax.fori_loop(0, tiles, direct, 0)
    for copy in loads[7:]:
        copy.wait()
    side_out(pool_ring)
    side_out(out_ring)

    def crossed(j, carry):
        @pl.when(by_x(j))
        def _():
            over_x(1, 1 - x, tp_y, j).wait_recv()

        @pl.when(jnp.logical_not(by_x(j)))
        def _():
            over_y(1, 1 - x, tp_y, j).wait_recv()

        over_core(3, 1 - x, tp_y, j).start()
        events(in_ring, reached(16 + 6 * j // tiles), reached(16 + 6 * (j + 1) // tiles))
        return carry

    lax.fori_loop(0, tiles, crossed, 0)
    own_out(pool_ring)

    def from_core(j, carry):
        over_core(0, x, tp_c, j).wait_recv()
        over_core(1, 1 - x, tp_c, j).wait_recv()
        over_core(2, x, tp_yc, j).wait_recv()
        over_core(3, 1 - x, tp_yc, j).wait_recv()
        return carry

    lax.fori_loop(0, tiles, from_core, 0)

    tile_rows = 256 if rows % 256 == 0 else 128
    per_side = rows // tile_rows

    def project(result, weights, level, first=False):
        def body(i, carry):
            part = pl.ds(pl.multiple_of(i * tile_rows, tile_rows), tile_rows)
            within = pl.ds(pl.multiple_of(i % per_side * tile_rows, tile_rows), tile_rows)
            value = None if first else result[part, :]
            for j in range(2):
                term = jnp.dot(
                    normed[i // per_side, level * 2 + j, within, :],
                    weights[level * 2 + j],
                    preferred_element_type=f32,
                )
                value = term if value is None else value + term
            result[part, :] = value
            return carry

        lax.fori_loop(0, 2 * per_side, body, 0)

    def project_step(result, weights, step):
        @pl.when(z - step >= 0)
        def _():
            project(result, weights, z - step)

        @pl.when(z + step < deep)
        def _():
            project(result, weights, z + step)

    project(total, w_in, z, first=True)

    def in_step(step, carry):
        each = 2 * in_parts
        events(in_ring, jnp.maximum((step - 1) * each, reached(22)), step * each)
        project_step(total, w_in, step)
        return carry

    lax.fori_loop(1, deep, in_step, 0)

    lane = lax.broadcasted_iota(jnp.int32, (WINDOW, 2 * HEAD), 1)
    low_half = lane < HEAD
    lead = lane % (HEAD // 2) < HEAD // 4
    blocks = plane // WINDOW

    def prepare(i, carry):
        part = pl.ds(pl.multiple_of(i * WINDOW, WINDOW), WINDOW)
        shifted = pl.ds(pl.multiple_of((i + 1) * WINDOW, WINDOW), WINDOW)
        for h in range(hk // (2 * HEAD)):
            lanes = slice(h * 2 * HEAD, (h + 1) * 2 * HEAD)
            key = norm_rope(
                total[part, lanes], key_gain[...], cosines[part, :], sines[part, :], low_half, lead
            )
            band[shifted, lanes] = key.astype(bf16)
        band[shifted, hk:] = total[part, hk : 2 * hk].astype(bf16)
        return carry

    lax.fori_loop(0, blocks, prepare, 0)

    def halo(index, buffer, size, upwards):
        if upwards:
            source, target, device = plane, 0, (up, tp)
        else:
            source, target, device = size, plane + size, (down, tp)
        return remote(
            buffer.at[pl.ds(source, size), :],
            buffer.at[pl.ds(target, size), :],
            halo_send.at[index],
            halo_recv.at[index],
            device,
        )

    def halo_out(index, buffer, size):
        @pl.when(has_down)
        def _():
            halo(index, buffer, size, False).start()

        @pl.when(has_up)
        def _():
            halo(index + 1, buffer, size, True).start()

        empty = jnp.zeros((size, buffer.shape[1]), bf16)

        @pl.when(jnp.logical_not(has_down))
        def _():
            buffer[0:size, :] = empty

        @pl.when(jnp.logical_not(has_up))
        def _():
            buffer[plane + size :, :] = empty

    def halo_in(index, buffer, size):
        @pl.when(has_up)
        def _():
            halo(index, buffer, size, False).wait_recv()

        @pl.when(has_down)
        def _():
            halo(index + 1, buffer, size, True).wait_recv()

    halo_out(0, band, WINDOW)

    def pool_stage():
        side_in(pool_ring)
        project(pool_total, w_pool, z, first=True)

        def step_body(step, carry):
            events(pool_ring, (step - 1) * 2, step * 2)
            project_step(pool_total, w_pool, step)
            return carry

        lax.fori_loop(1, deep, step_body, 0)
        pool_band[pool_pad : pool_pad + plane, :] = pool_total[...].astype(bf16)
        halo_out(2, pool_band, pool_pad)

    @pl.when(inner)
    def _():
        pool_stage()

    own_out(out_ring)
    side_in(out_ring)

    row = lax.broadcasted_iota(jnp.int32, (2 * WINDOW, 3 * WINDOW), 0) % WINDOW
    column = lax.broadcasted_iota(jnp.int32, (2 * WINDOW, 3 * WINDOW), 1)
    top_row = lax.broadcasted_iota(jnp.int32, (2 * WINDOW, 1), 0) < WINDOW

    def attend(turn, carry):
        @pl.when(turn == blocks - 2)
        def _():
            halo_in(0, band, WINDOW)

        i = (turn + 1) % blocks
        part = pl.ds(pl.multiple_of(i * WINDOW, WINDOW), WINDOW)
        key_rows = pl.ds(pl.multiple_of(i * WINDOW, WINDOW), 3 * WINDOW)
        key_pos = z * plane + i * WINDOW - WINDOW + column
        inside = (column >= row) & (column - row <= 2 * WINDOW) & (key_pos >= 0) & (key_pos < seq)
        for head in range(heads_k):
            lanes = slice(2 * hk + head * 2 * HEAD, 2 * hk + (head + 1) * 2 * HEAD)
            rotated = norm_rope(
                total[part, lanes],
                query_gain[...],
                cosines[part, :],
                sines[part, :],
                low_half,
                lead,
            ) * HEAD ** (-0.5)
            swapped = pltpu.roll(rotated, HEAD, 1)
            if head % 2 == 0:
                pair = (jnp.where(low_half, rotated, 0.0), jnp.where(low_half, swapped, 0.0))
            else:
                pair = (jnp.where(low_half, 0.0, swapped), jnp.where(low_half, 0.0, rotated))
            stacked = jnp.concatenate(pair, axis=0).astype(bf16)
            tile = head // 2 * 2 * HEAD
            keys = band[key_rows, tile : tile + 2 * HEAD]
            values = band[key_rows, hk + tile : hk + tile + 2 * HEAD]
            scores = lax.dot_general(
                stacked, keys, (((1,), (1,)), ((), ())), preferred_element_type=f32
            )
            scores = jnp.where(inside, scores, neg_big)
            first = x * 2 * heads_k + 2 * head
            limit = jnp.where(top_row, sink[first], sink[first + 1])
            top = jnp.maximum(jnp.max(scores, axis=1, keepdims=True), limit)
            raised = jnp.exp(scores - top)
            totals = jnp.sum(raised, axis=1, keepdims=True) + jnp.exp(limit - top)
            weights = (raised * (1.0 / totals)).astype(bf16)
            result = jnp.dot(weights, values, preferred_element_type=f32)
            one, two = result[:WINDOW], result[WINDOW:]
            if head % 2 == 0:
                joined = jnp.where(low_half, one, pltpu.roll(two, HEAD, 1))
            else:
                joined = jnp.where(low_half, pltpu.roll(one, HEAD, 1), two)
            mixer[part, hp + head * 2 * HEAD : hp + (head + 1) * 2 * HEAD] = joined.astype(bf16)
        return carry

    lax.fori_loop(0, blocks, attend, 0)

    @pl.when(jnp.logical_not(inner))
    def _():
        pool_stage()

    halo_in(2, pool_band, pool_pad)
    level = (tp * 2 + x) * hp // (POOL // 4)
    reach = jnp.where(level == 0, 1, jnp.where(level == 1, 2, jnp.where(level == 2, 4, 8)))

    def pool(i, carry):
        wide = WINDOW + 2 * pool_pad
        part = pl.ds(pl.multiple_of(i * WINDOW, WINDOW), WINDOW)
        running = pool_band[pl.ds(pl.multiple_of(i * WINDOW, pool_pad), wide), :].astype(f32)
        chosen = None
        for step in range(4):
            size = 2**step
            running = running + pltpu.roll(running, wide - size, 0)
            shifted = pltpu.roll(running, size, 0)[pool_pad : pool_pad + WINDOW]
            chosen = shifted if chosen is None else jnp.where(level == step, shifted, chosen)
        spot = z * plane + i * WINDOW + lax.broadcasted_iota(jnp.int32, (WINDOW, 1), 0)
        low = jnp.maximum(spot - reach, 0)
        high = jnp.minimum(spot + reach - 1, seq - 1)
        mixer[part, 0:hp] = (chosen / (high - low + 1).astype(f32)).astype(bf16)
        return carry

    lax.fori_loop(0, blocks, pool, 0)

    def source_of(b):
        group = b // 2
        paired = jnp.minimum(z, deep - 1 - z)
        step = jnp.where(group > 2 * paired, group - paired, (group + 1) // 2)
        downwards = jnp.where(group > 2 * paired, 2 * z > deep - 1, group % 2 == 1)
        return jnp.where(downwards, z - step, z + step) * 2 + b % 2

    slots = kept.shape[0]

    def product(source, c, which):
        left = jnp.concatenate(
            [
                mixer[pl.ds(pl.multiple_of((unit * 2 + which) * share, 16), share), :]
                for unit in range(4)
            ],
            axis=0,
        )
        return jnp.dot(left, w_out[source, c], preferred_element_type=f32).astype(bf16)

    def met_copy(b, c):
        return remote(
            away.at[b % slots, c], met.at[b, c], met_send.at[b, c], met_recv.at[b, c], (me, tp_c)
        )

    def axes(c):
        return (x, y) if c % 2 == 0 else (y, x)

    def unit_rows(c, first, second):
        unit = first * 2 + second if c % 2 == 0 else second * 2 + first
        return pl.ds(pl.multiple_of(unit * share, 16), share)

    def hop_copy(b, c, hop):
        over = (c + hop) % 2 == 0
        device = (me_x, tp) if over else (me, tp_y)
        send, recv = (one_send, one_recv) if hop == 0 else (two_send, two_recv)
        return remote(
            send.at[b, c], recv.at[b, c], hop_send.at[hop, b, c], hop_recv.at[hop, b, c], device
        )

    def chip_sum(b, c, first, second):
        part = unit_rows(c, first, second)
        return kept[b % slots, c, part, :].astype(f32) + met[b, c, part, :].astype(f32)

    def columns_of(b, c):
        first = source_of(b) * width + c * narrow
        return pl.ds(pl.multiple_of(first, narrow), narrow)

    def done_copy(b, c):
        return pltpu.make_async_copy(done.at[b, c], out.at[:, columns_of(b, c)], done_sem.at[b, c])

    def multiply(b):
        source = source_of(b)

        @pl.when(b >= slots)
        def _():
            for c in range(out_parts):
                met_copy(b - slots, c).wait_send()

        for c in range(out_parts):
            away[b % slots, c] = product(source, c, 1 - core)
            met_copy(b, c).start()
        for c in range(out_parts):
            kept[b % slots, c] = product(source, c, core)

    def first_hop(b):
        for c in range(out_parts):
            met_copy(b, c).wait_recv()
            first, _ = axes(c)
            for second in range(2):
                one_send[b, c, second] = chip_sum(b, c, 1 - first, second).astype(bf16)
            hop_copy(b, c, 0).start()

    def second_hop(b):
        for c in range(out_parts):
            hop_copy(b, c, 0).wait_recv()
            first, second = axes(c)
            value = chip_sum(b, c, first, 1 - second) + one_recv[b, c, 1 - second].astype(f32)
            two_send[b, c] = value.astype(bf16)
            hop_copy(b, c, 1).start()

    def finish(b):
        for c in range(out_parts):
            first, second = axes(c)
            value = chip_sum(b, c, first, second) + one_recv[b, c, second].astype(f32)
            hop_copy(b, c, 1).wait_recv()
            done[b, c] = (value + two_recv[b, c].astype(f32)).astype(bf16)
            done_copy(b, c).start()

    ahead = jnp.where(inner, 0, 2 * out_parts)

    def out_block(b, carry):
        @pl.when(b < count)
        def _():
            low = jnp.maximum(b * out_parts - ahead, 0)
            high = jnp.minimum((b + 1) * out_parts - ahead, all_events(out_ring))
            events(out_ring, low, high)
            multiply(b)
            first_hop(b)

        @pl.when((b >= 1) & (b < count + 1))
        def _():
            second_hop(b - 1)

        @pl.when(b >= 2)
        def _():
            finish(b - 2)

        return carry

    lax.fori_loop(0, count + 2, out_block, 0)

    for ring in (in_ring, pool_ring, out_ring):
        sends_done(ring)
    for hop in range(1, members):
        sum_copy(tp, hop).wait_send()

    def tokens_sent(j, carry):
        over_y(0, x, tp, j).wait_send()
        over_x(0, x, tp, j).wait_send()
        over_core(0, x, tp, j).wait_send()
        over_core(1, 1 - x, tp, j).wait_send()
        over_core(2, x, tp_y, j).wait_send()
        over_core(3, 1 - x, tp_y, j).wait_send()

        @pl.when(by_x(j))
        def _():
            over_x(1, x, tp_y, j).wait_send()

        @pl.when(jnp.logical_not(by_x(j)))
        def _():
            over_y(1, 1 - x, tp, j).wait_send()

        return carry

    lax.fori_loop(0, tiles, tokens_sent, 0)
    for index, buffer, size in ((0, band, WINDOW), (2, pool_band, pool_pad)):

        @pl.when(has_down)
        def _(index=index, buffer=buffer, size=size):
            halo(index, buffer, size, False).wait_send()

        @pl.when(has_up)
        def _(index=index, buffer=buffer, size=size):
            halo(index + 1, buffer, size, True).wait_send()

    def blocks_sent(b, carry):
        for c in range(out_parts):

            @pl.when(b >= count - slots)
            def _(c=c):
                met_copy(b, c).wait_send()

            hop_copy(b, c, 0).wait_send()
            hop_copy(b, c, 1).wait_send()
            done_copy(b, c).wait()
        return carry

    lax.fori_loop(0, count, blocks_sent, 0)


def plane_scratch(count, members, rows, features, depth, kw, qw, pw, width):
    hk, hq, hp = kw // 2, qw // 2, pw // 2
    share, narrow, plane, slots = rows // members, width // out_parts, 2 * rows, 4
    tiles = rows // WINDOW
    dma = pltpu.SemaphoreType.DMA
    return [
        pltpu.VMEM((rows, features), bf16),
        pltpu.VMEM((members, -(-tiles // 8) * 8, WINDOW), f32),
        pltpu.VMEM((2, count, rows, depth), bf16),
        pltpu.VMEM((count, depth, 2 * hk + hq), bf16),
        pltpu.VMEM((count, depth, hp), bf16),
        pltpu.VMEM((count, out_parts, hp + hq, narrow), bf16),
        pltpu.VMEM((depth, 2 * hk + hq), bf16),
        pltpu.VMEM((depth, hp), bf16),
        pltpu.VMEM((out_parts, hp + hq, narrow), bf16),
        pltpu.VMEM((plane, 2 * hk + hq), f32),
        pltpu.VMEM((plane, hp), f32),
        pltpu.VMEM((plane + 2 * WINDOW, 2 * hk), bf16),
        pltpu.VMEM((plane + 2 * pool_pad, hp), bf16),
        pltpu.VMEM((plane, 2 * HEAD), f32),
        pltpu.VMEM((plane, 2 * HEAD), f32),
        pltpu.VMEM((plane, hp + hq), bf16),
        pltpu.VMEM((slots, out_parts, 4 * share, narrow), bf16),
        pltpu.VMEM((count, out_parts, 4 * share, narrow), bf16),
        pltpu.VMEM((slots, out_parts, 4 * share, narrow), bf16),
        pltpu.VMEM((count, out_parts, 2, share, narrow), bf16),
        pltpu.VMEM((count, out_parts, 2, share, narrow), bf16),
        pltpu.VMEM((count, out_parts, share, narrow), bf16),
        pltpu.VMEM((count, out_parts, share, narrow), bf16),
        pltpu.VMEM((count, out_parts, share, narrow), bf16),
        dma((9 + 4 * out_parts,)),
        dma((members - 1,)),
        dma((members - 1,)),
        dma((3, count, in_parts)),
        dma((3, count, 1)),
        dma((3, count, out_parts)),
        dma((in_parts + 1 + out_parts,)),
        dma((2, tiles)),
        dma((2, tiles)),
        dma((2, tiles)),
        dma((2, tiles)),
        dma((4, tiles)),
        dma((4, tiles)),
        dma((4,)),
        dma((4,)),
        dma((count, out_parts)),
        dma((count, out_parts)),
        dma((2, count, out_parts)),
        dma((2, count, out_parts)),
        dma((count, out_parts)),
    ]


def ring_scratch(count, members, rows, features, depth, kw, qw, pw, width):
    chips, share = members // 2, rows // members
    far = max(chips - 1, 1)
    dma = pltpu.SemaphoreType.DMA
    return [
        pltpu.VMEM((members, rows, features), bf16),
        pltpu.VMEM((count, rows, depth), bf16),
        pltpu.VMEM((count, depth, 2 * kw + pw), bf16),
        pltpu.VMEM((count, depth, qw), bf16),
        pltpu.VMEM((count, pw + qw, width), bf16),
        pltpu.VMEM((rows, 2 * kw + pw), f32),
        pltpu.VMEM((rows, qw), f32),
        pltpu.VMEM((rows + 2 * WINDOW, 2 * kw), bf16),
        pltpu.VMEM((rows + 2 * pool_pad, pw), bf16),
        pltpu.VMEM((rows, 2 * HEAD), f32),
        pltpu.VMEM((rows, 2 * HEAD), f32),
        pltpu.VMEM((rows, pw + qw), bf16),
        pltpu.VMEM((count, chips * share, width), bf16),
        pltpu.VMEM((count, chips * share, width), bf16),
        pltpu.VMEM((count, chips * share, width), bf16),
        pltpu.VMEM((count, far, share, width), bf16),
        pltpu.VMEM((count, far, share, width), bf16),
        pltpu.VMEM((count, share, width), bf16),
        dma((7,)),
        dma((2, count, chunks)),
        dma((count, chunks)),
        dma((2, count, chunks)),
        dma((count, chunks)),
        dma((2, count, chunks)),
        dma((count, chunks)),
        dma((far, token_chunks)),
        dma((far, token_chunks)),
        dma((chips, token_chunks)),
        dma((chips, token_chunks)),
        dma((4,)),
        dma((4,)),
        dma((count,)),
        dma((count,)),
        dma((count, far)),
        dma((count, far)),
        dma((count,)),
    ]


def shards(
    tokens,
    norm_gain,
    w_query,
    w_key,
    w_value,
    w_pool,
    query_gain,
    key_gain,
    sink_logit,
    w_out_pool,
    w_out_attn,
):
    count, members = lax.axis_size("sp"), lax.axis_size("tp")
    rows, features = tokens.shape
    depth, kw = w_key.shape
    qw, pw, width = w_query.shape[1], w_pool.shape[1], w_out_pool.shape[1]
    tables = [jnp.asarray(table) for table in rope_parts(count * rows)]
    twice = lambda gain: jnp.concatenate([gain, gain]).reshape(1, 2 * HEAD)
    anywhere = pl.BlockSpec(memory_space=pl.ANY)
    in_vmem = pl.BlockSpec(memory_space=pltpu.VMEM)
    sizes = (count, members, rows, features, depth, kw, qw, pw, width)
    shared = (
        members == 4
        and count % 2 == 0
        and count >= 4
        and rows % (2 * WINDOW) == 0
        and depth % (16 * in_parts) == 0
        and all(size % 256 == 0 for size in (kw, qw, pw, width))
    )
    kernel, scratch = (plane_kernel, plane_scratch) if shared else (layer_kernel, ring_scratch)
    return pl.pallas_call(
        functools.partial(kernel, count, members),
        out_shape=jax.ShapeDtypeStruct((rows // members, count * width), bf16),
        in_specs=[anywhere] * 7 + [in_vmem] * 7 + [pl.BlockSpec(memory_space=pltpu.SMEM)],
        out_specs=anywhere,
        scratch_shapes=scratch(*sizes),
        compiler_params=pltpu.CompilerParams(
            collective_id=0, has_side_effects=True, vmem_limit_bytes=62 * 1024 * 1024
        ),
    )(
        tokens,
        w_query,
        w_key,
        w_value,
        w_pool,
        w_out_pool,
        w_out_attn,
        norm_gain.reshape(members, -1) if shared else norm_gain.reshape(1, -1),
        twice(query_gain),
        twice(key_gain),
        *tables,
        sink_logit,
    )


def solution(mesh):
    placed = (
        P("sp", "tp"),
        P(),
        P("sp", "tp"),
        P("sp", "tp"),
        P("sp", "tp"),
        P("sp", "tp"),
        P(),
        P(),
        P("tp"),
        P("tp", "sp"),
        P("tp", "sp"),
    )
    return jax.shard_map(
        shards, mesh=mesh, in_specs=placed, out_specs=P(("sp", "tp"), None), check_vma=False
    )
```

```python
import functools

import jax
import jax.numpy as jnp
import numpy as np
from jax import lax
from jax.experimental import pallas as pl
from jax.experimental.pallas import tpu as pltpu
from jax.sharding import PartitionSpec as P

HEAD = 64
POOL = 1024
WINDOW = 128
GRID_W = 64

eps = 1e-06
rope_base = 10000.0
neg_big = -1e30
pool_pad = 16
chunks = 4
token_chunks = 8
in_parts = 4
pooled_parts = 4
MESH = pl.DeviceIdType.MESH
f32, bf16 = jnp.float32, jnp.bfloat16


def rope_parts(rows_total):
    quarter = HEAD // 4
    steps = np.arange(quarter, dtype=np.float32) * np.float32(2.0) / np.float32(HEAD // 2)
    freqs = (np.float32(1.0) / np.float32(rope_base) ** steps).astype(np.float32)

    def table(count, first):
        angle = np.arange(count, dtype=np.float32)[:, None] * freqs
        twice = np.concatenate([angle, angle], axis=1).astype(np.float64)
        none = np.zeros_like(twice)
        made = []
        for part in (np.cos(twice), np.sin(twice)):
            head = [part, none] if first else [none, part]
            made.append(np.concatenate(head + head, axis=1).astype(np.float32))
        return made

    return table(rows_total // GRID_W, True) + table(GRID_W, False)


def ring_place(index, count, across):
    deep = count // across
    if across == 1 or deep % 2:
        return index
    z, x = index // across, index % across
    turn = deep - 1 - z
    inner = jnp.where(turn % 2 == 0, x - 1, across - 1 - x)
    return jnp.where(x == 0, z, deep + turn * (across - 1) + inner)


def ring_index(place, count, across):
    deep = count // across
    if across == 1 or deep % 2:
        return place
    rest = jnp.maximum(place - deep, 0)
    turn, inner = rest // (across - 1), rest % (across - 1)
    x = jnp.where(turn % 2 == 0, inner + 1, across - 1 - inner)
    return jnp.where(place < deep, place * across, (deep - 1 - turn) * across + x)


def norm_rope(raw, gain, cosine, sine, low_half, lead):
    squares = raw * raw
    low_sum = jnp.sum(jnp.where(low_half, squares, 0.0), axis=1, keepdims=True)
    high_sum = jnp.sum(jnp.where(low_half, 0.0, squares), axis=1, keepdims=True)
    mean = jnp.where(low_half, low_sum, high_sum) * (1.0 / HEAD)
    scaled = raw * lax.rsqrt(mean + eps) * gain
    turned = jnp.where(
        lead,
        -pltpu.roll(scaled, 2 * HEAD - HEAD // 4, 1),
        pltpu.roll(scaled, HEAD // 4, 1),
    )
    return scaled * cosine + turned * sine


def layer_kernel(
    count,
    members,
    tokens,
    wq,
    wk,
    wv,
    wp,
    wop,
    woa,
    norm_gain,
    query_gain,
    key_gain,
    row_cos,
    row_sin,
    col_cos,
    col_sin,
    sink,
    out,
    tok,
    normed,
    w_side,
    w_query,
    w_out,
    side,
    query,
    band,
    pool_band,
    cosines,
    sines,
    mixer,
    away,
    met,
    kept,
    y_send,
    y_recv,
    done,
    load_sem,
    side_send,
    side_recv,
    query_send,
    query_recv,
    out_send,
    out_recv,
    ty_send,
    ty_recv,
    td_send,
    td_recv,
    halo_send,
    halo_recv,
    met_send,
    met_recv,
    yy_send,
    yy_recv,
    done_sem,
):
    rows, features = tokens.shape
    depth, kw = wk.shape
    qw, pw, width = wq.shape[1], wp.shape[1], wop.shape[1]
    chips = members // 2
    share = rows // members
    half = (count - 1) // 2
    heads_k = kw // HEAD
    seq = count * rows
    across = chips

    me, tp = lax.axis_index("sp"), lax.axis_index("tp")
    chip, core = tp // 2, tp % 2
    partner = chip * 2 + 1 - core
    place = ring_place(me, count, across)
    owner_of = lambda spot: ring_index(spot, count, across)
    at = lambda offset: (place + offset + count) % count
    following, previous = owner_of(at(1)), owner_of(at(-1))

    loads = [
        pltpu.make_async_copy(wk, w_side.at[place, :, pl.ds(0, kw)], load_sem.at[0]),
        pltpu.make_async_copy(wv, w_side.at[place, :, pl.ds(kw, kw)], load_sem.at[1]),
        pltpu.make_async_copy(wp, w_side.at[place, :, pl.ds(2 * kw, pw)], load_sem.at[2]),
        pltpu.make_async_copy(tokens, tok.at[tp], load_sem.at[3]),
        pltpu.make_async_copy(wq, w_query.at[place], load_sem.at[4]),
        pltpu.make_async_copy(wop, w_out.at[place, pl.ds(0, pw), :], load_sem.at[5]),
        pltpu.make_async_copy(woa, w_out.at[place, pl.ds(pw, qw), :], load_sem.at[6]),
    ]
    for load in loads:
        load.start()

    barrier = pltpu.get_barrier_semaphore()
    greeted = [
        (following, tp),
        (previous, tp),
        (me, partner),
        ((me + 1) % count, tp),
        ((me + count - 1) % count, tp),
    ]
    greeted += [(me, (chip + hop) % chips * 2 + core) for hop in range(1, chips)]
    for device in greeted:
        pl.semaphore_signal(barrier, inc=1, device_id=device, device_id_type=MESH)
    pl.semaphore_wait(barrier, len(greeted))

    def remote(source, target, send_sem, recv_sem, device):
        return pltpu.make_async_remote_copy(
            src_ref=source,
            dst_ref=target,
            send_sem=send_sem,
            recv_sem=recv_sem,
            device_id=device,
            device_id_type=MESH,
        )

    def hop_copy(ring, way, spot, c):
        buffer, send_sem, recv_sem = ring
        size = buffer.shape[1] // chunks
        part = buffer.at[spot, pl.ds(pl.multiple_of(c * size, 16), size), :]
        device = (following if way == 0 else previous, tp)
        return remote(part, part, send_sem.at[way, spot, c], recv_sem.at[spot, c], device)

    def send_own(ring):
        for c in range(chunks):
            hop_copy(ring, 0, place, c).start()
            hop_copy(ring, 1, place, c).start()

    def event(ring, step, c):
        low, high = at(-step), at(step)
        hop_copy(ring, 0, low, c).wait_recv()

        @pl.when((step < half) | (c < chunks // 2))
        def _():
            hop_copy(ring, 0, low, c).start()

        hop_copy(ring, 1, high, c).wait_recv()

        @pl.when((step < half) | (c >= chunks // 2))
        def _():
            hop_copy(ring, 1, high, c).start()

    def events(ring, step):
        def body(c, carry):
            event(ring, step, c)
            return carry

        lax.fori_loop(0, chunks, body, 0)

    def opposite(ring):
        def body(c, carry):
            hop_copy(ring, 0, at(count // 2), c).wait_recv()
            return carry

        lax.fori_loop(0, chunks, body, 0)

    def sends_done(ring):
        def each(c, carry):
            hop_copy(ring, 0, place, c).wait_send()
            hop_copy(ring, 1, place, c).wait_send()

            def steps(step, inner):
                @pl.when((step < half) | (c < chunks // 2))
                def _():
                    hop_copy(ring, 0, at(-step), c).wait_send()

                @pl.when((step < half) | (c >= chunks // 2))
                def _():
                    hop_copy(ring, 1, at(step), c).wait_send()

                return inner

            return lax.fori_loop(1, half + 1, steps, carry)

        lax.fori_loop(0, chunks, each, 0)

    side_ring = (w_side, side_send, side_recv)
    query_ring = (w_query, query_send, query_recv)
    out_ring = (w_out, out_send, out_recv)

    for load in loads[:3]:
        load.wait()
    send_own(side_ring)
    loads[3].wait()

    token_rows = rows // token_chunks

    def token_part(owner, j):
        return tok.at[owner, pl.ds(pl.multiple_of(j * token_rows, 16), token_rows), :]

    def token_far(hop, owner, j):
        part = token_part(owner, j)
        target = (chip + hop) % chips * 2 + core
        return remote(
            part, part, ty_send.at[hop - 1, j], ty_recv.at[hop - 1, j], (me, target)
        )

    def token_near(slot, owner, j):
        part = token_part(owner, j)
        return remote(part, part, td_send.at[slot, j], td_recv.at[slot, j], (me, partner))

    def start_tokens(j, carry):
        for hop in range(1, chips):
            token_far(hop, tp, j).start()
        token_near(0, tp, j).start()
        return carry

    lax.fori_loop(0, token_chunks, start_tokens, 0)

    for g in range(rows // GRID_W):
        spot = pl.ds(me * (rows // GRID_W) + g, 1)
        grid_rows = pl.ds(g * GRID_W, GRID_W)
        cosines[grid_rows, :] = col_cos[...] + row_cos[spot, :]
        sines[grid_rows, :] = col_sin[...] + row_sin[spot, :]

    pieces = features // depth
    norm_rows = 32 if token_rows % 32 == 0 else 16

    def normalise(j):
        token_near(0, partner, j).wait_recv()
        for hop in range(1, chips):
            token_near(hop, (chip - hop + chips) % chips * 2 + 1 - core, j).wait_recv()

        def tile(i, carry):
            at_rows = pl.ds(pl.multiple_of(j * token_rows + i * norm_rows, 16), norm_rows)
            squares = jnp.zeros((norm_rows, 1), f32)
            for t in range(members):
                block = tok[t, at_rows, :].astype(f32)
                squares = squares + jnp.sum(block * block, axis=1, keepdims=True)
            scale = lax.rsqrt(squares / (members * features) + eps)
            for t in range(members):
                for piece in range(pieces):
                    first = piece * depth
                    gain = norm_gain[:, t * features + first : t * features + first + depth]
                    block = tok[t, at_rows, first : first + depth].astype(f32)
                    normed[t * pieces + piece, at_rows, :] = (block * scale * gain).astype(bf16)
            return carry

        lax.fori_loop(0, token_rows // norm_rows, tile, 0)

    def token_step(j, carry):
        for hop in range(1, chips):
            source = (chip - hop + chips) % chips * 2 + core
            token_far(hop, source, j).wait_recv()
            token_near(hop, source, j).start()

        @pl.when(j < half * chunks)
        def _():
            event(side_ring, j // chunks + 1, j % chunks)

        @pl.when(j >= 1)
        def _():
            normalise(j - 1)

        return carry

    lax.fori_loop(0, token_chunks, token_step, 0)
    normalise(token_chunks - 1)

    tile_rows = 256 if rows % 256 == 0 else 128

    def project(total, weights, spots, first=False):
        def body(i, carry):
            part = pl.ds(pl.multiple_of(i * tile_rows, tile_rows), tile_rows)
            terms = [
                jnp.dot(
                    normed[owner_of(spot), part, :], weights[spot], preferred_element_type=f32
                )
                for spot in spots
            ]
            value = functools.reduce(lambda a, b: a + b, terms)
            total[part, :] = value if first else total[part, :] + value
            return carry

        lax.fori_loop(0, rows // tile_rows, body, 0)

    project(side, w_side, [place], first=True)
    early = token_chunks // chunks

    def side_step(step, carry):
        @pl.when(step > early)
        def _():
            events(side_ring, step)

        project(side, w_side, [at(-step), at(step)])
        return carry

    lax.fori_loop(1, half + 1, side_step, 0)
    loads[4].wait()
    send_own(query_ring)
    opposite(side_ring)
    project(side, w_side, [at(count // 2)])

    lane = lax.broadcasted_iota(jnp.int32, (WINDOW, 2 * HEAD), 1)
    low_half = lane < HEAD
    lead = lane % (HEAD // 2) < HEAD // 4

    def prepare(i, carry):
        part = pl.ds(pl.multiple_of(i * WINDOW, WINDOW), WINDOW)
        shifted = pl.ds(pl.multiple_of((i + 1) * WINDOW, WINDOW), WINDOW)
        for h in range(kw // (2 * HEAD)):
            lanes = slice(h * 2 * HEAD, (h + 1) * 2 * HEAD)
            key = norm_rope(
                side[part, lanes], key_gain[...], cosines[part, :], sines[part, :], low_half, lead
            )
            band[shifted, lanes] = key.astype(bf16)
        band[shifted, kw : 2 * kw] = side[part, kw : 2 * kw].astype(bf16)
        pooled_rows = pl.ds(pl.multiple_of(i * WINDOW + pool_pad, pool_pad), WINDOW)
        pool_band[pooled_rows, :] = side[part, 2 * kw :].astype(bf16)
        return carry

    lax.fori_loop(0, rows // WINDOW, prepare, 0)

    before, behind = (me + count - 1) % count, (me + 1) % count

    def halo(index, buffer, size, upwards):
        if upwards:
            source, target, device = rows, 0, (behind, tp)
        else:
            source, target, device = size, rows + size, (before, tp)
        return remote(
            buffer.at[pl.ds(source, size), :],
            buffer.at[pl.ds(target, size), :],
            halo_send.at[index],
            halo_recv.at[index],
            device,
        )

    lower = [halo(0, band, WINDOW, False), halo(1, pool_band, pool_pad, False)]
    upper = [halo(2, band, WINDOW, True), halo(3, pool_band, pool_pad, True)]
    has_lower, has_upper = me > 0, me < count - 1

    @pl.when(has_lower)
    def _():
        for copy in lower:
            copy.start()

    @pl.when(has_upper)
    def _():
        for copy in upper:
            copy.start()

    @pl.when(jnp.logical_not(has_lower))
    def _():
        band[0:WINDOW, :] = jnp.zeros((WINDOW, 2 * kw), bf16)
        pool_band[0:pool_pad, :] = jnp.zeros((pool_pad, pw), bf16)

    @pl.when(jnp.logical_not(has_upper))
    def _():
        band[rows + WINDOW :, :] = jnp.zeros((WINDOW, 2 * kw), bf16)
        pool_band[rows + pool_pad :, :] = jnp.zeros((pool_pad, pw), bf16)

    project(query, w_query, [place], first=True)

    def query_step(step, carry):
        events(query_ring, step)
        project(query, w_query, [at(-step), at(step)])
        return carry

    lax.fori_loop(1, half + 1, query_step, 0)
    loads[5].wait()
    loads[6].wait()
    send_own(out_ring)

    @pl.when(has_lower)
    def _():
        for copy in upper:
            copy.wait_recv()

    @pl.when(has_upper)
    def _():
        for copy in lower:
            copy.wait_recv()

    level = tp * pw // (POOL // 4)
    reach = jnp.where(level == 0, 1, jnp.where(level == 1, 2, jnp.where(level == 2, 4, 8)))

    def pool(i, carry):
        wide = WINDOW + 2 * pool_pad
        part = pl.ds(pl.multiple_of(i * WINDOW, WINDOW), WINDOW)
        values = pool_band[pl.ds(pl.multiple_of(i * WINDOW, pool_pad), wide), :].astype(f32)
        total, chosen = values, None
        for step in range(4):
            size = 2**step
            total = total + pltpu.roll(total, wide - size, 0)
            shifted = pltpu.roll(total, size, 0)[pool_pad : pool_pad + WINDOW]
            chosen = shifted if chosen is None else jnp.where(level == step, shifted, chosen)
        spot = me * rows + i * WINDOW + lax.broadcasted_iota(jnp.int32, (WINDOW, 1), 0)
        low = jnp.maximum(spot - reach, 0)
        high = jnp.minimum(spot + reach - 1, seq - 1)
        mixer[part, 0:pw] = (chosen / (high - low + 1).astype(f32)).astype(bf16)
        return carry

    lax.fori_loop(0, rows // WINDOW, pool, 0)

    opposite(query_ring)
    project(query, w_query, [at(count // 2)])

    blocks = rows // WINDOW
    row = lax.broadcasted_iota(jnp.int32, (2 * WINDOW, 3 * WINDOW), 0) % WINDOW
    column = lax.broadcasted_iota(jnp.int32, (2 * WINDOW, 3 * WINDOW), 1)
    top_row = lax.broadcasted_iota(jnp.int32, (2 * WINDOW, 1), 0) < WINDOW

    def attend(i, carry):
        part = pl.ds(pl.multiple_of(i * WINDOW, WINDOW), WINDOW)
        key_rows = pl.ds(pl.multiple_of(i * WINDOW, WINDOW), 3 * WINDOW)
        key_pos = me * rows + i * WINDOW - WINDOW + column
        inside = (column >= row) & (column - row <= 2 * WINDOW) & (key_pos >= 0) & (key_pos < seq)
        for head in range(heads_k):
            lanes = slice(head * 2 * HEAD, (head + 1) * 2 * HEAD)
            rotated = norm_rope(
                query[part, lanes],
                query_gain[...],
                cosines[part, :],
                sines[part, :],
                low_half,
                lead,
            ) * HEAD ** (-0.5)
            other = pltpu.roll(rotated, HEAD, 1)
            if head % 2 == 0:
                pair = (jnp.where(low_half, rotated, 0.0), jnp.where(low_half, other, 0.0))
            else:
                pair = (jnp.where(low_half, 0.0, other), jnp.where(low_half, 0.0, rotated))
            stacked = jnp.concatenate(pair, axis=0).astype(bf16)
            tile = head // 2 * 2 * HEAD
            keys = band[key_rows, tile : tile + 2 * HEAD]
            values = band[key_rows, kw + tile : kw + tile + 2 * HEAD]
            scores = lax.dot_general(
                stacked, keys, (((1,), (1,)), ((), ())), preferred_element_type=f32
            )
            scores = jnp.where(inside, scores, neg_big)
            limit = jnp.where(top_row, sink[2 * head], sink[2 * head + 1])
            top = jnp.maximum(jnp.max(scores, axis=1, keepdims=True), limit)
            raised = jnp.exp(scores - top)
            totals = jnp.sum(raised, axis=1, keepdims=True) + jnp.exp(limit - top)
            weights = (raised * (1.0 / totals)).astype(bf16)
            result = jnp.dot(weights, values, preferred_element_type=f32)
            one, two = result[:WINDOW], result[WINDOW:]
            if head % 2 == 0:
                joined = jnp.where(low_half, one, pltpu.roll(two, HEAD, 1))
            else:
                joined = jnp.where(low_half, pltpu.roll(one, HEAD, 1), two)
            mixer[part, pw + head * 2 * HEAD : pw + (head + 1) * 2 * HEAD] = joined.astype(bf16)

        for c in range(chunks):

            @pl.when(i == ((c + 1) * blocks + chunks - 1) // chunks - 1)
            def _(c=c):
                event(out_ring, 1, c)

        return carry

    lax.fori_loop(0, blocks, attend, 0)

    def product(spot, which):
        left = jnp.concatenate(
            [
                mixer[pl.ds(pl.multiple_of((y * 2 + which) * share, 16), share), :]
                for y in range(chips)
            ],
            axis=0,
        )
        return jnp.dot(left, w_out[spot], preferred_element_type=f32).astype(bf16)

    def met_copy(spot):
        return remote(
            away.at[spot], met.at[spot], met_send.at[spot], met_recv.at[spot], (me, partner)
        )

    def y_copy(spot, hop):
        target = (chip + hop) % chips * 2 + core
        return remote(
            y_send.at[spot, hop - 1],
            y_recv.at[spot, hop - 1],
            yy_send.at[spot, hop - 1],
            yy_recv.at[spot, hop - 1],
            (me, target),
        )

    def done_copy(spot):
        columns = pl.ds(pl.multiple_of(owner_of(spot) * width, width), width)
        return pltpu.make_async_copy(done.at[spot], out.at[:, columns], done_sem.at[spot])

    def both_rows(spot, y):
        part = pl.ds(pl.multiple_of(y * share, 16), share)
        return kept[spot, part, :].astype(f32) + met[spot, part, :].astype(f32)

    def group(spots):
        def first(spot):
            away[spot] = product(spot, 1 - core)
            met_copy(spot).start()

        def second(spot):
            kept[spot] = product(spot, core)

        def third(spot):
            met_copy(spot).wait_recv()
            for hop in range(1, chips):
                y_send[spot, hop - 1] = both_rows(spot, (chip + hop) % chips).astype(bf16)
                y_copy(spot, hop).start()

        for part in (first, second, third):
            for spot in spots:
                part(spot)

    def finish(spot):
        total = both_rows(spot, chip)
        for hop in range(1, chips):
            y_copy(spot, hop).wait_recv()
            total = total + y_recv[spot, hop - 1].astype(f32)
        done[spot] = total.astype(bf16)
        done_copy(spot).start()

    group([place])

    def out_step(step, carry):
        @pl.when(step > 1)
        def _():
            events(out_ring, step)

        group([at(-step), at(step)])

        @pl.when(step == 1)
        def _():
            finish(place)

        @pl.when(step > 1)
        def _():
            finish(at(1 - step))
            finish(at(step - 1))

        return carry

    lax.fori_loop(1, half + 1, out_step, 0)
    opposite(out_ring)
    group([at(count // 2)])
    finish(at(-half))
    finish(at(half))
    finish(at(count // 2))

    for ring in (side_ring, query_ring, out_ring):
        sends_done(ring)

    def tokens_sent(j, carry):
        token_near(0, tp, j).wait_send()
        for hop in range(1, chips):
            token_far(hop, tp, j).wait_send()
            token_near(hop, (chip - hop + chips) % chips * 2 + core, j).wait_send()
        return carry

    lax.fori_loop(0, token_chunks, tokens_sent, 0)

    @pl.when(has_lower)
    def _():
        for copy in lower:
            copy.wait_send()

    @pl.when(has_upper)
    def _():
        for copy in upper:
            copy.wait_send()

    def blocks_sent(spot, carry):
        met_copy(spot).wait_send()
        for hop in range(1, chips):
            y_copy(spot, hop).wait_send()
        done_copy(spot).wait()
        return carry

    lax.fori_loop(0, count, blocks_sent, 0)


def plane_kernel(
    count,
    members,
    tokens,
    wq,
    wk,
    wv,
    wp,
    wop,
    woa,
    norm_gain,
    query_gain,
    key_gain,
    row_cos,
    row_sin,
    col_cos,
    col_sin,
    sink,
    out,
    raw,
    sums,
    normed,
    w_in,
    w_pool,
    w_out,
    in_spare,
    pool_spare,
    out_spare,
    total,
    pool_total,
    band,
    pool_band,
    cosines,
    sines,
    mixer,
    result,
    rounded,
    load_sem,
    sum_send,
    sum_recv,
    in_sems,
    pool_sems,
    out_sems,
    x_sems,
    spread_sems,
    token_sems,
    attend_sems,
    pooled_sems,
    halo_send,
    halo_recv,
    result_send,
    result_recv,
):
    rows, features = tokens.shape
    depth = wk.shape[0]
    hk, hq, hp = wk.shape[1] // 2, wq.shape[1] // 2, wp.shape[1] // 2
    width = wop.shape[1]
    narrow = width // members
    share = rows // members
    plane = 2 * rows
    heads_k = hk // HEAD
    seq = count * rows
    deep = count // 2
    pieces = features // depth
    tiles = rows // WINDOW

    me, tp = lax.axis_index("sp"), lax.axis_index("tp")
    z, x = me // 2, me % 2
    y, core = tp // 2, tp % 2
    me_x, tp_y, tp_c = me + 1 - 2 * x, (1 - y) * 2 + core, y * 2 + 1 - core
    tp_yc = (1 - y) * 2 + 1 - core
    up, down = (me + 2) % count, (me + count - 2) % count
    has_up, has_down = z < deep - 1, z > 0
    inner = has_up & has_down

    mine = lambda size: pl.ds(pl.multiple_of(x * size, 128), size)
    other = lambda size: pl.ds(pl.multiple_of((1 - x) * size, 128), size)
    loads = []

    def load(source, target):
        loads.append(pltpu.make_async_copy(source, target, load_sem.at[len(loads)]))
        loads[-1].start()

    for target, pick in ((w_in.at[me], mine), (in_spare, other)):
        load(wk.at[:, pick(hk)], target.at[:, pl.ds(0, hk)])
        load(wv.at[:, pick(hk)], target.at[:, pl.ds(hk, hk)])
        load(wq.at[:, pick(hq)], target.at[:, pl.ds(2 * hk, hq)])
    load(tokens, raw)
    for target, pick in ((w_pool.at[me], mine), (pool_spare, other)):
        load(wp.at[:, pick(hp)], target)
    strip = lambda t: pl.ds(pl.multiple_of(t * narrow, narrow), narrow)
    for target, t in [(w_out.at[z, tp], tp)] + [(out_spare.at[t], t) for t in range(members)]:
        for h in range(2):
            first = h * (hp + hq)
            load(wop.at[pl.ds(h * hp, hp), strip(t)], target.at[pl.ds(first, hp), :])
            load(woa.at[pl.ds(h * hq, hq), strip(t)], target.at[pl.ds(first + hp, hq), :])

    barrier = pltpu.get_barrier_semaphore()
    greeted = [(up, tp), (down, tp), (me_x, tp)]
    for t in (tp_y, tp_c, tp_yc):
        greeted += [(me, t), (me_x, t)]
    for device in greeted:
        pl.semaphore_signal(barrier, inc=1, device_id=device, device_id_type=MESH)
    pl.semaphore_wait(barrier, len(greeted))

    def remote(source, target, send_sem, recv_sem, device):
        return pltpu.make_async_remote_copy(
            src_ref=source,
            dst_ref=target,
            send_sem=send_sem,
            recv_sem=recv_sem,
            device_id=device,
            device_id_type=MESH,
        )

    def by_rows(parts):
        def view(buffer, c):
            size = buffer.shape[0] // parts
            return buffer.at[pl.ds(pl.multiple_of(c * size, 16), size), :]

        return view

    in_ring = (w_in, in_spare, in_sems, 0, in_parts, by_rows(in_parts))
    pool_ring = (w_pool, pool_spare, pool_sems, in_parts, 1, by_rows(1))
    def z_copy(ring, way, source, c):
        buffer, _, sems, _, _, view = ring
        part = view(buffer.at[source], c)
        return remote(
            part, part, sems.at[way, source, c], sems.at[2, source, c], ((up, down)[way], tp)
        )

    def x_copy(ring, source, c):
        buffer, spare, sems, first, _, view = ring
        return remote(
            view(spare, c),
            view(buffer.at[source], c),
            x_sems.at[first + c],
            sems.at[2, source, c],
            (me_x, tp),
        )

    def both_ways(ring, source, c, act):
        @pl.when(has_up)
        def _():
            act(z_copy(ring, 0, source, c))

        @pl.when(has_down)
        def _():
            act(z_copy(ring, 1, source, c))

    start = lambda copy: copy.start()
    sent = lambda copy: copy.wait_send()

    def own_out(ring):
        for c in range(ring[4]):
            both_ways(ring, me, c, start)

    def side_out(ring):
        for c in range(ring[4]):
            x_copy(ring, me, c).start()

    def side_in(ring):
        for c in range(ring[4]):
            x_copy(ring, me_x, c).wait_recv()
            both_ways(ring, me_x, c, start)

    def passing(ring, n):
        parts = ring[4]
        step, j, c = n // (2 * parts) + 1, n // parts % 2, n % parts
        column = (x + j) % 2
        low, high = z - step, z + step
        return (low >= 0, low * 2 + column), (high < deep, high * 2 + column), c

    def event(ring, n):
        (is_low, low), (is_high, high), c = passing(ring, n)

        @pl.when(is_low)
        def _():
            z_copy(ring, 0, low, c).wait_recv()

            @pl.when(has_up)
            def _():
                z_copy(ring, 0, low, c).start()

        @pl.when(is_high)
        def _():
            z_copy(ring, 1, high, c).wait_recv()

            @pl.when(has_down)
            def _():
                z_copy(ring, 1, high, c).start()

    def events(ring, first, last):
        def body(n, carry):
            event(ring, n)
            return carry

        lax.fori_loop(first, last, body, 0)

    def all_events(ring):
        return (deep - 1) * 2 * ring[4]

    def sends_done(ring):
        for c in range(ring[4]):
            both_ways(ring, me, c, sent)
            both_ways(ring, me_x, c, sent)
            x_copy(ring, me, c).wait_send()

        def body(n, carry):
            (is_low, low), (is_high, high), c = passing(ring, n)

            @pl.when(is_low & has_up)
            def _():
                z_copy(ring, 0, low, c).wait_send()

            @pl.when(is_high & has_down)
            def _():
                z_copy(ring, 1, high, c).wait_send()

            return carry

        lax.fori_loop(0, all_events(ring), body, 0)

    def out_copy(way, level, c):
        part = w_out.at[level, (tp - c + members) % members]
        device = ((up, down)[way], tp)
        return remote(part, part, out_sems.at[way, level, c], out_sems.at[2, level, c], device)

    def spread(c):
        target = (tp + c) % members
        return remote(
            out_spare.at[target],
            w_out.at[z, tp],
            spread_sems.at[c],
            out_sems.at[2, z, c],
            (me, target),
        )

    def spread_in(c):
        owner = (tp - c + members) % members
        return remote(
            out_spare.at[owner],
            w_out.at[z, owner],
            spread_sems.at[c],
            out_sems.at[2, z, c],
            (me, owner),
        )

    def out_both(c, act):
        @pl.when(has_up)
        def _():
            act(out_copy(0, z, c))

        @pl.when(has_down)
        def _():
            act(out_copy(1, z, c))

    def out_event(n):
        step, c = n // members + 1, n % members
        low, high = z - step, z + step

        @pl.when(low >= 0)
        def _():
            out_copy(0, low, c).wait_recv()

            @pl.when(has_up)
            def _():
                out_copy(0, low, c).start()

        @pl.when(high < deep)
        def _():
            out_copy(1, high, c).wait_recv()

            @pl.when(has_down)
            def _():
                out_copy(1, high, c).start()

    def out_events(first, last):
        def body(n, carry):
            out_event(n)
            return carry

        lax.fori_loop(first, last, body, 0)

    def out_sent(n, carry):
        step, c = n // members + 1, n % members
        low, high = z - step, z + step

        @pl.when((low >= 0) & has_up)
        def _():
            out_copy(0, low, c).wait_send()

        @pl.when((high < deep) & has_down)
        def _():
            out_copy(1, high, c).wait_send()

        return carry

    for copy in loads[:6]:
        copy.wait()
    for c in range(in_parts):
        x_copy(in_ring, me, c).start()
        both_ways(in_ring, me, c, start)

    loads[6].wait()
    sums[tp] = jnp.zeros_like(sums[tp])
    for i in range(tiles):
        block = raw[i * WINDOW : (i + 1) * WINDOW, :].astype(f32)
        square = jnp.sum(block * block, axis=1, keepdims=True)
        turned = jnp.transpose(jnp.broadcast_to(square, (WINDOW, WINDOW)))
        sums[tp, i : i + 1, :] = turned[0:1, :]

    def sum_copy(owner, hop):
        target = (tp + hop) % members
        return remote(
            sums.at[owner],
            sums.at[owner],
            sum_send.at[hop - 1],
            sum_recv.at[hop - 1],
            (me, target),
        )

    for hop in range(1, members):
        sum_copy(tp, hop).start()
    for g in range(plane // GRID_W):
        spot = pl.ds(z * (plane // GRID_W) + g, 1)
        grid_rows = pl.ds(g * GRID_W, GRID_W)
        cosines[grid_rows, :] = col_cos[...] + row_cos[spot, :]
        sines[grid_rows, :] = col_sin[...] + row_sin[spot, :]
    for hop in range(1, members):
        sum_copy((tp - hop + members) % members, hop).wait_recv()
    squares = sums[0]
    for t in range(1, members):
        squares = squares + sums[t]
    scales = lax.rsqrt(squares / (members * features) + eps)

    class Stream:
        def __init__(self, view, sems, by_x):
            self.view, self.sems, self.by_x = view, sems, by_x

        def copy(self, base, count_of, slot, side, owner, j, device):
            part = self.view(side, owner, j)
            send, recv = self.sems.at[base + slot, j], self.sems.at[base + count_of + slot, j]
            return remote(part, part, send, recv, device)

        def over_x(self, slot, side, owner, j):
            return self.copy(0, 2, slot, side, owner, j, (me_x, tp))

        def over_y(self, slot, side, owner, j):
            return self.copy(4, 2, slot, side, owner, j, (me, tp_y))

        def over_core(self, slot, side, owner, j):
            return self.copy(8, 4, slot, side, owner, j, (me, tp_c))

        def start(self, j):
            self.over_y(0, x, tp, j).start()
            self.over_x(0, x, tp, j).start()
            self.over_core(0, x, tp, j).start()

        def direct(self, j):
            self.over_y(0, x, tp_y, j).wait_recv()
            self.over_core(2, x, tp_y, j).start()

            @pl.when(self.by_x(j))
            def _():
                self.over_x(1, x, tp_y, j).start()

            self.over_x(0, 1 - x, tp, j).wait_recv()
            self.over_core(1, 1 - x, tp, j).start()

            @pl.when(jnp.logical_not(self.by_x(j)))
            def _():
                self.over_y(1, 1 - x, tp, j).start()

        def crossed(self, j):
            @pl.when(self.by_x(j))
            def _():
                self.over_x(1, 1 - x, tp_y, j).wait_recv()

            @pl.when(jnp.logical_not(self.by_x(j)))
            def _():
                self.over_y(1, 1 - x, tp_y, j).wait_recv()

            self.over_core(3, 1 - x, tp_y, j).start()

        def near_side(self, j):
            self.over_core(0, x, tp_c, j).wait_recv()
            self.over_core(2, x, tp_yc, j).wait_recv()

        def far_side(self, j):
            self.over_core(1, 1 - x, tp_c, j).wait_recv()
            self.over_core(3, 1 - x, tp_yc, j).wait_recv()

        def sent(self, j):
            self.over_y(0, x, tp, j).wait_send()
            self.over_x(0, x, tp, j).wait_send()
            self.over_core(0, x, tp, j).wait_send()
            self.over_core(1, 1 - x, tp, j).wait_send()
            self.over_core(2, x, tp_y, j).wait_send()
            self.over_core(3, 1 - x, tp_y, j).wait_send()

            @pl.when(self.by_x(j))
            def _():
                self.over_x(1, x, tp_y, j).wait_send()

            @pl.when(jnp.logical_not(self.by_x(j)))
            def _():
                self.over_y(1, 1 - x, tp, j).wait_send()

        def every(self, act):
            def body(j, carry):
                act(j)
                return carry

            lax.fori_loop(0, self.sems.shape[1], body, 0)

    def block_rows(j, size):
        return pl.ds(pl.multiple_of(j * size, 16), size)

    def token_view(side, owner, j):
        return normed.at[side, pl.ds(owner * pieces, pieces), block_rows(j, WINDOW), :]

    def attend_view(side, owner, j):
        return mixer.at[owner, side, block_rows(j, WINDOW), pl.ds(hp, hq)]

    def pooled_view(side, owner, j):
        return mixer.at[owner, side, block_rows(j, plane // pooled_parts), pl.ds(0, hp)]

    token_stream = Stream(token_view, token_sems, lambda j: j % 3 == 0)
    attend_stream = Stream(attend_view, attend_sems, lambda j: j % 2 == 0)
    pooled_stream = Stream(pooled_view, pooled_sems, lambda j: j % 2 == 0)

    gains = norm_gain[pl.ds(tp, 1), :]
    for i in range(tiles):
        here = slice(i * WINDOW, (i + 1) * WINDOW)
        scale = jnp.transpose(jnp.broadcast_to(scales[i : i + 1, :], (WINDOW, WINDOW)))
        for first in range(0, features, WINDOW):
            block = raw[here, first : first + WINDOW].astype(f32)
            value = (block * scale * gains[:, first : first + WINDOW]).astype(bf16)
            inside = first % depth
            normed[x, tp * pieces + first // depth, here, inside : inside + WINDOW] = value
        token_stream.start(i)

    side_in(in_ring)
    whole = all_events(in_ring)
    reached = lambda part: whole * part // 24
    events(in_ring, 0, reached(4))

    def direct(j, carry):
        token_stream.direct(j)
        events(in_ring, reached(4 + 12 * j // tiles), reached(4 + 12 * (j + 1) // tiles))
        return carry

    lax.fori_loop(0, tiles, direct, 0)
    for copy in loads[7:]:
        copy.wait()
    side_out(pool_ring)
    for c in range(1, members):
        spread(c).start()
    token_stream.every(token_stream.near_side)

    tile_rows = 256 if rows % 256 == 0 else 128
    per_side = rows // tile_rows

    def project(result, weights, level, side, first=False):
        def body(i, carry):
            within = pl.ds(pl.multiple_of(i * tile_rows, tile_rows), tile_rows)
            part = pl.ds(pl.multiple_of(side * rows + i * tile_rows, tile_rows), tile_rows)
            value = None if first else result[part, :]
            for j in range(2):
                term = jnp.dot(
                    normed[side, level * 2 + j, within, :],
                    weights[level * 2 + j],
                    preferred_element_type=f32,
                )
                value = term if value is None else value + term
            result[part, :] = value
            return carry

        lax.fori_loop(0, per_side, body, 0)

    def project_step(result, weights, step, side):
        @pl.when(z - step >= 0)
        def _():
            project(result, weights, z - step, side)

        @pl.when(z + step < deep)
        def _():
            project(result, weights, z + step, side)

    early = max(reached(16) // (2 * in_parts), 0)

    def crossed(j, carry):
        token_stream.crossed(j)

        @pl.when(j == 0)
        def _():
            project(total, w_in, z, x, first=True)

        @pl.when((j >= 1) & (j <= early))
        def _():
            project_step(total, w_in, j, x)

        events(in_ring, reached(16 + 6 * j // tiles), reached(16 + 6 * (j + 1) // tiles))
        return carry

    lax.fori_loop(0, tiles, crossed, 0)
    own_out(pool_ring)
    side_in(pool_ring)
    token_stream.every(token_stream.far_side)
    project(total, w_in, z, 1 - x, first=True)

    def in_step(step, carry):
        each = 2 * in_parts
        events(in_ring, jnp.maximum((step - 1) * each, reached(22)), step * each)

        @pl.when(step > min(early, tiles - 1))
        def _():
            project_step(total, w_in, step, x)

        project_step(total, w_in, step, 1 - x)
        return carry

    lax.fori_loop(1, deep, in_step, 0)

    lane = lax.broadcasted_iota(jnp.int32, (WINDOW, 2 * HEAD), 1)
    low_half = lane < HEAD
    lead = lane % (HEAD // 2) < HEAD // 4
    blocks = plane // WINDOW

    def prepare(i, carry):
        part = pl.ds(pl.multiple_of(i * WINDOW, WINDOW), WINDOW)
        shifted = pl.ds(pl.multiple_of((i + 1) * WINDOW, WINDOW), WINDOW)
        for h in range(hk // (2 * HEAD)):
            lanes = slice(h * 2 * HEAD, (h + 1) * 2 * HEAD)
            key = norm_rope(
                total[part, lanes], key_gain[...], cosines[part, :], sines[part, :], low_half, lead
            )
            band[shifted, lanes] = key.astype(bf16)
        band[shifted, hk:] = total[part, hk : 2 * hk].astype(bf16)
        return carry

    lax.fori_loop(0, blocks, prepare, 0)

    def halo(index, buffer, size, upwards):
        if upwards:
            source, target, device = plane, 0, (up, tp)
        else:
            source, target, device = size, plane + size, (down, tp)
        return remote(
            buffer.at[pl.ds(source, size), :],
            buffer.at[pl.ds(target, size), :],
            halo_send.at[index],
            halo_recv.at[index],
            device,
        )

    def halo_out(index, buffer, size):
        @pl.when(has_down)
        def _():
            halo(index, buffer, size, False).start()

        @pl.when(has_up)
        def _():
            halo(index + 1, buffer, size, True).start()

        empty = jnp.zeros((size, buffer.shape[1]), bf16)

        @pl.when(jnp.logical_not(has_down))
        def _():
            buffer[0:size, :] = empty

        @pl.when(jnp.logical_not(has_up))
        def _():
            buffer[plane + size :, :] = empty

    def halo_in(index, buffer, size):
        @pl.when(has_up)
        def _():
            halo(index, buffer, size, False).wait_recv()

        @pl.when(has_down)
        def _():
            halo(index + 1, buffer, size, True).wait_recv()

    halo_out(0, band, WINDOW)

    def pool_stage():
        for side in range(2):
            project(pool_total, w_pool, z, side, first=True)

        def step_body(step, carry):
            events(pool_ring, (step - 1) * 2, step * 2)
            for side in range(2):
                project_step(pool_total, w_pool, step, side)
            return carry

        lax.fori_loop(1, deep, step_body, 0)
        pool_band[pool_pad : pool_pad + plane, :] = pool_total[...].astype(bf16)
        halo_out(2, pool_band, pool_pad)

    @pl.when(inner)
    def _():
        pool_stage()

    out_both(0, start)
    for c in range(1, members):
        spread_in(c).wait_recv()
        out_both(c, start)

    row = lax.broadcasted_iota(jnp.int32, (2 * WINDOW, 3 * WINDOW), 0) % WINDOW
    column = lax.broadcasted_iota(jnp.int32, (2 * WINDOW, 3 * WINDOW), 1)
    top_row = lax.broadcasted_iota(jnp.int32, (2 * WINDOW, 1), 0) < WINDOW

    def attend(turn, carry):
        @pl.when(turn == blocks - 2)
        def _():
            halo_in(0, band, WINDOW)

        i = (turn + 1) % blocks
        part = pl.ds(pl.multiple_of(i * WINDOW, WINDOW), WINDOW)
        key_rows = pl.ds(pl.multiple_of(i * WINDOW, WINDOW), 3 * WINDOW)
        key_pos = z * plane + i * WINDOW - WINDOW + column
        inside = (column >= row) & (column - row <= 2 * WINDOW) & (key_pos >= 0) & (key_pos < seq)
        for head in range(heads_k):
            lanes = slice(2 * hk + head * 2 * HEAD, 2 * hk + (head + 1) * 2 * HEAD)
            rotated = norm_rope(
                total[part, lanes],
                query_gain[...],
                cosines[part, :],
                sines[part, :],
                low_half,
                lead,
            ) * HEAD ** (-0.5)
            swapped = pltpu.roll(rotated, HEAD, 1)
            if head % 2 == 0:
                pair = (jnp.where(low_half, rotated, 0.0), jnp.where(low_half, swapped, 0.0))
            else:
                pair = (jnp.where(low_half, 0.0, swapped), jnp.where(low_half, 0.0, rotated))
            stacked = jnp.concatenate(pair, axis=0).astype(bf16)
            tile = head // 2 * 2 * HEAD
            keys = band[key_rows, tile : tile + 2 * HEAD]
            values = band[key_rows, hk + tile : hk + tile + 2 * HEAD]
            scores = lax.dot_general(
                stacked, keys, (((1,), (1,)), ((), ())), preferred_element_type=f32
            )
            scores = jnp.where(inside, scores, neg_big)
            first = x * 2 * heads_k + 2 * head
            limit = jnp.where(top_row, sink[first], sink[first + 1])
            top = jnp.maximum(jnp.max(scores, axis=1, keepdims=True), limit)
            raised = jnp.exp(scores - top)
            totals = jnp.sum(raised, axis=1, keepdims=True) + jnp.exp(limit - top)
            weights = (raised * (1.0 / totals)).astype(bf16)
            result = jnp.dot(weights, values, preferred_element_type=f32)
            one, two = result[:WINDOW], result[WINDOW:]
            if head % 2 == 0:
                joined = jnp.where(low_half, one, pltpu.roll(two, HEAD, 1))
            else:
                joined = jnp.where(low_half, pltpu.roll(one, HEAD, 1), two)
            lanes = slice(hp + head * 2 * HEAD, hp + (head + 1) * 2 * HEAD)
            mixer[tp, x, part, lanes] = joined.astype(bf16)
        attend_stream.start(i)

        @pl.when(turn >= behind)
        def _():
            attend_stream.direct((turn - behind + 1) % blocks)

        return carry

    behind = 2
    lax.fori_loop(0, blocks, attend, 0)
    for turn in range(blocks - behind, blocks):
        attend_stream.direct((turn + 1) % blocks)

    @pl.when(inner)
    def _():
        out_events(0, members)

    @pl.when(jnp.logical_not(inner))
    def _():
        pool_stage()

    halo_in(2, pool_band, pool_pad)
    level = (tp * 2 + x) * hp // (POOL // 4)
    reach = jnp.where(level == 0, 1, jnp.where(level == 1, 2, jnp.where(level == 2, 4, 8)))

    def pool(i, carry):
        wide = WINDOW + 2 * pool_pad
        part = pl.ds(pl.multiple_of(i * WINDOW, WINDOW), WINDOW)
        running = pool_band[pl.ds(pl.multiple_of(i * WINDOW, pool_pad), wide), :].astype(f32)
        chosen = None
        for step in range(4):
            size = 2**step
            running = running + pltpu.roll(running, wide - size, 0)
            shifted = pltpu.roll(running, size, 0)[pool_pad : pool_pad + WINDOW]
            chosen = shifted if chosen is None else jnp.where(level == step, shifted, chosen)
        spot = z * plane + i * WINDOW + lax.broadcasted_iota(jnp.int32, (WINDOW, 1), 0)
        low = jnp.maximum(spot - reach, 0)
        high = jnp.minimum(spot + reach - 1, seq - 1)
        mixer[tp, x, part, 0:hp] = (chosen / (high - low + 1).astype(f32)).astype(bf16)
        return carry

    lax.fori_loop(0, blocks, pool, 0)

    pooled_stream.every(pooled_stream.start)
    attend_stream.every(attend_stream.crossed)
    pooled_stream.every(pooled_stream.direct)
    pooled_stream.every(pooled_stream.crossed)
    for stream in (attend_stream, pooled_stream):
        stream.every(stream.near_side)
        stream.every(stream.far_side)

    def level_of(group):
        paired = jnp.minimum(z, deep - 1 - z)
        step = jnp.where(group > 2 * paired, group - paired, (group + 1) // 2)
        downwards = jnp.where(group > 2 * paired, 2 * z > deep - 1, group % 2 == 1)
        return jnp.where(downwards, z - step, z + step)

    here = x * members + tp
    out_steps = (deep - 1) * members

    def columns_of(level, side, t):
        first = (level * 2 + side) * width + t * narrow
        return pl.ds(pl.multiple_of(first, narrow), narrow)

    def result_copy(level, hop):
        target = (here + hop) % (2 * members)
        return remote(
            rounded.at[level, pl.ds(pl.multiple_of(target * share, 16), share), :],
            out.at[:, columns_of(level, x, tp)],
            result_send.at[level, hop],
            result_recv.at[level, hop],
            (z * 2 + target // members, target % members),
        )

    def result_in(level, hop):
        source = (here - hop + 2 * members) % (2 * members)
        return remote(
            rounded.at[level, pl.ds(0, share), :],
            out.at[:, columns_of(level, source // members, source % members)],
            result_send.at[level, hop],
            result_recv.at[level, hop],
            (z * 2 + source // members, source % members),
        )

    def result_own(level):
        return pltpu.make_async_copy(
            rounded.at[level, pl.ds(pl.multiple_of(here * share, 16), share), :],
            out.at[:, columns_of(level, x, tp)],
            result_send.at[level, 0],
        )

    def out_level(group, carry):
        level = level_of(group)
        for c in range(members):
            first_event = jnp.where(inner, out_steps, (group - 1) * members + c)

            @pl.when((first_event >= 0) & (first_event < out_steps))
            def _():
                out_event(first_event)

            t = (tp - c + members) % members

            def body(i, inner_carry):
                part = pl.ds(pl.multiple_of(i * tile_rows, tile_rows), tile_rows)
                value = None if c == 0 else result[part, :]
                for h in range(2):
                    term = jnp.dot(
                        mixer[t, h, part, :],
                        w_out[level, t, h * (hp + hq) : (h + 1) * (hp + hq), :],
                        preferred_element_type=f32,
                    )
                    value = term if value is None else value + term
                if c == members - 1:
                    rounded[level, part, :] = value.astype(bf16)
                else:
                    result[part, :] = value
                return inner_carry

            lax.fori_loop(0, plane // tile_rows, body, 0)
        for hop in range(1, 2 * members):
            result_copy(level, hop).start()
        result_own(level).start()
        return carry

    @pl.when(inner)
    def _():
        out_events(members, out_steps)

    lax.fori_loop(0, deep, out_level, 0)

    def results(level, carry):
        for hop in range(1, 2 * members):
            result_in(level, hop).wait_recv()
        return carry

    lax.fori_loop(0, deep, results, 0)

    for ring in (in_ring, pool_ring):
        sends_done(ring)
    for c in range(members):
        out_both(c, sent)
    for c in range(1, members):
        spread(c).wait_send()
    lax.fori_loop(0, out_steps, out_sent, 0)
    for hop in range(1, members):
        sum_copy(tp, hop).wait_send()

    for stream in (token_stream, attend_stream, pooled_stream):
        stream.every(stream.sent)
    for index, buffer, size in ((0, band, WINDOW), (2, pool_band, pool_pad)):

        @pl.when(has_down)
        def _(index=index, buffer=buffer, size=size):
            halo(index, buffer, size, False).wait_send()

        @pl.when(has_up)
        def _(index=index, buffer=buffer, size=size):
            halo(index + 1, buffer, size, True).wait_send()

    def results_sent(level, carry):
        for hop in range(1, 2 * members):
            result_copy(level, hop).wait_send()
        result_own(level).wait()
        return carry

    lax.fori_loop(0, deep, results_sent, 0)


def plane_scratch(count, members, rows, features, depth, kw, qw, pw, width):
    hk, hq, hp = kw // 2, qw // 2, pw // 2
    narrow, plane, deep, tiles = width // members, 2 * rows, count // 2, rows // WINDOW
    dma = pltpu.SemaphoreType.DMA
    return [
        pltpu.VMEM((rows, features), bf16),
        pltpu.VMEM((members, -(-tiles // 8) * 8, WINDOW), f32),
        pltpu.VMEM((2, count, rows, depth), bf16),
        pltpu.VMEM((count, depth, 2 * hk + hq), bf16),
        pltpu.VMEM((count, depth, hp), bf16),
        pltpu.VMEM((deep, members, 2 * (hp + hq), narrow), bf16),
        pltpu.VMEM((depth, 2 * hk + hq), bf16),
        pltpu.VMEM((depth, hp), bf16),
        pltpu.VMEM((members, 2 * (hp + hq), narrow), bf16),
        pltpu.VMEM((plane, 2 * hk + hq), f32),
        pltpu.VMEM((plane, hp), f32),
        pltpu.VMEM((plane + 2 * WINDOW, 2 * hk), bf16),
        pltpu.VMEM((plane + 2 * pool_pad, hp), bf16),
        pltpu.VMEM((plane, 2 * HEAD), f32),
        pltpu.VMEM((plane, 2 * HEAD), f32),
        pltpu.VMEM((members, 2, plane, hp + hq), bf16),
        pltpu.VMEM((plane, narrow), f32),
        pltpu.VMEM((deep, plane, narrow), bf16),
        dma((13 + 4 * members,)),
        dma((members - 1,)),
        dma((members - 1,)),
        dma((3, count, in_parts)),
        dma((3, count, 1)),
        dma((3, deep, members)),
        dma((in_parts + 1,)),
        dma((members,)),
        dma((16, tiles)),
        dma((16, 2 * tiles)),
        dma((16, pooled_parts)),
        dma((4,)),
        dma((4,)),
        dma((deep, 2 * members)),
        dma((deep, 2 * members)),
    ]


def ring_scratch(count, members, rows, features, depth, kw, qw, pw, width):
    chips, share = members // 2, rows // members
    far = max(chips - 1, 1)
    dma = pltpu.SemaphoreType.DMA
    return [
        pltpu.VMEM((members, rows, features), bf16),
        pltpu.VMEM((count, rows, depth), bf16),
        pltpu.VMEM((count, depth, 2 * kw + pw), bf16),
        pltpu.VMEM((count, depth, qw), bf16),
        pltpu.VMEM((count, pw + qw, width), bf16),
        pltpu.VMEM((rows, 2 * kw + pw), f32),
        pltpu.VMEM((rows, qw), f32),
        pltpu.VMEM((rows + 2 * WINDOW, 2 * kw), bf16),
        pltpu.VMEM((rows + 2 * pool_pad, pw), bf16),
        pltpu.VMEM((rows, 2 * HEAD), f32),
        pltpu.VMEM((rows, 2 * HEAD), f32),
        pltpu.VMEM((rows, pw + qw), bf16),
        pltpu.VMEM((count, chips * share, width), bf16),
        pltpu.VMEM((count, chips * share, width), bf16),
        pltpu.VMEM((count, chips * share, width), bf16),
        pltpu.VMEM((count, far, share, width), bf16),
        pltpu.VMEM((count, far, share, width), bf16),
        pltpu.VMEM((count, share, width), bf16),
        dma((7,)),
        dma((2, count, chunks)),
        dma((count, chunks)),
        dma((2, count, chunks)),
        dma((count, chunks)),
        dma((2, count, chunks)),
        dma((count, chunks)),
        dma((far, token_chunks)),
        dma((far, token_chunks)),
        dma((chips, token_chunks)),
        dma((chips, token_chunks)),
        dma((4,)),
        dma((4,)),
        dma((count,)),
        dma((count,)),
        dma((count, far)),
        dma((count, far)),
        dma((count,)),
    ]


def shards(
    tokens,
    norm_gain,
    w_query,
    w_key,
    w_value,
    w_pool,
    query_gain,
    key_gain,
    sink_logit,
    w_out_pool,
    w_out_attn,
):
    count, members = lax.axis_size("sp"), lax.axis_size("tp")
    rows, features = tokens.shape
    depth, kw = w_key.shape
    qw, pw, width = w_query.shape[1], w_pool.shape[1], w_out_pool.shape[1]
    tables = [jnp.asarray(table) for table in rope_parts(count * rows)]
    twice = lambda gain: jnp.concatenate([gain, gain]).reshape(1, 2 * HEAD)
    anywhere = pl.BlockSpec(memory_space=pl.ANY)
    in_vmem = pl.BlockSpec(memory_space=pltpu.VMEM)
    sizes = (count, members, rows, features, depth, kw, qw, pw, width)
    shared = (
        members == 4
        and count % 2 == 0
        and count >= 4
        and rows % (2 * WINDOW) == 0
        and depth % (16 * in_parts) == 0
        and all(size % 256 == 0 for size in (kw, qw, pw))
        and width % (128 * members) == 0
    )
    kernel, scratch = (plane_kernel, plane_scratch) if shared else (layer_kernel, ring_scratch)
    return pl.pallas_call(
        functools.partial(kernel, count, members),
        out_shape=jax.ShapeDtypeStruct((rows // members, count * width), bf16),
        in_specs=[anywhere] * 7 + [in_vmem] * 7 + [pl.BlockSpec(memory_space=pltpu.SMEM)],
        out_specs=anywhere,
        scratch_shapes=scratch(*sizes),
        compiler_params=pltpu.CompilerParams(
            collective_id=0, has_side_effects=True, vmem_limit_bytes=62 * 1024 * 1024
        ),
    )(
        tokens,
        w_query,
        w_key,
        w_value,
        w_pool,
        w_out_pool,
        w_out_attn,
        norm_gain.reshape(members, -1) if shared else norm_gain.reshape(1, -1),
        twice(query_gain),
        twice(key_gain),
        *tables,
        sink_logit,
    )


def solution(mesh):
    placed = (
        P("sp", "tp"),
        P(),
        P("sp", "tp"),
        P("sp", "tp"),
        P("sp", "tp"),
        P("sp", "tp"),
        P(),
        P(),
        P("tp"),
        P("tp", "sp"),
        P("tp", "sp"),
    )
    return jax.shard_map(
        shards, mesh=mesh, in_specs=placed, out_specs=P(("sp", "tp"), None), check_vma=False
    )
```

```python
import functools

import jax
import jax.numpy as jnp
import numpy as np
from jax import lax
from jax.experimental import pallas as pl
from jax.experimental.pallas import tpu as pltpu
from jax.sharding import PartitionSpec as P

HEAD = 64
POOL = 1024
WINDOW = 128
GRID_W = 64

eps = 1e-06
rope_base = 10000.0
neg_big = -1e30
pool_pad = 16
chunks = 4
token_chunks = 8
in_parts = 4
pooled_parts = 4
MESH = pl.DeviceIdType.MESH
f32, bf16 = jnp.float32, jnp.bfloat16


def rope_parts(rows_total):
    quarter = HEAD // 4
    steps = np.arange(quarter, dtype=np.float32) * np.float32(2.0) / np.float32(HEAD // 2)
    freqs = (np.float32(1.0) / np.float32(rope_base) ** steps).astype(np.float32)

    def table(count, first):
        angle = np.arange(count, dtype=np.float32)[:, None] * freqs
        twice = np.concatenate([angle, angle], axis=1).astype(np.float64)
        none = np.zeros_like(twice)
        made = []
        for part in (np.cos(twice), np.sin(twice)):
            head = [part, none] if first else [none, part]
            made.append(np.concatenate(head + head, axis=1).astype(np.float32))
        return made

    return table(rows_total // GRID_W, True) + table(GRID_W, False)


def ring_place(index, count, across):
    deep = count // across
    if across == 1 or deep % 2:
        return index
    z, x = index // across, index % across
    turn = deep - 1 - z
    inner = jnp.where(turn % 2 == 0, x - 1, across - 1 - x)
    return jnp.where(x == 0, z, deep + turn * (across - 1) + inner)


def ring_index(place, count, across):
    deep = count // across
    if across == 1 or deep % 2:
        return place
    rest = jnp.maximum(place - deep, 0)
    turn, inner = rest // (across - 1), rest % (across - 1)
    x = jnp.where(turn % 2 == 0, inner + 1, across - 1 - inner)
    return jnp.where(place < deep, place * across, (deep - 1 - turn) * across + x)


def norm_rope(raw, gain, cosine, sine, low_half, lead):
    squares = raw * raw
    low_sum = jnp.sum(jnp.where(low_half, squares, 0.0), axis=1, keepdims=True)
    high_sum = jnp.sum(jnp.where(low_half, 0.0, squares), axis=1, keepdims=True)
    mean = jnp.where(low_half, low_sum, high_sum) * (1.0 / HEAD)
    scaled = raw * lax.rsqrt(mean + eps) * gain
    turned = jnp.where(
        lead,
        -pltpu.roll(scaled, 2 * HEAD - HEAD // 4, 1),
        pltpu.roll(scaled, HEAD // 4, 1),
    )
    return scaled * cosine + turned * sine


def layer_kernel(
    count,
    members,
    tokens,
    wq,
    wk,
    wv,
    wp,
    wop,
    woa,
    norm_gain,
    query_gain,
    key_gain,
    row_cos,
    row_sin,
    col_cos,
    col_sin,
    sink,
    out,
    tok,
    normed,
    w_side,
    w_query,
    w_out,
    side,
    query,
    band,
    pool_band,
    cosines,
    sines,
    mixer,
    away,
    met,
    kept,
    y_send,
    y_recv,
    done,
    load_sem,
    side_send,
    side_recv,
    query_send,
    query_recv,
    out_send,
    out_recv,
    ty_send,
    ty_recv,
    td_send,
    td_recv,
    halo_send,
    halo_recv,
    met_send,
    met_recv,
    yy_send,
    yy_recv,
    done_sem,
):
    rows, features = tokens.shape
    depth, kw = wk.shape
    qw, pw, width = wq.shape[1], wp.shape[1], wop.shape[1]
    chips = members // 2
    share = rows // members
    half = (count - 1) // 2
    heads_k = kw // HEAD
    seq = count * rows
    across = chips

    me, tp = lax.axis_index("sp"), lax.axis_index("tp")
    chip, core = tp // 2, tp % 2
    partner = chip * 2 + 1 - core
    place = ring_place(me, count, across)
    owner_of = lambda spot: ring_index(spot, count, across)
    at = lambda offset: (place + offset + count) % count
    following, previous = owner_of(at(1)), owner_of(at(-1))

    loads = [
        pltpu.make_async_copy(wk, w_side.at[place, :, pl.ds(0, kw)], load_sem.at[0]),
        pltpu.make_async_copy(wv, w_side.at[place, :, pl.ds(kw, kw)], load_sem.at[1]),
        pltpu.make_async_copy(wp, w_side.at[place, :, pl.ds(2 * kw, pw)], load_sem.at[2]),
        pltpu.make_async_copy(tokens, tok.at[tp], load_sem.at[3]),
        pltpu.make_async_copy(wq, w_query.at[place], load_sem.at[4]),
        pltpu.make_async_copy(wop, w_out.at[place, pl.ds(0, pw), :], load_sem.at[5]),
        pltpu.make_async_copy(woa, w_out.at[place, pl.ds(pw, qw), :], load_sem.at[6]),
    ]
    for load in loads:
        load.start()

    barrier = pltpu.get_barrier_semaphore()
    greeted = [
        (following, tp),
        (previous, tp),
        (me, partner),
        ((me + 1) % count, tp),
        ((me + count - 1) % count, tp),
    ]
    greeted += [(me, (chip + hop) % chips * 2 + core) for hop in range(1, chips)]
    for device in greeted:
        pl.semaphore_signal(barrier, inc=1, device_id=device, device_id_type=MESH)
    pl.semaphore_wait(barrier, len(greeted))

    def remote(source, target, send_sem, recv_sem, device):
        return pltpu.make_async_remote_copy(
            src_ref=source,
            dst_ref=target,
            send_sem=send_sem,
            recv_sem=recv_sem,
            device_id=device,
            device_id_type=MESH,
        )

    def hop_copy(ring, way, spot, c):
        buffer, send_sem, recv_sem = ring
        size = buffer.shape[1] // chunks
        part = buffer.at[spot, pl.ds(pl.multiple_of(c * size, 16), size), :]
        device = (following if way == 0 else previous, tp)
        return remote(part, part, send_sem.at[way, spot, c], recv_sem.at[spot, c], device)

    def send_own(ring):
        for c in range(chunks):
            hop_copy(ring, 0, place, c).start()
            hop_copy(ring, 1, place, c).start()

    def event(ring, step, c):
        low, high = at(-step), at(step)
        hop_copy(ring, 0, low, c).wait_recv()

        @pl.when((step < half) | (c < chunks // 2))
        def _():
            hop_copy(ring, 0, low, c).start()

        hop_copy(ring, 1, high, c).wait_recv()

        @pl.when((step < half) | (c >= chunks // 2))
        def _():
            hop_copy(ring, 1, high, c).start()

    def events(ring, step):
        def body(c, carry):
            event(ring, step, c)
            return carry

        lax.fori_loop(0, chunks, body, 0)

    def opposite(ring):
        def body(c, carry):
            hop_copy(ring, 0, at(count // 2), c).wait_recv()
            return carry

        lax.fori_loop(0, chunks, body, 0)

    def sends_done(ring):
        def each(c, carry):
            hop_copy(ring, 0, place, c).wait_send()
            hop_copy(ring, 1, place, c).wait_send()

            def steps(step, inner):
                @pl.when((step < half) | (c < chunks // 2))
                def _():
                    hop_copy(ring, 0, at(-step), c).wait_send()

                @pl.when((step < half) | (c >= chunks // 2))
                def _():
                    hop_copy(ring, 1, at(step), c).wait_send()

                return inner

            return lax.fori_loop(1, half + 1, steps, carry)

        lax.fori_loop(0, chunks, each, 0)

    side_ring = (w_side, side_send, side_recv)
    query_ring = (w_query, query_send, query_recv)
    out_ring = (w_out, out_send, out_recv)

    for load in loads[:3]:
        load.wait()
    send_own(side_ring)
    loads[3].wait()

    token_rows = rows // token_chunks

    def token_part(owner, j):
        return tok.at[owner, pl.ds(pl.multiple_of(j * token_rows, 16), token_rows), :]

    def token_far(hop, owner, j):
        part = token_part(owner, j)
        target = (chip + hop) % chips * 2 + core
        return remote(
            part, part, ty_send.at[hop - 1, j], ty_recv.at[hop - 1, j], (me, target)
        )

    def token_near(slot, owner, j):
        part = token_part(owner, j)
        return remote(part, part, td_send.at[slot, j], td_recv.at[slot, j], (me, partner))

    def start_tokens(j, carry):
        for hop in range(1, chips):
            token_far(hop, tp, j).start()
        token_near(0, tp, j).start()
        return carry

    lax.fori_loop(0, token_chunks, start_tokens, 0)

    for g in range(rows // GRID_W):
        spot = pl.ds(me * (rows // GRID_W) + g, 1)
        grid_rows = pl.ds(g * GRID_W, GRID_W)
        cosines[grid_rows, :] = col_cos[...] + row_cos[spot, :]
        sines[grid_rows, :] = col_sin[...] + row_sin[spot, :]

    pieces = features // depth
    norm_rows = 32 if token_rows % 32 == 0 else 16

    def normalise(j):
        token_near(0, partner, j).wait_recv()
        for hop in range(1, chips):
            token_near(hop, (chip - hop + chips) % chips * 2 + 1 - core, j).wait_recv()

        def tile(i, carry):
            at_rows = pl.ds(pl.multiple_of(j * token_rows + i * norm_rows, 16), norm_rows)
            squares = jnp.zeros((norm_rows, 1), f32)
            for t in range(members):
                block = tok[t, at_rows, :].astype(f32)
                squares = squares + jnp.sum(block * block, axis=1, keepdims=True)
            scale = lax.rsqrt(squares / (members * features) + eps)
            for t in range(members):
                for piece in range(pieces):
                    first = piece * depth
                    gain = norm_gain[:, t * features + first : t * features + first + depth]
                    block = tok[t, at_rows, first : first + depth].astype(f32)
                    normed[t * pieces + piece, at_rows, :] = (block * scale * gain).astype(bf16)
            return carry

        lax.fori_loop(0, token_rows // norm_rows, tile, 0)

    def token_step(j, carry):
        for hop in range(1, chips):
            source = (chip - hop + chips) % chips * 2 + core
            token_far(hop, source, j).wait_recv()
            token_near(hop, source, j).start()

        @pl.when(j < half * chunks)
        def _():
            event(side_ring, j // chunks + 1, j % chunks)

        @pl.when(j >= 1)
        def _():
            normalise(j - 1)

        return carry

    lax.fori_loop(0, token_chunks, token_step, 0)
    normalise(token_chunks - 1)

    tile_rows = 256 if rows % 256 == 0 else 128

    def project(total, weights, spots, first=False):
        def body(i, carry):
            part = pl.ds(pl.multiple_of(i * tile_rows, tile_rows), tile_rows)
            terms = [
                jnp.dot(
                    normed[owner_of(spot), part, :], weights[spot], preferred_element_type=f32
                )
                for spot in spots
            ]
            value = functools.reduce(lambda a, b: a + b, terms)
            total[part, :] = value if first else total[part, :] + value
            return carry

        lax.fori_loop(0, rows // tile_rows, body, 0)

    project(side, w_side, [place], first=True)
    early = token_chunks // chunks

    def side_step(step, carry):
        @pl.when(step > early)
        def _():
            events(side_ring, step)

        project(side, w_side, [at(-step), at(step)])
        return carry

    lax.fori_loop(1, half + 1, side_step, 0)
    loads[4].wait()
    send_own(query_ring)
    opposite(side_ring)
    project(side, w_side, [at(count // 2)])

    twice = lambda gain: jnp.concatenate([gain[...], gain[...]], axis=1)
    query_gains, key_gains = twice(query_gain), twice(key_gain)
    lane = lax.broadcasted_iota(jnp.int32, (WINDOW, 2 * HEAD), 1)
    low_half = lane < HEAD
    lead = lane % (HEAD // 2) < HEAD // 4

    def prepare(i, carry):
        part = pl.ds(pl.multiple_of(i * WINDOW, WINDOW), WINDOW)
        shifted = pl.ds(pl.multiple_of((i + 1) * WINDOW, WINDOW), WINDOW)
        for h in range(kw // (2 * HEAD)):
            lanes = slice(h * 2 * HEAD, (h + 1) * 2 * HEAD)
            key = norm_rope(
                side[part, lanes], key_gains, cosines[part, :], sines[part, :], low_half, lead
            )
            band[shifted, lanes] = key.astype(bf16)
        band[shifted, kw : 2 * kw] = side[part, kw : 2 * kw].astype(bf16)
        pooled_rows = pl.ds(pl.multiple_of(i * WINDOW + pool_pad, pool_pad), WINDOW)
        pool_band[pooled_rows, :] = side[part, 2 * kw :].astype(bf16)
        return carry

    lax.fori_loop(0, rows // WINDOW, prepare, 0)

    before, behind = (me + count - 1) % count, (me + 1) % count

    def halo(index, buffer, size, upwards):
        if upwards:
            source, target, device = rows, 0, (behind, tp)
        else:
            source, target, device = size, rows + size, (before, tp)
        return remote(
            buffer.at[pl.ds(source, size), :],
            buffer.at[pl.ds(target, size), :],
            halo_send.at[index],
            halo_recv.at[index],
            device,
        )

    lower = [halo(0, band, WINDOW, False), halo(1, pool_band, pool_pad, False)]
    upper = [halo(2, band, WINDOW, True), halo(3, pool_band, pool_pad, True)]
    has_lower, has_upper = me > 0, me < count - 1

    @pl.when(has_lower)
    def _():
        for copy in lower:
            copy.start()

    @pl.when(has_upper)
    def _():
        for copy in upper:
            copy.start()

    @pl.when(jnp.logical_not(has_lower))
    def _():
        band[0:WINDOW, :] = jnp.zeros((WINDOW, 2 * kw), bf16)
        pool_band[0:pool_pad, :] = jnp.zeros((pool_pad, pw), bf16)

    @pl.when(jnp.logical_not(has_upper))
    def _():
        band[rows + WINDOW :, :] = jnp.zeros((WINDOW, 2 * kw), bf16)
        pool_band[rows + pool_pad :, :] = jnp.zeros((pool_pad, pw), bf16)

    project(query, w_query, [place], first=True)

    def query_step(step, carry):
        events(query_ring, step)
        project(query, w_query, [at(-step), at(step)])
        return carry

    lax.fori_loop(1, half + 1, query_step, 0)
    loads[5].wait()
    loads[6].wait()
    send_own(out_ring)

    @pl.when(has_lower)
    def _():
        for copy in upper:
            copy.wait_recv()

    @pl.when(has_upper)
    def _():
        for copy in lower:
            copy.wait_recv()

    level = tp * pw // (POOL // 4)
    reach = jnp.where(level == 0, 1, jnp.where(level == 1, 2, jnp.where(level == 2, 4, 8)))

    def pool(i, carry):
        wide = WINDOW + 2 * pool_pad
        part = pl.ds(pl.multiple_of(i * WINDOW, WINDOW), WINDOW)
        values = pool_band[pl.ds(pl.multiple_of(i * WINDOW, pool_pad), wide), :].astype(f32)
        total, chosen = values, None
        for step in range(4):
            size = 2**step
            total = total + pltpu.roll(total, wide - size, 0)
            shifted = pltpu.roll(total, size, 0)[pool_pad : pool_pad + WINDOW]
            chosen = shifted if chosen is None else jnp.where(level == step, shifted, chosen)
        spot = me * rows + i * WINDOW + lax.broadcasted_iota(jnp.int32, (WINDOW, 1), 0)
        low = jnp.maximum(spot - reach, 0)
        high = jnp.minimum(spot + reach - 1, seq - 1)
        mixer[part, 0:pw] = (chosen / (high - low + 1).astype(f32)).astype(bf16)
        return carry

    lax.fori_loop(0, rows // WINDOW, pool, 0)

    opposite(query_ring)
    project(query, w_query, [at(count // 2)])

    blocks = rows // WINDOW
    row = lax.broadcasted_iota(jnp.int32, (2 * WINDOW, 3 * WINDOW), 0) % WINDOW
    column = lax.broadcasted_iota(jnp.int32, (2 * WINDOW, 3 * WINDOW), 1)
    top_row = lax.broadcasted_iota(jnp.int32, (2 * WINDOW, 1), 0) < WINDOW

    def attend(i, carry):
        part = pl.ds(pl.multiple_of(i * WINDOW, WINDOW), WINDOW)
        key_rows = pl.ds(pl.multiple_of(i * WINDOW, WINDOW), 3 * WINDOW)
        key_pos = me * rows + i * WINDOW - WINDOW + column
        inside = (column >= row) & (column - row <= 2 * WINDOW) & (key_pos >= 0) & (key_pos < seq)
        for head in range(heads_k):
            lanes = slice(head * 2 * HEAD, (head + 1) * 2 * HEAD)
            rotated = norm_rope(
                query[part, lanes],
                query_gains,
                cosines[part, :],
                sines[part, :],
                low_half,
                lead,
            ) * HEAD ** (-0.5)
            other = pltpu.roll(rotated, HEAD, 1)
            if head % 2 == 0:
                pair = (jnp.where(low_half, rotated, 0.0), jnp.where(low_half, other, 0.0))
            else:
                pair = (jnp.where(low_half, 0.0, other), jnp.where(low_half, 0.0, rotated))
            stacked = jnp.concatenate(pair, axis=0).astype(bf16)
            tile = head // 2 * 2 * HEAD
            keys = band[key_rows, tile : tile + 2 * HEAD]
            values = band[key_rows, kw + tile : kw + tile + 2 * HEAD]
            scores = lax.dot_general(
                stacked, keys, (((1,), (1,)), ((), ())), preferred_element_type=f32
            )
            scores = jnp.where(inside, scores, neg_big)
            limit = jnp.where(top_row, sink[2 * head], sink[2 * head + 1])
            top = jnp.maximum(jnp.max(scores, axis=1, keepdims=True), limit)
            raised = jnp.exp(scores - top)
            totals = jnp.sum(raised, axis=1, keepdims=True) + jnp.exp(limit - top)
            weights = (raised * (1.0 / totals)).astype(bf16)
            result = jnp.dot(weights, values, preferred_element_type=f32)
            one, two = result[:WINDOW], result[WINDOW:]
            if head % 2 == 0:
                joined = jnp.where(low_half, one, pltpu.roll(two, HEAD, 1))
            else:
                joined = jnp.where(low_half, pltpu.roll(one, HEAD, 1), two)
            mixer[part, pw + head * 2 * HEAD : pw + (head + 1) * 2 * HEAD] = joined.astype(bf16)

        for c in range(chunks):

            @pl.when(i == ((c + 1) * blocks + chunks - 1) // chunks - 1)
            def _(c=c):
                event(out_ring, 1, c)

        return carry

    lax.fori_loop(0, blocks, attend, 0)

    def product(spot, which):
        left = jnp.concatenate(
            [
                mixer[pl.ds(pl.multiple_of((y * 2 + which) * share, 16), share), :]
                for y in range(chips)
            ],
            axis=0,
        )
        return jnp.dot(left, w_out[spot], preferred_element_type=f32).astype(bf16)

    def met_copy(spot):
        return remote(
            away.at[spot], met.at[spot], met_send.at[spot], met_recv.at[spot], (me, partner)
        )

    def y_copy(spot, hop):
        target = (chip + hop) % chips * 2 + core
        return remote(
            y_send.at[spot, hop - 1],
            y_recv.at[spot, hop - 1],
            yy_send.at[spot, hop - 1],
            yy_recv.at[spot, hop - 1],
            (me, target),
        )

    def done_copy(spot):
        columns = pl.ds(pl.multiple_of(owner_of(spot) * width, width), width)
        return pltpu.make_async_copy(done.at[spot], out.at[:, columns], done_sem.at[spot])

    def both_rows(spot, y):
        part = pl.ds(pl.multiple_of(y * share, 16), share)
        return kept[spot, part, :].astype(f32) + met[spot, part, :].astype(f32)

    def group(spots):
        def first(spot):
            away[spot] = product(spot, 1 - core)
            met_copy(spot).start()

        def second(spot):
            kept[spot] = product(spot, core)

        def third(spot):
            met_copy(spot).wait_recv()
            for hop in range(1, chips):
                y_send[spot, hop - 1] = both_rows(spot, (chip + hop) % chips).astype(bf16)
                y_copy(spot, hop).start()

        for part in (first, second, third):
            for spot in spots:
                part(spot)

    def finish(spot):
        total = both_rows(spot, chip)
        for hop in range(1, chips):
            y_copy(spot, hop).wait_recv()
            total = total + y_recv[spot, hop - 1].astype(f32)
        done[spot] = total.astype(bf16)
        done_copy(spot).start()

    group([place])

    def out_step(step, carry):
        @pl.when(step > 1)
        def _():
            events(out_ring, step)

        group([at(-step), at(step)])

        @pl.when(step == 1)
        def _():
            finish(place)

        @pl.when(step > 1)
        def _():
            finish(at(1 - step))
            finish(at(step - 1))

        return carry

    lax.fori_loop(1, half + 1, out_step, 0)
    opposite(out_ring)
    group([at(count // 2)])
    finish(at(-half))
    finish(at(half))
    finish(at(count // 2))

    for ring in (side_ring, query_ring, out_ring):
        sends_done(ring)

    def tokens_sent(j, carry):
        token_near(0, tp, j).wait_send()
        for hop in range(1, chips):
            token_far(hop, tp, j).wait_send()
            token_near(hop, (chip - hop + chips) % chips * 2 + core, j).wait_send()
        return carry

    lax.fori_loop(0, token_chunks, tokens_sent, 0)

    @pl.when(has_lower)
    def _():
        for copy in lower:
            copy.wait_send()

    @pl.when(has_upper)
    def _():
        for copy in upper:
            copy.wait_send()

    def blocks_sent(spot, carry):
        met_copy(spot).wait_send()
        for hop in range(1, chips):
            y_copy(spot, hop).wait_send()
        done_copy(spot).wait()
        return carry

    lax.fori_loop(0, count, blocks_sent, 0)


def plane_kernel(
    count,
    members,
    tokens,
    wq,
    wk,
    wv,
    wp,
    wop,
    woa,
    norm_gain,
    query_gain,
    key_gain,
    row_cos,
    row_sin,
    col_cos,
    col_sin,
    sink,
    out,
    raw,
    sums,
    normed,
    w_in,
    w_pool,
    w_out,
    in_spare,
    pool_spare,
    out_spare,
    total,
    band,
    pool_band,
    cosines,
    sines,
    attended,
    pooled,
    result,
    rounded,
    load_sem,
    sum_send,
    sum_recv,
    in_sems,
    pool_sems,
    out_sems,
    x_sems,
    spread_sems,
    token_sems,
    attend_sems,
    pooled_sems,
    halo_send,
    halo_recv,
    result_send,
    result_recv,
):
    rows, features = tokens.shape
    depth = wk.shape[0]
    hk, hq, hp = wk.shape[1] // 2, wq.shape[1] // 2, wp.shape[1] // 2
    width = wop.shape[1]
    narrow = width // members
    share = rows // members
    plane = 2 * rows
    heads_k = hk // HEAD
    seq = count * rows
    deep = count // 2
    pieces = features // depth
    tiles = rows // WINDOW

    me, tp = lax.axis_index("sp"), lax.axis_index("tp")
    z, x = me // 2, me % 2
    y, core = tp // 2, tp % 2
    me_x, tp_y, tp_c = me + 1 - 2 * x, (1 - y) * 2 + core, y * 2 + 1 - core
    tp_yc = (1 - y) * 2 + 1 - core
    up, down = (me + 2) % count, (me + count - 2) % count
    has_up, has_down = z < deep - 1, z > 0
    inner = has_up & has_down

    mine = lambda size: pl.ds(pl.multiple_of(x * size, 128), size)
    other = lambda size: pl.ds(pl.multiple_of((1 - x) * size, 128), size)
    loads = []

    def load(source, target):
        loads.append(pltpu.make_async_copy(source, target, load_sem.at[len(loads)]))
        loads[-1].start()

    for target, pick in ((w_in.at[me], mine), (in_spare, other)):
        load(wk.at[:, pick(hk)], target.at[:, pl.ds(0, hk)])
        load(wv.at[:, pick(hk)], target.at[:, pl.ds(hk, hk)])
        load(wq.at[:, pick(hq)], target.at[:, pl.ds(2 * hk, hq)])
    load(tokens, raw)
    for target, pick in ((w_pool.at[me], mine), (pool_spare, other)):
        load(wp.at[:, pick(hp)], target)
    strip = lambda t: pl.ds(pl.multiple_of(t * narrow, narrow), narrow)
    for target, t in [(w_out.at[z, tp], tp)] + [(out_spare.at[t], t) for t in range(members)]:
        load(woa.at[:, strip(t)], target.at[pl.ds(0, 2 * hq), :])
        load(wop.at[:, strip(t)], target.at[pl.ds(2 * hq, 2 * hp), :])

    barrier = pltpu.get_barrier_semaphore()
    greeted = [(up, tp), (down, tp), (me_x, tp)]
    for t in (tp_y, tp_c, tp_yc):
        greeted += [(me, t), (me_x, t)]
    for device in greeted:
        pl.semaphore_signal(barrier, inc=1, device_id=device, device_id_type=MESH)
    pl.semaphore_wait(barrier, len(greeted))

    def remote(source, target, send_sem, recv_sem, device):
        return pltpu.make_async_remote_copy(
            src_ref=source,
            dst_ref=target,
            send_sem=send_sem,
            recv_sem=recv_sem,
            device_id=device,
            device_id_type=MESH,
        )

    def by_rows(parts):
        def view(buffer, c):
            size = buffer.shape[0] // parts
            return buffer.at[pl.ds(pl.multiple_of(c * size, 16), size), :]

        return view

    in_ring = (w_in, in_spare, in_sems, 0, in_parts, by_rows(in_parts))
    pool_ring = (w_pool, pool_spare, pool_sems, in_parts, 1, by_rows(1))
    def z_copy(ring, way, source, c):
        buffer, _, sems, _, _, view = ring
        part = view(buffer.at[source], c)
        return remote(
            part, part, sems.at[way, source, c], sems.at[2, source, c], ((up, down)[way], tp)
        )

    def x_copy(ring, source, c):
        buffer, spare, sems, first, _, view = ring
        return remote(
            view(spare, c),
            view(buffer.at[source], c),
            x_sems.at[first + c],
            sems.at[2, source, c],
            (me_x, tp),
        )

    def both_ways(ring, source, c, act):
        @pl.when(has_up)
        def _():
            act(z_copy(ring, 0, source, c))

        @pl.when(has_down)
        def _():
            act(z_copy(ring, 1, source, c))

    start = lambda copy: copy.start()
    sent = lambda copy: copy.wait_send()

    def own_out(ring):
        for c in range(ring[4]):
            both_ways(ring, me, c, start)

    def side_out(ring):
        for c in range(ring[4]):
            x_copy(ring, me, c).start()

    def side_in(ring):
        for c in range(ring[4]):
            x_copy(ring, me_x, c).wait_recv()
            both_ways(ring, me_x, c, start)

    def passing(ring, n):
        parts = ring[4]
        step, j, c = n // (2 * parts) + 1, n // parts % 2, n % parts
        column = (x + j) % 2
        low, high = z - step, z + step
        return (low >= 0, low * 2 + column), (high < deep, high * 2 + column), c

    def event(ring, n):
        (is_low, low), (is_high, high), c = passing(ring, n)

        @pl.when(is_low)
        def _():
            z_copy(ring, 0, low, c).wait_recv()

            @pl.when(has_up)
            def _():
                z_copy(ring, 0, low, c).start()

        @pl.when(is_high)
        def _():
            z_copy(ring, 1, high, c).wait_recv()

            @pl.when(has_down)
            def _():
                z_copy(ring, 1, high, c).start()

    def events(ring, first, last):
        def body(n, carry):
            event(ring, n)
            return carry

        lax.fori_loop(first, last, body, 0)

    def all_events(ring):
        return (deep - 1) * 2 * ring[4]

    def sends_done(ring):
        for c in range(ring[4]):
            both_ways(ring, me, c, sent)
            both_ways(ring, me_x, c, sent)
            x_copy(ring, me, c).wait_send()

        def body(n, carry):
            (is_low, low), (is_high, high), c = passing(ring, n)

            @pl.when(is_low & has_up)
            def _():
                z_copy(ring, 0, low, c).wait_send()

            @pl.when(is_high & has_down)
            def _():
                z_copy(ring, 1, high, c).wait_send()

            return carry

        lax.fori_loop(0, all_events(ring), body, 0)

    def out_copy(way, level, c):
        part = w_out.at[level, (tp - c + members) % members]
        device = ((up, down)[way], tp)
        return remote(part, part, out_sems.at[way, level, c], out_sems.at[2, level, c], device)

    def spread(c):
        target = (tp + c) % members
        return remote(
            out_spare.at[target],
            w_out.at[z, tp],
            spread_sems.at[c],
            out_sems.at[2, z, c],
            (me, target),
        )

    def spread_in(c):
        owner = (tp - c + members) % members
        return remote(
            out_spare.at[owner],
            w_out.at[z, owner],
            spread_sems.at[c],
            out_sems.at[2, z, c],
            (me, owner),
        )

    def out_both(c, act):
        @pl.when(has_up)
        def _():
            act(out_copy(0, z, c))

        @pl.when(has_down)
        def _():
            act(out_copy(1, z, c))

    def out_event(n):
        step, c = n // members + 1, n % members
        low, high = z - step, z + step

        @pl.when(low >= 0)
        def _():
            out_copy(0, low, c).wait_recv()

            @pl.when(has_up)
            def _():
                out_copy(0, low, c).start()

        @pl.when(high < deep)
        def _():
            out_copy(1, high, c).wait_recv()

            @pl.when(has_down)
            def _():
                out_copy(1, high, c).start()

    def out_events(first, last):
        def body(n, carry):
            out_event(n)
            return carry

        lax.fori_loop(first, last, body, 0)

    def out_sent(n, carry):
        step, c = n // members + 1, n % members
        low, high = z - step, z + step

        @pl.when((low >= 0) & has_up)
        def _():
            out_copy(0, low, c).wait_send()

        @pl.when((high < deep) & has_down)
        def _():
            out_copy(1, high, c).wait_send()

        return carry

    for copy in loads[:6]:
        copy.wait()
    for c in range(in_parts):
        x_copy(in_ring, me, c).start()
        both_ways(in_ring, me, c, start)

    loads[6].wait()
    sums[tp] = jnp.zeros_like(sums[tp])
    for i in range(tiles):
        block = raw[i * WINDOW : (i + 1) * WINDOW, :].astype(f32)
        square = jnp.sum(block * block, axis=1, keepdims=True)
        turned = jnp.transpose(jnp.broadcast_to(square, (WINDOW, WINDOW)))
        sums[tp, i : i + 1, :] = turned[0:1, :]

    def sum_copy(owner, hop):
        target = (tp + hop) % members
        return remote(
            sums.at[owner],
            sums.at[owner],
            sum_send.at[hop - 1],
            sum_recv.at[hop - 1],
            (me, target),
        )

    for hop in range(1, members):
        sum_copy(tp, hop).start()
    for g in range(plane // GRID_W):
        spot = pl.ds(z * (plane // GRID_W) + g, 1)
        grid_rows = pl.ds(g * GRID_W, GRID_W)
        cosines[grid_rows, :] = col_cos[...] + row_cos[spot, :]
        sines[grid_rows, :] = col_sin[...] + row_sin[spot, :]
    for hop in range(1, members):
        sum_copy((tp - hop + members) % members, hop).wait_recv()
    squares = sums[0]
    for t in range(1, members):
        squares = squares + sums[t]
    scales = lax.rsqrt(squares / (members * features) + eps)

    class Stream:
        def __init__(self, view, sems, by_x):
            self.view, self.sems, self.by_x = view, sems, by_x

        def copy(self, base, count_of, slot, side, owner, j, device):
            part = self.view(side, owner, j)
            send, recv = self.sems.at[base + slot, j], self.sems.at[base + count_of + slot, j]
            return remote(part, part, send, recv, device)

        def over_x(self, slot, side, owner, j):
            return self.copy(0, 2, slot, side, owner, j, (me_x, tp))

        def over_y(self, slot, side, owner, j):
            return self.copy(4, 2, slot, side, owner, j, (me, tp_y))

        def over_core(self, slot, side, owner, j):
            return self.copy(8, 4, slot, side, owner, j, (me, tp_c))

        def start(self, j):
            self.over_y(0, x, tp, j).start()
            self.over_x(0, x, tp, j).start()
            self.over_core(0, x, tp, j).start()

        def direct(self, j):
            self.over_y(0, x, tp_y, j).wait_recv()
            self.over_core(2, x, tp_y, j).start()

            @pl.when(self.by_x(j))
            def _():
                self.over_x(1, x, tp_y, j).start()

            self.over_x(0, 1 - x, tp, j).wait_recv()
            self.over_core(1, 1 - x, tp, j).start()

            @pl.when(jnp.logical_not(self.by_x(j)))
            def _():
                self.over_y(1, 1 - x, tp, j).start()

        def crossed(self, j):
            @pl.when(self.by_x(j))
            def _():
                self.over_x(1, 1 - x, tp_y, j).wait_recv()

            @pl.when(jnp.logical_not(self.by_x(j)))
            def _():
                self.over_y(1, 1 - x, tp_y, j).wait_recv()

            self.over_core(3, 1 - x, tp_y, j).start()

        def near_side(self, j):
            self.over_core(0, x, tp_c, j).wait_recv()
            self.over_core(2, x, tp_yc, j).wait_recv()

        def far_side(self, j):
            self.over_core(1, 1 - x, tp_c, j).wait_recv()
            self.over_core(3, 1 - x, tp_yc, j).wait_recv()

        def sent(self, j):
            self.over_y(0, x, tp, j).wait_send()
            self.over_x(0, x, tp, j).wait_send()
            self.over_core(0, x, tp, j).wait_send()
            self.over_core(1, 1 - x, tp, j).wait_send()
            self.over_core(2, x, tp_y, j).wait_send()
            self.over_core(3, 1 - x, tp_y, j).wait_send()

            @pl.when(self.by_x(j))
            def _():
                self.over_x(1, x, tp_y, j).wait_send()

            @pl.when(jnp.logical_not(self.by_x(j)))
            def _():
                self.over_y(1, 1 - x, tp, j).wait_send()

        def every(self, act):
            def body(j, carry):
                act(j)
                return carry

            lax.fori_loop(0, self.sems.shape[1], body, 0)

    def block_rows(j, size):
        return pl.ds(pl.multiple_of(j * size, 16), size)

    def token_view(side, owner, j):
        return normed.at[side, pl.ds(owner * pieces, pieces), block_rows(j, WINDOW), :]

    def attend_view(side, owner, j):
        return attended.at[owner, side, block_rows(j, WINDOW), :]

    def pooled_view(side, owner, j):
        return pooled.at[owner, side, block_rows(j, plane // pooled_parts), :]

    token_stream = Stream(token_view, token_sems, lambda j: j % 3 == 0)
    attend_stream = Stream(attend_view, attend_sems, lambda j: j % 2 == 0)
    pooled_stream = Stream(pooled_view, pooled_sems, lambda j: j % 2 == 0)

    gains = norm_gain[pl.ds(tp, 1), :]
    for i in range(tiles):
        here = slice(i * WINDOW, (i + 1) * WINDOW)
        scale = jnp.transpose(jnp.broadcast_to(scales[i : i + 1, :], (WINDOW, WINDOW)))
        for first in range(0, features, WINDOW):
            block = raw[here, first : first + WINDOW].astype(f32)
            value = (block * scale * gains[:, first : first + WINDOW]).astype(bf16)
            inside = first % depth
            normed[x, tp * pieces + first // depth, here, inside : inside + WINDOW] = value
        token_stream.start(i)

    side_in(in_ring)
    whole = all_events(in_ring)
    reached = lambda part: whole * part // 24
    events(in_ring, 0, reached(4))

    def direct(j, carry):
        token_stream.direct(j)
        events(in_ring, reached(4 + 12 * j // tiles), reached(4 + 12 * (j + 1) // tiles))
        return carry

    lax.fori_loop(0, tiles, direct, 0)
    for copy in loads[7:]:
        copy.wait()
    side_out(pool_ring)
    for c in range(1, members):
        spread(c).start()
    token_stream.every(token_stream.near_side)

    tile_rows = 256 if rows % 256 == 0 else 128
    per_side = rows // tile_rows

    def project(result, weights, level, side, first=False):
        def body(i, carry):
            within = pl.ds(pl.multiple_of(i * tile_rows, tile_rows), tile_rows)
            part = pl.ds(pl.multiple_of(side * rows + i * tile_rows, tile_rows), tile_rows)
            value = None if first else result[part, :]
            for j in range(2):
                term = jnp.dot(
                    normed[side, level * 2 + j, within, :],
                    weights[level * 2 + j],
                    preferred_element_type=f32,
                )
                value = term if value is None else value + term
            result[part, :] = value
            return carry

        lax.fori_loop(0, per_side, body, 0)

    def project_step(result, weights, step, side):
        @pl.when(z - step >= 0)
        def _():
            project(result, weights, z - step, side)

        @pl.when(z + step < deep)
        def _():
            project(result, weights, z + step, side)

    early = max(reached(16) // (2 * in_parts), 0)

    def crossed(j, carry):
        token_stream.crossed(j)

        @pl.when(j == 0)
        def _():
            project(total, w_in, z, x, first=True)

        @pl.when((j >= 1) & (j <= early))
        def _():
            project_step(total, w_in, j, x)

        events(in_ring, reached(16 + 4 * j // tiles), reached(16 + 4 * (j + 1) // tiles))
        return carry

    lax.fori_loop(0, tiles, crossed, 0)
    own_out(pool_ring)
    side_in(pool_ring)
    token_stream.every(token_stream.far_side)
    project(total, w_in, z, 1 - x, first=True)

    @pl.when(inner)
    def _():
        events(pool_ring, 0, 2)


    def in_step(step, carry):
        each = 2 * in_parts
        events(in_ring, jnp.maximum((step - 1) * each, reached(20)), step * each)

        @pl.when(step > min(early, tiles - 1))
        def _():
            project_step(total, w_in, step, x)

        project_step(total, w_in, step, 1 - x)
        return carry

    lax.fori_loop(1, deep, in_step, 0)

    twice = lambda gain: jnp.concatenate([gain[...], gain[...]], axis=1)
    query_gains, key_gains = twice(query_gain), twice(key_gain)
    lane = lax.broadcasted_iota(jnp.int32, (WINDOW, 2 * HEAD), 1)
    low_half = lane < HEAD
    lead = lane % (HEAD // 2) < HEAD // 4
    blocks = plane // WINDOW

    def prepare(i, carry):
        part = pl.ds(pl.multiple_of(i * WINDOW, WINDOW), WINDOW)
        shifted = pl.ds(pl.multiple_of((i + 1) * WINDOW, WINDOW), WINDOW)
        for h in range(hk // (2 * HEAD)):
            lanes = slice(h * 2 * HEAD, (h + 1) * 2 * HEAD)
            key = norm_rope(
                total[part, lanes], key_gains, cosines[part, :], sines[part, :], low_half, lead
            )
            band[shifted, lanes] = key.astype(bf16)
        band[shifted, hk:] = total[part, hk : 2 * hk].astype(bf16)
        return carry

    lax.fori_loop(0, blocks, prepare, 0)

    def halo(index, buffer, size, upwards):
        if upwards:
            source, target, device = plane, 0, (up, tp)
        else:
            source, target, device = size, plane + size, (down, tp)
        return remote(
            buffer.at[pl.ds(source, size), :],
            buffer.at[pl.ds(target, size), :],
            halo_send.at[index],
            halo_recv.at[index],
            device,
        )

    def halo_out(index, buffer, size):
        @pl.when(has_down)
        def _():
            halo(index, buffer, size, False).start()

        @pl.when(has_up)
        def _():
            halo(index + 1, buffer, size, True).start()

        empty = jnp.zeros((size, buffer.shape[1]), bf16)

        @pl.when(jnp.logical_not(has_down))
        def _():
            buffer[0:size, :] = empty

        @pl.when(jnp.logical_not(has_up))
        def _():
            buffer[plane + size :, :] = empty

    def halo_in(index, buffer, size):
        @pl.when(has_up)
        def _():
            halo(index, buffer, size, False).wait_recv()

        @pl.when(has_down)
        def _():
            halo(index + 1, buffer, size, True).wait_recv()

    halo_out(0, band, WINDOW)

    @pl.when(inner)
    def _():
        events(pool_ring, 2, all_events(pool_ring))

    for c in range(members - 1):
        if c > 0:
            spread_in(c).wait_recv()
        out_both(c, start)

    row = lax.broadcasted_iota(jnp.int32, (2 * WINDOW, 3 * WINDOW), 0) % WINDOW
    column = lax.broadcasted_iota(jnp.int32, (2 * WINDOW, 3 * WINDOW), 1)
    top_row = lax.broadcasted_iota(jnp.int32, (2 * WINDOW, 1), 0) < WINDOW

    def attend(turn, carry):
        @pl.when(turn == blocks - 2)
        def _():
            halo_in(0, band, WINDOW)

        i = (turn + 1) % blocks
        part = pl.ds(pl.multiple_of(i * WINDOW, WINDOW), WINDOW)
        key_rows = pl.ds(pl.multiple_of(i * WINDOW, WINDOW), 3 * WINDOW)
        key_pos = z * plane + i * WINDOW - WINDOW + column
        inside = (column >= row) & (column - row <= 2 * WINDOW) & (key_pos >= 0) & (key_pos < seq)
        for head in range(heads_k):
            lanes = slice(2 * hk + head * 2 * HEAD, 2 * hk + (head + 1) * 2 * HEAD)
            rotated = norm_rope(
                total[part, lanes],
                query_gains,
                cosines[part, :],
                sines[part, :],
                low_half,
                lead,
            ) * HEAD ** (-0.5)
            swapped = pltpu.roll(rotated, HEAD, 1)
            if head % 2 == 0:
                pair = (jnp.where(low_half, rotated, 0.0), jnp.where(low_half, swapped, 0.0))
            else:
                pair = (jnp.where(low_half, 0.0, swapped), jnp.where(low_half, 0.0, rotated))
            stacked = jnp.concatenate(pair, axis=0).astype(bf16)
            tile = head // 2 * 2 * HEAD
            keys = band[key_rows, tile : tile + 2 * HEAD]
            values = band[key_rows, hk + tile : hk + tile + 2 * HEAD]
            scores = lax.dot_general(
                stacked, keys, (((1,), (1,)), ((), ())), preferred_element_type=f32
            )
            scores = jnp.where(inside, scores, neg_big)
            first = x * 2 * heads_k + 2 * head
            limit = jnp.where(top_row, sink[first], sink[first + 1])
            top = jnp.maximum(jnp.max(scores, axis=1, keepdims=True), limit)
            raised = jnp.exp(scores - top)
            totals = jnp.sum(raised, axis=1, keepdims=True) + jnp.exp(limit - top)
            weights = (raised * (1.0 / totals)).astype(bf16)
            result = jnp.dot(weights, values, preferred_element_type=f32)
            one, two = result[:WINDOW], result[WINDOW:]
            if head % 2 == 0:
                joined = jnp.where(low_half, one, pltpu.roll(two, HEAD, 1))
            else:
                joined = jnp.where(low_half, pltpu.roll(one, HEAD, 1), two)
            attended[tp, x, part, head * 2 * HEAD : (head + 1) * 2 * HEAD] = joined.astype(bf16)
        attend_stream.start(i)

        @pl.when(turn >= behind)
        def _():
            attend_stream.direct((turn - behind + 1) % blocks)

        return carry

    behind = 5
    lax.fori_loop(0, blocks, attend, 0)

    events(pool_ring, jnp.where(inner, all_events(pool_ring), 0), all_events(pool_ring))

    for side in range(2):

        def pool_project(i, carry, side=side):
            part = pl.ds(pl.multiple_of(i * tile_rows, tile_rows), tile_rows)
            first = side * rows + pool_pad + i * tile_rows
            left = jnp.concatenate([normed[side, source, part, :] for source in range(count)], axis=1)
            right = w_pool[...].reshape(count * depth, hp)
            value = jnp.dot(left, right, preferred_element_type=f32)
            pool_band[pl.ds(pl.multiple_of(first, pool_pad), tile_rows), :] = value.astype(bf16)
            return carry

        lax.fori_loop(0, per_side, pool_project, 0)
    halo_out(2, pool_band, pool_pad)
    spread_in(members - 1).wait_recv()
    out_both(members - 1, start)

    @pl.when(inner)
    def _():
        out_events(0, members - 1)

    level = (tp * 2 + x) * hp // (POOL // 4)
    reach = jnp.where(level == 0, 1, jnp.where(level == 1, 2, jnp.where(level == 2, 4, 8)))

    def pool(i, carry):
        wide = WINDOW + 2 * pool_pad
        part = pl.ds(pl.multiple_of(i * WINDOW, WINDOW), WINDOW)
        running = pool_band[pl.ds(pl.multiple_of(i * WINDOW, pool_pad), wide), :].astype(f32)
        chosen = None
        for step in range(4):
            size = 2**step
            running = running + pltpu.roll(running, wide - size, 0)
            shifted = pltpu.roll(running, size, 0)[pool_pad : pool_pad + WINDOW]
            chosen = shifted if chosen is None else jnp.where(level == step, shifted, chosen)
        spot = z * plane + i * WINDOW + lax.broadcasted_iota(jnp.int32, (WINDOW, 1), 0)
        low = jnp.maximum(spot - reach, 0)
        high = jnp.minimum(spot + reach - 1, seq - 1)
        pooled[tp, x, part, :] = (chosen / (high - low + 1).astype(f32)).astype(bf16)
        return carry

    edge = blocks // pooled_parts
    lax.fori_loop(edge, blocks - edge, pool, 0)
    for part in range(1, pooled_parts - 1):
        pooled_stream.start(part)
    for turn in range(blocks - behind, blocks):
        attend_stream.direct((turn + 1) % blocks)
    halo_in(2, pool_band, pool_pad)
    lax.fori_loop(0, edge, pool, 0)
    lax.fori_loop(blocks - edge, blocks, pool, 0)
    pooled_stream.start(0)
    pooled_stream.start(pooled_parts - 1)

    @pl.when(inner)
    def _():
        out_events(members - 1, members)

    attend_stream.every(attend_stream.crossed)
    for stream_side in (attend_stream.near_side, attend_stream.far_side):
        attend_stream.every(stream_side)

    def level_of(group):
        paired = jnp.minimum(z, deep - 1 - z)
        step = jnp.where(group > 2 * paired, group - paired, (group + 1) // 2)
        downwards = jnp.where(group > 2 * paired, 2 * z > deep - 1, group % 2 == 1)
        return jnp.where(downwards, z - step, z + step)

    here = x * members + tp
    out_steps = (deep - 1) * members

    def columns_of(level, side, t):
        first = (level * 2 + side) * width + t * narrow
        return pl.ds(pl.multiple_of(first, narrow), narrow)

    def result_copy(level, hop):
        target = (here + hop) % (2 * members)
        return remote(
            rounded.at[level, pl.ds(pl.multiple_of(target * share, 16), share), :],
            out.at[:, columns_of(level, x, tp)],
            result_send.at[level, hop],
            result_recv.at[level, hop],
            (z * 2 + target // members, target % members),
        )

    def result_in(level, hop):
        source = (here - hop + 2 * members) % (2 * members)
        return remote(
            rounded.at[level, pl.ds(0, share), :],
            out.at[:, columns_of(level, source // members, source % members)],
            result_send.at[level, hop],
            result_recv.at[level, hop],
            (z * 2 + source // members, source % members),
        )

    def result_own(level):
        return pltpu.make_async_copy(
            rounded.at[level, pl.ds(pl.multiple_of(here * share, 16), share), :],
            out.at[:, columns_of(level, x, tp)],
            result_send.at[level, 0],
        )

    def send_level(level):
        for hop in range(1, 2 * members):
            result_copy(level, hop).start()
        result_own(level).start()

    span = 2 * tile_rows if plane % (2 * tile_rows) == 0 else tile_rows
    ends_event = lambda n: jnp.where(inner, out_steps, n)

    def end_events(first, last):
        out_events(ends_event(first), ends_event(last))

    def by_span(act):
        def body(i, carry):
            act(pl.ds(pl.multiple_of(i * span, span), span))
            return carry

        lax.fori_loop(0, plane // span, body, 0)

    all_blocks = [(t, h) for t in range(members) for h in range(2)]

    def attended_term(part, levels):
        left = jnp.concatenate([attended[t, h, part, :] for t, h in all_blocks], axis=1)
        right = jnp.concatenate(
            [
                jnp.concatenate([w_out[level, t, 0 : 2 * hq, :] for t in range(members)], axis=0)
                for level in levels
            ],
            axis=1,
        )
        return jnp.dot(left, right, preferred_element_type=f32)

    def pooled_term(part, levels):
        left = jnp.concatenate([pooled[t, h, part, :] for t, h in all_blocks], axis=1)
        right = jnp.concatenate(
            [
                jnp.concatenate([w_out[level, t, 2 * hq :, :] for t in range(members)], axis=0)
                for level in levels
            ],
            axis=1,
        )
        return jnp.dot(left, right, preferred_element_type=f32)

    firsts = (level_of(0), level_of(1))
    end_events(0, members)

    def first_attended(part):
        result[part, :] = attended_term(part, firsts)

    by_span(first_attended)

    inner_parts = list(range(1, pooled_parts - 1)) + [0, pooled_parts - 1]
    for part in inner_parts:
        pooled_stream.direct(part)

    @pl.when(inner)
    def _():
        out_events(members, out_steps)

    for part in inner_parts:
        pooled_stream.crossed(part)
    for stream_side in (pooled_stream.near_side, pooled_stream.far_side):
        pooled_stream.every(stream_side)

    def first_pooled(part):
        value = (result[part, :] + pooled_term(part, firsts)).astype(bf16)
        for index, level in enumerate(firsts):
            rounded[level, part, :] = value[:, index * narrow : (index + 1) * narrow]

    by_span(first_pooled)
    for level in firsts:
        send_level(level)

    def middle_level(group, carry):
        end_events((group - 1) * members, group * members)
        level = level_of(group)

        def whole_level(part):
            value = attended_term(part, [level]) + pooled_term(part, [level])
            rounded[level, part, :] = value.astype(bf16)

        by_span(whole_level)
        send_level(level)
        return carry

    lax.fori_loop(2, deep - 1, middle_level, 0)

    for ring in (in_ring, pool_ring):
        sends_done(ring)
    for c in range(members):
        out_both(c, sent)
    for c in range(1, members):
        spread(c).wait_send()
    for hop in range(1, members):
        sum_copy(tp, hop).wait_send()
    for stream in (token_stream, attend_stream, pooled_stream):
        stream.every(stream.sent)

    level = level_of(deep - 1)
    for c in range(members):
        n = (deep - 2) * members + c
        end_events(n, n + 1)
        t = (tp - c + members) % members

        def last_level(part, c=c, t=t):
            left = jnp.concatenate(
                [attended[t, h, part, :] for h in range(2)]
                + [pooled[t, h, part, :] for h in range(2)],
                axis=1,
            )
            value = jnp.dot(left, w_out[level, t], preferred_element_type=f32)
            if c > 0:
                value = result[part, 0:narrow] + value
            if c == members - 1:
                rounded[level, part, :] = value.astype(bf16)
            else:
                result[part, 0:narrow] = value

        by_span(last_level)
    send_level(level)

    def results(level, carry):
        for hop in range(1, 2 * members):
            result_in(level, hop).wait_recv()
        return carry

    lax.fori_loop(0, deep, results, 0)

    lax.fori_loop(0, out_steps, out_sent, 0)
    for index, buffer, size in ((0, band, WINDOW), (2, pool_band, pool_pad)):

        @pl.when(has_down)
        def _(index=index, buffer=buffer, size=size):
            halo(index, buffer, size, False).wait_send()

        @pl.when(has_up)
        def _(index=index, buffer=buffer, size=size):
            halo(index + 1, buffer, size, True).wait_send()

    def results_sent(level, carry):
        for hop in range(1, 2 * members):
            result_copy(level, hop).wait_send()
        result_own(level).wait()
        return carry

    lax.fori_loop(0, deep, results_sent, 0)


def plane_scratch(count, members, rows, features, depth, kw, qw, pw, width):
    hk, hq, hp = kw // 2, qw // 2, pw // 2
    narrow, plane, deep, tiles = width // members, 2 * rows, count // 2, rows // WINDOW
    dma = pltpu.SemaphoreType.DMA
    return [
        pltpu.VMEM((rows, features), bf16),
        pltpu.VMEM((members, -(-tiles // 8) * 8, WINDOW), f32),
        pltpu.VMEM((2, count, rows, depth), bf16),
        pltpu.VMEM((count, depth, 2 * hk + hq), bf16),
        pltpu.VMEM((count, depth, hp), bf16),
        pltpu.VMEM((deep, members, 2 * (hp + hq), narrow), bf16),
        pltpu.VMEM((depth, 2 * hk + hq), bf16),
        pltpu.VMEM((depth, hp), bf16),
        pltpu.VMEM((members, 2 * (hp + hq), narrow), bf16),
        pltpu.VMEM((plane, 2 * hk + hq), f32),
        pltpu.VMEM((plane + 2 * WINDOW, 2 * hk), bf16),
        pltpu.VMEM((plane + 2 * pool_pad, hp), bf16),
        pltpu.VMEM((plane, 2 * HEAD), f32),
        pltpu.VMEM((plane, 2 * HEAD), f32),
        pltpu.VMEM((members, 2, plane, hq), bf16),
        pltpu.VMEM((members, 2, plane, hp), bf16),
        pltpu.VMEM((plane, 2 * narrow), f32),
        pltpu.VMEM((deep, plane, narrow), bf16),
        dma((11 + 2 * members,)),
        dma((members - 1,)),
        dma((members - 1,)),
        dma((3, count, in_parts)),
        dma((3, count, 1)),
        dma((3, deep, members)),
        dma((in_parts + 1,)),
        dma((members,)),
        dma((16, tiles)),
        dma((16, 2 * tiles)),
        dma((16, pooled_parts)),
        dma((4,)),
        dma((4,)),
        dma((deep, 2 * members)),
        dma((deep, 2 * members)),
    ]


def ring_scratch(count, members, rows, features, depth, kw, qw, pw, width):
    chips, share = members // 2, rows // members
    far = max(chips - 1, 1)
    dma = pltpu.SemaphoreType.DMA
    return [
        pltpu.VMEM((members, rows, features), bf16),
        pltpu.VMEM((count, rows, depth), bf16),
        pltpu.VMEM((count, depth, 2 * kw + pw), bf16),
        pltpu.VMEM((count, depth, qw), bf16),
        pltpu.VMEM((count, pw + qw, width), bf16),
        pltpu.VMEM((rows, 2 * kw + pw), f32),
        pltpu.VMEM((rows, qw), f32),
        pltpu.VMEM((rows + 2 * WINDOW, 2 * kw), bf16),
        pltpu.VMEM((rows + 2 * pool_pad, pw), bf16),
        pltpu.VMEM((rows, 2 * HEAD), f32),
        pltpu.VMEM((rows, 2 * HEAD), f32),
        pltpu.VMEM((rows, pw + qw), bf16),
        pltpu.VMEM((count, chips * share, width), bf16),
        pltpu.VMEM((count, chips * share, width), bf16),
        pltpu.VMEM((count, chips * share, width), bf16),
        pltpu.VMEM((count, far, share, width), bf16),
        pltpu.VMEM((count, far, share, width), bf16),
        pltpu.VMEM((count, share, width), bf16),
        dma((7,)),
        dma((2, count, chunks)),
        dma((count, chunks)),
        dma((2, count, chunks)),
        dma((count, chunks)),
        dma((2, count, chunks)),
        dma((count, chunks)),
        dma((far, token_chunks)),
        dma((far, token_chunks)),
        dma((chips, token_chunks)),
        dma((chips, token_chunks)),
        dma((4,)),
        dma((4,)),
        dma((count,)),
        dma((count,)),
        dma((count, far)),
        dma((count, far)),
        dma((count,)),
    ]


def shards(
    tokens,
    norm_gain,
    w_query,
    w_key,
    w_value,
    w_pool,
    query_gain,
    key_gain,
    sink_logit,
    w_out_pool,
    w_out_attn,
):
    count, members = lax.axis_size("sp"), lax.axis_size("tp")
    rows, features = tokens.shape
    depth, kw = w_key.shape
    qw, pw, width = w_query.shape[1], w_pool.shape[1], w_out_pool.shape[1]
    tables = [jnp.asarray(table) for table in rope_parts(count * rows)]
    anywhere = pl.BlockSpec(memory_space=pl.ANY)
    in_vmem = pl.BlockSpec(memory_space=pltpu.VMEM)
    sizes = (count, members, rows, features, depth, kw, qw, pw, width)
    shared = (
        members == 4
        and count % 2 == 0
        and count >= 4
        and rows % (2 * WINDOW) == 0
        and depth % (16 * in_parts) == 0
        and all(size % 256 == 0 for size in (kw, qw, pw))
        and width % (128 * members) == 0
    )
    as_row = lambda gain: gain.reshape(1, HEAD)
    kernel, scratch = (plane_kernel, plane_scratch) if shared else (layer_kernel, ring_scratch)
    return pl.pallas_call(
        functools.partial(kernel, count, members),
        out_shape=jax.ShapeDtypeStruct((rows // members, count * width), bf16),
        in_specs=[anywhere] * 7 + [in_vmem] * 7 + [pl.BlockSpec(memory_space=pltpu.SMEM)],
        out_specs=anywhere,
        scratch_shapes=scratch(*sizes),
        compiler_params=pltpu.CompilerParams(
            collective_id=0, has_side_effects=True, vmem_limit_bytes=62 * 1024 * 1024
        ),
    )(
        tokens,
        w_query,
        w_key,
        w_value,
        w_pool,
        w_out_pool,
        w_out_attn,
        norm_gain.reshape(members, -1) if shared else norm_gain.reshape(1, -1),
        as_row(query_gain),
        as_row(key_gain),
        *tables,
        sink_logit,
    )


def solution(mesh):
    placed = (
        P("sp", "tp"),
        P(),
        P("sp", "tp"),
        P("sp", "tp"),
        P("sp", "tp"),
        P("sp", "tp"),
        P(),
        P(),
        P("tp"),
        P("tp", "sp"),
        P("tp", "sp"),
    )
    return jax.shard_map(
        shards, mesh=mesh, in_specs=placed, out_specs=P(("sp", "tp"), None), check_vma=False
    )
```

```python
import functools

import jax
import jax.numpy as jnp
import numpy as np
from jax import lax
from jax.experimental import pallas as pl
from jax.experimental.pallas import tpu as pltpu
from jax.sharding import PartitionSpec as P

HEAD = 64
POOL = 1024
WINDOW = 128
GRID_W = 64

eps = 1e-06
rope_base = 10000.0
neg_big = -1e30
pool_pad = 16
chunks = 4
token_chunks = 8
in_parts = 2
pooled_parts = 4
MESH = pl.DeviceIdType.MESH
f32, bf16 = jnp.float32, jnp.bfloat16


def rope_parts(rows_total):
    quarter = HEAD // 4
    steps = np.arange(quarter, dtype=np.float32) * np.float32(2.0) / np.float32(HEAD // 2)
    freqs = (np.float32(1.0) / np.float32(rope_base) ** steps).astype(np.float32)

    def table(count, first):
        angle = np.arange(count, dtype=np.float32)[:, None] * freqs
        twice = np.concatenate([angle, angle], axis=1).astype(np.float64)
        none = np.zeros_like(twice)
        made = []
        for part in (np.cos(twice), np.sin(twice)):
            head = [part, none] if first else [none, part]
            made.append(np.concatenate(head + head, axis=1).astype(np.float32))
        return made

    return table(rows_total // GRID_W, True) + table(GRID_W, False)


def ring_place(index, count, across):
    deep = count // across
    if across == 1 or deep % 2:
        return index
    z, x = index // across, index % across
    turn = deep - 1 - z
    inner = jnp.where(turn % 2 == 0, x - 1, across - 1 - x)
    return jnp.where(x == 0, z, deep + turn * (across - 1) + inner)


def ring_index(place, count, across):
    deep = count // across
    if across == 1 or deep % 2:
        return place
    rest = jnp.maximum(place - deep, 0)
    turn, inner = rest // (across - 1), rest % (across - 1)
    x = jnp.where(turn % 2 == 0, inner + 1, across - 1 - inner)
    return jnp.where(place < deep, place * across, (deep - 1 - turn) * across + x)


def norm_rope(raw, gain, cosine, sine, low_half, lead):
    squares = raw * raw
    low_sum = jnp.sum(jnp.where(low_half, squares, 0.0), axis=1, keepdims=True)
    high_sum = jnp.sum(jnp.where(low_half, 0.0, squares), axis=1, keepdims=True)
    mean = jnp.where(low_half, low_sum, high_sum) * (1.0 / HEAD)
    scaled = raw * lax.rsqrt(mean + eps) * gain
    turned = jnp.where(
        lead,
        -pltpu.roll(scaled, 2 * HEAD - HEAD // 4, 1),
        pltpu.roll(scaled, HEAD // 4, 1),
    )
    return scaled * cosine + turned * sine


def layer_kernel(
    count,
    members,
    tokens,
    wq,
    wk,
    wv,
    wp,
    wop,
    woa,
    norm_gain,
    query_gain,
    key_gain,
    row_cos,
    row_sin,
    col_cos,
    col_sin,
    sink,
    out,
    tok,
    normed,
    w_side,
    w_query,
    w_out,
    side,
    query,
    band,
    pool_band,
    cosines,
    sines,
    mixer,
    away,
    met,
    kept,
    y_send,
    y_recv,
    done,
    load_sem,
    side_send,
    side_recv,
    query_send,
    query_recv,
    out_send,
    out_recv,
    ty_send,
    ty_recv,
    td_send,
    td_recv,
    halo_send,
    halo_recv,
    met_send,
    met_recv,
    yy_send,
    yy_recv,
    done_sem,
):
    rows, features = tokens.shape
    depth, kw = wk.shape
    qw, pw, width = wq.shape[1], wp.shape[1], wop.shape[1]
    chips = members // 2
    share = rows // members
    half = (count - 1) // 2
    heads_k = kw // HEAD
    seq = count * rows
    across = chips

    me, tp = lax.axis_index("sp"), lax.axis_index("tp")
    chip, core = tp // 2, tp % 2
    partner = chip * 2 + 1 - core
    place = ring_place(me, count, across)
    owner_of = lambda spot: ring_index(spot, count, across)
    at = lambda offset: (place + offset + count) % count
    following, previous = owner_of(at(1)), owner_of(at(-1))

    loads = [
        pltpu.make_async_copy(wk, w_side.at[place, :, pl.ds(0, kw)], load_sem.at[0]),
        pltpu.make_async_copy(wv, w_side.at[place, :, pl.ds(kw, kw)], load_sem.at[1]),
        pltpu.make_async_copy(wp, w_side.at[place, :, pl.ds(2 * kw, pw)], load_sem.at[2]),
        pltpu.make_async_copy(tokens, tok.at[tp], load_sem.at[3]),
        pltpu.make_async_copy(wq, w_query.at[place], load_sem.at[4]),
        pltpu.make_async_copy(wop, w_out.at[place, pl.ds(0, pw), :], load_sem.at[5]),
        pltpu.make_async_copy(woa, w_out.at[place, pl.ds(pw, qw), :], load_sem.at[6]),
    ]
    for load in loads:
        load.start()

    barrier = pltpu.get_barrier_semaphore()
    greeted = [
        (following, tp),
        (previous, tp),
        (me, partner),
        ((me + 1) % count, tp),
        ((me + count - 1) % count, tp),
    ]
    greeted += [(me, (chip + hop) % chips * 2 + core) for hop in range(1, chips)]
    for device in greeted:
        pl.semaphore_signal(barrier, inc=1, device_id=device, device_id_type=MESH)
    pl.semaphore_wait(barrier, len(greeted))

    def remote(source, target, send_sem, recv_sem, device):
        return pltpu.make_async_remote_copy(
            src_ref=source,
            dst_ref=target,
            send_sem=send_sem,
            recv_sem=recv_sem,
            device_id=device,
            device_id_type=MESH,
        )

    def hop_copy(ring, way, spot, c):
        buffer, send_sem, recv_sem = ring
        size = buffer.shape[1] // chunks
        part = buffer.at[spot, pl.ds(pl.multiple_of(c * size, 16), size), :]
        device = (following if way == 0 else previous, tp)
        return remote(part, part, send_sem.at[way, spot, c], recv_sem.at[spot, c], device)

    def send_own(ring):
        for c in range(chunks):
            hop_copy(ring, 0, place, c).start()
            hop_copy(ring, 1, place, c).start()

    def event(ring, step, c):
        low, high = at(-step), at(step)
        hop_copy(ring, 0, low, c).wait_recv()

        @pl.when((step < half) | (c < chunks // 2))
        def _():
            hop_copy(ring, 0, low, c).start()

        hop_copy(ring, 1, high, c).wait_recv()

        @pl.when((step < half) | (c >= chunks // 2))
        def _():
            hop_copy(ring, 1, high, c).start()

    def events(ring, step):
        def body(c, carry):
            event(ring, step, c)
            return carry

        lax.fori_loop(0, chunks, body, 0)

    def opposite(ring):
        def body(c, carry):
            hop_copy(ring, 0, at(count // 2), c).wait_recv()
            return carry

        lax.fori_loop(0, chunks, body, 0)

    def sends_done(ring):
        def each(c, carry):
            hop_copy(ring, 0, place, c).wait_send()
            hop_copy(ring, 1, place, c).wait_send()

            def steps(step, inner):
                @pl.when((step < half) | (c < chunks // 2))
                def _():
                    hop_copy(ring, 0, at(-step), c).wait_send()

                @pl.when((step < half) | (c >= chunks // 2))
                def _():
                    hop_copy(ring, 1, at(step), c).wait_send()

                return inner

            return lax.fori_loop(1, half + 1, steps, carry)

        lax.fori_loop(0, chunks, each, 0)

    side_ring = (w_side, side_send, side_recv)
    query_ring = (w_query, query_send, query_recv)
    out_ring = (w_out, out_send, out_recv)

    for load in loads[:3]:
        load.wait()
    send_own(side_ring)
    loads[3].wait()

    token_rows = rows // token_chunks

    def token_part(owner, j):
        return tok.at[owner, pl.ds(pl.multiple_of(j * token_rows, 16), token_rows), :]

    def token_far(hop, owner, j):
        part = token_part(owner, j)
        target = (chip + hop) % chips * 2 + core
        return remote(
            part, part, ty_send.at[hop - 1, j], ty_recv.at[hop - 1, j], (me, target)
        )

    def token_near(slot, owner, j):
        part = token_part(owner, j)
        return remote(part, part, td_send.at[slot, j], td_recv.at[slot, j], (me, partner))

    def start_tokens(j, carry):
        for hop in range(1, chips):
            token_far(hop, tp, j).start()
        token_near(0, tp, j).start()
        return carry

    lax.fori_loop(0, token_chunks, start_tokens, 0)

    for g in range(rows // GRID_W):
        spot = pl.ds(me * (rows // GRID_W) + g, 1)
        grid_rows = pl.ds(g * GRID_W, GRID_W)
        cosines[grid_rows, :] = col_cos[...] + row_cos[spot, :]
        sines[grid_rows, :] = col_sin[...] + row_sin[spot, :]

    pieces = features // depth
    norm_rows = 32 if token_rows % 32 == 0 else 16

    def normalise(j):
        token_near(0, partner, j).wait_recv()
        for hop in range(1, chips):
            token_near(hop, (chip - hop + chips) % chips * 2 + 1 - core, j).wait_recv()

        def tile(i, carry):
            at_rows = pl.ds(pl.multiple_of(j * token_rows + i * norm_rows, 16), norm_rows)
            squares = jnp.zeros((norm_rows, 1), f32)
            for t in range(members):
                block = tok[t, at_rows, :].astype(f32)
                squares = squares + jnp.sum(block * block, axis=1, keepdims=True)
            scale = lax.rsqrt(squares / (members * features) + eps)
            for t in range(members):
                for piece in range(pieces):
                    first = piece * depth
                    gain = norm_gain[:, t * features + first : t * features + first + depth]
                    block = tok[t, at_rows, first : first + depth].astype(f32)
                    normed[t * pieces + piece, at_rows, :] = (block * scale * gain).astype(bf16)
            return carry

        lax.fori_loop(0, token_rows // norm_rows, tile, 0)

    def token_step(j, carry):
        for hop in range(1, chips):
            source = (chip - hop + chips) % chips * 2 + core
            token_far(hop, source, j).wait_recv()
            token_near(hop, source, j).start()

        @pl.when(j < half * chunks)
        def _():
            event(side_ring, j // chunks + 1, j % chunks)

        @pl.when(j >= 1)
        def _():
            normalise(j - 1)

        return carry

    lax.fori_loop(0, token_chunks, token_step, 0)
    normalise(token_chunks - 1)

    tile_rows = 256 if rows % 256 == 0 else 128

    def project(total, weights, spots, first=False):
        def body(i, carry):
            part = pl.ds(pl.multiple_of(i * tile_rows, tile_rows), tile_rows)
            terms = [
                jnp.dot(
                    normed[owner_of(spot), part, :], weights[spot], preferred_element_type=f32
                )
                for spot in spots
            ]
            value = functools.reduce(lambda a, b: a + b, terms)
            total[part, :] = value if first else total[part, :] + value
            return carry

        lax.fori_loop(0, rows // tile_rows, body, 0)

    project(side, w_side, [place], first=True)
    early = token_chunks // chunks

    def side_step(step, carry):
        @pl.when(step > early)
        def _():
            events(side_ring, step)

        project(side, w_side, [at(-step), at(step)])
        return carry

    lax.fori_loop(1, half + 1, side_step, 0)
    loads[4].wait()
    send_own(query_ring)
    opposite(side_ring)
    project(side, w_side, [at(count // 2)])

    twice = lambda gain: jnp.concatenate([gain[...], gain[...]], axis=1)
    query_gains, key_gains = twice(query_gain), twice(key_gain)
    lane = lax.broadcasted_iota(jnp.int32, (WINDOW, 2 * HEAD), 1)
    low_half = lane < HEAD
    lead = lane % (HEAD // 2) < HEAD // 4

    def prepare(i, carry):
        part = pl.ds(pl.multiple_of(i * WINDOW, WINDOW), WINDOW)
        shifted = pl.ds(pl.multiple_of((i + 1) * WINDOW, WINDOW), WINDOW)
        for h in range(kw // (2 * HEAD)):
            lanes = slice(h * 2 * HEAD, (h + 1) * 2 * HEAD)
            key = norm_rope(
                side[part, lanes], key_gains, cosines[part, :], sines[part, :], low_half, lead
            )
            band[shifted, lanes] = key.astype(bf16)
        band[shifted, kw : 2 * kw] = side[part, kw : 2 * kw].astype(bf16)
        pooled_rows = pl.ds(pl.multiple_of(i * WINDOW + pool_pad, pool_pad), WINDOW)
        pool_band[pooled_rows, :] = side[part, 2 * kw :].astype(bf16)
        return carry

    lax.fori_loop(0, rows // WINDOW, prepare, 0)

    before, behind = (me + count - 1) % count, (me + 1) % count

    def halo(index, buffer, size, upwards):
        if upwards:
            source, target, device = rows, 0, (behind, tp)
        else:
            source, target, device = size, rows + size, (before, tp)
        return remote(
            buffer.at[pl.ds(source, size), :],
            buffer.at[pl.ds(target, size), :],
            halo_send.at[index],
            halo_recv.at[index],
            device,
        )

    lower = [halo(0, band, WINDOW, False), halo(1, pool_band, pool_pad, False)]
    upper = [halo(2, band, WINDOW, True), halo(3, pool_band, pool_pad, True)]
    has_lower, has_upper = me > 0, me < count - 1

    @pl.when(has_lower)
    def _():
        for copy in lower:
            copy.start()

    @pl.when(has_upper)
    def _():
        for copy in upper:
            copy.start()

    @pl.when(jnp.logical_not(has_lower))
    def _():
        band[0:WINDOW, :] = jnp.zeros((WINDOW, 2 * kw), bf16)
        pool_band[0:pool_pad, :] = jnp.zeros((pool_pad, pw), bf16)

    @pl.when(jnp.logical_not(has_upper))
    def _():
        band[rows + WINDOW :, :] = jnp.zeros((WINDOW, 2 * kw), bf16)
        pool_band[rows + pool_pad :, :] = jnp.zeros((pool_pad, pw), bf16)

    project(query, w_query, [place], first=True)

    def query_step(step, carry):
        events(query_ring, step)
        project(query, w_query, [at(-step), at(step)])
        return carry

    lax.fori_loop(1, half + 1, query_step, 0)
    loads[5].wait()
    loads[6].wait()
    send_own(out_ring)

    @pl.when(has_lower)
    def _():
        for copy in upper:
            copy.wait_recv()

    @pl.when(has_upper)
    def _():
        for copy in lower:
            copy.wait_recv()

    level = tp * pw // (POOL // 4)
    reach = jnp.where(level == 0, 1, jnp.where(level == 1, 2, jnp.where(level == 2, 4, 8)))

    def pool(i, carry):
        wide = WINDOW + 2 * pool_pad
        part = pl.ds(pl.multiple_of(i * WINDOW, WINDOW), WINDOW)
        values = pool_band[pl.ds(pl.multiple_of(i * WINDOW, pool_pad), wide), :].astype(f32)
        total, chosen = values, None
        for step in range(4):
            size = 2**step
            total = total + pltpu.roll(total, wide - size, 0)
            shifted = pltpu.roll(total, size, 0)[pool_pad : pool_pad + WINDOW]
            chosen = shifted if chosen is None else jnp.where(level == step, shifted, chosen)
        spot = me * rows + i * WINDOW + lax.broadcasted_iota(jnp.int32, (WINDOW, 1), 0)
        low = jnp.maximum(spot - reach, 0)
        high = jnp.minimum(spot + reach - 1, seq - 1)
        mixer[part, 0:pw] = (chosen / (high - low + 1).astype(f32)).astype(bf16)
        return carry

    lax.fori_loop(0, rows // WINDOW, pool, 0)

    opposite(query_ring)
    project(query, w_query, [at(count // 2)])

    blocks = rows // WINDOW
    row = lax.broadcasted_iota(jnp.int32, (2 * WINDOW, 3 * WINDOW), 0) % WINDOW
    column = lax.broadcasted_iota(jnp.int32, (2 * WINDOW, 3 * WINDOW), 1)
    top_row = lax.broadcasted_iota(jnp.int32, (2 * WINDOW, 1), 0) < WINDOW

    def attend(i, carry):
        part = pl.ds(pl.multiple_of(i * WINDOW, WINDOW), WINDOW)
        key_rows = pl.ds(pl.multiple_of(i * WINDOW, WINDOW), 3 * WINDOW)
        key_pos = me * rows + i * WINDOW - WINDOW + column
        inside = (column >= row) & (column - row <= 2 * WINDOW) & (key_pos >= 0) & (key_pos < seq)
        for head in range(heads_k):
            lanes = slice(head * 2 * HEAD, (head + 1) * 2 * HEAD)
            rotated = norm_rope(
                query[part, lanes],
                query_gains,
                cosines[part, :],
                sines[part, :],
                low_half,
                lead,
            ) * HEAD ** (-0.5)
            other = pltpu.roll(rotated, HEAD, 1)
            if head % 2 == 0:
                pair = (jnp.where(low_half, rotated, 0.0), jnp.where(low_half, other, 0.0))
            else:
                pair = (jnp.where(low_half, 0.0, other), jnp.where(low_half, 0.0, rotated))
            stacked = jnp.concatenate(pair, axis=0).astype(bf16)
            tile = head // 2 * 2 * HEAD
            keys = band[key_rows, tile : tile + 2 * HEAD]
            values = band[key_rows, kw + tile : kw + tile + 2 * HEAD]
            scores = lax.dot_general(
                stacked, keys, (((1,), (1,)), ((), ())), preferred_element_type=f32
            )
            scores = jnp.where(inside, scores, neg_big)
            limit = jnp.where(top_row, sink[2 * head], sink[2 * head + 1])
            top = jnp.maximum(jnp.max(scores, axis=1, keepdims=True), limit)
            raised = jnp.exp(scores - top)
            totals = jnp.sum(raised, axis=1, keepdims=True) + jnp.exp(limit - top)
            weights = (raised * (1.0 / totals)).astype(bf16)
            result = jnp.dot(weights, values, preferred_element_type=f32)
            one, two = result[:WINDOW], result[WINDOW:]
            if head % 2 == 0:
                joined = jnp.where(low_half, one, pltpu.roll(two, HEAD, 1))
            else:
                joined = jnp.where(low_half, pltpu.roll(one, HEAD, 1), two)
            mixer[part, pw + head * 2 * HEAD : pw + (head + 1) * 2 * HEAD] = joined.astype(bf16)

        for c in range(chunks):

            @pl.when(i == ((c + 1) * blocks + chunks - 1) // chunks - 1)
            def _(c=c):
                event(out_ring, 1, c)

        return carry

    lax.fori_loop(0, blocks, attend, 0)

    def product(spot, which):
        left = jnp.concatenate(
            [
                mixer[pl.ds(pl.multiple_of((y * 2 + which) * share, 16), share), :]
                for y in range(chips)
            ],
            axis=0,
        )
        return jnp.dot(left, w_out[spot], preferred_element_type=f32).astype(bf16)

    def met_copy(spot):
        return remote(
            away.at[spot], met.at[spot], met_send.at[spot], met_recv.at[spot], (me, partner)
        )

    def y_copy(spot, hop):
        target = (chip + hop) % chips * 2 + core
        return remote(
            y_send.at[spot, hop - 1],
            y_recv.at[spot, hop - 1],
            yy_send.at[spot, hop - 1],
            yy_recv.at[spot, hop - 1],
            (me, target),
        )

    def done_copy(spot):
        columns = pl.ds(pl.multiple_of(owner_of(spot) * width, width), width)
        return pltpu.make_async_copy(done.at[spot], out.at[:, columns], done_sem.at[spot])

    def both_rows(spot, y):
        part = pl.ds(pl.multiple_of(y * share, 16), share)
        return kept[spot, part, :].astype(f32) + met[spot, part, :].astype(f32)

    def group(spots):
        def first(spot):
            away[spot] = product(spot, 1 - core)
            met_copy(spot).start()

        def second(spot):
            kept[spot] = product(spot, core)

        def third(spot):
            met_copy(spot).wait_recv()
            for hop in range(1, chips):
                y_send[spot, hop - 1] = both_rows(spot, (chip + hop) % chips).astype(bf16)
                y_copy(spot, hop).start()

        for part in (first, second, third):
            for spot in spots:
                part(spot)

    def finish(spot):
        total = both_rows(spot, chip)
        for hop in range(1, chips):
            y_copy(spot, hop).wait_recv()
            total = total + y_recv[spot, hop - 1].astype(f32)
        done[spot] = total.astype(bf16)
        done_copy(spot).start()

    group([place])

    def out_step(step, carry):
        @pl.when(step > 1)
        def _():
            events(out_ring, step)

        group([at(-step), at(step)])

        @pl.when(step == 1)
        def _():
            finish(place)

        @pl.when(step > 1)
        def _():
            finish(at(1 - step))
            finish(at(step - 1))

        return carry

    lax.fori_loop(1, half + 1, out_step, 0)
    opposite(out_ring)
    group([at(count // 2)])
    finish(at(-half))
    finish(at(half))
    finish(at(count // 2))

    for ring in (side_ring, query_ring, out_ring):
        sends_done(ring)

    def tokens_sent(j, carry):
        token_near(0, tp, j).wait_send()
        for hop in range(1, chips):
            token_far(hop, tp, j).wait_send()
            token_near(hop, (chip - hop + chips) % chips * 2 + core, j).wait_send()
        return carry

    lax.fori_loop(0, token_chunks, tokens_sent, 0)

    @pl.when(has_lower)
    def _():
        for copy in lower:
            copy.wait_send()

    @pl.when(has_upper)
    def _():
        for copy in upper:
            copy.wait_send()

    def blocks_sent(spot, carry):
        met_copy(spot).wait_send()
        for hop in range(1, chips):
            y_copy(spot, hop).wait_send()
        done_copy(spot).wait()
        return carry

    lax.fori_loop(0, count, blocks_sent, 0)


def plane_kernel(
    count,
    members,
    tokens,
    wq,
    wk,
    wv,
    wp,
    wop,
    woa,
    norm_gain_in,
    query_gain_in,
    key_gain_in,
    row_cos_in,
    row_sin_in,
    col_cos_in,
    col_sin_in,
    sink_in,
    out,
    norm_gain,
    query_gain,
    key_gain,
    row_cos,
    row_sin,
    col_cos,
    col_sin,
    sink,
    small_sem,
    raw,
    sums,
    normed,
    w_in,
    w_pool,
    w_out,
    in_spare,
    pool_spare,
    out_spare,
    total,
    band,
    pool_band,
    cosines,
    sines,
    attended,
    pooled,
    result,
    rounded,
    load_sem,
    sum_sems,
    in_sems,
    pool_sems,
    out_sems,
    x_sems,
    spread_sems,
    token_sems,
    token_bulk,
    attend_sems,
    attend_bulk,
    pooled_sems,
    pooled_bulk,
    halo_send,
    halo_recv,
    result_sems,
):
    rows, features = tokens.shape
    depth = wk.shape[0]
    hk, hq, hp = wk.shape[1] // 2, wq.shape[1] // 2, wp.shape[1] // 2
    width = wop.shape[1]
    narrow = width // members
    share = rows // members
    plane = 2 * rows
    heads_k = hk // HEAD
    seq = count * rows
    deep = count // 2
    pieces = features // depth
    tiles = rows // WINDOW
    grid = plane // GRID_W

    me, tp = lax.axis_index("sp"), lax.axis_index("tp")
    z, x = me // 2, me % 2
    y, core = tp // 2, tp % 2
    me_x, tp_y, tp_c = me + 1 - 2 * x, (1 - y) * 2 + core, y * 2 + 1 - core
    tp_yc = (1 - y) * 2 + 1 - core
    up, down = (me + 2) % count, (me + count - 2) % count
    has_up, has_down = z < deep - 1, z > 0
    inner = has_up & has_down

    mine = lambda size: pl.ds(pl.multiple_of(x * size, 128), size)
    other = lambda size: pl.ds(pl.multiple_of((1 - x) * size, 128), size)

    def load(group, source, target):
        pltpu.make_async_copy(source, target, load_sem.at[group]).start()

    def loaded(group, whole):
        pltpu.make_async_copy(whole, whole, load_sem.at[group]).wait()

    for target, pick in ((w_in.at[me], mine), (in_spare, other)):
        load(0, wk.at[:, pick(hk)], target.at[:, pl.ds(0, hk)])
        load(0, wv.at[:, pick(hk)], target.at[:, pl.ds(hk, hk)])
        load(0, wq.at[:, pick(hq)], target.at[:, pl.ds(2 * hk, hq)])
    load(1, tokens, raw)
    small = [
        pltpu.make_async_copy(source, target, small_sem.at[index])
        for index, (source, target) in enumerate(
            (
                (norm_gain_in, norm_gain),
                (query_gain_in, query_gain),
                (key_gain_in, key_gain),
                (row_cos_in.at[pl.ds(z * grid, grid), :], row_cos),
                (row_sin_in.at[pl.ds(z * grid, grid), :], row_sin),
                (col_cos_in, col_cos),
                (col_sin_in, col_sin),
                (sink_in, sink),
            )
        )
    ]
    for copy in small:
        copy.start()
    for target, pick in ((w_pool.at[me], mine), (pool_spare, other)):
        load(2, wp.at[:, pick(hp)], target)
    strip = lambda t: pl.ds(pl.multiple_of(t * narrow, narrow), narrow)
    strips = [(3, w_out.at[z, tp], tp)] + [(4, out_spare.at[t], t) for t in range(members)]
    for group, target, t in strips:
        load(group, woa.at[:, strip(t)], target.at[pl.ds(0, 2 * hq), :])
        load(group, wop.at[:, strip(t)], target.at[pl.ds(2 * hq, 2 * hp), :])

    barrier = pltpu.get_barrier_semaphore()
    greeted = [(up, tp), (down, tp), (me_x, tp)]
    for t in (tp_y, tp_c, tp_yc):
        greeted += [(me, t), (me_x, t)]
    for device in greeted:
        pl.semaphore_signal(barrier, inc=1, device_id=device, device_id_type=MESH)
    pl.semaphore_wait(barrier, len(greeted))

    def remote(source, target, send_sem, recv_sem, device):
        return pltpu.make_async_remote_copy(
            src_ref=source,
            dst_ref=target,
            send_sem=send_sem,
            recv_sem=recv_sem,
            device_id=device,
            device_id_type=MESH,
        )

    def by_rows(parts):
        def view(buffer, c):
            size = buffer.shape[0] // parts
            return buffer.at[pl.ds(pl.multiple_of(c * size, 16), size), :]

        return view

    in_ring = (w_in, in_spare, in_sems, 0, in_parts, by_rows(in_parts))
    pool_ring = (w_pool, pool_spare, pool_sems, 1, 1, by_rows(1))
    def z_copy(ring, way, source, c, own=False):
        buffer, _, sems, _, _, view = ring
        part = view(buffer.at[source], c)
        send = sems.at[int(own and way == 1), source, c]
        return remote(part, part, send, sems.at[1, source, c], ((up, down)[way], tp))

    def x_copy(ring, source, c):
        buffer, spare, sems, first, _, view = ring
        return remote(
            view(spare, c),
            view(buffer.at[source], c),
            x_sems.at[first],
            sems.at[1, source, c],
            (me_x, tp),
        )

    def both_ways(ring, source, c, act):
        @pl.when(has_up)
        def _():
            act(z_copy(ring, 0, source, c, own=True))

        @pl.when(has_down)
        def _():
            act(z_copy(ring, 1, source, c, own=True))

    start = lambda copy: copy.start()
    sent = lambda copy: copy.wait_send()

    def own_out(ring):
        for c in range(ring[4]):
            both_ways(ring, me, c, start)

    def side_out(ring):
        for c in range(ring[4]):
            x_copy(ring, me, c).start()

    def side_in(ring):
        for c in range(ring[4]):
            x_copy(ring, me_x, c).wait_recv()
            both_ways(ring, me_x, c, start)

    def passing(ring, n):
        parts = ring[4]
        step, j, c = n // (2 * parts) + 1, n // parts % 2, n % parts
        column = (x + j) % 2
        low, high = z - step, z + step
        return (low >= 0, low * 2 + column), (high < deep, high * 2 + column), c

    def event(ring, n):
        (is_low, low), (is_high, high), c = passing(ring, n)

        @pl.when(is_low)
        def _():
            z_copy(ring, 0, low, c).wait_recv()

            @pl.when(has_up)
            def _():
                z_copy(ring, 0, low, c).start()

        @pl.when(is_high)
        def _():
            z_copy(ring, 1, high, c).wait_recv()

            @pl.when(has_down)
            def _():
                z_copy(ring, 1, high, c).start()

    def events(ring, first, last):
        def body(n, carry):
            event(ring, n)
            return carry

        lax.fori_loop(first, last, body, 0)

    def all_events(ring):
        return (deep - 1) * 2 * ring[4]

    def bulk(whole, sem):
        return remote(whole, whole, sem, sem, (me_x, tp))

    def sends_done(ring):
        bulk(ring[1], x_sems.at[ring[3]]).wait_send()
        for c in range(ring[4]):
            both_ways(ring, me, c, sent)
            both_ways(ring, me_x, c, sent)

        def body(n, carry):
            (is_low, low), (is_high, high), c = passing(ring, n)

            @pl.when(is_low & has_up)
            def _():
                z_copy(ring, 0, low, c).wait_send()

            @pl.when(is_high & has_down)
            def _():
                z_copy(ring, 1, high, c).wait_send()

            return carry

        lax.fori_loop(0, all_events(ring), body, 0)

    def out_copy(way, level, c, own=False):
        part = w_out.at[level, (tp - c + members) % members]
        send = out_sems.at[int(own and way == 1), level, c]
        return remote(part, part, send, out_sems.at[1, level, c], ((up, down)[way], tp))

    def spread(c):
        target = (tp + c) % members
        return remote(
            out_spare.at[target],
            w_out.at[z, tp],
            spread_sems.at[0],
            out_sems.at[1, z, c],
            (me, target),
        )

    def spread_in(c):
        owner = (tp - c + members) % members
        return remote(
            out_spare.at[owner],
            w_out.at[z, owner],
            spread_sems.at[0],
            out_sems.at[1, z, c],
            (me, owner),
        )

    def out_both(c, act):
        @pl.when(has_up)
        def _():
            act(out_copy(0, z, c, own=True))

        @pl.when(has_down)
        def _():
            act(out_copy(1, z, c, own=True))

    def out_event(n):
        step, c = n // members + 1, n % members
        low, high = z - step, z + step

        @pl.when(low >= 0)
        def _():
            out_copy(0, low, c).wait_recv()

            @pl.when(has_up)
            def _():
                out_copy(0, low, c).start()

        @pl.when(high < deep)
        def _():
            out_copy(1, high, c).wait_recv()

            @pl.when(has_down)
            def _():
                out_copy(1, high, c).start()

    def out_events(first, last):
        def body(n, carry):
            out_event(n)
            return carry

        lax.fori_loop(first, last, body, 0)

    def out_sent(n, carry):
        step, c = n // members + 1, n % members
        low, high = z - step, z + step

        @pl.when((low >= 0) & has_up)
        def _():
            out_copy(0, low, c).wait_send()

        @pl.when((high < deep) & has_down)
        def _():
            out_copy(1, high, c).wait_send()

        return carry

    loaded(0, w_in.at[pl.ds(0, 2)])
    for c in range(in_parts):
        x_copy(in_ring, me, c).start()
        both_ways(in_ring, me, c, start)

    loaded(1, raw)
    for copy in small:
        copy.wait()
    sums[tp] = jnp.zeros_like(sums[tp])
    for i in range(tiles):
        block = raw[i * WINDOW : (i + 1) * WINDOW, :].astype(f32)
        square = jnp.sum(block * block, axis=1, keepdims=True)
        turned = jnp.transpose(jnp.broadcast_to(square, (WINDOW, WINDOW)))
        sums[tp, i : i + 1, :] = turned[0:1, :]

    def sum_copy(owner, hop):
        target = (tp + hop) % members
        return remote(
            sums.at[owner],
            sums.at[owner],
            sum_sems.at[0],
            sum_sems.at[1],
            (me, target),
        )

    for hop in range(1, members):
        sum_copy(tp, hop).start()
    for g in range(grid):
        grid_rows = pl.ds(g * GRID_W, GRID_W)
        cosines[grid_rows, :] = col_cos[...] + row_cos[g : g + 1, :]
        sines[grid_rows, :] = col_sin[...] + row_sin[g : g + 1, :]
    bulk(sums.at[pl.ds(0, members - 1)], sum_sems.at[1]).wait_recv()
    squares = sums[0]
    for t in range(1, members):
        squares = squares + sums[t]
    scales = lax.rsqrt(squares / (members * features) + eps)

    class Stream:
        def __init__(self, view, all_sent, side, sems, bulk_sems, by_x):
            self.view, self.all_sent, self.side = view, all_sent, side
            self.sems, self.bulk_sems, self.by_x = sems, bulk_sems, by_x

        def copy(self, recv, side, owner, j, device):
            part = self.view(side, owner, j)
            return remote(part, part, self.bulk_sems.at[0], recv, device)

        def over_x(self, slot, side, owner, j):
            return self.copy(self.sems.at[2 * slot, j], side, owner, j, (me_x, tp))

        def over_y(self, slot, side, owner, j):
            return self.copy(self.sems.at[1 + slot, j], side, owner, j, (me, tp_y))

        def over_core(self, slot, side, owner, j):
            return self.copy(self.bulk_sems.at[1 + slot % 2], side, owner, j, (me, tp_c))

        def start(self, j):
            self.over_y(0, x, tp, j).start()
            self.over_x(0, x, tp, j).start()
            self.over_core(0, x, tp, j).start()

        def direct(self, j):
            self.over_y(0, x, tp_y, j).wait_recv()
            self.over_core(2, x, tp_y, j).start()

            @pl.when(self.by_x(j))
            def _():
                self.over_x(1, x, tp_y, j).start()

            self.over_x(0, 1 - x, tp, j).wait_recv()
            self.over_core(1, 1 - x, tp, j).start()

            @pl.when(jnp.logical_not(self.by_x(j)))
            def _():
                self.over_y(1, 1 - x, tp, j).start()

        def crossed(self, j):
            @pl.when(self.by_x(j))
            def _():
                self.over_x(1, 1 - x, tp_y, j).wait_recv()

            @pl.when(jnp.logical_not(self.by_x(j)))
            def _():
                self.over_y(1, 1 - x, tp_y, j).wait_recv()

            self.over_core(3, 1 - x, tp_y, j).start()

        def near_side(self):
            bulk(self.side, self.bulk_sems.at[1]).wait_recv()

        def far_side(self):
            bulk(self.side, self.bulk_sems.at[2]).wait_recv()

        def sent(self):
            bulk(self.all_sent, self.bulk_sems.at[0]).wait_send()

        def every(self, act):
            def body(j, carry):
                act(j)
                return carry

            lax.fori_loop(0, self.sems.shape[1], body, 0)

    def block_rows(j, size):
        return pl.ds(pl.multiple_of(j * size, 16), size)

    def token_view(side, owner, j):
        return normed.at[side, pl.ds(owner * pieces, pieces), block_rows(j, WINDOW), :]

    def attend_view(side, owner, j):
        return attended.at[owner, side, block_rows(j, WINDOW), :]

    def pooled_view(side, owner, j):
        return pooled.at[owner, side, block_rows(j, plane // pooled_parts), :]

    most = lambda size: pl.ds(0, size * (2 * members - 1) // (2 * members))
    token_stream = Stream(
        token_view,
        normed.at[:, :, most(rows), :],
        normed.at[0, pl.ds(0, count // 2)],
        token_sems,
        token_bulk,
        lambda j: j % 3 == 0,
    )
    attend_stream, pooled_stream = [
        Stream(
            view,
            buffer.at[:, :, most(plane), :],
            buffer.at[0],
            sems,
            bulk_sems,
            lambda j: j % 2 == 0,
        )
        for view, buffer, sems, bulk_sems in (
            (attend_view, attended, attend_sems, attend_bulk),
            (pooled_view, pooled, pooled_sems, pooled_bulk),
        )
    ]

    for i in range(tiles):
        here = slice(i * WINDOW, (i + 1) * WINDOW)
        scale = jnp.transpose(jnp.broadcast_to(scales[i : i + 1, :], (WINDOW, WINDOW)))
        for first in range(0, features, WINDOW):
            block = raw[here, first : first + WINDOW].astype(f32)
            gain = norm_gain[:, pl.ds(pl.multiple_of(tp * features + first, WINDOW), WINDOW)]
            value = (block * scale * gain).astype(bf16)
            inside = first % depth
            normed[x, tp * pieces + first // depth, here, inside : inside + WINDOW] = value
        token_stream.start(i)

    side_in(in_ring)
    whole = all_events(in_ring)
    reached = lambda part: whole * part // 24
    events(in_ring, 0, reached(4))

    def direct(j, carry):
        token_stream.direct(j)
        events(in_ring, reached(4 + 12 * j // tiles), reached(4 + 12 * (j + 1) // tiles))
        return carry

    lax.fori_loop(0, tiles, direct, 0)
    loaded(2, w_pool.at[pl.ds(0, 2)])
    loaded(3, w_out.at[0, 0])
    loaded(4, out_spare)
    side_out(pool_ring)
    for c in range(1, members):
        spread(c).start()
    token_stream.near_side()

    tile_rows = 256 if rows % 256 == 0 else 128
    per_side = rows // tile_rows

    def project(result, weights, level, side, first=False):
        def body(i, carry):
            within = pl.ds(pl.multiple_of(i * tile_rows, tile_rows), tile_rows)
            part = pl.ds(pl.multiple_of(side * rows + i * tile_rows, tile_rows), tile_rows)
            value = None if first else result[part, :]
            for j in range(2):
                term = jnp.dot(
                    normed[side, level * 2 + j, within, :],
                    weights[level * 2 + j],
                    preferred_element_type=f32,
                )
                value = term if value is None else value + term
            result[part, :] = value
            return carry

        lax.fori_loop(0, per_side, body, 0)

    def project_step(result, weights, step, side):
        @pl.when(z - step >= 0)
        def _():
            project(result, weights, z - step, side)

        @pl.when(z + step < deep)
        def _():
            project(result, weights, z + step, side)

    early = max(reached(16) // (2 * in_parts), 0)

    def crossed(j, carry):
        token_stream.crossed(j)

        @pl.when(j == 0)
        def _():
            project(total, w_in, z, x, first=True)

        @pl.when((j >= 1) & (j <= early))
        def _():
            project_step(total, w_in, j, x)

        events(in_ring, reached(16 + 4 * j // tiles), reached(16 + 4 * (j + 1) // tiles))
        return carry

    lax.fori_loop(0, tiles, crossed, 0)
    own_out(pool_ring)
    side_in(pool_ring)
    token_stream.far_side()
    project(total, w_in, z, 1 - x, first=True)

    @pl.when(inner)
    def _():
        events(pool_ring, 0, 2)


    def in_step(step, carry):
        each = 2 * in_parts
        events(in_ring, jnp.maximum((step - 1) * each, reached(20)), step * each)

        @pl.when(step > min(early, tiles - 1))
        def _():
            project_step(total, w_in, step, x)

        project_step(total, w_in, step, 1 - x)
        return carry

    lax.fori_loop(1, deep, in_step, 0)

    twice = lambda gain: jnp.concatenate([gain[...], gain[...]], axis=1)
    query_gains, key_gains = twice(query_gain), twice(key_gain)
    lane = lax.broadcasted_iota(jnp.int32, (WINDOW, 2 * HEAD), 1)
    low_half = lane < HEAD
    lead = lane % (HEAD // 2) < HEAD // 4
    blocks = plane // WINDOW

    def prepare(i, carry):
        part = pl.ds(pl.multiple_of(i * WINDOW, WINDOW), WINDOW)
        shifted = pl.ds(pl.multiple_of((i + 1) * WINDOW, WINDOW), WINDOW)
        for h in range(hk // (2 * HEAD)):
            lanes = slice(h * 2 * HEAD, (h + 1) * 2 * HEAD)
            key = norm_rope(
                total[part, lanes], key_gains, cosines[part, :], sines[part, :], low_half, lead
            )
            band[shifted, lanes] = key.astype(bf16)
        band[shifted, hk:] = total[part, hk : 2 * hk].astype(bf16)
        return carry

    lax.fori_loop(0, blocks, prepare, 0)

    def halo(index, buffer, size, upwards):
        if upwards:
            source, target, device = plane, 0, (up, tp)
        else:
            source, target, device = size, plane + size, (down, tp)
        return remote(
            buffer.at[pl.ds(source, size), :],
            buffer.at[pl.ds(target, size), :],
            halo_send.at[index],
            halo_recv.at[index],
            device,
        )

    def halo_out(index, buffer, size):
        @pl.when(has_down)
        def _():
            halo(index, buffer, size, False).start()

        @pl.when(has_up)
        def _():
            halo(index + 1, buffer, size, True).start()

        empty = jnp.zeros((size, buffer.shape[1]), bf16)

        @pl.when(jnp.logical_not(has_down))
        def _():
            buffer[0:size, :] = empty

        @pl.when(jnp.logical_not(has_up))
        def _():
            buffer[plane + size :, :] = empty

    def halo_in(index, buffer, size):
        @pl.when(has_up)
        def _():
            halo(index, buffer, size, False).wait_recv()

        @pl.when(has_down)
        def _():
            halo(index + 1, buffer, size, True).wait_recv()

    halo_out(0, band, WINDOW)

    @pl.when(inner)
    def _():
        events(pool_ring, 2, all_events(pool_ring))

    for c in range(members - 1):
        if c > 0:
            spread_in(c).wait_recv()
        out_both(c, start)

    row = lax.broadcasted_iota(jnp.int32, (2 * WINDOW, 3 * WINDOW), 0) % WINDOW
    column = lax.broadcasted_iota(jnp.int32, (2 * WINDOW, 3 * WINDOW), 1)
    top_row = lax.broadcasted_iota(jnp.int32, (2 * WINDOW, 1), 0) < WINDOW

    def attend(turn, carry):
        @pl.when(turn == blocks - 2)
        def _():
            halo_in(0, band, WINDOW)

        i = (turn + 1) % blocks
        part = pl.ds(pl.multiple_of(i * WINDOW, WINDOW), WINDOW)
        key_rows = pl.ds(pl.multiple_of(i * WINDOW, WINDOW), 3 * WINDOW)
        key_pos = z * plane + i * WINDOW - WINDOW + column
        inside = (column >= row) & (column - row <= 2 * WINDOW) & (key_pos >= 0) & (key_pos < seq)
        for head in range(heads_k):
            lanes = slice(2 * hk + head * 2 * HEAD, 2 * hk + (head + 1) * 2 * HEAD)
            rotated = norm_rope(
                total[part, lanes],
                query_gains,
                cosines[part, :],
                sines[part, :],
                low_half,
                lead,
            ) * HEAD ** (-0.5)
            swapped = pltpu.roll(rotated, HEAD, 1)
            if head % 2 == 0:
                pair = (jnp.where(low_half, rotated, 0.0), jnp.where(low_half, swapped, 0.0))
            else:
                pair = (jnp.where(low_half, 0.0, swapped), jnp.where(low_half, 0.0, rotated))
            stacked = jnp.concatenate(pair, axis=0).astype(bf16)
            tile = head // 2 * 2 * HEAD
            keys = band[key_rows, tile : tile + 2 * HEAD]
            values = band[key_rows, hk + tile : hk + tile + 2 * HEAD]
            scores = lax.dot_general(
                stacked, keys, (((1,), (1,)), ((), ())), preferred_element_type=f32
            )
            scores = jnp.where(inside, scores, neg_big)
            first = x * 2 * heads_k + 2 * head
            limit = jnp.where(top_row, sink[first], sink[first + 1])
            top = jnp.maximum(jnp.max(scores, axis=1, keepdims=True), limit)
            raised = jnp.exp(scores - top)
            totals = jnp.sum(raised, axis=1, keepdims=True) + jnp.exp(limit - top)
            weights = (raised * (1.0 / totals)).astype(bf16)
            result = jnp.dot(weights, values, preferred_element_type=f32)
            one, two = result[:WINDOW], result[WINDOW:]
            if head % 2 == 0:
                joined = jnp.where(low_half, one, pltpu.roll(two, HEAD, 1))
            else:
                joined = jnp.where(low_half, pltpu.roll(one, HEAD, 1), two)
            attended[tp, x, part, head * 2 * HEAD : (head + 1) * 2 * HEAD] = joined.astype(bf16)
        attend_stream.start(i)

        @pl.when(turn >= behind)
        def _():
            attend_stream.direct((turn - behind + 1) % blocks)

        return carry

    behind = 5
    lax.fori_loop(0, blocks, attend, 0)

    events(pool_ring, jnp.where(inner, all_events(pool_ring), 0), all_events(pool_ring))

    for side in range(2):

        def pool_project(i, carry, side=side):
            part = pl.ds(pl.multiple_of(i * tile_rows, tile_rows), tile_rows)
            first = side * rows + pool_pad + i * tile_rows
            left = jnp.concatenate([normed[side, source, part, :] for source in range(count)], axis=1)
            right = w_pool[...].reshape(count * depth, hp)
            value = jnp.dot(left, right, preferred_element_type=f32)
            pool_band[pl.ds(pl.multiple_of(first, pool_pad), tile_rows), :] = value.astype(bf16)
            return carry

        lax.fori_loop(0, per_side, pool_project, 0)
    halo_out(2, pool_band, pool_pad)
    spread_in(members - 1).wait_recv()
    out_both(members - 1, start)

    @pl.when(inner)
    def _():
        out_events(0, members - 1)

    level = (tp * 2 + x) * hp // (POOL // 4)
    reach = jnp.where(level == 0, 1, jnp.where(level == 1, 2, jnp.where(level == 2, 4, 8)))

    def pool(i, carry):
        wide = WINDOW + 2 * pool_pad
        part = pl.ds(pl.multiple_of(i * WINDOW, WINDOW), WINDOW)
        running = pool_band[pl.ds(pl.multiple_of(i * WINDOW, pool_pad), wide), :].astype(f32)
        chosen = None
        for step in range(4):
            size = 2**step
            running = running + pltpu.roll(running, wide - size, 0)
            shifted = pltpu.roll(running, size, 0)[pool_pad : pool_pad + WINDOW]
            chosen = shifted if chosen is None else jnp.where(level == step, shifted, chosen)
        spot = z * plane + i * WINDOW + lax.broadcasted_iota(jnp.int32, (WINDOW, 1), 0)
        low = jnp.maximum(spot - reach, 0)
        high = jnp.minimum(spot + reach - 1, seq - 1)
        pooled[tp, x, part, :] = (chosen / (high - low + 1).astype(f32)).astype(bf16)
        return carry

    edge = blocks // pooled_parts
    lax.fori_loop(edge, blocks - edge, pool, 0)
    for part in range(1, pooled_parts - 1):
        pooled_stream.start(part)
    for turn in range(blocks - behind, blocks):
        attend_stream.direct((turn + 1) % blocks)
    halo_in(2, pool_band, pool_pad)
    lax.fori_loop(0, edge, pool, 0)
    lax.fori_loop(blocks - edge, blocks, pool, 0)
    pooled_stream.start(0)
    pooled_stream.start(pooled_parts - 1)

    @pl.when(inner)
    def _():
        out_events(members - 1, members)

    attend_stream.every(attend_stream.crossed)
    attend_stream.near_side()
    attend_stream.far_side()

    def level_of(group):
        paired = jnp.minimum(z, deep - 1 - z)
        step = jnp.where(group > 2 * paired, group - paired, (group + 1) // 2)
        downwards = jnp.where(group > 2 * paired, 2 * z > deep - 1, group % 2 == 1)
        return jnp.where(downwards, z - step, z + step)

    here = x * members + tp
    out_steps = (deep - 1) * members

    def columns_of(level, side, t):
        first = (level * 2 + side) * width + t * narrow
        return pl.ds(pl.multiple_of(first, narrow), narrow)

    def result_copy(level, hop):
        target = (here + hop) % (2 * members)
        return remote(
            rounded.at[level, pl.ds(pl.multiple_of(target * share, 16), share), :],
            out.at[:, columns_of(level, x, tp)],
            result_sems.at[0, level],
            result_sems.at[1, level],
            (z * 2 + target // members, target % members),
        )

    def result_own(level):
        return pltpu.make_async_copy(
            rounded.at[level, pl.ds(pl.multiple_of(here * share, 16), share), :],
            out.at[:, columns_of(level, x, tp)],
            result_sems.at[2, level],
        )

    def send_level(level):
        for hop in range(1, 2 * members):
            result_copy(level, hop).start()
        result_own(level).start()

    span = 2 * tile_rows if plane % (2 * tile_rows) == 0 else tile_rows
    ends_event = lambda n: jnp.where(inner, out_steps, n)

    def end_events(first, last):
        out_events(ends_event(first), ends_event(last))

    def by_span(act):
        def body(i, carry):
            act(pl.ds(pl.multiple_of(i * span, span), span))
            return carry

        lax.fori_loop(0, plane // span, body, 0)

    all_blocks = [(t, h) for t in range(members) for h in range(2)]

    def attended_term(part, levels):
        left = jnp.concatenate([attended[t, h, part, :] for t, h in all_blocks], axis=1)
        right = jnp.concatenate(
            [
                jnp.concatenate([w_out[level, t, 0 : 2 * hq, :] for t in range(members)], axis=0)
                for level in levels
            ],
            axis=1,
        )
        return jnp.dot(left, right, preferred_element_type=f32)

    def pooled_term(part, levels):
        left = jnp.concatenate([pooled[t, h, part, :] for t, h in all_blocks], axis=1)
        right = jnp.concatenate(
            [
                jnp.concatenate([w_out[level, t, 2 * hq :, :] for t in range(members)], axis=0)
                for level in levels
            ],
            axis=1,
        )
        return jnp.dot(left, right, preferred_element_type=f32)

    firsts = (level_of(0), level_of(1))
    end_events(0, members)

    def first_attended(part):
        result[part, :] = attended_term(part, firsts)

    by_span(first_attended)

    inner_parts = list(range(1, pooled_parts - 1)) + [0, pooled_parts - 1]
    for part in inner_parts:
        pooled_stream.direct(part)

    @pl.when(inner)
    def _():
        out_events(members, out_steps)

    for part in inner_parts:
        pooled_stream.crossed(part)
    pooled_stream.near_side()
    pooled_stream.far_side()

    def first_pooled(part):
        value = (result[part, :] + pooled_term(part, firsts)).astype(bf16)
        for index, level in enumerate(firsts):
            rounded[level, part, :] = value[:, index * narrow : (index + 1) * narrow]

    by_span(first_pooled)
    for level in firsts:
        send_level(level)

    def middle_level(group, carry):
        end_events((group - 1) * members, group * members)
        level = level_of(group)

        def whole_level(part):
            value = attended_term(part, [level]) + pooled_term(part, [level])
            rounded[level, part, :] = value.astype(bf16)

        by_span(whole_level)
        send_level(level)
        return carry

    lax.fori_loop(2, deep - 1, middle_level, 0)

    for ring in (in_ring, pool_ring):
        sends_done(ring)
    for c in range(members):
        out_both(c, sent)
    bulk(out_spare.at[pl.ds(0, members - 1)], spread_sems.at[0]).wait_send()
    bulk(sums.at[pl.ds(0, members - 1)], sum_sems.at[0]).wait_send()
    for stream in (token_stream, attend_stream, pooled_stream):
        stream.sent()

    level = level_of(deep - 1)
    for c in range(members):
        n = (deep - 2) * members + c
        end_events(n, n + 1)
        t = (tp - c + members) % members

        def last_level(part, c=c, t=t):
            left = jnp.concatenate(
                [attended[t, h, part, :] for h in range(2)]
                + [pooled[t, h, part, :] for h in range(2)],
                axis=1,
            )
            value = jnp.dot(left, w_out[level, t], preferred_element_type=f32)
            if c > 0:
                value = result[part, 0:narrow] + value
            if c == members - 1:
                rounded[level, part, :] = value.astype(bf16)
            else:
                result[part, 0:narrow] = value

        by_span(last_level)
    send_level(level)

    arrivals = out.at[:, pl.ds(0, (2 * members - 1) * narrow)]

    def results(level, carry):
        bulk(arrivals, result_sems.at[1, level]).wait_recv()
        return carry

    lax.fori_loop(0, deep, results, 0)

    lax.fori_loop(0, out_steps, out_sent, 0)
    for index, buffer, size in ((0, band, WINDOW), (2, pool_band, pool_pad)):

        @pl.when(has_down)
        def _(index=index, buffer=buffer, size=size):
            halo(index, buffer, size, False).wait_send()

        @pl.when(has_up)
        def _(index=index, buffer=buffer, size=size):
            halo(index + 1, buffer, size, True).wait_send()

    def results_sent(level, carry):
        bulk(rounded.at[level, most(plane), :], result_sems.at[0, level]).wait_send()
        result_own(level).wait()
        return carry

    lax.fori_loop(0, deep, results_sent, 0)


def plane_scratch(count, members, rows, features, depth, kw, qw, pw, width):
    hk, hq, hp = kw // 2, qw // 2, pw // 2
    narrow, plane, deep, tiles = width // members, 2 * rows, count // 2, rows // WINDOW
    dma = pltpu.SemaphoreType.DMA
    return [
        pltpu.VMEM((1, members * features), f32),
        pltpu.VMEM((1, HEAD), f32),
        pltpu.VMEM((1, HEAD), f32),
        pltpu.VMEM((plane // GRID_W, 2 * HEAD), f32),
        pltpu.VMEM((plane // GRID_W, 2 * HEAD), f32),
        pltpu.VMEM((GRID_W, 2 * HEAD), f32),
        pltpu.VMEM((GRID_W, 2 * HEAD), f32),
        pltpu.SMEM((2 * hq // HEAD,), f32),
        dma((8,)),
        pltpu.VMEM((rows, features), bf16),
        pltpu.VMEM((members, -(-tiles // 8) * 8, WINDOW), f32),
        pltpu.VMEM((2, count, rows, depth), bf16),
        pltpu.VMEM((count, depth, 2 * hk + hq), bf16),
        pltpu.VMEM((count, depth, hp), bf16),
        pltpu.VMEM((deep, members, 2 * (hp + hq), narrow), bf16),
        pltpu.VMEM((depth, 2 * hk + hq), bf16),
        pltpu.VMEM((depth, hp), bf16),
        pltpu.VMEM((members, 2 * (hp + hq), narrow), bf16),
        pltpu.VMEM((plane, 2 * hk + hq), f32),
        pltpu.VMEM((plane + 2 * WINDOW, 2 * hk), bf16),
        pltpu.VMEM((plane + 2 * pool_pad, hp), bf16),
        pltpu.VMEM((plane, 2 * HEAD), f32),
        pltpu.VMEM((plane, 2 * HEAD), f32),
        pltpu.VMEM((members, 2, plane, hq), bf16),
        pltpu.VMEM((members, 2, plane, hp), bf16),
        pltpu.VMEM((plane, 2 * narrow), f32),
        pltpu.VMEM((deep, plane, narrow), bf16),
        dma((5,)),
        dma((2,)),
        dma((2, count, in_parts)),
        dma((2, count, 1)),
        dma((2, deep, members)),
        dma((2,)),
        dma((1,)),
        dma((3, tiles)),
        dma((3,)),
        dma((3, 2 * tiles)),
        dma((3,)),
        dma((3, pooled_parts)),
        dma((3,)),
        dma((4,)),
        dma((4,)),
        dma((3, deep)),
    ]


def ring_scratch(count, members, rows, features, depth, kw, qw, pw, width):
    chips, share = members // 2, rows // members
    far = max(chips - 1, 1)
    dma = pltpu.SemaphoreType.DMA
    return [
        pltpu.VMEM((members, rows, features), bf16),
        pltpu.VMEM((count, rows, depth), bf16),
        pltpu.VMEM((count, depth, 2 * kw + pw), bf16),
        pltpu.VMEM((count, depth, qw), bf16),
        pltpu.VMEM((count, pw + qw, width), bf16),
        pltpu.VMEM((rows, 2 * kw + pw), f32),
        pltpu.VMEM((rows, qw), f32),
        pltpu.VMEM((rows + 2 * WINDOW, 2 * kw), bf16),
        pltpu.VMEM((rows + 2 * pool_pad, pw), bf16),
        pltpu.VMEM((rows, 2 * HEAD), f32),
        pltpu.VMEM((rows, 2 * HEAD), f32),
        pltpu.VMEM((rows, pw + qw), bf16),
        pltpu.VMEM((count, chips * share, width), bf16),
        pltpu.VMEM((count, chips * share, width), bf16),
        pltpu.VMEM((count, chips * share, width), bf16),
        pltpu.VMEM((count, far, share, width), bf16),
        pltpu.VMEM((count, far, share, width), bf16),
        pltpu.VMEM((count, share, width), bf16),
        dma((7,)),
        dma((2, count, chunks)),
        dma((count, chunks)),
        dma((2, count, chunks)),
        dma((count, chunks)),
        dma((2, count, chunks)),
        dma((count, chunks)),
        dma((far, token_chunks)),
        dma((far, token_chunks)),
        dma((chips, token_chunks)),
        dma((chips, token_chunks)),
        dma((4,)),
        dma((4,)),
        dma((count,)),
        dma((count,)),
        dma((count, far)),
        dma((count, far)),
        dma((count,)),
    ]


def shards(
    tokens,
    norm_gain,
    w_query,
    w_key,
    w_value,
    w_pool,
    query_gain,
    key_gain,
    sink_logit,
    w_out_pool,
    w_out_attn,
):
    count, members = lax.axis_size("sp"), lax.axis_size("tp")
    rows, features = tokens.shape
    depth, kw = w_key.shape
    qw, pw, width = w_query.shape[1], w_pool.shape[1], w_out_pool.shape[1]
    tables = [jnp.asarray(table) for table in rope_parts(count * rows)]
    anywhere = pl.BlockSpec(memory_space=pl.ANY)
    in_vmem = pl.BlockSpec(memory_space=pltpu.VMEM)
    sizes = (count, members, rows, features, depth, kw, qw, pw, width)
    shared = (
        members == 4
        and count % 2 == 0
        and count >= 4
        and rows % (2 * WINDOW) == 0
        and depth % (16 * in_parts) == 0
        and all(size % 256 == 0 for size in (kw, qw, pw))
        and width % (128 * members) == 0
    )
    grant = (46 if shared else 60) * 1024 * 1024
    specs = [anywhere] * 7 + [in_vmem] * 7 + [pl.BlockSpec(memory_space=pltpu.SMEM)]
    if shared:
        specs = [pl.BlockSpec(memory_space=pltpu.HBM)] * 15
    as_row = lambda gain: gain.reshape(1, HEAD)
    kernel, scratch = (plane_kernel, plane_scratch) if shared else (layer_kernel, ring_scratch)
    operands = (
        tokens,
        w_query,
        w_key,
        w_value,
        w_pool,
        w_out_pool,
        w_out_attn,
        norm_gain.reshape(1, -1),
        as_row(query_gain),
        as_row(key_gain),
        *tables,
        sink_logit,
    )
    shape = (rows // members, count * width)
    result = jax.ShapeDtypeStruct(shape, bf16)
    if shared:
        operands = [pltpu.with_memory_space_constraint(each, pltpu.HBM) for each in operands]
        result = pltpu.VMEM(shape, bf16)
    return pl.pallas_call(
        functools.partial(kernel, count, members),
        out_shape=result,
        in_specs=specs,
        out_specs=anywhere,
        scratch_shapes=scratch(*sizes),
        compiler_params=pltpu.CompilerParams(
            collective_id=0, has_side_effects=True, vmem_limit_bytes=grant
        ),
    )(*operands)


def solution(mesh):
    placed = (
        P("sp", "tp"),
        P(),
        P("sp", "tp"),
        P("sp", "tp"),
        P("sp", "tp"),
        P("sp", "tp"),
        P(),
        P(),
        P("tp"),
        P("tp", "sp"),
        P("tp", "sp"),
    )
    return jax.shard_map(
        shards, mesh=mesh, in_specs=placed, out_specs=P(("sp", "tp"), None), check_vma=False
    )
```

```python
import functools

import jax
import jax.numpy as jnp
import numpy as np
from jax import lax
from jax.experimental import pallas as pl
from jax.experimental.pallas import tpu as pltpu
from jax.sharding import PartitionSpec as P

HEAD = 64
POOL = 1024
WINDOW = 128
GRID_W = 64

eps = 1e-06
rope_base = 10000.0
neg_big = -1e30
pool_pad = 16
chunks = 4
token_chunks = 8
in_parts = 2
pooled_parts = 4
MESH = pl.DeviceIdType.MESH
f32, bf16 = jnp.float32, jnp.bfloat16


def rope_parts(rows_total):
    quarter = HEAD // 4
    steps = np.arange(quarter, dtype=np.float32) * np.float32(2.0) / np.float32(HEAD // 2)
    freqs = (np.float32(1.0) / np.float32(rope_base) ** steps).astype(np.float32)

    def table(count, first):
        angle = np.arange(count, dtype=np.float32)[:, None] * freqs
        twice = np.concatenate([angle, angle], axis=1).astype(np.float64)
        none = np.zeros_like(twice)
        made = []
        for part in (np.cos(twice), np.sin(twice)):
            head = [part, none] if first else [none, part]
            made.append(np.concatenate(head + head, axis=1).astype(np.float32))
        return made

    return table(rows_total // GRID_W, True) + table(GRID_W, False)


def ring_place(index, count, across):
    deep = count // across
    if across == 1 or deep % 2:
        return index
    z, x = index // across, index % across
    turn = deep - 1 - z
    inner = jnp.where(turn % 2 == 0, x - 1, across - 1 - x)
    return jnp.where(x == 0, z, deep + turn * (across - 1) + inner)


def ring_index(place, count, across):
    deep = count // across
    if across == 1 or deep % 2:
        return place
    rest = jnp.maximum(place - deep, 0)
    turn, inner = rest // (across - 1), rest % (across - 1)
    x = jnp.where(turn % 2 == 0, inner + 1, across - 1 - inner)
    return jnp.where(place < deep, place * across, (deep - 1 - turn) * across + x)


def norm_rope(raw, gain, cosine, sine, low_half, lead):
    squares = raw * raw
    low_sum = jnp.sum(jnp.where(low_half, squares, 0.0), axis=1, keepdims=True)
    high_sum = jnp.sum(jnp.where(low_half, 0.0, squares), axis=1, keepdims=True)
    mean = jnp.where(low_half, low_sum, high_sum) * (1.0 / HEAD)
    scaled = raw * lax.rsqrt(mean + eps) * gain
    turned = jnp.where(
        lead,
        -pltpu.roll(scaled, 2 * HEAD - HEAD // 4, 1),
        pltpu.roll(scaled, HEAD // 4, 1),
    )
    return scaled * cosine + turned * sine


def layer_kernel(
    count,
    members,
    tokens,
    wq,
    wk,
    wv,
    wp,
    wop,
    woa,
    norm_gain,
    query_gain,
    key_gain,
    row_cos,
    row_sin,
    col_cos,
    col_sin,
    sink,
    out,
    tok,
    normed,
    w_side,
    w_query,
    w_out,
    side,
    query,
    band,
    pool_band,
    cosines,
    sines,
    mixer,
    away,
    met,
    kept,
    y_send,
    y_recv,
    done,
    load_sem,
    side_send,
    side_recv,
    query_send,
    query_recv,
    out_send,
    out_recv,
    ty_send,
    ty_recv,
    td_send,
    td_recv,
    halo_send,
    halo_recv,
    met_send,
    met_recv,
    yy_send,
    yy_recv,
    done_sem,
):
    rows, features = tokens.shape
    depth, kw = wk.shape
    qw, pw, width = wq.shape[1], wp.shape[1], wop.shape[1]
    chips = members // 2
    share = rows // members
    half = (count - 1) // 2
    heads_k = kw // HEAD
    seq = count * rows
    across = chips

    me, tp = lax.axis_index("sp"), lax.axis_index("tp")
    chip, core = tp // 2, tp % 2
    partner = chip * 2 + 1 - core
    place = ring_place(me, count, across)
    owner_of = lambda spot: ring_index(spot, count, across)
    at = lambda offset: (place + offset + count) % count
    following, previous = owner_of(at(1)), owner_of(at(-1))

    loads = [
        pltpu.make_async_copy(wk, w_side.at[place, :, pl.ds(0, kw)], load_sem.at[0]),
        pltpu.make_async_copy(wv, w_side.at[place, :, pl.ds(kw, kw)], load_sem.at[1]),
        pltpu.make_async_copy(wp, w_side.at[place, :, pl.ds(2 * kw, pw)], load_sem.at[2]),
        pltpu.make_async_copy(tokens, tok.at[tp], load_sem.at[3]),
        pltpu.make_async_copy(wq, w_query.at[place], load_sem.at[4]),
        pltpu.make_async_copy(wop, w_out.at[place, pl.ds(0, pw), :], load_sem.at[5]),
        pltpu.make_async_copy(woa, w_out.at[place, pl.ds(pw, qw), :], load_sem.at[6]),
    ]
    for load in loads:
        load.start()

    barrier = pltpu.get_barrier_semaphore()
    greeted = [
        (following, tp),
        (previous, tp),
        (me, partner),
        ((me + 1) % count, tp),
        ((me + count - 1) % count, tp),
    ]
    greeted += [(me, (chip + hop) % chips * 2 + core) for hop in range(1, chips)]
    for device in greeted:
        pl.semaphore_signal(barrier, inc=1, device_id=device, device_id_type=MESH)
    pl.semaphore_wait(barrier, len(greeted))

    def remote(source, target, send_sem, recv_sem, device):
        return pltpu.make_async_remote_copy(
            src_ref=source,
            dst_ref=target,
            send_sem=send_sem,
            recv_sem=recv_sem,
            device_id=device,
            device_id_type=MESH,
        )

    def hop_copy(ring, way, spot, c):
        buffer, send_sem, recv_sem = ring
        size = buffer.shape[1] // chunks
        part = buffer.at[spot, pl.ds(pl.multiple_of(c * size, 16), size), :]
        device = (following if way == 0 else previous, tp)
        return remote(part, part, send_sem.at[way, spot, c], recv_sem.at[spot, c], device)

    def send_own(ring):
        for c in range(chunks):
            hop_copy(ring, 0, place, c).start()
            hop_copy(ring, 1, place, c).start()

    def event(ring, step, c):
        low, high = at(-step), at(step)
        hop_copy(ring, 0, low, c).wait_recv()

        @pl.when((step < half) | (c < chunks // 2))
        def _():
            hop_copy(ring, 0, low, c).start()

        hop_copy(ring, 1, high, c).wait_recv()

        @pl.when((step < half) | (c >= chunks // 2))
        def _():
            hop_copy(ring, 1, high, c).start()

    def events(ring, step):
        def body(c, carry):
            event(ring, step, c)
            return carry

        lax.fori_loop(0, chunks, body, 0)

    def opposite(ring):
        def body(c, carry):
            hop_copy(ring, 0, at(count // 2), c).wait_recv()
            return carry

        lax.fori_loop(0, chunks, body, 0)

    def sends_done(ring):
        def each(c, carry):
            hop_copy(ring, 0, place, c).wait_send()
            hop_copy(ring, 1, place, c).wait_send()

            def steps(step, inner):
                @pl.when((step < half) | (c < chunks // 2))
                def _():
                    hop_copy(ring, 0, at(-step), c).wait_send()

                @pl.when((step < half) | (c >= chunks // 2))
                def _():
                    hop_copy(ring, 1, at(step), c).wait_send()

                return inner

            return lax.fori_loop(1, half + 1, steps, carry)

        lax.fori_loop(0, chunks, each, 0)

    side_ring = (w_side, side_send, side_recv)
    query_ring = (w_query, query_send, query_recv)
    out_ring = (w_out, out_send, out_recv)

    for load in loads[:3]:
        load.wait()
    send_own(side_ring)
    loads[3].wait()

    token_rows = rows // token_chunks

    def token_part(owner, j):
        return tok.at[owner, pl.ds(pl.multiple_of(j * token_rows, 16), token_rows), :]

    def token_far(hop, owner, j):
        part = token_part(owner, j)
        target = (chip + hop) % chips * 2 + core
        return remote(
            part, part, ty_send.at[hop - 1, j], ty_recv.at[hop - 1, j], (me, target)
        )

    def token_near(slot, owner, j):
        part = token_part(owner, j)
        return remote(part, part, td_send.at[slot, j], td_recv.at[slot, j], (me, partner))

    def start_tokens(j, carry):
        for hop in range(1, chips):
            token_far(hop, tp, j).start()
        token_near(0, tp, j).start()
        return carry

    lax.fori_loop(0, token_chunks, start_tokens, 0)

    for g in range(rows // GRID_W):
        spot = pl.ds(me * (rows // GRID_W) + g, 1)
        grid_rows = pl.ds(g * GRID_W, GRID_W)
        cosines[grid_rows, :] = col_cos[...] + row_cos[spot, :]
        sines[grid_rows, :] = col_sin[...] + row_sin[spot, :]

    pieces = features // depth
    norm_rows = 32 if token_rows % 32 == 0 else 16

    def normalise(j):
        token_near(0, partner, j).wait_recv()
        for hop in range(1, chips):
            token_near(hop, (chip - hop + chips) % chips * 2 + 1 - core, j).wait_recv()

        def tile(i, carry):
            at_rows = pl.ds(pl.multiple_of(j * token_rows + i * norm_rows, 16), norm_rows)
            squares = jnp.zeros((norm_rows, 1), f32)
            for t in range(members):
                block = tok[t, at_rows, :].astype(f32)
                squares = squares + jnp.sum(block * block, axis=1, keepdims=True)
            scale = lax.rsqrt(squares / (members * features) + eps)
            for t in range(members):
                for piece in range(pieces):
                    first = piece * depth
                    gain = norm_gain[:, t * features + first : t * features + first + depth]
                    block = tok[t, at_rows, first : first + depth].astype(f32)
                    normed[t * pieces + piece, at_rows, :] = (block * scale * gain).astype(bf16)
            return carry

        lax.fori_loop(0, token_rows // norm_rows, tile, 0)

    def token_step(j, carry):
        for hop in range(1, chips):
            source = (chip - hop + chips) % chips * 2 + core
            token_far(hop, source, j).wait_recv()
            token_near(hop, source, j).start()

        @pl.when(j < half * chunks)
        def _():
            event(side_ring, j // chunks + 1, j % chunks)

        @pl.when(j >= 1)
        def _():
            normalise(j - 1)

        return carry

    lax.fori_loop(0, token_chunks, token_step, 0)
    normalise(token_chunks - 1)

    tile_rows = 256 if rows % 256 == 0 else 128

    def project(total, weights, spots, first=False):
        def body(i, carry):
            part = pl.ds(pl.multiple_of(i * tile_rows, tile_rows), tile_rows)
            terms = [
                jnp.dot(
                    normed[owner_of(spot), part, :], weights[spot], preferred_element_type=f32
                )
                for spot in spots
            ]
            value = functools.reduce(lambda a, b: a + b, terms)
            total[part, :] = value if first else total[part, :] + value
            return carry

        lax.fori_loop(0, rows // tile_rows, body, 0)

    project(side, w_side, [place], first=True)
    early = token_chunks // chunks

    def side_step(step, carry):
        @pl.when(step > early)
        def _():
            events(side_ring, step)

        project(side, w_side, [at(-step), at(step)])
        return carry

    lax.fori_loop(1, half + 1, side_step, 0)
    loads[4].wait()
    send_own(query_ring)
    opposite(side_ring)
    project(side, w_side, [at(count // 2)])

    twice = lambda gain: jnp.concatenate([gain[...], gain[...]], axis=1)
    query_gains, key_gains = twice(query_gain), twice(key_gain)
    lane = lax.broadcasted_iota(jnp.int32, (WINDOW, 2 * HEAD), 1)
    low_half = lane < HEAD
    lead = lane % (HEAD // 2) < HEAD // 4

    def prepare(i, carry):
        part = pl.ds(pl.multiple_of(i * WINDOW, WINDOW), WINDOW)
        shifted = pl.ds(pl.multiple_of((i + 1) * WINDOW, WINDOW), WINDOW)
        for h in range(kw // (2 * HEAD)):
            lanes = slice(h * 2 * HEAD, (h + 1) * 2 * HEAD)
            key = norm_rope(
                side[part, lanes], key_gains, cosines[part, :], sines[part, :], low_half, lead
            )
            band[shifted, lanes] = key.astype(bf16)
        band[shifted, kw : 2 * kw] = side[part, kw : 2 * kw].astype(bf16)
        pooled_rows = pl.ds(pl.multiple_of(i * WINDOW + pool_pad, pool_pad), WINDOW)
        pool_band[pooled_rows, :] = side[part, 2 * kw :].astype(bf16)
        return carry

    lax.fori_loop(0, rows // WINDOW, prepare, 0)

    before, behind = (me + count - 1) % count, (me + 1) % count

    def halo(index, buffer, size, upwards):
        if upwards:
            source, target, device = rows, 0, (behind, tp)
        else:
            source, target, device = size, rows + size, (before, tp)
        return remote(
            buffer.at[pl.ds(source, size), :],
            buffer.at[pl.ds(target, size), :],
            halo_send.at[index],
            halo_recv.at[index],
            device,
        )

    lower = [halo(0, band, WINDOW, False), halo(1, pool_band, pool_pad, False)]
    upper = [halo(2, band, WINDOW, True), halo(3, pool_band, pool_pad, True)]
    has_lower, has_upper = me > 0, me < count - 1

    @pl.when(has_lower)
    def _():
        for copy in lower:
            copy.start()

    @pl.when(has_upper)
    def _():
        for copy in upper:
            copy.start()

    @pl.when(jnp.logical_not(has_lower))
    def _():
        band[0:WINDOW, :] = jnp.zeros((WINDOW, 2 * kw), bf16)
        pool_band[0:pool_pad, :] = jnp.zeros((pool_pad, pw), bf16)

    @pl.when(jnp.logical_not(has_upper))
    def _():
        band[rows + WINDOW :, :] = jnp.zeros((WINDOW, 2 * kw), bf16)
        pool_band[rows + pool_pad :, :] = jnp.zeros((pool_pad, pw), bf16)

    project(query, w_query, [place], first=True)

    def query_step(step, carry):
        events(query_ring, step)
        project(query, w_query, [at(-step), at(step)])
        return carry

    lax.fori_loop(1, half + 1, query_step, 0)
    loads[5].wait()
    loads[6].wait()
    send_own(out_ring)

    @pl.when(has_lower)
    def _():
        for copy in upper:
            copy.wait_recv()

    @pl.when(has_upper)
    def _():
        for copy in lower:
            copy.wait_recv()

    level = tp * pw // (POOL // 4)
    reach = jnp.where(level == 0, 1, jnp.where(level == 1, 2, jnp.where(level == 2, 4, 8)))

    def pool(i, carry):
        wide = WINDOW + 2 * pool_pad
        part = pl.ds(pl.multiple_of(i * WINDOW, WINDOW), WINDOW)
        values = pool_band[pl.ds(pl.multiple_of(i * WINDOW, pool_pad), wide), :].astype(f32)
        total, chosen = values, None
        for step in range(4):
            size = 2**step
            total = total + pltpu.roll(total, wide - size, 0)
            shifted = pltpu.roll(total, size, 0)[pool_pad : pool_pad + WINDOW]
            chosen = shifted if chosen is None else jnp.where(level == step, shifted, chosen)
        spot = me * rows + i * WINDOW + lax.broadcasted_iota(jnp.int32, (WINDOW, 1), 0)
        low = jnp.maximum(spot - reach, 0)
        high = jnp.minimum(spot + reach - 1, seq - 1)
        mixer[part, 0:pw] = (chosen / (high - low + 1).astype(f32)).astype(bf16)
        return carry

    lax.fori_loop(0, rows // WINDOW, pool, 0)

    opposite(query_ring)
    project(query, w_query, [at(count // 2)])

    blocks = rows // WINDOW
    row = lax.broadcasted_iota(jnp.int32, (2 * WINDOW, 3 * WINDOW), 0) % WINDOW
    column = lax.broadcasted_iota(jnp.int32, (2 * WINDOW, 3 * WINDOW), 1)
    top_row = lax.broadcasted_iota(jnp.int32, (2 * WINDOW, 1), 0) < WINDOW

    def attend(i, carry):
        part = pl.ds(pl.multiple_of(i * WINDOW, WINDOW), WINDOW)
        key_rows = pl.ds(pl.multiple_of(i * WINDOW, WINDOW), 3 * WINDOW)
        key_pos = me * rows + i * WINDOW - WINDOW + column
        inside = (column >= row) & (column - row <= 2 * WINDOW) & (key_pos >= 0) & (key_pos < seq)
        for head in range(heads_k):
            lanes = slice(head * 2 * HEAD, (head + 1) * 2 * HEAD)
            rotated = norm_rope(
                query[part, lanes],
                query_gains,
                cosines[part, :],
                sines[part, :],
                low_half,
                lead,
            ) * HEAD ** (-0.5)
            other = pltpu.roll(rotated, HEAD, 1)
            if head % 2 == 0:
                pair = (jnp.where(low_half, rotated, 0.0), jnp.where(low_half, other, 0.0))
            else:
                pair = (jnp.where(low_half, 0.0, other), jnp.where(low_half, 0.0, rotated))
            stacked = jnp.concatenate(pair, axis=0).astype(bf16)
            tile = head // 2 * 2 * HEAD
            keys = band[key_rows, tile : tile + 2 * HEAD]
            values = band[key_rows, kw + tile : kw + tile + 2 * HEAD]
            scores = lax.dot_general(
                stacked, keys, (((1,), (1,)), ((), ())), preferred_element_type=f32
            )
            scores = jnp.where(inside, scores, neg_big)
            limit = jnp.where(top_row, sink[2 * head], sink[2 * head + 1])
            top = jnp.maximum(jnp.max(scores, axis=1, keepdims=True), limit)
            raised = jnp.exp(scores - top)
            totals = jnp.sum(raised, axis=1, keepdims=True) + jnp.exp(limit - top)
            weights = (raised * (1.0 / totals)).astype(bf16)
            result = jnp.dot(weights, values, preferred_element_type=f32)
            one, two = result[:WINDOW], result[WINDOW:]
            if head % 2 == 0:
                joined = jnp.where(low_half, one, pltpu.roll(two, HEAD, 1))
            else:
                joined = jnp.where(low_half, pltpu.roll(one, HEAD, 1), two)
            mixer[part, pw + head * 2 * HEAD : pw + (head + 1) * 2 * HEAD] = joined.astype(bf16)

        for c in range(chunks):

            @pl.when(i == ((c + 1) * blocks + chunks - 1) // chunks - 1)
            def _(c=c):
                event(out_ring, 1, c)

        return carry

    lax.fori_loop(0, blocks, attend, 0)

    def product(spot, which):
        left = jnp.concatenate(
            [
                mixer[pl.ds(pl.multiple_of((y * 2 + which) * share, 16), share), :]
                for y in range(chips)
            ],
            axis=0,
        )
        return jnp.dot(left, w_out[spot], preferred_element_type=f32).astype(bf16)

    def met_copy(spot):
        return remote(
            away.at[spot], met.at[spot], met_send.at[spot], met_recv.at[spot], (me, partner)
        )

    def y_copy(spot, hop):
        target = (chip + hop) % chips * 2 + core
        return remote(
            y_send.at[spot, hop - 1],
            y_recv.at[spot, hop - 1],
            yy_send.at[spot, hop - 1],
            yy_recv.at[spot, hop - 1],
            (me, target),
        )

    def done_copy(spot):
        columns = pl.ds(pl.multiple_of(owner_of(spot) * width, width), width)
        return pltpu.make_async_copy(done.at[spot], out.at[:, columns], done_sem.at[spot])

    def both_rows(spot, y):
        part = pl.ds(pl.multiple_of(y * share, 16), share)
        return kept[spot, part, :].astype(f32) + met[spot, part, :].astype(f32)

    def group(spots):
        def first(spot):
            away[spot] = product(spot, 1 - core)
            met_copy(spot).start()

        def second(spot):
            kept[spot] = product(spot, core)

        def third(spot):
            met_copy(spot).wait_recv()
            for hop in range(1, chips):
                y_send[spot, hop - 1] = both_rows(spot, (chip + hop) % chips).astype(bf16)
                y_copy(spot, hop).start()

        for part in (first, second, third):
            for spot in spots:
                part(spot)

    def finish(spot):
        total = both_rows(spot, chip)
        for hop in range(1, chips):
            y_copy(spot, hop).wait_recv()
            total = total + y_recv[spot, hop - 1].astype(f32)
        done[spot] = total.astype(bf16)
        done_copy(spot).start()

    group([place])

    def out_step(step, carry):
        @pl.when(step > 1)
        def _():
            events(out_ring, step)

        group([at(-step), at(step)])

        @pl.when(step == 1)
        def _():
            finish(place)

        @pl.when(step > 1)
        def _():
            finish(at(1 - step))
            finish(at(step - 1))

        return carry

    lax.fori_loop(1, half + 1, out_step, 0)
    opposite(out_ring)
    group([at(count // 2)])
    finish(at(-half))
    finish(at(half))
    finish(at(count // 2))

    for ring in (side_ring, query_ring, out_ring):
        sends_done(ring)

    def tokens_sent(j, carry):
        token_near(0, tp, j).wait_send()
        for hop in range(1, chips):
            token_far(hop, tp, j).wait_send()
            token_near(hop, (chip - hop + chips) % chips * 2 + core, j).wait_send()
        return carry

    lax.fori_loop(0, token_chunks, tokens_sent, 0)

    @pl.when(has_lower)
    def _():
        for copy in lower:
            copy.wait_send()

    @pl.when(has_upper)
    def _():
        for copy in upper:
            copy.wait_send()

    def blocks_sent(spot, carry):
        met_copy(spot).wait_send()
        for hop in range(1, chips):
            y_copy(spot, hop).wait_send()
        done_copy(spot).wait()
        return carry

    lax.fori_loop(0, count, blocks_sent, 0)


def plane_kernel(
    count,
    members,
    tokens,
    wq,
    wk,
    wv,
    wp,
    wop,
    woa,
    norm_gain_in,
    query_gain_in,
    key_gain_in,
    row_cos_in,
    row_sin_in,
    col_cos_in,
    col_sin_in,
    sink_in,
    out,
    norm_gain,
    query_gain,
    key_gain,
    row_cos,
    row_sin,
    col_cos,
    col_sin,
    sink,
    small_sem,
    raw,
    sums,
    normed,
    w_in,
    w_pool,
    w_out,
    in_spare,
    pool_spare,
    out_spare,
    total,
    band,
    pool_band,
    cosines,
    sines,
    attended,
    pooled,
    result,
    rounded,
    load_sem,
    sum_sems,
    in_sems,
    pool_sems,
    out_sems,
    x_sems,
    ring_sems,
    spread_sems,
    token_sems,
    token_bulk,
    attend_sems,
    attend_bulk,
    pooled_sems,
    pooled_bulk,
    halo_send,
    halo_recv,
    result_sems,
):
    rows, features = tokens.shape
    depth = wk.shape[0]
    hk, hq, hp = wk.shape[1] // 2, wq.shape[1] // 2, wp.shape[1] // 2
    width = wop.shape[1]
    narrow = width // members
    share = rows // members
    plane = 2 * rows
    heads_k = hk // HEAD
    seq = count * rows
    deep = count // 2
    pieces = features // depth
    tiles = rows // WINDOW
    grid = plane // GRID_W

    me, tp = lax.axis_index("sp"), lax.axis_index("tp")
    z, x = me // 2, me % 2
    y, core = tp // 2, tp % 2
    me_x, tp_y, tp_c = me + 1 - 2 * x, (1 - y) * 2 + core, y * 2 + 1 - core
    tp_yc = (1 - y) * 2 + 1 - core
    up, down = (me + 2) % count, (me + count - 2) % count
    has_up, has_down = z < deep - 1, z > 0
    inner = has_up & has_down

    mine = lambda size: pl.ds(pl.multiple_of(x * size, 128), size)
    other = lambda size: pl.ds(pl.multiple_of((1 - x) * size, 128), size)

    def load(group, source, target):
        pltpu.make_async_copy(source, target, load_sem.at[group]).start()

    def loaded(group, whole):
        pltpu.make_async_copy(whole, whole, load_sem.at[group]).wait()

    for target, pick in ((w_in.at[me], mine), (in_spare, other)):
        load(0, wk.at[:, pick(hk)], target.at[:, pl.ds(0, hk)])
        load(0, wv.at[:, pick(hk)], target.at[:, pl.ds(hk, hk)])
        load(0, wq.at[:, pick(hq)], target.at[:, pl.ds(2 * hk, hq)])
    load(1, tokens, raw)
    small = [
        pltpu.make_async_copy(source, target, small_sem.at[index])
        for index, (source, target) in enumerate(
            (
                (norm_gain_in, norm_gain),
                (query_gain_in, query_gain),
                (key_gain_in, key_gain),
                (row_cos_in.at[pl.ds(z * grid, grid), :], row_cos),
                (row_sin_in.at[pl.ds(z * grid, grid), :], row_sin),
                (col_cos_in, col_cos),
                (col_sin_in, col_sin),
                (sink_in, sink),
            )
        )
    ]
    for copy in small:
        copy.start()
    for target, pick in ((w_pool.at[me], mine), (pool_spare, other)):
        load(2, wp.at[:, pick(hp)], target)
    strip = lambda t: pl.ds(pl.multiple_of(t * narrow, narrow), narrow)
    strips = [(3, w_out.at[z, tp], tp)] + [(4, out_spare.at[t], t) for t in range(members)]
    for group, target, t in strips:
        load(group, woa.at[:, strip(t)], target.at[pl.ds(0, 2 * hq), :])
        load(group, wop.at[:, strip(t)], target.at[pl.ds(2 * hq, 2 * hp), :])

    barrier = pltpu.get_barrier_semaphore()
    greeted = [(up, tp), (down, tp), (me_x, tp)]
    for t in (tp_y, tp_c, tp_yc):
        greeted += [(me, t), (me_x, t)]
    for device in greeted:
        pl.semaphore_signal(barrier, inc=1, device_id=device, device_id_type=MESH)
    pl.semaphore_wait(barrier, len(greeted))

    def remote(source, target, send_sem, recv_sem, device):
        return pltpu.make_async_remote_copy(
            src_ref=source,
            dst_ref=target,
            send_sem=send_sem,
            recv_sem=recv_sem,
            device_id=device,
            device_id_type=MESH,
        )

    def by_rows(parts):
        def view(buffer, c):
            size = buffer.shape[0] // parts
            return buffer.at[pl.ds(pl.multiple_of(c * size, 16), size), :]

        return view

    in_ring = (w_in, in_spare, in_sems, 0, in_parts, by_rows(in_parts))
    pool_ring = (w_pool, pool_spare, pool_sems, 1, 1, by_rows(1))
    def z_copy(ring, way, source, c):
        buffer, _, sems, _, _, view = ring
        part = view(buffer.at[source], c)
        send = ring_sems.at[ring[3], way]
        return remote(part, part, send, sems.at[source, c], ((up, down)[way], tp))

    def x_copy(ring, source, c):
        buffer, spare, sems, first, _, view = ring
        return remote(
            view(spare, c),
            view(buffer.at[source], c),
            x_sems.at[first],
            sems.at[source, c],
            (me_x, tp),
        )

    def both_ways(ring, source, c, act):
        @pl.when(has_up)
        def _():
            act(z_copy(ring, 0, source, c))

        @pl.when(has_down)
        def _():
            act(z_copy(ring, 1, source, c))

    start = lambda copy: copy.start()

    def own_out(ring):
        for c in range(ring[4]):
            both_ways(ring, me, c, start)

    def side_out(ring):
        for c in range(ring[4]):
            x_copy(ring, me, c).start()

    def side_in(ring):
        for c in range(ring[4]):
            x_copy(ring, me_x, c).wait_recv()
            both_ways(ring, me_x, c, start)

    def passing(ring, n):
        parts = ring[4]
        step, j, c = n // (2 * parts) + 1, n // parts % 2, n % parts
        column = (x + j) % 2
        low, high = z - step, z + step
        return (low >= 0, low * 2 + column), (high < deep, high * 2 + column), c

    def event(ring, n):
        (is_low, low), (is_high, high), c = passing(ring, n)

        @pl.when(is_low)
        def _():
            z_copy(ring, 0, low, c).wait_recv()

            @pl.when(has_up)
            def _():
                z_copy(ring, 0, low, c).start()

        @pl.when(is_high)
        def _():
            z_copy(ring, 1, high, c).wait_recv()

            @pl.when(has_down)
            def _():
                z_copy(ring, 1, high, c).start()

    def events(ring, first, last):
        def body(n, carry):
            event(ring, n)
            return carry

        lax.fori_loop(first, last, body, 0)

    def all_events(ring):
        return (deep - 1) * 2 * ring[4]

    def bulk(whole, sem):
        return remote(whole, whole, sem, sem, (me_x, tp))

    def sends_done(buffer, sem, each):
        for level in range(deep):

            @pl.when(z == level)
            def _(level=level):
                if level < deep - 1:
                    whole = buffer.at[pl.ds(0, (level + 1) * each)]
                    bulk(whole, ring_sems.at[sem, 0]).wait_send()
                if level > 0:
                    whole = buffer.at[pl.ds(0, (deep - level) * each)]
                    bulk(whole, ring_sems.at[sem, 1]).wait_send()

    def out_copy(way, level, c):
        part = w_out.at[level, (tp - c + members) % members]
        send = ring_sems.at[2, way]
        return remote(part, part, send, out_sems.at[level, c], ((up, down)[way], tp))

    def spread(c):
        target = (tp + c) % members
        return remote(
            out_spare.at[target],
            w_out.at[z, tp],
            spread_sems.at[0],
            out_sems.at[z, c],
            (me, target),
        )

    def spread_in(c):
        owner = (tp - c + members) % members
        return remote(
            out_spare.at[owner],
            w_out.at[z, owner],
            spread_sems.at[0],
            out_sems.at[z, c],
            (me, owner),
        )

    def out_both(c, act):
        @pl.when(has_up)
        def _():
            act(out_copy(0, z, c))

        @pl.when(has_down)
        def _():
            act(out_copy(1, z, c))

    def out_event(n):
        step, c = n // members + 1, n % members
        low, high = z - step, z + step

        @pl.when(low >= 0)
        def _():
            out_copy(0, low, c).wait_recv()

            @pl.when(has_up)
            def _():
                out_copy(0, low, c).start()

        @pl.when(high < deep)
        def _():
            out_copy(1, high, c).wait_recv()

            @pl.when(has_down)
            def _():
                out_copy(1, high, c).start()

    def out_events(first, last):
        def body(n, carry):
            out_event(n)
            return carry

        lax.fori_loop(first, last, body, 0)

    loaded(0, w_in.at[pl.ds(0, 2)])
    for c in range(in_parts):
        x_copy(in_ring, me, c).start()
        both_ways(in_ring, me, c, start)

    loaded(1, raw)
    for copy in small:
        copy.wait()
    sums[tp] = jnp.zeros_like(sums[tp])
    for i in range(tiles):
        block = raw[i * WINDOW : (i + 1) * WINDOW, :].astype(f32)
        square = jnp.sum(block * block, axis=1, keepdims=True)
        turned = jnp.transpose(jnp.broadcast_to(square, (WINDOW, WINDOW)))
        sums[tp, i : i + 1, :] = turned[0:1, :]

    def sum_copy(owner, hop):
        target = (tp + hop) % members
        return remote(
            sums.at[owner],
            sums.at[owner],
            sum_sems.at[0],
            sum_sems.at[1],
            (me, target),
        )

    for hop in range(1, members):
        sum_copy(tp, hop).start()
    for g in range(grid):
        grid_rows = pl.ds(g * GRID_W, GRID_W)
        cosines[grid_rows, :] = col_cos[...] + row_cos[g : g + 1, :]
        sines[grid_rows, :] = col_sin[...] + row_sin[g : g + 1, :]
    bulk(sums.at[pl.ds(0, members - 1)], sum_sems.at[1]).wait_recv()
    squares = sums[0]
    for t in range(1, members):
        squares = squares + sums[t]
    scales = lax.rsqrt(squares / (members * features) + eps)

    class Stream:
        def __init__(self, view, all_sent, side, sems, bulk_sems, by_x):
            self.view, self.all_sent, self.side = view, all_sent, side
            self.sems, self.bulk_sems, self.by_x = sems, bulk_sems, by_x

        def copy(self, recv, side, owner, j, device):
            part = self.view(side, owner, j)
            return remote(part, part, self.bulk_sems.at[0], recv, device)

        def over_x(self, slot, side, owner, j):
            return self.copy(self.sems.at[2 * slot, j], side, owner, j, (me_x, tp))

        def over_y(self, slot, side, owner, j):
            return self.copy(self.sems.at[1 + slot, j], side, owner, j, (me, tp_y))

        def over_core(self, slot, side, owner, j):
            return self.copy(self.bulk_sems.at[1 + slot % 2], side, owner, j, (me, tp_c))

        def start(self, j):
            self.over_y(0, x, tp, j).start()
            self.over_x(0, x, tp, j).start()
            self.over_core(0, x, tp, j).start()

        def direct(self, j):
            self.over_y(0, x, tp_y, j).wait_recv()
            self.over_core(2, x, tp_y, j).start()

            @pl.when(self.by_x(j))
            def _():
                self.over_x(1, x, tp_y, j).start()

            self.over_x(0, 1 - x, tp, j).wait_recv()
            self.over_core(1, 1 - x, tp, j).start()

            @pl.when(jnp.logical_not(self.by_x(j)))
            def _():
                self.over_y(1, 1 - x, tp, j).start()

        def crossed(self, j):
            @pl.when(self.by_x(j))
            def _():
                self.over_x(1, 1 - x, tp_y, j).wait_recv()

            @pl.when(jnp.logical_not(self.by_x(j)))
            def _():
                self.over_y(1, 1 - x, tp_y, j).wait_recv()

            self.over_core(3, 1 - x, tp_y, j).start()

        def near_side(self):
            bulk(self.side, self.bulk_sems.at[1]).wait_recv()

        def far_side(self):
            bulk(self.side, self.bulk_sems.at[2]).wait_recv()

        def sent(self):
            bulk(self.all_sent, self.bulk_sems.at[0]).wait_send()

        def every(self, act):
            def body(j, carry):
                act(j)
                return carry

            lax.fori_loop(0, self.sems.shape[1], body, 0)

    def block_rows(j, size):
        return pl.ds(pl.multiple_of(j * size, 16), size)

    def token_view(side, owner, j):
        return normed.at[side, pl.ds(owner * pieces, pieces), block_rows(j, WINDOW), :]

    def attend_view(side, owner, j):
        return attended.at[owner, side, block_rows(j, WINDOW), :]

    def pooled_view(side, owner, j):
        return pooled.at[owner, side, block_rows(j, plane // pooled_parts), :]

    most = lambda size: pl.ds(0, size * (2 * members - 1) // (2 * members))
    token_stream = Stream(
        token_view,
        normed.at[:, :, most(rows), :],
        normed.at[0, pl.ds(0, count // 2)],
        token_sems,
        token_bulk,
        lambda j: j % 3 == 0,
    )
    attend_stream, pooled_stream = [
        Stream(
            view,
            buffer.at[:, :, most(plane), :],
            buffer.at[0],
            sems,
            bulk_sems,
            lambda j: j % 2 == 0,
        )
        for view, buffer, sems, bulk_sems in (
            (attend_view, attended, attend_sems, attend_bulk),
            (pooled_view, pooled, pooled_sems, pooled_bulk),
        )
    ]

    for i in range(tiles):
        here = slice(i * WINDOW, (i + 1) * WINDOW)
        scale = jnp.transpose(jnp.broadcast_to(scales[i : i + 1, :], (WINDOW, WINDOW)))
        for first in range(0, features, WINDOW):
            block = raw[here, first : first + WINDOW].astype(f32)
            gain = norm_gain[:, pl.ds(pl.multiple_of(tp * features + first, WINDOW), WINDOW)]
            value = (block * scale * gain).astype(bf16)
            inside = first % depth
            normed[x, tp * pieces + first // depth, here, inside : inside + WINDOW] = value
        token_stream.start(i)

    side_in(in_ring)
    whole = all_events(in_ring)
    reached = lambda part: whole * part // 24
    events(in_ring, 0, reached(4))

    def direct(j, carry):
        token_stream.direct(j)
        events(in_ring, reached(4 + 12 * j // tiles), reached(4 + 12 * (j + 1) // tiles))
        return carry

    lax.fori_loop(0, tiles, direct, 0)
    loaded(2, w_pool.at[pl.ds(0, 2)])
    loaded(3, w_out.at[0, 0])
    loaded(4, out_spare)
    side_out(pool_ring)
    for c in range(1, members):
        spread(c).start()
    token_stream.near_side()

    tile_rows = 256 if rows % 256 == 0 else 128
    per_side = rows // tile_rows

    def project(result, weights, level, side, first=False):
        def body(i, carry):
            within = pl.ds(pl.multiple_of(i * tile_rows, tile_rows), tile_rows)
            part = pl.ds(pl.multiple_of(side * rows + i * tile_rows, tile_rows), tile_rows)
            value = None if first else result[part, :]
            for j in range(2):
                term = jnp.dot(
                    normed[side, level * 2 + j, within, :],
                    weights[level * 2 + j],
                    preferred_element_type=f32,
                )
                value = term if value is None else value + term
            result[part, :] = value
            return carry

        lax.fori_loop(0, per_side, body, 0)

    def project_step(result, weights, step, side):
        @pl.when(z - step >= 0)
        def _():
            project(result, weights, z - step, side)

        @pl.when(z + step < deep)
        def _():
            project(result, weights, z + step, side)

    early = max(reached(16) // (2 * in_parts), 0)

    def crossed(j, carry):
        token_stream.crossed(j)

        @pl.when(j == 0)
        def _():
            project(total, w_in, z, x, first=True)

        @pl.when((j >= 1) & (j <= early))
        def _():
            project_step(total, w_in, j, x)

        events(in_ring, reached(16 + 4 * j // tiles), reached(16 + 4 * (j + 1) // tiles))
        return carry

    lax.fori_loop(0, tiles, crossed, 0)
    own_out(pool_ring)
    side_in(pool_ring)
    token_stream.far_side()
    project(total, w_in, z, 1 - x, first=True)

    @pl.when(inner)
    def _():
        events(pool_ring, 0, 2)


    def in_step(step, carry):
        each = 2 * in_parts
        events(in_ring, jnp.maximum((step - 1) * each, reached(20)), step * each)

        @pl.when(step > min(early, tiles - 1))
        def _():
            project_step(total, w_in, step, x)

        project_step(total, w_in, step, 1 - x)
        return carry

    lax.fori_loop(1, deep, in_step, 0)

    twice = lambda gain: jnp.concatenate([gain[...], gain[...]], axis=1)
    query_gains, key_gains = twice(query_gain), twice(key_gain)
    lane = lax.broadcasted_iota(jnp.int32, (WINDOW, 2 * HEAD), 1)
    low_half = lane < HEAD
    lead = lane % (HEAD // 2) < HEAD // 4
    blocks = plane // WINDOW

    def prepare(i, carry):
        part = pl.ds(pl.multiple_of(i * WINDOW, WINDOW), WINDOW)
        shifted = pl.ds(pl.multiple_of((i + 1) * WINDOW, WINDOW), WINDOW)
        for h in range(hk // (2 * HEAD)):
            lanes = slice(h * 2 * HEAD, (h + 1) * 2 * HEAD)
            key = norm_rope(
                total[part, lanes], key_gains, cosines[part, :], sines[part, :], low_half, lead
            )
            band[shifted, lanes] = key.astype(bf16)
        band[shifted, hk:] = total[part, hk : 2 * hk].astype(bf16)
        return carry

    lax.fori_loop(0, blocks, prepare, 0)

    def halo(index, buffer, size, upwards):
        if upwards:
            source, target, device = plane, 0, (up, tp)
        else:
            source, target, device = size, plane + size, (down, tp)
        return remote(
            buffer.at[pl.ds(source, size), :],
            buffer.at[pl.ds(target, size), :],
            halo_send.at[index],
            halo_recv.at[index],
            device,
        )

    def halo_out(index, buffer, size):
        @pl.when(has_down)
        def _():
            halo(index, buffer, size, False).start()

        @pl.when(has_up)
        def _():
            halo(index + 1, buffer, size, True).start()

        empty = jnp.zeros((size, buffer.shape[1]), bf16)

        @pl.when(jnp.logical_not(has_down))
        def _():
            buffer[0:size, :] = empty

        @pl.when(jnp.logical_not(has_up))
        def _():
            buffer[plane + size :, :] = empty

    def halo_in(index, buffer, size):
        @pl.when(has_up)
        def _():
            halo(index, buffer, size, False).wait_recv()

        @pl.when(has_down)
        def _():
            halo(index + 1, buffer, size, True).wait_recv()

    halo_out(0, band, WINDOW)

    @pl.when(inner)
    def _():
        events(pool_ring, 2, all_events(pool_ring))

    for c in range(members - 1):
        if c > 0:
            spread_in(c).wait_recv()
        out_both(c, start)

    row = lax.broadcasted_iota(jnp.int32, (2 * WINDOW, 3 * WINDOW), 0) % WINDOW
    column = lax.broadcasted_iota(jnp.int32, (2 * WINDOW, 3 * WINDOW), 1)
    top_row = lax.broadcasted_iota(jnp.int32, (2 * WINDOW, 1), 0) < WINDOW

    def attend(turn, carry):
        @pl.when(turn == blocks - 2)
        def _():
            halo_in(0, band, WINDOW)

        i = (turn + 1) % blocks
        part = pl.ds(pl.multiple_of(i * WINDOW, WINDOW), WINDOW)
        key_rows = pl.ds(pl.multiple_of(i * WINDOW, WINDOW), 3 * WINDOW)
        key_pos = z * plane + i * WINDOW - WINDOW + column
        inside = (column >= row) & (column - row <= 2 * WINDOW) & (key_pos >= 0) & (key_pos < seq)
        for head in range(heads_k):
            lanes = slice(2 * hk + head * 2 * HEAD, 2 * hk + (head + 1) * 2 * HEAD)
            rotated = norm_rope(
                total[part, lanes],
                query_gains,
                cosines[part, :],
                sines[part, :],
                low_half,
                lead,
            ) * HEAD ** (-0.5)
            swapped = pltpu.roll(rotated, HEAD, 1)
            if head % 2 == 0:
                pair = (jnp.where(low_half, rotated, 0.0), jnp.where(low_half, swapped, 0.0))
            else:
                pair = (jnp.where(low_half, 0.0, swapped), jnp.where(low_half, 0.0, rotated))
            stacked = jnp.concatenate(pair, axis=0).astype(bf16)
            tile = head // 2 * 2 * HEAD
            keys = band[key_rows, tile : tile + 2 * HEAD]
            values = band[key_rows, hk + tile : hk + tile + 2 * HEAD]
            scores = lax.dot_general(
                stacked, keys, (((1,), (1,)), ((), ())), preferred_element_type=f32
            )
            scores = jnp.where(inside, scores, neg_big)
            first = x * 2 * heads_k + 2 * head
            limit = jnp.where(top_row, sink[first], sink[first + 1])
            top = jnp.maximum(jnp.max(scores, axis=1, keepdims=True), limit)
            raised = jnp.exp(scores - top)
            totals = jnp.sum(raised, axis=1, keepdims=True) + jnp.exp(limit - top)
            weights = (raised * (1.0 / totals)).astype(bf16)
            result = jnp.dot(weights, values, preferred_element_type=f32)
            one, two = result[:WINDOW], result[WINDOW:]
            if head % 2 == 0:
                joined = jnp.where(low_half, one, pltpu.roll(two, HEAD, 1))
            else:
                joined = jnp.where(low_half, pltpu.roll(one, HEAD, 1), two)
            attended[tp, x, part, head * 2 * HEAD : (head + 1) * 2 * HEAD] = joined.astype(bf16)
        attend_stream.start(i)

        @pl.when(turn >= behind)
        def _():
            attend_stream.direct((turn - behind + 1) % blocks)

        return carry

    behind = 5
    lax.fori_loop(0, blocks, attend, 0)

    events(pool_ring, jnp.where(inner, all_events(pool_ring), 0), all_events(pool_ring))

    for side in range(2):

        def pool_project(i, carry, side=side):
            part = pl.ds(pl.multiple_of(i * tile_rows, tile_rows), tile_rows)
            first = side * rows + pool_pad + i * tile_rows
            left = jnp.concatenate([normed[side, source, part, :] for source in range(count)], axis=1)
            right = w_pool[...].reshape(count * depth, hp)
            value = jnp.dot(left, right, preferred_element_type=f32)
            pool_band[pl.ds(pl.multiple_of(first, pool_pad), tile_rows), :] = value.astype(bf16)
            return carry

        lax.fori_loop(0, per_side, pool_project, 0)
    halo_out(2, pool_band, pool_pad)
    spread_in(members - 1).wait_recv()
    out_both(members - 1, start)

    @pl.when(inner)
    def _():
        out_events(0, members - 1)

    level = (tp * 2 + x) * hp // (POOL // 4)
    reach = jnp.where(level == 0, 1, jnp.where(level == 1, 2, jnp.where(level == 2, 4, 8)))

    def pool(i, carry):
        wide = WINDOW + 2 * pool_pad
        part = pl.ds(pl.multiple_of(i * WINDOW, WINDOW), WINDOW)
        running = pool_band[pl.ds(pl.multiple_of(i * WINDOW, pool_pad), wide), :].astype(f32)
        chosen = None
        for step in range(4):
            size = 2**step
            running = running + pltpu.roll(running, wide - size, 0)
            shifted = pltpu.roll(running, size, 0)[pool_pad : pool_pad + WINDOW]
            chosen = shifted if chosen is None else jnp.where(level == step, shifted, chosen)
        spot = z * plane + i * WINDOW + lax.broadcasted_iota(jnp.int32, (WINDOW, 1), 0)
        low = jnp.maximum(spot - reach, 0)
        high = jnp.minimum(spot + reach - 1, seq - 1)
        pooled[tp, x, part, :] = (chosen / (high - low + 1).astype(f32)).astype(bf16)
        return carry

    edge = blocks // pooled_parts
    lax.fori_loop(edge, blocks - edge, pool, 0)
    for part in range(1, pooled_parts - 1):
        pooled_stream.start(part)
    for turn in range(blocks - behind, blocks):
        attend_stream.direct((turn + 1) % blocks)
    halo_in(2, pool_band, pool_pad)
    lax.fori_loop(0, edge, pool, 0)
    lax.fori_loop(blocks - edge, blocks, pool, 0)
    pooled_stream.start(0)
    pooled_stream.start(pooled_parts - 1)

    @pl.when(inner)
    def _():
        out_events(members - 1, members)

    attend_stream.every(attend_stream.crossed)
    attend_stream.near_side()
    attend_stream.far_side()

    def level_of(group):
        paired = jnp.minimum(z, deep - 1 - z)
        step = jnp.where(group > 2 * paired, group - paired, (group + 1) // 2)
        downwards = jnp.where(group > 2 * paired, 2 * z > deep - 1, group % 2 == 1)
        return jnp.where(downwards, z - step, z + step)

    here = x * members + tp
    out_steps = (deep - 1) * members

    def columns_of(level, side, t):
        first = (level * 2 + side) * width + t * narrow
        return pl.ds(pl.multiple_of(first, narrow), narrow)

    def result_copy(level, side, t):
        first = pl.multiple_of((side * members + t) * share, 16)
        return remote(
            rounded.at[level, pl.ds(first, share), :],
            out.at[:, columns_of(level, x, tp)],
            result_sems.at[0, level],
            result_sems.at[1, level],
            (z * 2 + side, t),
        )

    def result_own(level):
        return pltpu.make_async_copy(
            rounded.at[level, pl.ds(pl.multiple_of(here * share, 16), share), :],
            out.at[:, columns_of(level, x, tp)],
            result_sems.at[2, level],
        )

    def send_far(level):
        for hop in range(members):
            result_copy(level, 1 - x, (tp + hop) % members).start()

    def send_near(level):
        for hop in range(1, members):
            result_copy(level, x, (tp + hop) % members).start()
        result_own(level).start()

    def send_level(level):
        send_far(level)
        send_near(level)

    span = 2 * tile_rows if plane % (2 * tile_rows) == 0 else tile_rows
    ends_event = lambda n: jnp.where(inner, out_steps, n)

    def end_events(first, last):
        out_events(ends_event(first), ends_event(last))

    def by_span(act):
        def body(i, carry):
            act(pl.ds(pl.multiple_of(i * span, span), span))
            return carry

        lax.fori_loop(0, plane // span, body, 0)

    all_blocks = [(t, h) for t in range(members) for h in range(2)]

    def attended_term(part, levels):
        left = jnp.concatenate([attended[t, h, part, :] for t, h in all_blocks], axis=1)
        right = jnp.concatenate(
            [
                jnp.concatenate([w_out[level, t, 0 : 2 * hq, :] for t in range(members)], axis=0)
                for level in levels
            ],
            axis=1,
        )
        return jnp.dot(left, right, preferred_element_type=f32)

    def pooled_term(part, levels):
        left = jnp.concatenate([pooled[t, h, part, :] for t, h in all_blocks], axis=1)
        right = jnp.concatenate(
            [
                jnp.concatenate([w_out[level, t, 2 * hq :, :] for t in range(members)], axis=0)
                for level in levels
            ],
            axis=1,
        )
        return jnp.dot(left, right, preferred_element_type=f32)

    firsts = (level_of(0), level_of(1))
    end_events(0, members)

    def first_attended(part):
        result[part, :] = attended_term(part, firsts)

    by_span(first_attended)

    inner_parts = list(range(1, pooled_parts - 1)) + [0, pooled_parts - 1]
    for part in inner_parts:
        pooled_stream.direct(part)

    @pl.when(inner)
    def _():
        out_events(members, out_steps)

    for part in inner_parts:
        pooled_stream.crossed(part)
    pooled_stream.near_side()
    pooled_stream.far_side()

    def first_pooled(part):
        value = (result[part, :] + pooled_term(part, firsts)).astype(bf16)
        for index, level in enumerate(firsts):
            rounded[level, part, :] = value[:, index * narrow : (index + 1) * narrow]

    by_span(first_pooled)
    for level in firsts:
        send_level(level)

    def middle_level(group, carry):
        end_events((group - 1) * members, group * members)
        level = level_of(group)

        def whole_level(part):
            value = attended_term(part, [level]) + pooled_term(part, [level])
            rounded[level, part, :] = value.astype(bf16)

        by_span(whole_level)
        send_level(level)
        return carry

    lax.fori_loop(2, deep - 1, middle_level, 0)

    for ring in (in_ring, pool_ring):
        bulk(ring[1], x_sems.at[ring[3]]).wait_send()
        sends_done(ring[0], ring[3], 2)
    bulk(out_spare.at[pl.ds(0, members - 1)], spread_sems.at[0]).wait_send()
    bulk(sums.at[pl.ds(0, members - 1)], sum_sems.at[0]).wait_send()
    for stream in (token_stream, attend_stream, pooled_stream):
        stream.sent()

    level = level_of(deep - 1)
    for c in range(members):
        n = (deep - 2) * members + c
        end_events(n, n + 1)
        t = (tp - c + members) % members

        def last_level(part, c=c, t=t):
            left = jnp.concatenate(
                [attended[t, h, part, :] for h in range(2)]
                + [pooled[t, h, part, :] for h in range(2)],
                axis=1,
            )
            value = jnp.dot(left, w_out[level, t], preferred_element_type=f32)
            if c > 0:
                value = result[part, 0:narrow] + value
            if c == members - 1:
                rounded[level, part, :] = value.astype(bf16)
            else:
                result[part, 0:narrow] = value

        if c < members - 1:
            by_span(last_level)
            continue
        for side, send in ((1 - x, send_far), (x, send_near)):
            for start_row in range(0, rows, rows // 2):
                first = pl.multiple_of(side * rows + start_row, rows // 2)
                last_level(pl.ds(first, rows // 2))
            send(level)

    arrivals = out.at[:, pl.ds(0, (2 * members - 1) * narrow)]

    def results(level, carry):
        bulk(arrivals, result_sems.at[1, level]).wait_recv()
        return carry

    lax.fori_loop(0, deep, results, 0)

    sends_done(w_out, 2, 1)
    for index, buffer, size in ((0, band, WINDOW), (2, pool_band, pool_pad)):

        @pl.when(has_down)
        def _(index=index, buffer=buffer, size=size):
            halo(index, buffer, size, False).wait_send()

        @pl.when(has_up)
        def _(index=index, buffer=buffer, size=size):
            halo(index + 1, buffer, size, True).wait_send()

    def results_sent(level, carry):
        bulk(rounded.at[level, most(plane), :], result_sems.at[0, level]).wait_send()
        result_own(level).wait()
        return carry

    lax.fori_loop(0, deep, results_sent, 0)


def plane_scratch(count, members, rows, features, depth, kw, qw, pw, width):
    hk, hq, hp = kw // 2, qw // 2, pw // 2
    narrow, plane, deep, tiles = width // members, 2 * rows, count // 2, rows // WINDOW
    dma = pltpu.SemaphoreType.DMA
    return [
        pltpu.VMEM((1, members * features), f32),
        pltpu.VMEM((1, HEAD), f32),
        pltpu.VMEM((1, HEAD), f32),
        pltpu.VMEM((plane // GRID_W, 2 * HEAD), f32),
        pltpu.VMEM((plane // GRID_W, 2 * HEAD), f32),
        pltpu.VMEM((GRID_W, 2 * HEAD), f32),
        pltpu.VMEM((GRID_W, 2 * HEAD), f32),
        pltpu.SMEM((2 * hq // HEAD,), f32),
        dma((8,)),
        pltpu.VMEM((rows, features), bf16),
        pltpu.VMEM((members, -(-tiles // 8) * 8, WINDOW), f32),
        pltpu.VMEM((2, count, rows, depth), bf16),
        pltpu.VMEM((count, depth, 2 * hk + hq), bf16),
        pltpu.VMEM((count, depth, hp), bf16),
        pltpu.VMEM((deep, members, 2 * (hp + hq), narrow), bf16),
        pltpu.VMEM((depth, 2 * hk + hq), bf16),
        pltpu.VMEM((depth, hp), bf16),
        pltpu.VMEM((members, 2 * (hp + hq), narrow), bf16),
        pltpu.VMEM((plane, 2 * hk + hq), f32),
        pltpu.VMEM((plane + 2 * WINDOW, 2 * hk), bf16),
        pltpu.VMEM((plane + 2 * pool_pad, hp), bf16),
        pltpu.VMEM((plane, 2 * HEAD), f32),
        pltpu.VMEM((plane, 2 * HEAD), f32),
        pltpu.VMEM((members, 2, plane, hq), bf16),
        pltpu.VMEM((members, 2, plane, hp), bf16),
        pltpu.VMEM((plane, 2 * narrow), f32),
        pltpu.VMEM((deep, plane, narrow), bf16),
        dma((5,)),
        dma((2,)),
        dma((count, in_parts)),
        dma((count, 1)),
        dma((deep, members)),
        dma((2,)),
        dma((3, 2)),
        dma((1,)),
        dma((3, tiles)),
        dma((3,)),
        dma((3, 2 * tiles)),
        dma((3,)),
        dma((3, pooled_parts)),
        dma((3,)),
        dma((4,)),
        dma((4,)),
        dma((3, deep)),
    ]


def ring_scratch(count, members, rows, features, depth, kw, qw, pw, width):
    chips, share = members // 2, rows // members
    far = max(chips - 1, 1)
    dma = pltpu.SemaphoreType.DMA
    return [
        pltpu.VMEM((members, rows, features), bf16),
        pltpu.VMEM((count, rows, depth), bf16),
        pltpu.VMEM((count, depth, 2 * kw + pw), bf16),
        pltpu.VMEM((count, depth, qw), bf16),
        pltpu.VMEM((count, pw + qw, width), bf16),
        pltpu.VMEM((rows, 2 * kw + pw), f32),
        pltpu.VMEM((rows, qw), f32),
        pltpu.VMEM((rows + 2 * WINDOW, 2 * kw), bf16),
        pltpu.VMEM((rows + 2 * pool_pad, pw), bf16),
        pltpu.VMEM((rows, 2 * HEAD), f32),
        pltpu.VMEM((rows, 2 * HEAD), f32),
        pltpu.VMEM((rows, pw + qw), bf16),
        pltpu.VMEM((count, chips * share, width), bf16),
        pltpu.VMEM((count, chips * share, width), bf16),
        pltpu.VMEM((count, chips * share, width), bf16),
        pltpu.VMEM((count, far, share, width), bf16),
        pltpu.VMEM((count, far, share, width), bf16),
        pltpu.VMEM((count, share, width), bf16),
        dma((7,)),
        dma((2, count, chunks)),
        dma((count, chunks)),
        dma((2, count, chunks)),
        dma((count, chunks)),
        dma((2, count, chunks)),
        dma((count, chunks)),
        dma((far, token_chunks)),
        dma((far, token_chunks)),
        dma((chips, token_chunks)),
        dma((chips, token_chunks)),
        dma((4,)),
        dma((4,)),
        dma((count,)),
        dma((count,)),
        dma((count, far)),
        dma((count, far)),
        dma((count,)),
    ]


def shards(
    tokens,
    norm_gain,
    w_query,
    w_key,
    w_value,
    w_pool,
    query_gain,
    key_gain,
    sink_logit,
    w_out_pool,
    w_out_attn,
):
    count, members = lax.axis_size("sp"), lax.axis_size("tp")
    rows, features = tokens.shape
    depth, kw = w_key.shape
    qw, pw, width = w_query.shape[1], w_pool.shape[1], w_out_pool.shape[1]
    tables = [jnp.asarray(table) for table in rope_parts(count * rows)]
    anywhere = pl.BlockSpec(memory_space=pl.ANY)
    in_vmem = pl.BlockSpec(memory_space=pltpu.VMEM)
    sizes = (count, members, rows, features, depth, kw, qw, pw, width)
    shared = (
        members == 4
        and count % 2 == 0
        and count >= 4
        and rows % (2 * WINDOW) == 0
        and depth % (16 * in_parts) == 0
        and all(size % 256 == 0 for size in (kw, qw, pw))
        and width % (128 * members) == 0
    )
    grant = (46 if shared else 60) * 1024 * 1024
    specs = [anywhere] * 7 + [in_vmem] * 7 + [pl.BlockSpec(memory_space=pltpu.SMEM)]
    if shared:
        specs = [pl.BlockSpec(memory_space=pltpu.HBM)] * 15
    as_row = lambda gain: gain.reshape(1, HEAD)
    kernel, scratch = (plane_kernel, plane_scratch) if shared else (layer_kernel, ring_scratch)
    operands = (
        tokens,
        w_query,
        w_key,
        w_value,
        w_pool,
        w_out_pool,
        w_out_attn,
        norm_gain.reshape(1, -1),
        as_row(query_gain),
        as_row(key_gain),
        *tables,
        sink_logit,
    )
    shape = (rows // members, count * width)
    result = jax.ShapeDtypeStruct(shape, bf16)
    if shared:
        operands = [pltpu.with_memory_space_constraint(each, pltpu.HBM) for each in operands]
        result = pltpu.VMEM(shape, bf16)
    return pl.pallas_call(
        functools.partial(kernel, count, members),
        out_shape=result,
        in_specs=specs,
        out_specs=anywhere,
        scratch_shapes=scratch(*sizes),
        compiler_params=pltpu.CompilerParams(
            collective_id=0, has_side_effects=True, vmem_limit_bytes=grant
        ),
    )(*operands)


def solution(mesh):
    placed = (
        P("sp", "tp"),
        P(),
        P("sp", "tp"),
        P("sp", "tp"),
        P("sp", "tp"),
        P("sp", "tp"),
        P(),
        P(),
        P("tp"),
        P("tp", "sp"),
        P("tp", "sp"),
    )
    return jax.shard_map(
        shards, mesh=mesh, in_specs=placed, out_specs=P(("sp", "tp"), None), check_vma=False
    )
```

```python
import functools

import jax
import jax.numpy as jnp
import numpy as np
from jax import lax
from jax.experimental import pallas as pl
from jax.experimental.pallas import tpu as pltpu
from jax.sharding import PartitionSpec as P

HEAD = 64
POOL = 1024
WINDOW = 128
GRID_W = 64

eps = 1e-06
rope_base = 10000.0
neg_big = -1e30
pool_pad = 16
chunks = 4
token_chunks = 8
in_parts = 2
pooled_parts = 4
MESH = pl.DeviceIdType.MESH
f32, bf16 = jnp.float32, jnp.bfloat16


def rope_parts(rows_total):
    quarter = HEAD // 4
    steps = np.arange(quarter, dtype=np.float32) * np.float32(2.0) / np.float32(HEAD // 2)
    freqs = (np.float32(1.0) / np.float32(rope_base) ** steps).astype(np.float32)

    def table(count, first):
        angle = np.arange(count, dtype=np.float32)[:, None] * freqs
        twice = np.concatenate([angle, angle], axis=1).astype(np.float64)
        none = np.zeros_like(twice)
        made = []
        for part in (np.cos(twice), np.sin(twice)):
            head = [part, none] if first else [none, part]
            made.append(np.concatenate(head + head, axis=1).astype(np.float32))
        return made

    return table(rows_total // GRID_W, True) + table(GRID_W, False)


def ring_place(index, count, across):
    deep = count // across
    if across == 1 or deep % 2:
        return index
    z, x = index // across, index % across
    turn = deep - 1 - z
    inner = jnp.where(turn % 2 == 0, x - 1, across - 1 - x)
    return jnp.where(x == 0, z, deep + turn * (across - 1) + inner)


def ring_index(place, count, across):
    deep = count // across
    if across == 1 or deep % 2:
        return place
    rest = jnp.maximum(place - deep, 0)
    turn, inner = rest // (across - 1), rest % (across - 1)
    x = jnp.where(turn % 2 == 0, inner + 1, across - 1 - inner)
    return jnp.where(place < deep, place * across, (deep - 1 - turn) * across + x)


def norm_rope(raw, gain, cosine, sine, low_half, lead):
    squares = raw * raw
    low_sum = jnp.sum(jnp.where(low_half, squares, 0.0), axis=1, keepdims=True)
    high_sum = jnp.sum(jnp.where(low_half, 0.0, squares), axis=1, keepdims=True)
    mean = jnp.where(low_half, low_sum, high_sum) * (1.0 / HEAD)
    scaled = raw * lax.rsqrt(mean + eps) * gain
    turned = jnp.where(
        lead,
        -pltpu.roll(scaled, 2 * HEAD - HEAD // 4, 1),
        pltpu.roll(scaled, HEAD // 4, 1),
    )
    return scaled * cosine + turned * sine


def layer_kernel(
    count,
    members,
    tokens,
    wq,
    wk,
    wv,
    wp,
    wop,
    woa,
    norm_gain,
    query_gain,
    key_gain,
    row_cos,
    row_sin,
    col_cos,
    col_sin,
    sink,
    out,
    tok,
    normed,
    w_side,
    w_query,
    w_out,
    side,
    query,
    band,
    pool_band,
    cosines,
    sines,
    mixer,
    away,
    met,
    kept,
    y_send,
    y_recv,
    done,
    load_sem,
    side_send,
    side_recv,
    query_send,
    query_recv,
    out_send,
    out_recv,
    ty_send,
    ty_recv,
    td_send,
    td_recv,
    halo_send,
    halo_recv,
    met_send,
    met_recv,
    yy_send,
    yy_recv,
    done_sem,
):
    rows, features = tokens.shape
    depth, kw = wk.shape
    qw, pw, width = wq.shape[1], wp.shape[1], wop.shape[1]
    chips = members // 2
    share = rows // members
    half = (count - 1) // 2
    heads_k = kw // HEAD
    seq = count * rows
    across = chips

    me, tp = lax.axis_index("sp"), lax.axis_index("tp")
    chip, core = tp // 2, tp % 2
    partner = chip * 2 + 1 - core
    place = ring_place(me, count, across)
    owner_of = lambda spot: ring_index(spot, count, across)
    at = lambda offset: (place + offset + count) % count
    following, previous = owner_of(at(1)), owner_of(at(-1))

    loads = [
        pltpu.make_async_copy(wk, w_side.at[place, :, pl.ds(0, kw)], load_sem.at[0]),
        pltpu.make_async_copy(wv, w_side.at[place, :, pl.ds(kw, kw)], load_sem.at[1]),
        pltpu.make_async_copy(wp, w_side.at[place, :, pl.ds(2 * kw, pw)], load_sem.at[2]),
        pltpu.make_async_copy(tokens, tok.at[tp], load_sem.at[3]),
        pltpu.make_async_copy(wq, w_query.at[place], load_sem.at[4]),
        pltpu.make_async_copy(wop, w_out.at[place, pl.ds(0, pw), :], load_sem.at[5]),
        pltpu.make_async_copy(woa, w_out.at[place, pl.ds(pw, qw), :], load_sem.at[6]),
    ]
    for load in loads:
        load.start()

    barrier = pltpu.get_barrier_semaphore()
    greeted = [
        (following, tp),
        (previous, tp),
        (me, partner),
        ((me + 1) % count, tp),
        ((me + count - 1) % count, tp),
    ]
    greeted += [(me, (chip + hop) % chips * 2 + core) for hop in range(1, chips)]
    for device in greeted:
        pl.semaphore_signal(barrier, inc=1, device_id=device, device_id_type=MESH)
    pl.semaphore_wait(barrier, len(greeted))

    def remote(source, target, send_sem, recv_sem, device):
        return pltpu.make_async_remote_copy(
            src_ref=source,
            dst_ref=target,
            send_sem=send_sem,
            recv_sem=recv_sem,
            device_id=device,
            device_id_type=MESH,
        )

    def hop_copy(ring, way, spot, c):
        buffer, send_sem, recv_sem = ring
        size = buffer.shape[1] // chunks
        part = buffer.at[spot, pl.ds(pl.multiple_of(c * size, 16), size), :]
        device = (following if way == 0 else previous, tp)
        return remote(part, part, send_sem.at[way, spot, c], recv_sem.at[spot, c], device)

    def send_own(ring):
        for c in range(chunks):
            hop_copy(ring, 0, place, c).start()
            hop_copy(ring, 1, place, c).start()

    def event(ring, step, c):
        low, high = at(-step), at(step)
        hop_copy(ring, 0, low, c).wait_recv()

        @pl.when((step < half) | (c < chunks // 2))
        def _():
            hop_copy(ring, 0, low, c).start()

        hop_copy(ring, 1, high, c).wait_recv()

        @pl.when((step < half) | (c >= chunks // 2))
        def _():
            hop_copy(ring, 1, high, c).start()

    def events(ring, step):
        def body(c, carry):
            event(ring, step, c)
            return carry

        lax.fori_loop(0, chunks, body, 0)

    def opposite(ring):
        def body(c, carry):
            hop_copy(ring, 0, at(count // 2), c).wait_recv()
            return carry

        lax.fori_loop(0, chunks, body, 0)

    def sends_done(ring):
        def each(c, carry):
            hop_copy(ring, 0, place, c).wait_send()
            hop_copy(ring, 1, place, c).wait_send()

            def steps(step, inner):
                @pl.when((step < half) | (c < chunks // 2))
                def _():
                    hop_copy(ring, 0, at(-step), c).wait_send()

                @pl.when((step < half) | (c >= chunks // 2))
                def _():
                    hop_copy(ring, 1, at(step), c).wait_send()

                return inner

            return lax.fori_loop(1, half + 1, steps, carry)

        lax.fori_loop(0, chunks, each, 0)

    side_ring = (w_side, side_send, side_recv)
    query_ring = (w_query, query_send, query_recv)
    out_ring = (w_out, out_send, out_recv)

    for load in loads[:3]:
        load.wait()
    send_own(side_ring)
    loads[3].wait()

    token_rows = rows // token_chunks

    def token_part(owner, j):
        return tok.at[owner, pl.ds(pl.multiple_of(j * token_rows, 16), token_rows), :]

    def token_far(hop, owner, j):
        part = token_part(owner, j)
        target = (chip + hop) % chips * 2 + core
        return remote(
            part, part, ty_send.at[hop - 1, j], ty_recv.at[hop - 1, j], (me, target)
        )

    def token_near(slot, owner, j):
        part = token_part(owner, j)
        return remote(part, part, td_send.at[slot, j], td_recv.at[slot, j], (me, partner))

    def start_tokens(j, carry):
        for hop in range(1, chips):
            token_far(hop, tp, j).start()
        token_near(0, tp, j).start()
        return carry

    lax.fori_loop(0, token_chunks, start_tokens, 0)

    for g in range(rows // GRID_W):
        spot = pl.ds(me * (rows // GRID_W) + g, 1)
        grid_rows = pl.ds(g * GRID_W, GRID_W)
        cosines[grid_rows, :] = col_cos[...] + row_cos[spot, :]
        sines[grid_rows, :] = col_sin[...] + row_sin[spot, :]

    pieces = features // depth
    norm_rows = 32 if token_rows % 32 == 0 else 16

    def normalise(j):
        token_near(0, partner, j).wait_recv()
        for hop in range(1, chips):
            token_near(hop, (chip - hop + chips) % chips * 2 + 1 - core, j).wait_recv()

        def tile(i, carry):
            at_rows = pl.ds(pl.multiple_of(j * token_rows + i * norm_rows, 16), norm_rows)
            squares = jnp.zeros((norm_rows, 1), f32)
            for t in range(members):
                block = tok[t, at_rows, :].astype(f32)
                squares = squares + jnp.sum(block * block, axis=1, keepdims=True)
            scale = lax.rsqrt(squares / (members * features) + eps)
            for t in range(members):
                for piece in range(pieces):
                    first = piece * depth
                    gain = norm_gain[:, t * features + first : t * features + first + depth]
                    block = tok[t, at_rows, first : first + depth].astype(f32)
                    normed[t * pieces + piece, at_rows, :] = (block * scale * gain).astype(bf16)
            return carry

        lax.fori_loop(0, token_rows // norm_rows, tile, 0)

    def token_step(j, carry):
        for hop in range(1, chips):
            source = (chip - hop + chips) % chips * 2 + core
            token_far(hop, source, j).wait_recv()
            token_near(hop, source, j).start()

        @pl.when(j < half * chunks)
        def _():
            event(side_ring, j // chunks + 1, j % chunks)

        @pl.when(j >= 1)
        def _():
            normalise(j - 1)

        return carry

    lax.fori_loop(0, token_chunks, token_step, 0)
    normalise(token_chunks - 1)

    tile_rows = 256 if rows % 256 == 0 else 128

    def project(total, weights, spots, first=False):
        def body(i, carry):
            part = pl.ds(pl.multiple_of(i * tile_rows, tile_rows), tile_rows)
            terms = [
                jnp.dot(
                    normed[owner_of(spot), part, :], weights[spot], preferred_element_type=f32
                )
                for spot in spots
            ]
            value = functools.reduce(lambda a, b: a + b, terms)
            total[part, :] = value if first else total[part, :] + value
            return carry

        lax.fori_loop(0, rows // tile_rows, body, 0)

    project(side, w_side, [place], first=True)
    early = token_chunks // chunks

    def side_step(step, carry):
        @pl.when(step > early)
        def _():
            events(side_ring, step)

        project(side, w_side, [at(-step), at(step)])
        return carry

    lax.fori_loop(1, half + 1, side_step, 0)
    loads[4].wait()
    send_own(query_ring)
    opposite(side_ring)
    project(side, w_side, [at(count // 2)])

    twice = lambda gain: jnp.concatenate([gain[...], gain[...]], axis=1)
    query_gains, key_gains = twice(query_gain), twice(key_gain)
    lane = lax.broadcasted_iota(jnp.int32, (WINDOW, 2 * HEAD), 1)
    low_half = lane < HEAD
    lead = lane % (HEAD // 2) < HEAD // 4

    def prepare(i, carry):
        part = pl.ds(pl.multiple_of(i * WINDOW, WINDOW), WINDOW)
        shifted = pl.ds(pl.multiple_of((i + 1) * WINDOW, WINDOW), WINDOW)
        for h in range(kw // (2 * HEAD)):
            lanes = slice(h * 2 * HEAD, (h + 1) * 2 * HEAD)
            key = norm_rope(
                side[part, lanes], key_gains, cosines[part, :], sines[part, :], low_half, lead
            )
            band[shifted, lanes] = key.astype(bf16)
        band[shifted, kw : 2 * kw] = side[part, kw : 2 * kw].astype(bf16)
        pooled_rows = pl.ds(pl.multiple_of(i * WINDOW + pool_pad, pool_pad), WINDOW)
        pool_band[pooled_rows, :] = side[part, 2 * kw :].astype(bf16)
        return carry

    lax.fori_loop(0, rows // WINDOW, prepare, 0)

    before, behind = (me + count - 1) % count, (me + 1) % count

    def halo(index, buffer, size, upwards):
        if upwards:
            source, target, device = rows, 0, (behind, tp)
        else:
            source, target, device = size, rows + size, (before, tp)
        return remote(
            buffer.at[pl.ds(source, size), :],
            buffer.at[pl.ds(target, size), :],
            halo_send.at[index],
            halo_recv.at[index],
            device,
        )

    lower = [halo(0, band, WINDOW, False), halo(1, pool_band, pool_pad, False)]
    upper = [halo(2, band, WINDOW, True), halo(3, pool_band, pool_pad, True)]
    has_lower, has_upper = me > 0, me < count - 1

    @pl.when(has_lower)
    def _():
        for copy in lower:
            copy.start()

    @pl.when(has_upper)
    def _():
        for copy in upper:
            copy.start()

    @pl.when(jnp.logical_not(has_lower))
    def _():
        band[0:WINDOW, :] = jnp.zeros((WINDOW, 2 * kw), bf16)
        pool_band[0:pool_pad, :] = jnp.zeros((pool_pad, pw), bf16)

    @pl.when(jnp.logical_not(has_upper))
    def _():
        band[rows + WINDOW :, :] = jnp.zeros((WINDOW, 2 * kw), bf16)
        pool_band[rows + pool_pad :, :] = jnp.zeros((pool_pad, pw), bf16)

    project(query, w_query, [place], first=True)

    def query_step(step, carry):
        events(query_ring, step)
        project(query, w_query, [at(-step), at(step)])
        return carry

    lax.fori_loop(1, half + 1, query_step, 0)
    loads[5].wait()
    loads[6].wait()
    send_own(out_ring)

    @pl.when(has_lower)
    def _():
        for copy in upper:
            copy.wait_recv()

    @pl.when(has_upper)
    def _():
        for copy in lower:
            copy.wait_recv()

    level = tp * pw // (POOL // 4)
    reach = jnp.where(level == 0, 1, jnp.where(level == 1, 2, jnp.where(level == 2, 4, 8)))

    def pool(i, carry):
        wide = WINDOW + 2 * pool_pad
        part = pl.ds(pl.multiple_of(i * WINDOW, WINDOW), WINDOW)
        values = pool_band[pl.ds(pl.multiple_of(i * WINDOW, pool_pad), wide), :].astype(f32)
        total, chosen = values, None
        for step in range(4):
            size = 2**step
            total = total + pltpu.roll(total, wide - size, 0)
            shifted = pltpu.roll(total, size, 0)[pool_pad : pool_pad + WINDOW]
            chosen = shifted if chosen is None else jnp.where(level == step, shifted, chosen)
        spot = me * rows + i * WINDOW + lax.broadcasted_iota(jnp.int32, (WINDOW, 1), 0)
        low = jnp.maximum(spot - reach, 0)
        high = jnp.minimum(spot + reach - 1, seq - 1)
        mixer[part, 0:pw] = (chosen / (high - low + 1).astype(f32)).astype(bf16)
        return carry

    lax.fori_loop(0, rows // WINDOW, pool, 0)

    opposite(query_ring)
    project(query, w_query, [at(count // 2)])

    blocks = rows // WINDOW
    row = lax.broadcasted_iota(jnp.int32, (2 * WINDOW, 3 * WINDOW), 0) % WINDOW
    column = lax.broadcasted_iota(jnp.int32, (2 * WINDOW, 3 * WINDOW), 1)
    top_row = lax.broadcasted_iota(jnp.int32, (2 * WINDOW, 1), 0) < WINDOW

    def attend(i, carry):
        part = pl.ds(pl.multiple_of(i * WINDOW, WINDOW), WINDOW)
        key_rows = pl.ds(pl.multiple_of(i * WINDOW, WINDOW), 3 * WINDOW)
        key_pos = me * rows + i * WINDOW - WINDOW + column
        inside = (column >= row) & (column - row <= 2 * WINDOW) & (key_pos >= 0) & (key_pos < seq)
        for head in range(heads_k):
            lanes = slice(head * 2 * HEAD, (head + 1) * 2 * HEAD)
            rotated = norm_rope(
                query[part, lanes],
                query_gains,
                cosines[part, :],
                sines[part, :],
                low_half,
                lead,
            ) * HEAD ** (-0.5)
            other = pltpu.roll(rotated, HEAD, 1)
            if head % 2 == 0:
                pair = (jnp.where(low_half, rotated, 0.0), jnp.where(low_half, other, 0.0))
            else:
                pair = (jnp.where(low_half, 0.0, other), jnp.where(low_half, 0.0, rotated))
            stacked = jnp.concatenate(pair, axis=0).astype(bf16)
            tile = head // 2 * 2 * HEAD
            keys = band[key_rows, tile : tile + 2 * HEAD]
            values = band[key_rows, kw + tile : kw + tile + 2 * HEAD]
            scores = lax.dot_general(
                stacked, keys, (((1,), (1,)), ((), ())), preferred_element_type=f32
            )
            scores = jnp.where(inside, scores, neg_big)
            limit = jnp.where(top_row, sink[2 * head], sink[2 * head + 1])
            top = jnp.maximum(jnp.max(scores, axis=1, keepdims=True), limit)
            raised = jnp.exp(scores - top)
            totals = jnp.sum(raised, axis=1, keepdims=True) + jnp.exp(limit - top)
            weights = (raised * (1.0 / totals)).astype(bf16)
            result = jnp.dot(weights, values, preferred_element_type=f32)
            one, two = result[:WINDOW], result[WINDOW:]
            if head % 2 == 0:
                joined = jnp.where(low_half, one, pltpu.roll(two, HEAD, 1))
            else:
                joined = jnp.where(low_half, pltpu.roll(one, HEAD, 1), two)
            mixer[part, pw + head * 2 * HEAD : pw + (head + 1) * 2 * HEAD] = joined.astype(bf16)

        for c in range(chunks):

            @pl.when(i == ((c + 1) * blocks + chunks - 1) // chunks - 1)
            def _(c=c):
                event(out_ring, 1, c)

        return carry

    lax.fori_loop(0, blocks, attend, 0)

    def product(spot, which):
        left = jnp.concatenate(
            [
                mixer[pl.ds(pl.multiple_of((y * 2 + which) * share, 16), share), :]
                for y in range(chips)
            ],
            axis=0,
        )
        return jnp.dot(left, w_out[spot], preferred_element_type=f32).astype(bf16)

    def met_copy(spot):
        return remote(
            away.at[spot], met.at[spot], met_send.at[spot], met_recv.at[spot], (me, partner)
        )

    def y_copy(spot, hop):
        target = (chip + hop) % chips * 2 + core
        return remote(
            y_send.at[spot, hop - 1],
            y_recv.at[spot, hop - 1],
            yy_send.at[spot, hop - 1],
            yy_recv.at[spot, hop - 1],
            (me, target),
        )

    def done_copy(spot):
        columns = pl.ds(pl.multiple_of(owner_of(spot) * width, width), width)
        return pltpu.make_async_copy(done.at[spot], out.at[:, columns], done_sem.at[spot])

    def both_rows(spot, y):
        part = pl.ds(pl.multiple_of(y * share, 16), share)
        return kept[spot, part, :].astype(f32) + met[spot, part, :].astype(f32)

    def group(spots):
        def first(spot):
            away[spot] = product(spot, 1 - core)
            met_copy(spot).start()

        def second(spot):
            kept[spot] = product(spot, core)

        def third(spot):
            met_copy(spot).wait_recv()
            for hop in range(1, chips):
                y_send[spot, hop - 1] = both_rows(spot, (chip + hop) % chips).astype(bf16)
                y_copy(spot, hop).start()

        for part in (first, second, third):
            for spot in spots:
                part(spot)

    def finish(spot):
        total = both_rows(spot, chip)
        for hop in range(1, chips):
            y_copy(spot, hop).wait_recv()
            total = total + y_recv[spot, hop - 1].astype(f32)
        done[spot] = total.astype(bf16)
        done_copy(spot).start()

    group([place])

    def out_step(step, carry):
        @pl.when(step > 1)
        def _():
            events(out_ring, step)

        group([at(-step), at(step)])

        @pl.when(step == 1)
        def _():
            finish(place)

        @pl.when(step > 1)
        def _():
            finish(at(1 - step))
            finish(at(step - 1))

        return carry

    lax.fori_loop(1, half + 1, out_step, 0)
    opposite(out_ring)
    group([at(count // 2)])
    finish(at(-half))
    finish(at(half))
    finish(at(count // 2))

    for ring in (side_ring, query_ring, out_ring):
        sends_done(ring)

    def tokens_sent(j, carry):
        token_near(0, tp, j).wait_send()
        for hop in range(1, chips):
            token_far(hop, tp, j).wait_send()
            token_near(hop, (chip - hop + chips) % chips * 2 + core, j).wait_send()
        return carry

    lax.fori_loop(0, token_chunks, tokens_sent, 0)

    @pl.when(has_lower)
    def _():
        for copy in lower:
            copy.wait_send()

    @pl.when(has_upper)
    def _():
        for copy in upper:
            copy.wait_send()

    def blocks_sent(spot, carry):
        met_copy(spot).wait_send()
        for hop in range(1, chips):
            y_copy(spot, hop).wait_send()
        done_copy(spot).wait()
        return carry

    lax.fori_loop(0, count, blocks_sent, 0)


def plane_kernel(
    count,
    members,
    tokens,
    wq,
    wk,
    wv,
    wp,
    wop,
    woa,
    norm_gain_in,
    query_gain_in,
    key_gain_in,
    row_cos_in,
    row_sin_in,
    col_cos_in,
    col_sin_in,
    sink_in,
    out,
    norm_gain,
    query_gain,
    key_gain,
    row_cos,
    row_sin,
    col_cos,
    col_sin,
    sink,
    small_sem,
    raw,
    sums,
    normed,
    w_in,
    w_pool,
    w_out,
    in_spare,
    pool_spare,
    out_spare,
    total,
    band,
    pool_band,
    cosines,
    sines,
    attended,
    pooled,
    result,
    rounded,
    load_sem,
    sum_sems,
    in_sems,
    pool_sems,
    out_sems,
    x_sems,
    ring_sems,
    spread_sems,
    token_sems,
    token_bulk,
    attend_sems,
    attend_bulk,
    pooled_sems,
    pooled_bulk,
    halo_send,
    halo_recv,
    result_sems,
    go_sem,
):
    rows, features = tokens.shape
    depth = wk.shape[0]
    hk, hq, hp = wk.shape[1] // 2, wq.shape[1] // 2, wp.shape[1] // 2
    width = wop.shape[1]
    narrow = width // members
    share = rows // members
    plane = 2 * rows
    heads_k = hk // HEAD
    seq = count * rows
    deep = count // 2
    pieces = features // depth
    tiles = rows // WINDOW
    grid = plane // GRID_W

    me, tp = lax.axis_index("sp"), lax.axis_index("tp")
    z, x = me // 2, me % 2
    y, core = tp // 2, tp % 2
    me_x, tp_y, tp_c = me + 1 - 2 * x, (1 - y) * 2 + core, y * 2 + 1 - core
    tp_yc = (1 - y) * 2 + 1 - core
    up, down = (me + 2) % count, (me + count - 2) % count
    has_up, has_down = z < deep - 1, z > 0
    inner = has_up & has_down

    mine = lambda size: pl.ds(pl.multiple_of(x * size, 128), size)
    other = lambda size: pl.ds(pl.multiple_of((1 - x) * size, 128), size)

    def load(group, source, target):
        pltpu.make_async_copy(source, target, load_sem.at[group]).start()

    def loaded(group, whole):
        pltpu.make_async_copy(whole, whole, load_sem.at[group]).wait()

    for target, pick in ((w_in.at[me], mine), (in_spare, other)):
        load(0, wk.at[:, pick(hk)], target.at[:, pl.ds(0, hk)])
        load(0, wv.at[:, pick(hk)], target.at[:, pl.ds(hk, hk)])
        load(0, wq.at[:, pick(hq)], target.at[:, pl.ds(2 * hk, hq)])
    load(1, tokens, raw)
    small = [
        pltpu.make_async_copy(source, target, small_sem.at[index])
        for index, (source, target) in enumerate(
            (
                (norm_gain_in, norm_gain),
                (query_gain_in, query_gain),
                (key_gain_in, key_gain),
                (row_cos_in.at[pl.ds(z * grid, grid), :], row_cos),
                (row_sin_in.at[pl.ds(z * grid, grid), :], row_sin),
                (col_cos_in, col_cos),
                (col_sin_in, col_sin),
                (sink_in, sink),
            )
        )
    ]
    for copy in small:
        copy.start()
    for target, pick in ((w_pool.at[me], mine), (pool_spare, other)):
        load(2, wp.at[:, pick(hp)], target)
    strip = lambda t: pl.ds(pl.multiple_of(t * narrow, narrow), narrow)
    strips = [(3, w_out.at[z, tp], tp)] + [(4, out_spare.at[t], t) for t in range(members)]
    for group, target, t in strips:
        load(group, woa.at[:, strip(t)], target.at[pl.ds(0, 2 * hq), :])
        load(group, wop.at[:, strip(t)], target.at[pl.ds(2 * hq, 2 * hp), :])

    barrier = pltpu.get_barrier_semaphore()
    greeted = [(up, tp), (down, tp), (me_x, tp), (me, tp_y), (me, tp_c), (me, tp_yc)]
    for device in greeted:
        pl.semaphore_signal(barrier, inc=1, device_id=device, device_id_type=MESH)
    pl.semaphore_wait(barrier, len(greeted))

    def remote(source, target, send_sem, recv_sem, device):
        return pltpu.make_async_remote_copy(
            src_ref=source,
            dst_ref=target,
            send_sem=send_sem,
            recv_sem=recv_sem,
            device_id=device,
            device_id_type=MESH,
        )

    def by_rows(parts):
        def view(buffer, c):
            size = buffer.shape[0] // parts
            return buffer.at[pl.ds(pl.multiple_of(c * size, 16), size), :]

        return view

    in_ring = (w_in, in_spare, in_sems, 0, in_parts, by_rows(in_parts))
    pool_ring = (w_pool, pool_spare, pool_sems, 1, 1, by_rows(1))
    def z_copy(ring, way, source, c):
        buffer, _, sems, _, _, view = ring
        part = view(buffer.at[source], c)
        send = ring_sems.at[ring[3], way]
        return remote(part, part, send, sems.at[source, c], ((up, down)[way], tp))

    def x_copy(ring, source, c):
        buffer, spare, sems, first, _, view = ring
        return remote(
            view(spare, c),
            view(buffer.at[source], c),
            x_sems.at[first],
            sems.at[source, c],
            (me_x, tp),
        )

    def both_ways(ring, source, c, act):
        @pl.when(has_up)
        def _():
            act(z_copy(ring, 0, source, c))

        @pl.when(has_down)
        def _():
            act(z_copy(ring, 1, source, c))

    start = lambda copy: copy.start()

    def own_out(ring):
        for c in range(ring[4]):
            both_ways(ring, me, c, start)

    def side_out(ring):
        for c in range(ring[4]):
            x_copy(ring, me, c).start()

    def side_in(ring):
        for c in range(ring[4]):
            x_copy(ring, me_x, c).wait_recv()
            both_ways(ring, me_x, c, start)

    def passing(ring, n):
        parts = ring[4]
        step, j, c = n // (2 * parts) + 1, n // parts % 2, n % parts
        column = (x + j) % 2
        low, high = z - step, z + step
        return (low >= 0, low * 2 + column), (high < deep, high * 2 + column), c

    def event(ring, n):
        (is_low, low), (is_high, high), c = passing(ring, n)

        @pl.when(is_low)
        def _():
            z_copy(ring, 0, low, c).wait_recv()

            @pl.when(has_up)
            def _():
                z_copy(ring, 0, low, c).start()

        @pl.when(is_high)
        def _():
            z_copy(ring, 1, high, c).wait_recv()

            @pl.when(has_down)
            def _():
                z_copy(ring, 1, high, c).start()

    def events(ring, first, last):
        def body(n, carry):
            event(ring, n)
            return carry

        lax.fori_loop(first, last, body, 0)

    def all_events(ring):
        return (deep - 1) * 2 * ring[4]

    def bulk(whole, sem):
        return remote(whole, whole, sem, sem, (me_x, tp))

    def sends_done(buffer, sem, each):
        for level in range(deep):

            @pl.when(z == level)
            def _(level=level):
                if level < deep - 1:
                    whole = buffer.at[pl.ds(0, (level + 1) * each)]
                    bulk(whole, ring_sems.at[sem, 0]).wait_send()
                if level > 0:
                    whole = buffer.at[pl.ds(0, (deep - level) * each)]
                    bulk(whole, ring_sems.at[sem, 1]).wait_send()

    def out_copy(way, level, c):
        part = w_out.at[level, (tp - c + members) % members]
        send = ring_sems.at[2, way]
        return remote(part, part, send, out_sems.at[level, c], ((up, down)[way], tp))

    def spread(c):
        target = (tp + c) % members
        return remote(
            out_spare.at[target],
            w_out.at[z, tp],
            spread_sems.at[0],
            out_sems.at[z, c],
            (me, target),
        )

    def spread_in(c):
        owner = (tp - c + members) % members
        return remote(
            out_spare.at[owner],
            w_out.at[z, owner],
            spread_sems.at[0],
            out_sems.at[z, c],
            (me, owner),
        )

    def out_both(c, act):
        @pl.when(has_up)
        def _():
            act(out_copy(0, z, c))

        @pl.when(has_down)
        def _():
            act(out_copy(1, z, c))

    skewed = deep >= 4
    late_up = skewed & (core == 1) & (z == deep - 2)
    late_down = skewed & (core == 1) & (z == 1)

    def late_copies(act):
        @pl.when(late_up)
        def _():
            for c in range(members):
                act(out_copy(0, 0, c))

        @pl.when(late_down)
        def _():
            for c in range(members):
                act(out_copy(1, deep - 1, c))

    def out_event(n):
        step, c = n // members + 1, n % members
        low, high = z - step, z + step

        @pl.when(low >= 0)
        def _():
            out_copy(0, low, c).wait_recv()

            @pl.when(has_up & jnp.logical_not(late_up & (low == 0)))
            def _():
                out_copy(0, low, c).start()

        @pl.when(high < deep)
        def _():
            out_copy(1, high, c).wait_recv()

            @pl.when(has_down & jnp.logical_not(late_down & (high == deep - 1)))
            def _():
                out_copy(1, high, c).start()

    def out_events(first, last):
        def body(n, carry):
            out_event(n)
            return carry

        lax.fori_loop(first, last, body, 0)

    loaded(0, w_in.at[pl.ds(0, 2)])
    for c in range(in_parts):
        x_copy(in_ring, me, c).start()
        both_ways(in_ring, me, c, start)

    loaded(1, raw)
    for copy in small:
        copy.wait()
    sums[tp] = jnp.zeros_like(sums[tp])
    for i in range(tiles):
        block = raw[i * WINDOW : (i + 1) * WINDOW, :].astype(f32)
        square = jnp.sum(block * block, axis=1, keepdims=True)
        turned = jnp.transpose(jnp.broadcast_to(square, (WINDOW, WINDOW)))
        sums[tp, i : i + 1, :] = turned[0:1, :]

    def sum_copy(owner, hop):
        target = (tp + hop) % members
        return remote(
            sums.at[owner],
            sums.at[owner],
            sum_sems.at[0],
            sum_sems.at[1],
            (me, target),
        )

    for hop in range(1, members):
        sum_copy(tp, hop).start()
    for g in range(grid):
        grid_rows = pl.ds(g * GRID_W, GRID_W)
        cosines[grid_rows, :] = col_cos[...] + row_cos[g : g + 1, :]
        sines[grid_rows, :] = col_sin[...] + row_sin[g : g + 1, :]
    bulk(sums.at[pl.ds(0, members - 1)], sum_sems.at[1]).wait_recv()
    squares = sums[0]
    for t in range(1, members):
        squares = squares + sums[t]
    scales = lax.rsqrt(squares / (members * features) + eps)

    class Stream:
        def __init__(self, view, all_sent, side, sems, bulk_sems, by_x, pair=None):
            self.pair, self.crossing = pair, 1 if pair else 2
            self.view, self.all_sent, self.side = view, all_sent, side
            self.sems, self.bulk_sems, self.by_x = sems, bulk_sems, by_x

        def copy(self, recv, side, owner, j, device):
            part = self.view(side, owner, j)
            return remote(part, part, self.bulk_sems.at[0], recv, device)

        def over_x(self, slot, side, owner, j):
            return self.copy(self.sems.at[slot * self.crossing, j], side, owner, j, (me_x, tp))

        def over_y(self, slot, side, owner, j):
            index = slot * self.crossing if self.pair or slot else 1
            return self.copy(self.sems.at[index, j], side, owner, j, (me, tp_y))

        def over_core(self, slot, side, owner, j):
            return self.copy(self.bulk_sems.at[1 + slot % 2], side, owner, j, (me, tp_c))

        def start(self, j):
            self.over_y(0, x, tp, j).start()
            self.over_x(0, x, tp, j).start()
            self.over_core(0, x, tp, j).start()

        def direct(self, j):
            if self.pair:
                bulk(self.pair(j), self.sems.at[0, j]).wait_recv()
            else:
                self.over_y(0, x, tp_y, j).wait_recv()
            self.over_core(2, x, tp_y, j).start()

            @pl.when(self.by_x(j))
            def _():
                self.over_x(1, x, tp_y, j).start()

            if not self.pair:
                self.over_x(0, 1 - x, tp, j).wait_recv()
            self.over_core(1, 1 - x, tp, j).start()

            @pl.when(jnp.logical_not(self.by_x(j)))
            def _():
                self.over_y(1, 1 - x, tp, j).start()

        def crossed(self, j):
            @pl.when(self.by_x(j))
            def _():
                self.over_x(1, 1 - x, tp_y, j).wait_recv()

            @pl.when(jnp.logical_not(self.by_x(j)))
            def _():
                self.over_y(1, 1 - x, tp_y, j).wait_recv()

            self.over_core(3, 1 - x, tp_y, j).start()

        def near_side(self):
            bulk(self.side, self.bulk_sems.at[1]).wait_recv()

        def far_side(self):
            bulk(self.side, self.bulk_sems.at[2]).wait_recv()

        def sent(self):
            bulk(self.all_sent, self.bulk_sems.at[0]).wait_send()

        def every(self, act):
            def body(j, carry):
                act(j)
                return carry

            lax.fori_loop(0, self.sems.shape[1], body, 0)

    def block_rows(j, size):
        return pl.ds(pl.multiple_of(j * size, 16), size)

    def token_view(side, owner, j):
        return normed.at[side, pl.ds(owner * pieces, pieces), block_rows(j, WINDOW), :]

    def attend_view(side, owner, j):
        return attended.at[owner, side, block_rows(j, WINDOW), :]

    def pooled_view(side, owner, j):
        return pooled.at[owner, side, block_rows(j, plane // pooled_parts), :]

    most = lambda size: pl.ds(0, size * (2 * members - 1) // (2 * members))
    token_stream = Stream(
        token_view,
        normed.at[:, :, most(rows), :],
        normed.at[0, pl.ds(0, count // 2)],
        token_sems,
        token_bulk,
        lambda j: j % 3 == 0,
    )
    attend_stream, pooled_stream = [
        Stream(
            view,
            buffer.at[:, :, most(plane), :],
            buffer.at[0],
            sems,
            bulk_sems,
            lambda j: j % 2 == 0,
            lambda j, buffer=buffer, size=size: buffer.at[0, :, block_rows(j, size), :],
        )
        for view, buffer, sems, bulk_sems, size in (
            (attend_view, attended, attend_sems, attend_bulk, WINDOW),
            (pooled_view, pooled, pooled_sems, pooled_bulk, plane // pooled_parts),
        )
    ]

    for i in range(tiles):
        here = slice(i * WINDOW, (i + 1) * WINDOW)
        scale = jnp.transpose(jnp.broadcast_to(scales[i : i + 1, :], (WINDOW, WINDOW)))
        for first in range(0, features, WINDOW):
            block = raw[here, first : first + WINDOW].astype(f32)
            gain = norm_gain[:, pl.ds(pl.multiple_of(tp * features + first, WINDOW), WINDOW)]
            value = (block * scale * gain).astype(bf16)
            inside = first % depth
            normed[x, tp * pieces + first // depth, here, inside : inside + WINDOW] = value
        token_stream.start(i)

    side_in(in_ring)
    whole = all_events(in_ring)
    reached = lambda part: whole * part // 24
    events(in_ring, 0, reached(4))

    def direct(j, carry):
        token_stream.direct(j)
        events(in_ring, reached(4 + 12 * j // tiles), reached(4 + 12 * (j + 1) // tiles))
        return carry

    lax.fori_loop(0, tiles, direct, 0)
    loaded(2, w_pool.at[pl.ds(0, 2)])
    loaded(3, w_out.at[0, 0])
    loaded(4, out_spare)
    side_out(pool_ring)
    for c in range(1, members):
        spread(c).start()
    token_stream.near_side()

    tile_rows = 256 if rows % 256 == 0 else 128
    per_side = rows // tile_rows

    def project(result, weights, level, side, first=False):
        def body(i, carry):
            within = pl.ds(pl.multiple_of(i * tile_rows, tile_rows), tile_rows)
            part = pl.ds(pl.multiple_of(side * rows + i * tile_rows, tile_rows), tile_rows)
            value = None if first else result[part, :]
            for j in range(2):
                term = jnp.dot(
                    normed[side, level * 2 + j, within, :],
                    weights[level * 2 + j],
                    preferred_element_type=f32,
                )
                value = term if value is None else value + term
            result[part, :] = value
            return carry

        lax.fori_loop(0, per_side, body, 0)

    def project_step(result, weights, step, side):
        @pl.when(z - step >= 0)
        def _():
            project(result, weights, z - step, side)

        @pl.when(z + step < deep)
        def _():
            project(result, weights, z + step, side)

    early = max(reached(16) // (2 * in_parts), 0)

    def crossed(j, carry):
        token_stream.crossed(j)

        @pl.when(j == 0)
        def _():
            project(total, w_in, z, x, first=True)

        @pl.when((j >= 1) & (j <= early))
        def _():
            project_step(total, w_in, j, x)

        events(in_ring, reached(16 + 4 * j // tiles), reached(16 + 4 * (j + 1) // tiles))
        return carry

    lax.fori_loop(0, tiles, crossed, 0)
    own_out(pool_ring)
    side_in(pool_ring)
    token_stream.far_side()
    project(total, w_in, z, 1 - x, first=True)

    @pl.when(inner)
    def _():
        events(pool_ring, 0, 2)


    def in_step(step, carry):
        each = 2 * in_parts
        events(in_ring, jnp.maximum((step - 1) * each, reached(20)), step * each)

        @pl.when(step > min(early, tiles - 1))
        def _():
            project_step(total, w_in, step, x)

        project_step(total, w_in, step, 1 - x)
        return carry

    lax.fori_loop(1, deep, in_step, 0)

    twice = lambda gain: jnp.concatenate([gain[...], gain[...]], axis=1)
    query_gains, key_gains = twice(query_gain), twice(key_gain)
    lane = lax.broadcasted_iota(jnp.int32, (WINDOW, 2 * HEAD), 1)
    low_half = lane < HEAD
    lead = lane % (HEAD // 2) < HEAD // 4
    blocks = plane // WINDOW

    def prepare(i, carry):
        part = pl.ds(pl.multiple_of(i * WINDOW, WINDOW), WINDOW)
        shifted = pl.ds(pl.multiple_of((i + 1) * WINDOW, WINDOW), WINDOW)
        for h in range(hk // (2 * HEAD)):
            lanes = slice(h * 2 * HEAD, (h + 1) * 2 * HEAD)
            key = norm_rope(
                total[part, lanes], key_gains, cosines[part, :], sines[part, :], low_half, lead
            )
            band[shifted, lanes] = key.astype(bf16)
        band[shifted, hk:] = total[part, hk : 2 * hk].astype(bf16)
        return carry

    lax.fori_loop(0, blocks, prepare, 0)

    def halo(index, buffer, size, upwards):
        if upwards:
            source, target, device = plane, 0, (up, tp)
        else:
            source, target, device = size, plane + size, (down, tp)
        return remote(
            buffer.at[pl.ds(source, size), :],
            buffer.at[pl.ds(target, size), :],
            halo_send.at[index],
            halo_recv.at[index],
            device,
        )

    def halo_out(index, buffer, size):
        @pl.when(has_down)
        def _():
            halo(index, buffer, size, False).start()

        @pl.when(has_up)
        def _():
            halo(index + 1, buffer, size, True).start()

        empty = jnp.zeros((size, buffer.shape[1]), bf16)

        @pl.when(jnp.logical_not(has_down))
        def _():
            buffer[0:size, :] = empty

        @pl.when(jnp.logical_not(has_up))
        def _():
            buffer[plane + size :, :] = empty

    def halo_in(index, buffer, size):
        @pl.when(has_up)
        def _():
            halo(index, buffer, size, False).wait_recv()

        @pl.when(has_down)
        def _():
            halo(index + 1, buffer, size, True).wait_recv()

    halo_out(0, band, WINDOW)

    @pl.when(inner)
    def _():
        events(pool_ring, 2, all_events(pool_ring))

    for c in range(members - 1):
        if c > 0:
            spread_in(c).wait_recv()
        out_both(c, start)

    row = lax.broadcasted_iota(jnp.int32, (2 * WINDOW, 3 * WINDOW), 0) % WINDOW
    column = lax.broadcasted_iota(jnp.int32, (2 * WINDOW, 3 * WINDOW), 1)
    top_row = lax.broadcasted_iota(jnp.int32, (2 * WINDOW, 1), 0) < WINDOW

    def attend(turn, carry):
        @pl.when(turn == blocks - 2)
        def _():
            halo_in(0, band, WINDOW)

        i = (turn + 1) % blocks
        part = pl.ds(pl.multiple_of(i * WINDOW, WINDOW), WINDOW)
        key_rows = pl.ds(pl.multiple_of(i * WINDOW, WINDOW), 3 * WINDOW)
        key_pos = z * plane + i * WINDOW - WINDOW + column
        inside = (column >= row) & (column - row <= 2 * WINDOW) & (key_pos >= 0) & (key_pos < seq)
        for head in range(heads_k):
            lanes = slice(2 * hk + head * 2 * HEAD, 2 * hk + (head + 1) * 2 * HEAD)
            rotated = norm_rope(
                total[part, lanes],
                query_gains,
                cosines[part, :],
                sines[part, :],
                low_half,
                lead,
            ) * HEAD ** (-0.5)
            swapped = pltpu.roll(rotated, HEAD, 1)
            if head % 2 == 0:
                pair = (jnp.where(low_half, rotated, 0.0), jnp.where(low_half, swapped, 0.0))
            else:
                pair = (jnp.where(low_half, 0.0, swapped), jnp.where(low_half, 0.0, rotated))
            stacked = jnp.concatenate(pair, axis=0).astype(bf16)
            tile = head // 2 * 2 * HEAD
            keys = band[key_rows, tile : tile + 2 * HEAD]
            values = band[key_rows, hk + tile : hk + tile + 2 * HEAD]
            scores = lax.dot_general(
                stacked, keys, (((1,), (1,)), ((), ())), preferred_element_type=f32
            )
            scores = jnp.where(inside, scores, neg_big)
            first = x * 2 * heads_k + 2 * head
            limit = jnp.where(top_row, sink[first], sink[first + 1])
            top = jnp.maximum(jnp.max(scores, axis=1, keepdims=True), limit)
            raised = jnp.exp(scores - top)
            totals = jnp.sum(raised, axis=1, keepdims=True) + jnp.exp(limit - top)
            weights = (raised * (1.0 / totals)).astype(bf16)
            result = jnp.dot(weights, values, preferred_element_type=f32)
            one, two = result[:WINDOW], result[WINDOW:]
            if head % 2 == 0:
                joined = jnp.where(low_half, one, pltpu.roll(two, HEAD, 1))
            else:
                joined = jnp.where(low_half, pltpu.roll(one, HEAD, 1), two)
            attended[tp, x, part, head * 2 * HEAD : (head + 1) * 2 * HEAD] = joined.astype(bf16)
        attend_stream.start(i)

        @pl.when(turn >= behind)
        def _():
            attend_stream.direct((turn - behind + 1) % blocks)

        return carry

    behind = 5
    lax.fori_loop(0, blocks, attend, 0)

    events(pool_ring, jnp.where(inner, all_events(pool_ring), 0), all_events(pool_ring))

    for side in range(2):

        def pool_project(i, carry, side=side):
            part = pl.ds(pl.multiple_of(i * tile_rows, tile_rows), tile_rows)
            first = side * rows + pool_pad + i * tile_rows
            left = jnp.concatenate([normed[side, source, part, :] for source in range(count)], axis=1)
            right = w_pool[...].reshape(count * depth, hp)
            value = jnp.dot(left, right, preferred_element_type=f32)
            pool_band[pl.ds(pl.multiple_of(first, pool_pad), tile_rows), :] = value.astype(bf16)
            return carry

        lax.fori_loop(0, per_side, pool_project, 0)
    halo_out(2, pool_band, pool_pad)
    spread_in(members - 1).wait_recv()
    out_both(members - 1, start)

    @pl.when(inner)
    def _():
        out_events(0, members - 1)

    level = (tp * 2 + x) * hp // (POOL // 4)
    reach = jnp.where(level == 0, 1, jnp.where(level == 1, 2, jnp.where(level == 2, 4, 8)))

    def pool(i, carry):
        wide = WINDOW + 2 * pool_pad
        part = pl.ds(pl.multiple_of(i * WINDOW, WINDOW), WINDOW)
        running = pool_band[pl.ds(pl.multiple_of(i * WINDOW, pool_pad), wide), :].astype(f32)
        chosen = None
        for step in range(4):
            size = 2**step
            running = running + pltpu.roll(running, wide - size, 0)
            shifted = pltpu.roll(running, size, 0)[pool_pad : pool_pad + WINDOW]
            chosen = shifted if chosen is None else jnp.where(level == step, shifted, chosen)
        spot = z * plane + i * WINDOW + lax.broadcasted_iota(jnp.int32, (WINDOW, 1), 0)
        low = jnp.maximum(spot - reach, 0)
        high = jnp.minimum(spot + reach - 1, seq - 1)
        pooled[tp, x, part, :] = (chosen / (high - low + 1).astype(f32)).astype(bf16)
        return carry

    edge = blocks // pooled_parts
    lax.fori_loop(edge, blocks - edge, pool, 0)
    for part in range(1, pooled_parts - 1):
        pooled_stream.start(part)
    for turn in range(blocks - behind, blocks):
        attend_stream.direct((turn + 1) % blocks)
    halo_in(2, pool_band, pool_pad)
    lax.fori_loop(0, edge, pool, 0)
    lax.fori_loop(blocks - edge, blocks, pool, 0)
    pooled_stream.start(0)
    pooled_stream.start(pooled_parts - 1)

    @pl.when(inner)
    def _():
        out_events(members - 1, members)

    attend_stream.every(attend_stream.crossed)
    attend_stream.near_side()
    attend_stream.far_side()

    def level_of(group):
        paired = jnp.minimum(z, deep - 1 - z)
        step = jnp.where(group > 2 * paired, group - paired, (group + 1) // 2)
        downwards = jnp.where(group > 2 * paired, 2 * z > deep - 1, group % 2 == 1)
        return jnp.where(downwards, z - step, z + step)

    here = x * members + tp
    out_steps = (deep - 1) * members

    def columns_of(level, side, t):
        first = (level * 2 + side) * width + t * narrow
        return pl.ds(pl.multiple_of(first, narrow), narrow)

    def result_copy(level, side, t):
        first = pl.multiple_of((side * members + t) * share, 16)
        return remote(
            rounded.at[level, pl.ds(first, share), :],
            out.at[:, columns_of(level, x, tp)],
            result_sems.at[0],
            result_sems.at[1],
            (z * 2 + side, t),
        )

    def result_own(level):
        return pltpu.make_async_copy(
            rounded.at[level, pl.ds(pl.multiple_of(here * share, 16), share), :],
            out.at[:, columns_of(level, x, tp)],
            result_sems.at[2],
        )

    def send_far(level):
        for t in (tp_y, tp_yc, tp, tp_c):
            result_copy(level, 1 - x, t).start()

    def send_near(level):
        for t in (tp_y, tp_yc, tp_c):
            result_copy(level, x, t).start()
        result_own(level).start()

    def send_level(level):
        send_far(level)
        send_near(level)

    span = 2 * tile_rows if plane % (2 * tile_rows) == 0 else tile_rows
    ends_event = lambda n: jnp.where(inner, out_steps, n)

    def end_events(first, last):
        out_events(ends_event(first), ends_event(last))

    def by_span(act):
        def body(i, carry):
            act(pl.ds(pl.multiple_of(i * span, span), span))
            return carry

        lax.fori_loop(0, plane // span, body, 0)

    all_blocks = [(t, h) for t in range(members) for h in range(2)]

    def attended_term(part, levels):
        left = jnp.concatenate([attended[t, h, part, :] for t, h in all_blocks], axis=1)
        right = jnp.concatenate(
            [
                jnp.concatenate([w_out[level, t, 0 : 2 * hq, :] for t in range(members)], axis=0)
                for level in levels
            ],
            axis=1,
        )
        return jnp.dot(left, right, preferred_element_type=f32)

    def pooled_term(part, levels):
        left = jnp.concatenate([pooled[t, h, part, :] for t, h in all_blocks], axis=1)
        right = jnp.concatenate(
            [
                jnp.concatenate([w_out[level, t, 2 * hq :, :] for t in range(members)], axis=0)
                for level in levels
            ],
            axis=1,
        )
        return jnp.dot(left, right, preferred_element_type=f32)

    firsts = (level_of(0), level_of(1))
    end_events(0, members)

    def first_attended(part):
        result[part, :] = attended_term(part, firsts)

    by_span(first_attended)

    inner_parts = list(range(1, pooled_parts - 1)) + [0, pooled_parts - 1]
    for part in inner_parts:
        pooled_stream.direct(part)

    @pl.when(inner)
    def _():
        out_events(members, out_steps)

    for part in inner_parts:
        pooled_stream.crossed(part)
    pooled_stream.near_side()
    pooled_stream.far_side()

    def first_pooled(part):
        value = (result[part, :] + pooled_term(part, firsts)).astype(bf16)
        for index, level in enumerate(firsts):
            rounded[level, part, :] = value[:, index * narrow : (index + 1) * narrow]

    by_span(first_pooled)
    for level in firsts:
        send_level(level)

    def middle_level(group, carry):
        end_events((group - 1) * members, group * members)
        level = level_of(group)

        def whole_level(part):
            value = attended_term(part, [level]) + pooled_term(part, [level])
            rounded[level, part, :] = value.astype(bf16)

        by_span(whole_level)
        send_level(level)
        return carry

    lax.fori_loop(2, deep - 1, middle_level, 0)

    for ring in (in_ring, pool_ring):
        bulk(ring[1], x_sems.at[ring[3]]).wait_send()
        sends_done(ring[0], ring[3], 2)
    bulk(out_spare.at[pl.ds(0, members - 1)], spread_sems.at[0]).wait_send()
    bulk(sums.at[pl.ds(0, members - 1)], sum_sems.at[0]).wait_send()
    for stream in (token_stream, attend_stream, pooled_stream):
        stream.sent()

    @pl.when(late_up | late_down)
    def _():
        pl.semaphore_wait(go_sem, 1)
        late_copies(start)

    level = level_of(deep - 1)
    for c in range(members):
        n = (deep - 2) * members + c
        end_events(n, n + 1)
        t = (tp - c + members) % members

        def last_level(part, c=c, t=t):
            left = jnp.concatenate(
                [attended[t, h, part, :] for h in range(2)]
                + [pooled[t, h, part, :] for h in range(2)],
                axis=1,
            )
            value = jnp.dot(left, w_out[level, t], preferred_element_type=f32)
            if c > 0:
                value = result[part, 0:narrow] + value
            if c == members - 1:
                rounded[level, part, :] = value.astype(bf16)
            else:
                result[part, 0:narrow] = value

        if c == members - 3 and skewed:

            @pl.when(jnp.logical_not(inner) & (core == 0))
            def _():
                nearest = jnp.where(has_up, up, down)
                pl.semaphore_signal(
                    go_sem, inc=1, device_id=(nearest, tp_c), device_id_type=MESH
                )

        if c < members - 1:
            by_span(last_level)
            continue
        for side, send in ((1 - x, send_far), (x, send_near)):
            for start_row in range(0, rows, rows // 2):
                first = pl.multiple_of(side * rows + start_row, rows // 2)
                last_level(pl.ds(first, rows // 2))
            send(level)

    bulk(out.at[:, pl.ds(0, deep * (2 * members - 1) * narrow)], result_sems.at[1]).wait_recv()

    sends_done(w_out, 2, 1)
    for index, buffer, size in ((0, band, WINDOW), (2, pool_band, pool_pad)):

        @pl.when(has_down)
        def _(index=index, buffer=buffer, size=size):
            halo(index, buffer, size, False).wait_send()

        @pl.when(has_up)
        def _(index=index, buffer=buffer, size=size):
            halo(index + 1, buffer, size, True).wait_send()

    bulk(rounded.at[:, most(plane), :], result_sems.at[0]).wait_send()
    here_rows = rounded.at[:, pl.ds(0, share), :]
    pltpu.make_async_copy(here_rows, here_rows, result_sems.at[2]).wait()


def plane_scratch(count, members, rows, features, depth, kw, qw, pw, width):
    hk, hq, hp = kw // 2, qw // 2, pw // 2
    narrow, plane, deep, tiles = width // members, 2 * rows, count // 2, rows // WINDOW
    dma = pltpu.SemaphoreType.DMA
    return [
        pltpu.VMEM((1, members * features), f32),
        pltpu.VMEM((1, HEAD), f32),
        pltpu.VMEM((1, HEAD), f32),
        pltpu.VMEM((plane // GRID_W, 2 * HEAD), f32),
        pltpu.VMEM((plane // GRID_W, 2 * HEAD), f32),
        pltpu.VMEM((GRID_W, 2 * HEAD), f32),
        pltpu.VMEM((GRID_W, 2 * HEAD), f32),
        pltpu.SMEM((2 * hq // HEAD,), f32),
        dma((8,)),
        pltpu.VMEM((rows, features), bf16),
        pltpu.VMEM((members, -(-tiles // 8) * 8, WINDOW), f32),
        pltpu.VMEM((2, count, rows, depth), bf16),
        pltpu.VMEM((count, depth, 2 * hk + hq), bf16),
        pltpu.VMEM((count, depth, hp), bf16),
        pltpu.VMEM((deep, members, 2 * (hp + hq), narrow), bf16),
        pltpu.VMEM((depth, 2 * hk + hq), bf16),
        pltpu.VMEM((depth, hp), bf16),
        pltpu.VMEM((members, 2 * (hp + hq), narrow), bf16),
        pltpu.VMEM((plane, 2 * hk + hq), f32),
        pltpu.VMEM((plane + 2 * WINDOW, 2 * hk), bf16),
        pltpu.VMEM((plane + 2 * pool_pad, hp), bf16),
        pltpu.VMEM((plane, 2 * HEAD), f32),
        pltpu.VMEM((plane, 2 * HEAD), f32),
        pltpu.VMEM((members, 2, plane, hq), bf16),
        pltpu.VMEM((members, 2, plane, hp), bf16),
        pltpu.VMEM((plane, 2 * narrow), f32),
        pltpu.VMEM((deep, plane, narrow), bf16),
        dma((5,)),
        dma((2,)),
        dma((count, in_parts)),
        dma((count, 1)),
        dma((deep, members)),
        dma((2,)),
        dma((3, 2)),
        dma((1,)),
        dma((3, tiles)),
        dma((3,)),
        dma((2, 2 * tiles)),
        dma((3,)),
        dma((2, pooled_parts)),
        dma((3,)),
        dma((4,)),
        dma((4,)),
        dma((3,)),
        pltpu.SemaphoreType.REGULAR,
    ]


def ring_scratch(count, members, rows, features, depth, kw, qw, pw, width):
    chips, share = members // 2, rows // members
    far = max(chips - 1, 1)
    dma = pltpu.SemaphoreType.DMA
    return [
        pltpu.VMEM((members, rows, features), bf16),
        pltpu.VMEM((count, rows, depth), bf16),
        pltpu.VMEM((count, depth, 2 * kw + pw), bf16),
        pltpu.VMEM((count, depth, qw), bf16),
        pltpu.VMEM((count, pw + qw, width), bf16),
        pltpu.VMEM((rows, 2 * kw + pw), f32),
        pltpu.VMEM((rows, qw), f32),
        pltpu.VMEM((rows + 2 * WINDOW, 2 * kw), bf16),
        pltpu.VMEM((rows + 2 * pool_pad, pw), bf16),
        pltpu.VMEM((rows, 2 * HEAD), f32),
        pltpu.VMEM((rows, 2 * HEAD), f32),
        pltpu.VMEM((rows, pw + qw), bf16),
        pltpu.VMEM((count, chips * share, width), bf16),
        pltpu.VMEM((count, chips * share, width), bf16),
        pltpu.VMEM((count, chips * share, width), bf16),
        pltpu.VMEM((count, far, share, width), bf16),
        pltpu.VMEM((count, far, share, width), bf16),
        pltpu.VMEM((count, share, width), bf16),
        dma((7,)),
        dma((2, count, chunks)),
        dma((count, chunks)),
        dma((2, count, chunks)),
        dma((count, chunks)),
        dma((2, count, chunks)),
        dma((count, chunks)),
        dma((far, token_chunks)),
        dma((far, token_chunks)),
        dma((chips, token_chunks)),
        dma((chips, token_chunks)),
        dma((4,)),
        dma((4,)),
        dma((count,)),
        dma((count,)),
        dma((count, far)),
        dma((count, far)),
        dma((count,)),
    ]


def shards(
    tokens,
    norm_gain,
    w_query,
    w_key,
    w_value,
    w_pool,
    query_gain,
    key_gain,
    sink_logit,
    w_out_pool,
    w_out_attn,
):
    count, members = lax.axis_size("sp"), lax.axis_size("tp")
    rows, features = tokens.shape
    depth, kw = w_key.shape
    qw, pw, width = w_query.shape[1], w_pool.shape[1], w_out_pool.shape[1]
    tables = [jnp.asarray(table) for table in rope_parts(count * rows)]
    anywhere = pl.BlockSpec(memory_space=pl.ANY)
    in_vmem = pl.BlockSpec(memory_space=pltpu.VMEM)
    sizes = (count, members, rows, features, depth, kw, qw, pw, width)
    shared = (
        members == 4
        and count % 2 == 0
        and count >= 4
        and rows % (2 * WINDOW) == 0
        and depth % (16 * in_parts) == 0
        and all(size % 256 == 0 for size in (kw, qw, pw))
        and width % (128 * members) == 0
    )
    grant = (46 if shared else 60) * 1024 * 1024
    specs = [anywhere] * 7 + [in_vmem] * 7 + [pl.BlockSpec(memory_space=pltpu.SMEM)]
    if shared:
        specs = [pl.BlockSpec(memory_space=pltpu.HBM)] * 15
    as_row = lambda gain: gain.reshape(1, HEAD)
    kernel, scratch = (plane_kernel, plane_scratch) if shared else (layer_kernel, ring_scratch)
    operands = (
        tokens,
        w_query,
        w_key,
        w_value,
        w_pool,
        w_out_pool,
        w_out_attn,
        norm_gain.reshape(1, -1),
        as_row(query_gain),
        as_row(key_gain),
        *tables,
        sink_logit,
    )
    shape = (rows // members, count * width)
    result = jax.ShapeDtypeStruct(shape, bf16)
    if shared:
        operands = [pltpu.with_memory_space_constraint(each, pltpu.HBM) for each in operands]
        result = pltpu.VMEM(shape, bf16)
    return pl.pallas_call(
        functools.partial(kernel, count, members),
        out_shape=result,
        in_specs=specs,
        out_specs=anywhere,
        scratch_shapes=scratch(*sizes),
        compiler_params=pltpu.CompilerParams(
            collective_id=0, has_side_effects=True, vmem_limit_bytes=grant
        ),
    )(*operands)


def solution(mesh):
    placed = (
        P("sp", "tp"),
        P(),
        P("sp", "tp"),
        P("sp", "tp"),
        P("sp", "tp"),
        P("sp", "tp"),
        P(),
        P(),
        P("tp"),
        P("tp", "sp"),
        P("tp", "sp"),
    )
    return jax.shard_map(
        shards, mesh=mesh, in_specs=placed, out_specs=P(("sp", "tp"), None), check_vma=False
    )
```

```python
import functools

import jax
import jax.numpy as jnp
import numpy as np
from jax import lax
from jax.experimental import pallas as pl
from jax.experimental.pallas import tpu as pltpu
from jax.sharding import PartitionSpec as P

HEAD = 64
POOL = 1024
WINDOW = 128
GRID_W = 64

eps = 1e-06
rope_base = 10000.0
neg_big = -1e30
pool_pad = 16
chunks = 4
token_chunks = 8
in_parts = 2
pooled_parts = 4
MESH = pl.DeviceIdType.MESH
f32, bf16 = jnp.float32, jnp.bfloat16


def rope_parts(rows_total):
    quarter = HEAD // 4
    steps = np.arange(quarter, dtype=np.float32) * np.float32(2.0) / np.float32(HEAD // 2)
    freqs = (np.float32(1.0) / np.float32(rope_base) ** steps).astype(np.float32)

    def table(count, first):
        angle = np.arange(count, dtype=np.float32)[:, None] * freqs
        twice = np.concatenate([angle, angle], axis=1).astype(np.float64)
        none = np.zeros_like(twice)
        made = []
        for part in (np.cos(twice), np.sin(twice)):
            head = [part, none] if first else [none, part]
            made.append(np.concatenate(head + head, axis=1).astype(np.float32))
        return made

    return table(rows_total // GRID_W, True) + table(GRID_W, False)


def ring_place(index, count, across):
    deep = count // across
    if across == 1 or deep % 2:
        return index
    z, x = index // across, index % across
    turn = deep - 1 - z
    inner = jnp.where(turn % 2 == 0, x - 1, across - 1 - x)
    return jnp.where(x == 0, z, deep + turn * (across - 1) + inner)


def ring_index(place, count, across):
    deep = count // across
    if across == 1 or deep % 2:
        return place
    rest = jnp.maximum(place - deep, 0)
    turn, inner = rest // (across - 1), rest % (across - 1)
    x = jnp.where(turn % 2 == 0, inner + 1, across - 1 - inner)
    return jnp.where(place < deep, place * across, (deep - 1 - turn) * across + x)


def norm_rope(raw, gain, cosine, sine, low_half, lead):
    squares = raw * raw
    low_sum = jnp.sum(jnp.where(low_half, squares, 0.0), axis=1, keepdims=True)
    high_sum = jnp.sum(jnp.where(low_half, 0.0, squares), axis=1, keepdims=True)
    mean = jnp.where(low_half, low_sum, high_sum) * (1.0 / HEAD)
    scaled = raw * lax.rsqrt(mean + eps) * gain
    turned = jnp.where(
        lead,
        -pltpu.roll(scaled, 2 * HEAD - HEAD // 4, 1),
        pltpu.roll(scaled, HEAD // 4, 1),
    )
    return scaled * cosine + turned * sine


def layer_kernel(
    count,
    members,
    tokens,
    wq,
    wk,
    wv,
    wp,
    wop,
    woa,
    norm_gain,
    query_gain,
    key_gain,
    row_cos,
    row_sin,
    col_cos,
    col_sin,
    sink,
    out,
    tok,
    normed,
    w_side,
    w_query,
    w_out,
    side,
    query,
    band,
    pool_band,
    cosines,
    sines,
    mixer,
    away,
    met,
    kept,
    y_send,
    y_recv,
    done,
    load_sem,
    side_send,
    side_recv,
    query_send,
    query_recv,
    out_send,
    out_recv,
    ty_send,
    ty_recv,
    td_send,
    td_recv,
    halo_send,
    halo_recv,
    met_send,
    met_recv,
    yy_send,
    yy_recv,
    done_sem,
):
    rows, features = tokens.shape
    depth, kw = wk.shape
    qw, pw, width = wq.shape[1], wp.shape[1], wop.shape[1]
    chips = members // 2
    share = rows // members
    half = (count - 1) // 2
    heads_k = kw // HEAD
    seq = count * rows
    across = chips

    me, tp = lax.axis_index("sp"), lax.axis_index("tp")
    chip, core = tp // 2, tp % 2
    partner = chip * 2 + 1 - core
    place = ring_place(me, count, across)
    owner_of = lambda spot: ring_index(spot, count, across)
    at = lambda offset: (place + offset + count) % count
    following, previous = owner_of(at(1)), owner_of(at(-1))

    loads = [
        pltpu.make_async_copy(wk, w_side.at[place, :, pl.ds(0, kw)], load_sem.at[0]),
        pltpu.make_async_copy(wv, w_side.at[place, :, pl.ds(kw, kw)], load_sem.at[1]),
        pltpu.make_async_copy(wp, w_side.at[place, :, pl.ds(2 * kw, pw)], load_sem.at[2]),
        pltpu.make_async_copy(tokens, tok.at[tp], load_sem.at[3]),
        pltpu.make_async_copy(wq, w_query.at[place], load_sem.at[4]),
        pltpu.make_async_copy(wop, w_out.at[place, pl.ds(0, pw), :], load_sem.at[5]),
        pltpu.make_async_copy(woa, w_out.at[place, pl.ds(pw, qw), :], load_sem.at[6]),
    ]
    for load in loads:
        load.start()

    barrier = pltpu.get_barrier_semaphore()
    greeted = [
        (following, tp),
        (previous, tp),
        (me, partner),
        ((me + 1) % count, tp),
        ((me + count - 1) % count, tp),
    ]
    greeted += [(me, (chip + hop) % chips * 2 + core) for hop in range(1, chips)]
    for device in greeted:
        pl.semaphore_signal(barrier, inc=1, device_id=device, device_id_type=MESH)
    pl.semaphore_wait(barrier, len(greeted))

    def remote(source, target, send_sem, recv_sem, device):
        return pltpu.make_async_remote_copy(
            src_ref=source,
            dst_ref=target,
            send_sem=send_sem,
            recv_sem=recv_sem,
            device_id=device,
            device_id_type=MESH,
        )

    def hop_copy(ring, way, spot, c):
        buffer, send_sem, recv_sem = ring
        size = buffer.shape[1] // chunks
        part = buffer.at[spot, pl.ds(pl.multiple_of(c * size, 16), size), :]
        device = (following if way == 0 else previous, tp)
        return remote(part, part, send_sem.at[way, spot, c], recv_sem.at[spot, c], device)

    def send_own(ring):
        for c in range(chunks):
            hop_copy(ring, 0, place, c).start()
            hop_copy(ring, 1, place, c).start()

    def event(ring, step, c):
        low, high = at(-step), at(step)
        hop_copy(ring, 0, low, c).wait_recv()

        @pl.when((step < half) | (c < chunks // 2))
        def _():
            hop_copy(ring, 0, low, c).start()

        hop_copy(ring, 1, high, c).wait_recv()

        @pl.when((step < half) | (c >= chunks // 2))
        def _():
            hop_copy(ring, 1, high, c).start()

    def events(ring, step):
        def body(c, carry):
            event(ring, step, c)
            return carry

        lax.fori_loop(0, chunks, body, 0)

    def opposite(ring):
        def body(c, carry):
            hop_copy(ring, 0, at(count // 2), c).wait_recv()
            return carry

        lax.fori_loop(0, chunks, body, 0)

    def sends_done(ring):
        def each(c, carry):
            hop_copy(ring, 0, place, c).wait_send()
            hop_copy(ring, 1, place, c).wait_send()

            def steps(step, inner):
                @pl.when((step < half) | (c < chunks // 2))
                def _():
                    hop_copy(ring, 0, at(-step), c).wait_send()

                @pl.when((step < half) | (c >= chunks // 2))
                def _():
                    hop_copy(ring, 1, at(step), c).wait_send()

                return inner

            return lax.fori_loop(1, half + 1, steps, carry)

        lax.fori_loop(0, chunks, each, 0)

    side_ring = (w_side, side_send, side_recv)
    query_ring = (w_query, query_send, query_recv)
    out_ring = (w_out, out_send, out_recv)

    for load in loads[:3]:
        load.wait()
    send_own(side_ring)
    loads[3].wait()

    token_rows = rows // token_chunks

    def token_part(owner, j):
        return tok.at[owner, pl.ds(pl.multiple_of(j * token_rows, 16), token_rows), :]

    def token_far(hop, owner, j):
        part = token_part(owner, j)
        target = (chip + hop) % chips * 2 + core
        return remote(
            part, part, ty_send.at[hop - 1, j], ty_recv.at[hop - 1, j], (me, target)
        )

    def token_near(slot, owner, j):
        part = token_part(owner, j)
        return remote(part, part, td_send.at[slot, j], td_recv.at[slot, j], (me, partner))

    def start_tokens(j, carry):
        for hop in range(1, chips):
            token_far(hop, tp, j).start()
        token_near(0, tp, j).start()
        return carry

    lax.fori_loop(0, token_chunks, start_tokens, 0)

    for g in range(rows // GRID_W):
        spot = pl.ds(me * (rows // GRID_W) + g, 1)
        grid_rows = pl.ds(g * GRID_W, GRID_W)
        cosines[grid_rows, :] = col_cos[...] + row_cos[spot, :]
        sines[grid_rows, :] = col_sin[...] + row_sin[spot, :]

    pieces = features // depth
    norm_rows = 32 if token_rows % 32 == 0 else 16

    def normalise(j):
        token_near(0, partner, j).wait_recv()
        for hop in range(1, chips):
            token_near(hop, (chip - hop + chips) % chips * 2 + 1 - core, j).wait_recv()

        def tile(i, carry):
            at_rows = pl.ds(pl.multiple_of(j * token_rows + i * norm_rows, 16), norm_rows)
            squares = jnp.zeros((norm_rows, 1), f32)
            for t in range(members):
                block = tok[t, at_rows, :].astype(f32)
                squares = squares + jnp.sum(block * block, axis=1, keepdims=True)
            scale = lax.rsqrt(squares / (members * features) + eps)
            for t in range(members):
                for piece in range(pieces):
                    first = piece * depth
                    gain = norm_gain[:, t * features + first : t * features + first + depth]
                    block = tok[t, at_rows, first : first + depth].astype(f32)
                    normed[t * pieces + piece, at_rows, :] = (block * scale * gain).astype(bf16)
            return carry

        lax.fori_loop(0, token_rows // norm_rows, tile, 0)

    def token_step(j, carry):
        for hop in range(1, chips):
            source = (chip - hop + chips) % chips * 2 + core
            token_far(hop, source, j).wait_recv()
            token_near(hop, source, j).start()

        @pl.when(j < half * chunks)
        def _():
            event(side_ring, j // chunks + 1, j % chunks)

        @pl.when(j >= 1)
        def _():
            normalise(j - 1)

        return carry

    lax.fori_loop(0, token_chunks, token_step, 0)
    normalise(token_chunks - 1)

    tile_rows = 256 if rows % 256 == 0 else 128

    def project(total, weights, spots, first=False):
        def body(i, carry):
            part = pl.ds(pl.multiple_of(i * tile_rows, tile_rows), tile_rows)
            terms = [
                jnp.dot(
                    normed[owner_of(spot), part, :], weights[spot], preferred_element_type=f32
                )
                for spot in spots
            ]
            value = functools.reduce(lambda a, b: a + b, terms)
            total[part, :] = value if first else total[part, :] + value
            return carry

        lax.fori_loop(0, rows // tile_rows, body, 0)

    project(side, w_side, [place], first=True)
    early = token_chunks // chunks

    def side_step(step, carry):
        @pl.when(step > early)
        def _():
            events(side_ring, step)

        project(side, w_side, [at(-step), at(step)])
        return carry

    lax.fori_loop(1, half + 1, side_step, 0)
    loads[4].wait()
    send_own(query_ring)
    opposite(side_ring)
    project(side, w_side, [at(count // 2)])

    twice = lambda gain: jnp.concatenate([gain[...], gain[...]], axis=1)
    query_gains, key_gains = twice(query_gain), twice(key_gain)
    lane = lax.broadcasted_iota(jnp.int32, (WINDOW, 2 * HEAD), 1)
    low_half = lane < HEAD
    lead = lane % (HEAD // 2) < HEAD // 4

    def prepare(i, carry):
        part = pl.ds(pl.multiple_of(i * WINDOW, WINDOW), WINDOW)
        shifted = pl.ds(pl.multiple_of((i + 1) * WINDOW, WINDOW), WINDOW)
        for h in range(kw // (2 * HEAD)):
            lanes = slice(h * 2 * HEAD, (h + 1) * 2 * HEAD)
            key = norm_rope(
                side[part, lanes], key_gains, cosines[part, :], sines[part, :], low_half, lead
            )
            band[shifted, lanes] = key.astype(bf16)
        band[shifted, kw : 2 * kw] = side[part, kw : 2 * kw].astype(bf16)
        pooled_rows = pl.ds(pl.multiple_of(i * WINDOW + pool_pad, pool_pad), WINDOW)
        pool_band[pooled_rows, :] = side[part, 2 * kw :].astype(bf16)
        return carry

    lax.fori_loop(0, rows // WINDOW, prepare, 0)

    before, behind = (me + count - 1) % count, (me + 1) % count

    def halo(index, buffer, size, upwards):
        if upwards:
            source, target, device = rows, 0, (behind, tp)
        else:
            source, target, device = size, rows + size, (before, tp)
        return remote(
            buffer.at[pl.ds(source, size), :],
            buffer.at[pl.ds(target, size), :],
            halo_send.at[index],
            halo_recv.at[index],
            device,
        )

    lower = [halo(0, band, WINDOW, False), halo(1, pool_band, pool_pad, False)]
    upper = [halo(2, band, WINDOW, True), halo(3, pool_band, pool_pad, True)]
    has_lower, has_upper = me > 0, me < count - 1

    @pl.when(has_lower)
    def _():
        for copy in lower:
            copy.start()

    @pl.when(has_upper)
    def _():
        for copy in upper:
            copy.start()

    @pl.when(jnp.logical_not(has_lower))
    def _():
        band[0:WINDOW, :] = jnp.zeros((WINDOW, 2 * kw), bf16)
        pool_band[0:pool_pad, :] = jnp.zeros((pool_pad, pw), bf16)

    @pl.when(jnp.logical_not(has_upper))
    def _():
        band[rows + WINDOW :, :] = jnp.zeros((WINDOW, 2 * kw), bf16)
        pool_band[rows + pool_pad :, :] = jnp.zeros((pool_pad, pw), bf16)

    project(query, w_query, [place], first=True)

    def query_step(step, carry):
        events(query_ring, step)
        project(query, w_query, [at(-step), at(step)])
        return carry

    lax.fori_loop(1, half + 1, query_step, 0)
    loads[5].wait()
    loads[6].wait()
    send_own(out_ring)

    @pl.when(has_lower)
    def _():
        for copy in upper:
            copy.wait_recv()

    @pl.when(has_upper)
    def _():
        for copy in lower:
            copy.wait_recv()

    level = tp * pw // (POOL // 4)
    reach = jnp.where(level == 0, 1, jnp.where(level == 1, 2, jnp.where(level == 2, 4, 8)))

    def pool(i, carry):
        wide = WINDOW + 2 * pool_pad
        part = pl.ds(pl.multiple_of(i * WINDOW, WINDOW), WINDOW)
        values = pool_band[pl.ds(pl.multiple_of(i * WINDOW, pool_pad), wide), :].astype(f32)
        total, chosen = values, None
        for step in range(4):
            size = 2**step
            total = total + pltpu.roll(total, wide - size, 0)
            shifted = pltpu.roll(total, size, 0)[pool_pad : pool_pad + WINDOW]
            chosen = shifted if chosen is None else jnp.where(level == step, shifted, chosen)
        spot = me * rows + i * WINDOW + lax.broadcasted_iota(jnp.int32, (WINDOW, 1), 0)
        low = jnp.maximum(spot - reach, 0)
        high = jnp.minimum(spot + reach - 1, seq - 1)
        mixer[part, 0:pw] = (chosen / (high - low + 1).astype(f32)).astype(bf16)
        return carry

    lax.fori_loop(0, rows // WINDOW, pool, 0)

    opposite(query_ring)
    project(query, w_query, [at(count // 2)])

    blocks = rows // WINDOW
    row = lax.broadcasted_iota(jnp.int32, (2 * WINDOW, 3 * WINDOW), 0) % WINDOW
    column = lax.broadcasted_iota(jnp.int32, (2 * WINDOW, 3 * WINDOW), 1)
    top_row = lax.broadcasted_iota(jnp.int32, (2 * WINDOW, 1), 0) < WINDOW

    def attend(i, carry):
        part = pl.ds(pl.multiple_of(i * WINDOW, WINDOW), WINDOW)
        key_rows = pl.ds(pl.multiple_of(i * WINDOW, WINDOW), 3 * WINDOW)
        key_pos = me * rows + i * WINDOW - WINDOW + column
        inside = (column >= row) & (column - row <= 2 * WINDOW) & (key_pos >= 0) & (key_pos < seq)
        for head in range(heads_k):
            lanes = slice(head * 2 * HEAD, (head + 1) * 2 * HEAD)
            rotated = norm_rope(
                query[part, lanes],
                query_gains,
                cosines[part, :],
                sines[part, :],
                low_half,
                lead,
            ) * HEAD ** (-0.5)
            other = pltpu.roll(rotated, HEAD, 1)
            if head % 2 == 0:
                pair = (jnp.where(low_half, rotated, 0.0), jnp.where(low_half, other, 0.0))
            else:
                pair = (jnp.where(low_half, 0.0, other), jnp.where(low_half, 0.0, rotated))
            stacked = jnp.concatenate(pair, axis=0).astype(bf16)
            tile = head // 2 * 2 * HEAD
            keys = band[key_rows, tile : tile + 2 * HEAD]
            values = band[key_rows, kw + tile : kw + tile + 2 * HEAD]
            scores = lax.dot_general(
                stacked, keys, (((1,), (1,)), ((), ())), preferred_element_type=f32
            )
            scores = jnp.where(inside, scores, neg_big)
            limit = jnp.where(top_row, sink[2 * head], sink[2 * head + 1])
            top = jnp.maximum(jnp.max(scores, axis=1, keepdims=True), limit)
            raised = jnp.exp(scores - top)
            totals = jnp.sum(raised, axis=1, keepdims=True) + jnp.exp(limit - top)
            weights = (raised * (1.0 / totals)).astype(bf16)
            result = jnp.dot(weights, values, preferred_element_type=f32)
            one, two = result[:WINDOW], result[WINDOW:]
            if head % 2 == 0:
                joined = jnp.where(low_half, one, pltpu.roll(two, HEAD, 1))
            else:
                joined = jnp.where(low_half, pltpu.roll(one, HEAD, 1), two)
            mixer[part, pw + head * 2 * HEAD : pw + (head + 1) * 2 * HEAD] = joined.astype(bf16)

        for c in range(chunks):

            @pl.when(i == ((c + 1) * blocks + chunks - 1) // chunks - 1)
            def _(c=c):
                event(out_ring, 1, c)

        return carry

    lax.fori_loop(0, blocks, attend, 0)

    def product(spot, which):
        left = jnp.concatenate(
            [
                mixer[pl.ds(pl.multiple_of((y * 2 + which) * share, 16), share), :]
                for y in range(chips)
            ],
            axis=0,
        )
        return jnp.dot(left, w_out[spot], preferred_element_type=f32).astype(bf16)

    def met_copy(spot):
        return remote(
            away.at[spot], met.at[spot], met_send.at[spot], met_recv.at[spot], (me, partner)
        )

    def y_copy(spot, hop):
        target = (chip + hop) % chips * 2 + core
        return remote(
            y_send.at[spot, hop - 1],
            y_recv.at[spot, hop - 1],
            yy_send.at[spot, hop - 1],
            yy_recv.at[spot, hop - 1],
            (me, target),
        )

    def done_copy(spot):
        columns = pl.ds(pl.multiple_of(owner_of(spot) * width, width), width)
        return pltpu.make_async_copy(done.at[spot], out.at[:, columns], done_sem.at[spot])

    def both_rows(spot, y):
        part = pl.ds(pl.multiple_of(y * share, 16), share)
        return kept[spot, part, :].astype(f32) + met[spot, part, :].astype(f32)

    def group(spots):
        def first(spot):
            away[spot] = product(spot, 1 - core)
            met_copy(spot).start()

        def second(spot):
            kept[spot] = product(spot, core)

        def third(spot):
            met_copy(spot).wait_recv()
            for hop in range(1, chips):
                y_send[spot, hop - 1] = both_rows(spot, (chip + hop) % chips).astype(bf16)
                y_copy(spot, hop).start()

        for part in (first, second, third):
            for spot in spots:
                part(spot)

    def finish(spot):
        total = both_rows(spot, chip)
        for hop in range(1, chips):
            y_copy(spot, hop).wait_recv()
            total = total + y_recv[spot, hop - 1].astype(f32)
        done[spot] = total.astype(bf16)
        done_copy(spot).start()

    group([place])

    def out_step(step, carry):
        @pl.when(step > 1)
        def _():
            events(out_ring, step)

        group([at(-step), at(step)])

        @pl.when(step == 1)
        def _():
            finish(place)

        @pl.when(step > 1)
        def _():
            finish(at(1 - step))
            finish(at(step - 1))

        return carry

    lax.fori_loop(1, half + 1, out_step, 0)
    opposite(out_ring)
    group([at(count // 2)])
    finish(at(-half))
    finish(at(half))
    finish(at(count // 2))

    for ring in (side_ring, query_ring, out_ring):
        sends_done(ring)

    def tokens_sent(j, carry):
        token_near(0, tp, j).wait_send()
        for hop in range(1, chips):
            token_far(hop, tp, j).wait_send()
            token_near(hop, (chip - hop + chips) % chips * 2 + core, j).wait_send()
        return carry

    lax.fori_loop(0, token_chunks, tokens_sent, 0)

    @pl.when(has_lower)
    def _():
        for copy in lower:
            copy.wait_send()

    @pl.when(has_upper)
    def _():
        for copy in upper:
            copy.wait_send()

    def blocks_sent(spot, carry):
        met_copy(spot).wait_send()
        for hop in range(1, chips):
            y_copy(spot, hop).wait_send()
        done_copy(spot).wait()
        return carry

    lax.fori_loop(0, count, blocks_sent, 0)


def plane_kernel(
    count,
    members,
    tokens,
    wq,
    wk,
    wv,
    wp,
    wop,
    woa,
    norm_gain_in,
    query_gain_in,
    key_gain_in,
    row_cos_in,
    row_sin_in,
    col_cos_in,
    col_sin_in,
    sink_in,
    out,
    norm_gain,
    query_gain,
    key_gain,
    row_cos,
    row_sin,
    col_cos,
    col_sin,
    sink,
    small_sem,
    raw,
    sums,
    normed,
    w_in,
    w_pool,
    w_out,
    in_spare,
    pool_spare,
    out_spare,
    total,
    band,
    pool_band,
    cosines,
    sines,
    attended,
    pooled,
    result,
    rounded,
    load_sem,
    sum_sems,
    in_sems,
    pool_sems,
    out_sems,
    x_sems,
    ring_sems,
    spread_sems,
    token_sems,
    token_bulk,
    attend_sems,
    attend_bulk,
    pooled_sems,
    pooled_bulk,
    halo_send,
    halo_recv,
    result_sems,
    go_sem,
):
    rows, features = tokens.shape
    depth = wk.shape[0]
    hk, hq, hp = wk.shape[1] // 2, wq.shape[1] // 2, wp.shape[1] // 2
    width = wop.shape[1]
    narrow = width // members
    share = rows // members
    plane = 2 * rows
    heads_k = hk // HEAD
    seq = count * rows
    deep = count // 2
    pieces = features // depth
    tiles = rows // WINDOW
    grid = plane // GRID_W

    me, tp = lax.axis_index("sp"), lax.axis_index("tp")
    z, x = me // 2, me % 2
    y, core = tp // 2, tp % 2
    me_x, tp_y, tp_c = me + 1 - 2 * x, (1 - y) * 2 + core, y * 2 + 1 - core
    tp_yc = (1 - y) * 2 + 1 - core
    up, down = (me + 2) % count, (me + count - 2) % count
    has_up, has_down = z < deep - 1, z > 0
    inner = has_up & has_down

    mine = lambda size: pl.ds(pl.multiple_of(x * size, 128), size)
    other = lambda size: pl.ds(pl.multiple_of((1 - x) * size, 128), size)

    def load(group, source, target):
        pltpu.make_async_copy(source, target, load_sem.at[group]).start()

    def loaded(group, whole):
        pltpu.make_async_copy(whole, whole, load_sem.at[group]).wait()

    for target, pick in ((w_in.at[me], mine), (in_spare, other)):
        load(0, wk.at[:, pick(hk)], target.at[:, pl.ds(0, hk)])
        load(0, wv.at[:, pick(hk)], target.at[:, pl.ds(hk, hk)])
        load(0, wq.at[:, pick(hq)], target.at[:, pl.ds(2 * hk, hq)])
    load(1, tokens, raw)
    small = [
        pltpu.make_async_copy(source, target, small_sem.at[index])
        for index, (source, target) in enumerate(
            (
                (norm_gain_in, norm_gain),
                (query_gain_in, query_gain),
                (key_gain_in, key_gain),
                (row_cos_in.at[pl.ds(z * grid, grid), :], row_cos),
                (row_sin_in.at[pl.ds(z * grid, grid), :], row_sin),
                (col_cos_in, col_cos),
                (col_sin_in, col_sin),
                (sink_in, sink),
            )
        )
    ]
    for copy in small:
        copy.start()
    for target, pick in ((w_pool.at[me], mine), (pool_spare, other)):
        load(2, wp.at[:, pick(hp)], target)
    strip = lambda t: pl.ds(pl.multiple_of(t * narrow, narrow), narrow)
    strips = [(3, w_out.at[z, tp], tp)] + [(4, out_spare.at[t], t) for t in range(members)]
    for group, target, t in strips:
        load(group, woa.at[:, strip(t)], target.at[pl.ds(0, 2 * hq), :])
        load(group, wop.at[:, strip(t)], target.at[pl.ds(2 * hq, 2 * hp), :])

    barrier = pltpu.get_barrier_semaphore()
    greeted = [(up, tp), (down, tp), (me_x, tp), (me, tp_y), (me, tp_c), (me, tp_yc)]
    for device in greeted:
        pl.semaphore_signal(barrier, inc=1, device_id=device, device_id_type=MESH)
    pl.semaphore_wait(barrier, len(greeted))

    def remote(source, target, send_sem, recv_sem, device):
        return pltpu.make_async_remote_copy(
            src_ref=source,
            dst_ref=target,
            send_sem=send_sem,
            recv_sem=recv_sem,
            device_id=device,
            device_id_type=MESH,
        )

    def by_rows(parts):
        def view(buffer, c):
            size = buffer.shape[0] // parts
            return buffer.at[pl.ds(pl.multiple_of(c * size, 16), size), :]

        return view

    in_ring = (w_in, in_spare, in_sems, 0, in_parts, by_rows(in_parts))
    pool_ring = (w_pool, pool_spare, pool_sems, 1, 1, by_rows(1))
    def z_copy(ring, way, source, c):
        buffer, _, sems, _, _, view = ring
        part = view(buffer.at[source], c)
        send = ring_sems.at[ring[3], way]
        return remote(part, part, send, sems.at[source, c], ((up, down)[way], tp))

    def x_copy(ring, source, c):
        buffer, spare, sems, first, _, view = ring
        return remote(
            view(spare, c),
            view(buffer.at[source], c),
            x_sems.at[first],
            sems.at[source, c],
            (me_x, tp),
        )

    def both_ways(ring, source, c, act):
        @pl.when(has_up)
        def _():
            act(z_copy(ring, 0, source, c))

        @pl.when(has_down)
        def _():
            act(z_copy(ring, 1, source, c))

    start = lambda copy: copy.start()

    def own_out(ring):
        for c in range(ring[4]):
            both_ways(ring, me, c, start)

    def side_out(ring):
        for c in range(ring[4]):
            x_copy(ring, me, c).start()

    def side_in(ring):
        for c in range(ring[4]):
            x_copy(ring, me_x, c).wait_recv()
            both_ways(ring, me_x, c, start)

    def passing(ring, n):
        parts = ring[4]
        step, j, c = n // (2 * parts) + 1, n // parts % 2, n % parts
        column = (x + j) % 2
        low, high = z - step, z + step
        return (low >= 0, low * 2 + column), (high < deep, high * 2 + column), c

    def event(ring, n):
        (is_low, low), (is_high, high), c = passing(ring, n)

        @pl.when(is_low)
        def _():
            z_copy(ring, 0, low, c).wait_recv()

            @pl.when(has_up)
            def _():
                z_copy(ring, 0, low, c).start()

        @pl.when(is_high)
        def _():
            z_copy(ring, 1, high, c).wait_recv()

            @pl.when(has_down)
            def _():
                z_copy(ring, 1, high, c).start()

    def events(ring, first, last):
        def body(n, carry):
            event(ring, n)
            return carry

        lax.fori_loop(first, last, body, 0)

    def all_events(ring):
        return (deep - 1) * 2 * ring[4]

    def bulk(whole, sem):
        return remote(whole, whole, sem, sem, (me_x, tp))

    def sends_done(buffer, sem, each):
        for level in range(deep):

            @pl.when(z == level)
            def _(level=level):
                if level < deep - 1:
                    whole = buffer.at[pl.ds(0, (level + 1) * each)]
                    bulk(whole, ring_sems.at[sem, 0]).wait_send()
                if level > 0:
                    whole = buffer.at[pl.ds(0, (deep - level) * each)]
                    bulk(whole, ring_sems.at[sem, 1]).wait_send()

    def out_copy(way, level, c):
        part = w_out.at[level, (tp - c + members) % members]
        send = ring_sems.at[2, way]
        return remote(part, part, send, out_sems.at[level, c], ((up, down)[way], tp))

    def spread(c):
        target = (tp + c) % members
        return remote(
            out_spare.at[target],
            w_out.at[z, tp],
            spread_sems.at[0],
            out_sems.at[z, c],
            (me, target),
        )

    def spread_in(c):
        owner = (tp - c + members) % members
        return remote(
            out_spare.at[owner],
            w_out.at[z, owner],
            spread_sems.at[0],
            out_sems.at[z, c],
            (me, owner),
        )

    def out_both(c, act):
        @pl.when(has_up)
        def _():
            act(out_copy(0, z, c))

        @pl.when(has_down)
        def _():
            act(out_copy(1, z, c))

    skewed = deep >= 4
    late_up = skewed & (core == 1) & (z == deep - 2)
    late_down = skewed & (core == 1) & (z == 1)

    def late_copies(act):
        @pl.when(late_up)
        def _():
            for c in range(members):
                act(out_copy(0, 0, c))

        @pl.when(late_down)
        def _():
            for c in range(members):
                act(out_copy(1, deep - 1, c))

    def out_event(n):
        step, c = n // members + 1, n % members
        low, high = z - step, z + step

        @pl.when(low >= 0)
        def _():
            out_copy(0, low, c).wait_recv()

            @pl.when(has_up & jnp.logical_not(late_up & (low == 0)))
            def _():
                out_copy(0, low, c).start()

        @pl.when(high < deep)
        def _():
            out_copy(1, high, c).wait_recv()

            @pl.when(has_down & jnp.logical_not(late_down & (high == deep - 1)))
            def _():
                out_copy(1, high, c).start()

    def out_events(first, last):
        def body(n, carry):
            out_event(n)
            return carry

        lax.fori_loop(first, last, body, 0)

    loaded(0, w_in.at[pl.ds(0, 2)])
    for c in range(in_parts):
        x_copy(in_ring, me, c).start()
        both_ways(in_ring, me, c, start)

    loaded(1, raw)
    for copy in small:
        copy.wait()
    sums[tp] = jnp.zeros_like(sums[tp])
    for i in range(tiles):
        block = raw[i * WINDOW : (i + 1) * WINDOW, :].astype(f32)
        square = jnp.sum(block * block, axis=1, keepdims=True)
        turned = jnp.transpose(jnp.broadcast_to(square, (WINDOW, WINDOW)))
        sums[tp, i : i + 1, :] = turned[0:1, :]

    def sum_copy(owner, hop):
        target = (tp + hop) % members
        return remote(
            sums.at[owner],
            sums.at[owner],
            sum_sems.at[0],
            sum_sems.at[1],
            (me, target),
        )

    for hop in range(1, members):
        sum_copy(tp, hop).start()
    for g in range(grid):
        grid_rows = pl.ds(g * GRID_W, GRID_W)
        cosines[grid_rows, :] = col_cos[...] + row_cos[g : g + 1, :]
        sines[grid_rows, :] = col_sin[...] + row_sin[g : g + 1, :]
    bulk(sums.at[pl.ds(0, members - 1)], sum_sems.at[1]).wait_recv()
    squares = sums[0]
    for t in range(1, members):
        squares = squares + sums[t]
    scales = lax.rsqrt(squares / (members * features) + eps)

    class Stream:
        def __init__(self, view, all_sent, side, sems, bulk_sems, by_x, pair=None):
            self.pair, self.crossing = pair, 1 if pair else 2
            self.view, self.all_sent, self.side = view, all_sent, side
            self.sems, self.bulk_sems, self.by_x = sems, bulk_sems, by_x

        def copy(self, recv, side, owner, j, device):
            part = self.view(side, owner, j)
            return remote(part, part, self.bulk_sems.at[0], recv, device)

        def over_x(self, slot, side, owner, j):
            return self.copy(self.sems.at[slot * self.crossing, j], side, owner, j, (me_x, tp))

        def over_y(self, slot, side, owner, j):
            index = slot * self.crossing if self.pair or slot else 1
            return self.copy(self.sems.at[index, j], side, owner, j, (me, tp_y))

        def over_core(self, slot, side, owner, j):
            return self.copy(self.bulk_sems.at[1 + slot % 2], side, owner, j, (me, tp_c))

        def start(self, j):
            self.over_y(0, x, tp, j).start()
            self.over_x(0, x, tp, j).start()
            self.over_core(0, x, tp, j).start()

        def direct(self, j):
            if self.pair:
                bulk(self.pair(j), self.sems.at[0, j]).wait_recv()
            else:
                self.over_y(0, x, tp_y, j).wait_recv()
            self.over_core(2, x, tp_y, j).start()

            @pl.when(self.by_x(j))
            def _():
                self.over_x(1, x, tp_y, j).start()

            if not self.pair:
                self.over_x(0, 1 - x, tp, j).wait_recv()
            self.over_core(1, 1 - x, tp, j).start()

            @pl.when(jnp.logical_not(self.by_x(j)))
            def _():
                self.over_y(1, 1 - x, tp, j).start()

        def crossed(self, j):
            @pl.when(self.by_x(j))
            def _():
                self.over_x(1, 1 - x, tp_y, j).wait_recv()

            @pl.when(jnp.logical_not(self.by_x(j)))
            def _():
                self.over_y(1, 1 - x, tp_y, j).wait_recv()

            self.over_core(3, 1 - x, tp_y, j).start()

        def near_side(self):
            bulk(self.side, self.bulk_sems.at[1]).wait_recv()

        def far_side(self):
            bulk(self.side, self.bulk_sems.at[2]).wait_recv()

        def sent(self):
            bulk(self.all_sent, self.bulk_sems.at[0]).wait_send()

        def every(self, act):
            def body(j, carry):
                act(j)
                return carry

            lax.fori_loop(0, self.sems.shape[1], body, 0)

    def block_rows(j, size):
        return pl.ds(pl.multiple_of(j * size, 16), size)

    def token_view(side, owner, j):
        return normed.at[side, pl.ds(owner * pieces, pieces), block_rows(j, WINDOW), :]

    def attend_view(side, owner, j):
        return attended.at[owner, side, block_rows(j, WINDOW), :]

    def pooled_view(side, owner, j):
        return pooled.at[owner, side, block_rows(j, plane // pooled_parts), :]

    most = lambda size: pl.ds(0, size * (2 * members - 1) // (2 * members))
    token_stream = Stream(
        token_view,
        normed.at[:, :, most(rows), :],
        normed.at[0, pl.ds(0, count // 2)],
        token_sems,
        token_bulk,
        lambda j: j % 3 == 0,
    )
    attend_stream, pooled_stream = [
        Stream(
            view,
            buffer.at[:, :, most(plane), :],
            buffer.at[0],
            sems,
            bulk_sems,
            lambda j: j % 2 == 0,
            lambda j, buffer=buffer, size=size: buffer.at[0, :, block_rows(j, size), :],
        )
        for view, buffer, sems, bulk_sems, size in (
            (attend_view, attended, attend_sems, attend_bulk, WINDOW),
            (pooled_view, pooled, pooled_sems, pooled_bulk, plane // pooled_parts),
        )
    ]

    for i in range(tiles):
        here = slice(i * WINDOW, (i + 1) * WINDOW)
        scale = jnp.transpose(jnp.broadcast_to(scales[i : i + 1, :], (WINDOW, WINDOW)))
        for first in range(0, features, WINDOW):
            block = raw[here, first : first + WINDOW].astype(f32)
            gain = norm_gain[:, pl.ds(pl.multiple_of(tp * features + first, WINDOW), WINDOW)]
            value = (block * scale * gain).astype(bf16)
            inside = first % depth
            normed[x, tp * pieces + first // depth, here, inside : inside + WINDOW] = value
        token_stream.start(i)

    side_in(in_ring)
    whole = all_events(in_ring)
    reached = lambda part: whole * part // 24
    events(in_ring, 0, reached(4))

    def direct(j, carry):
        token_stream.direct(j)
        events(in_ring, reached(4 + 12 * j // tiles), reached(4 + 12 * (j + 1) // tiles))
        return carry

    lax.fori_loop(0, tiles, direct, 0)
    loaded(2, w_pool.at[pl.ds(0, 2)])
    loaded(3, w_out.at[0, 0])
    loaded(4, out_spare)
    side_out(pool_ring)
    for c in range(1, members):
        spread(c).start()
    token_stream.near_side()

    tile_rows = 256 if rows % 256 == 0 else 128
    per_side = rows // tile_rows

    def project(result, weights, level, side, first=False):
        def body(i, carry):
            within = pl.ds(pl.multiple_of(i * tile_rows, tile_rows), tile_rows)
            part = pl.ds(pl.multiple_of(side * rows + i * tile_rows, tile_rows), tile_rows)
            value = None if first else result[part, :]
            for j in range(2):
                term = jnp.dot(
                    normed[side, level * 2 + j, within, :],
                    weights[level * 2 + j],
                    preferred_element_type=f32,
                )
                value = term if value is None else value + term
            result[part, :] = value
            return carry

        lax.fori_loop(0, per_side, body, 0)

    def project_step(result, weights, step, side):
        @pl.when(z - step >= 0)
        def _():
            project(result, weights, z - step, side)

        @pl.when(z + step < deep)
        def _():
            project(result, weights, z + step, side)

    early = max(reached(16) // (2 * in_parts), 0)

    def crossed(j, carry):
        token_stream.crossed(j)

        @pl.when(j == 0)
        def _():
            project(total, w_in, z, x, first=True)

        @pl.when((j >= 1) & (j <= early))
        def _():
            project_step(total, w_in, j, x)

        events(in_ring, reached(16 + 4 * j // tiles), reached(16 + 4 * (j + 1) // tiles))
        return carry

    lax.fori_loop(0, tiles, crossed, 0)
    own_out(pool_ring)
    side_in(pool_ring)
    token_stream.far_side()
    project(total, w_in, z, 1 - x, first=True)

    @pl.when(inner)
    def _():
        events(pool_ring, 0, 2)


    def in_step(step, carry):
        each = 2 * in_parts
        events(in_ring, jnp.maximum((step - 1) * each, reached(20)), step * each)

        @pl.when(step > min(early, tiles - 1))
        def _():
            project_step(total, w_in, step, x)

        project_step(total, w_in, step, 1 - x)
        return carry

    lax.fori_loop(1, deep, in_step, 0)

    twice = lambda gain: jnp.concatenate([gain[...], gain[...]], axis=1)
    query_gains, key_gains = twice(query_gain), twice(key_gain)
    lane = lax.broadcasted_iota(jnp.int32, (WINDOW, 2 * HEAD), 1)
    low_half = lane < HEAD
    lead = lane % (HEAD // 2) < HEAD // 4
    blocks = plane // WINDOW

    def prepare(i, carry):
        part = pl.ds(pl.multiple_of(i * WINDOW, WINDOW), WINDOW)
        shifted = pl.ds(pl.multiple_of((i + 1) * WINDOW, WINDOW), WINDOW)
        for h in range(hk // (2 * HEAD)):
            lanes = slice(h * 2 * HEAD, (h + 1) * 2 * HEAD)
            key = norm_rope(
                total[part, lanes], key_gains, cosines[part, :], sines[part, :], low_half, lead
            )
            band[shifted, lanes] = key.astype(bf16)
        band[shifted, hk:] = total[part, hk : 2 * hk].astype(bf16)
        return carry

    lax.fori_loop(0, blocks, prepare, 0)

    def halo(index, buffer, size, upwards):
        if upwards:
            source, target, device = plane, 0, (up, tp)
        else:
            source, target, device = size, plane + size, (down, tp)
        return remote(
            buffer.at[pl.ds(source, size), :],
            buffer.at[pl.ds(target, size), :],
            halo_send.at[index],
            halo_recv.at[index],
            device,
        )

    def halo_out(index, buffer, size):
        @pl.when(has_down)
        def _():
            halo(index, buffer, size, False).start()

        @pl.when(has_up)
        def _():
            halo(index + 1, buffer, size, True).start()

        empty = jnp.zeros((size, buffer.shape[1]), bf16)

        @pl.when(jnp.logical_not(has_down))
        def _():
            buffer[0:size, :] = empty

        @pl.when(jnp.logical_not(has_up))
        def _():
            buffer[plane + size :, :] = empty

    def halo_in(index, buffer, size):
        @pl.when(has_up)
        def _():
            halo(index, buffer, size, False).wait_recv()

        @pl.when(has_down)
        def _():
            halo(index + 1, buffer, size, True).wait_recv()

    halo_out(0, band, WINDOW)

    @pl.when(inner)
    def _():
        events(pool_ring, 2, all_events(pool_ring))

    for c in range(members - 1):
        if c > 0:
            spread_in(c).wait_recv()
        out_both(c, start)

    row = lax.broadcasted_iota(jnp.int32, (2 * WINDOW, 3 * WINDOW), 0) % WINDOW
    column = lax.broadcasted_iota(jnp.int32, (2 * WINDOW, 3 * WINDOW), 1)
    top_row = lax.broadcasted_iota(jnp.int32, (2 * WINDOW, 1), 0) < WINDOW

    def attend(turn, carry):
        @pl.when(turn == blocks - 2)
        def _():
            halo_in(0, band, WINDOW)

        i = (turn + 1) % blocks
        part = pl.ds(pl.multiple_of(i * WINDOW, WINDOW), WINDOW)
        key_rows = pl.ds(pl.multiple_of(i * WINDOW, WINDOW), 3 * WINDOW)
        key_pos = z * plane + i * WINDOW - WINDOW + column
        inside = (column >= row) & (column - row <= 2 * WINDOW) & (key_pos >= 0) & (key_pos < seq)
        for head in range(heads_k):
            lanes = slice(2 * hk + head * 2 * HEAD, 2 * hk + (head + 1) * 2 * HEAD)
            rotated = norm_rope(
                total[part, lanes],
                query_gains,
                cosines[part, :],
                sines[part, :],
                low_half,
                lead,
            ) * HEAD ** (-0.5)
            swapped = pltpu.roll(rotated, HEAD, 1)
            if head % 2 == 0:
                pair = (jnp.where(low_half, rotated, 0.0), jnp.where(low_half, swapped, 0.0))
            else:
                pair = (jnp.where(low_half, 0.0, swapped), jnp.where(low_half, 0.0, rotated))
            stacked = jnp.concatenate(pair, axis=0).astype(bf16)
            tile = head // 2 * 2 * HEAD
            keys = band[key_rows, tile : tile + 2 * HEAD]
            values = band[key_rows, hk + tile : hk + tile + 2 * HEAD]
            scores = lax.dot_general(
                stacked, keys, (((1,), (1,)), ((), ())), preferred_element_type=f32
            )
            scores = jnp.where(inside, scores, neg_big)
            first = x * 2 * heads_k + 2 * head
            limit = jnp.where(top_row, sink[first], sink[first + 1])
            top = jnp.maximum(jnp.max(scores, axis=1, keepdims=True), limit)
            raised = jnp.exp(scores - top)
            totals = jnp.sum(raised, axis=1, keepdims=True) + jnp.exp(limit - top)
            weights = (raised * (1.0 / totals)).astype(bf16)
            result = jnp.dot(weights, values, preferred_element_type=f32)
            one, two = result[:WINDOW], result[WINDOW:]
            if head % 2 == 0:
                joined = jnp.where(low_half, one, pltpu.roll(two, HEAD, 1))
            else:
                joined = jnp.where(low_half, pltpu.roll(one, HEAD, 1), two)
            attended[tp, x, part, head * 2 * HEAD : (head + 1) * 2 * HEAD] = joined.astype(bf16)
        attend_stream.start(i)

        @pl.when(turn >= behind)
        def _():
            attend_stream.direct((turn - behind + 1) % blocks)

        return carry

    behind = 5
    lax.fori_loop(0, blocks, attend, 0)

    events(pool_ring, jnp.where(inner, all_events(pool_ring), 0), all_events(pool_ring))

    for side in range(2):

        def pool_project(i, carry, side=side):
            part = pl.ds(pl.multiple_of(i * tile_rows, tile_rows), tile_rows)
            first = side * rows + pool_pad + i * tile_rows
            left = jnp.concatenate([normed[side, source, part, :] for source in range(count)], axis=1)
            right = w_pool[...].reshape(count * depth, hp)
            value = jnp.dot(left, right, preferred_element_type=f32)
            pool_band[pl.ds(pl.multiple_of(first, pool_pad), tile_rows), :] = value.astype(bf16)
            return carry

        lax.fori_loop(0, per_side, pool_project, 0)
    halo_out(2, pool_band, pool_pad)
    spread_in(members - 1).wait_recv()
    out_both(members - 1, start)

    @pl.when(inner)
    def _():
        out_events(0, members - 1)

    level = (tp * 2 + x) * hp // (POOL // 4)
    reach = jnp.where(level == 0, 1, jnp.where(level == 1, 2, jnp.where(level == 2, 4, 8)))

    def pool(i, carry):
        wide = WINDOW + 2 * pool_pad
        part = pl.ds(pl.multiple_of(i * WINDOW, WINDOW), WINDOW)
        running = pool_band[pl.ds(pl.multiple_of(i * WINDOW, pool_pad), wide), :].astype(f32)
        chosen = None
        for step in range(4):
            size = 2**step
            running = running + pltpu.roll(running, wide - size, 0)
            shifted = pltpu.roll(running, size, 0)[pool_pad : pool_pad + WINDOW]
            chosen = shifted if chosen is None else jnp.where(level == step, shifted, chosen)
        spot = z * plane + i * WINDOW + lax.broadcasted_iota(jnp.int32, (WINDOW, 1), 0)
        low = jnp.maximum(spot - reach, 0)
        high = jnp.minimum(spot + reach - 1, seq - 1)
        pooled[tp, x, part, :] = (chosen / (high - low + 1).astype(f32)).astype(bf16)
        return carry

    edge = blocks // pooled_parts
    lax.fori_loop(edge, blocks - edge, pool, 0)
    for part in range(1, pooled_parts - 1):
        pooled_stream.start(part)
    for turn in range(blocks - behind, blocks):
        attend_stream.direct((turn + 1) % blocks)
    halo_in(2, pool_band, pool_pad)
    lax.fori_loop(0, edge, pool, 0)
    lax.fori_loop(blocks - edge, blocks, pool, 0)
    pooled_stream.start(0)
    pooled_stream.start(pooled_parts - 1)

    @pl.when(inner)
    def _():
        out_events(members - 1, members)

    attend_stream.every(attend_stream.crossed)
    attend_stream.near_side()
    attend_stream.far_side()

    def level_of(group):
        paired = jnp.minimum(z, deep - 1 - z)
        step = jnp.where(group > 2 * paired, group - paired, (group + 1) // 2)
        downwards = jnp.where(group > 2 * paired, 2 * z > deep - 1, group % 2 == 1)
        return jnp.where(downwards, z - step, z + step)

    here = x * members + tp
    out_steps = (deep - 1) * members

    def columns_of(level, side, t):
        first = (level * 2 + side) * width + t * narrow
        return pl.ds(pl.multiple_of(first, narrow), narrow)

    def result_copy(level, side, t):
        first = pl.multiple_of((side * members + t) * share, 16)
        return remote(
            rounded.at[level, pl.ds(first, share), :],
            out.at[:, columns_of(level, x, tp)],
            result_sems.at[0],
            result_sems.at[1],
            (z * 2 + side, t),
        )

    def result_own(level):
        return pltpu.make_async_copy(
            rounded.at[level, pl.ds(pl.multiple_of(here * share, 16), share), :],
            out.at[:, columns_of(level, x, tp)],
            result_sems.at[2],
        )

    def send_far(level):
        for t in (tp_y, tp_yc, tp, tp_c):
            result_copy(level, 1 - x, t).start()

    def send_near(level):
        for t in (tp_y, tp_yc, tp_c):
            result_copy(level, x, t).start()
        result_own(level).start()

    def send_level(level):
        send_far(level)
        send_near(level)

    span = 2 * tile_rows if plane % (2 * tile_rows) == 0 else tile_rows
    ends_event = lambda n: jnp.where(inner, out_steps, n)

    def end_events(first, last):
        out_events(ends_event(first), ends_event(last))

    def by_span(act):
        def body(i, carry):
            act(pl.ds(pl.multiple_of(i * span, span), span))
            return carry

        lax.fori_loop(0, plane // span, body, 0)

    all_blocks = [(t, h) for t in range(members) for h in range(2)]

    def attended_term(part, levels):
        left = jnp.concatenate([attended[t, h, part, :] for t, h in all_blocks], axis=1)
        right = jnp.concatenate(
            [
                jnp.concatenate([w_out[level, t, 0 : 2 * hq, :] for t in range(members)], axis=0)
                for level in levels
            ],
            axis=1,
        )
        return jnp.dot(left, right, preferred_element_type=f32)

    def pooled_term(part, levels):
        left = jnp.concatenate([pooled[t, h, part, :] for t, h in all_blocks], axis=1)
        right = jnp.concatenate(
            [
                jnp.concatenate([w_out[level, t, 2 * hq :, :] for t in range(members)], axis=0)
                for level in levels
            ],
            axis=1,
        )
        return jnp.dot(left, right, preferred_element_type=f32)

    firsts = (level_of(0), level_of(1))
    end_events(0, members)

    def first_attended(part):
        result[part, :] = attended_term(part, firsts)

    by_span(first_attended)

    inner_parts = list(range(1, pooled_parts - 1)) + [0, pooled_parts - 1]
    for part in inner_parts:
        pooled_stream.direct(part)

    @pl.when(inner)
    def _():
        out_events(members, out_steps)

    for part in inner_parts:
        pooled_stream.crossed(part)
    pooled_stream.near_side()
    pooled_stream.far_side()

    def first_pooled(part):
        value = (result[part, :] + pooled_term(part, firsts)).astype(bf16)
        for index, level in enumerate(firsts):
            rounded[level, part, :] = value[:, index * narrow : (index + 1) * narrow]

    by_span(first_pooled)
    for level in firsts:
        send_level(level)

    def middle_level(group, carry):
        end_events((group - 1) * members, group * members)
        level = level_of(group)

        def whole_level(part):
            value = attended_term(part, [level]) + pooled_term(part, [level])
            rounded[level, part, :] = value.astype(bf16)

        by_span(whole_level)
        send_level(level)
        return carry

    lax.fori_loop(2, deep - 1, middle_level, 0)

    for ring in (in_ring, pool_ring):
        bulk(ring[1], x_sems.at[ring[3]]).wait_send()
        sends_done(ring[0], ring[3], 2)
    bulk(out_spare.at[pl.ds(0, members - 1)], spread_sems.at[0]).wait_send()
    bulk(sums.at[pl.ds(0, members - 1)], sum_sems.at[0]).wait_send()
    for stream in (token_stream, attend_stream, pooled_stream):
        stream.sent()

    @pl.when(late_up | late_down)
    def _():
        pl.semaphore_wait(go_sem, 1)
        late_copies(start)

    level = level_of(deep - 1)
    for c in range(members):
        n = (deep - 2) * members + c
        end_events(n, n + 1)
        t = (tp - c + members) % members

        def last_level(part, c=c, t=t):
            left = jnp.concatenate(
                [attended[t, h, part, :] for h in range(2)]
                + [pooled[t, h, part, :] for h in range(2)],
                axis=1,
            )
            value = jnp.dot(left, w_out[level, t], preferred_element_type=f32)
            if c > 0:
                value = result[part, 0:narrow] + value
            if c == members - 1:
                rounded[level, part, :] = value.astype(bf16)
            else:
                result[part, 0:narrow] = value

        if c == members - 3 and skewed:

            @pl.when(jnp.logical_not(inner) & (core == 0))
            def _():
                nearest = jnp.where(has_up, up, down)
                pl.semaphore_signal(
                    go_sem, inc=1, device_id=(nearest, tp_c), device_id_type=MESH
                )

        if c < members - 1:
            by_span(last_level)
            continue
        for side in (1 - x, x):
            for chip in (1 - y, y):
                first = (side * members + chip * 2) * share
                last_level(pl.ds(pl.multiple_of(first, 2 * share), 2 * share))
                if side is x and chip is y:
                    result_copy(level, x, tp_c).start()
                    result_own(level).start()
                else:
                    result_copy(level, side, chip * 2 + core).start()
                    result_copy(level, side, chip * 2 + 1 - core).start()

    bulk(out.at[:, pl.ds(0, deep * (2 * members - 1) * narrow)], result_sems.at[1]).wait_recv()

    sends_done(w_out, 2, 1)
    for index, buffer, size in ((0, band, WINDOW), (2, pool_band, pool_pad)):

        @pl.when(has_down)
        def _(index=index, buffer=buffer, size=size):
            halo(index, buffer, size, False).wait_send()

        @pl.when(has_up)
        def _(index=index, buffer=buffer, size=size):
            halo(index + 1, buffer, size, True).wait_send()

    bulk(rounded.at[:, most(plane), :], result_sems.at[0]).wait_send()
    here_rows = rounded.at[:, pl.ds(0, share), :]
    pltpu.make_async_copy(here_rows, here_rows, result_sems.at[2]).wait()


def plane_scratch(count, members, rows, features, depth, kw, qw, pw, width):
    hk, hq, hp = kw // 2, qw // 2, pw // 2
    narrow, plane, deep, tiles = width // members, 2 * rows, count // 2, rows // WINDOW
    dma = pltpu.SemaphoreType.DMA
    return [
        pltpu.VMEM((1, members * features), f32),
        pltpu.VMEM((1, HEAD), f32),
        pltpu.VMEM((1, HEAD), f32),
        pltpu.VMEM((plane // GRID_W, 2 * HEAD), f32),
        pltpu.VMEM((plane // GRID_W, 2 * HEAD), f32),
        pltpu.VMEM((GRID_W, 2 * HEAD), f32),
        pltpu.VMEM((GRID_W, 2 * HEAD), f32),
        pltpu.SMEM((2 * hq // HEAD,), f32),
        dma((8,)),
        pltpu.VMEM((rows, features), bf16),
        pltpu.VMEM((members, -(-tiles // 8) * 8, WINDOW), f32),
        pltpu.VMEM((2, count, rows, depth), bf16),
        pltpu.VMEM((count, depth, 2 * hk + hq), bf16),
        pltpu.VMEM((count, depth, hp), bf16),
        pltpu.VMEM((deep, members, 2 * (hp + hq), narrow), bf16),
        pltpu.VMEM((depth, 2 * hk + hq), bf16),
        pltpu.VMEM((depth, hp), bf16),
        pltpu.VMEM((members, 2 * (hp + hq), narrow), bf16),
        pltpu.VMEM((plane, 2 * hk + hq), f32),
        pltpu.VMEM((plane + 2 * WINDOW, 2 * hk), bf16),
        pltpu.VMEM((plane + 2 * pool_pad, hp), bf16),
        pltpu.VMEM((plane, 2 * HEAD), f32),
        pltpu.VMEM((plane, 2 * HEAD), f32),
        pltpu.VMEM((members, 2, plane, hq), bf16),
        pltpu.VMEM((members, 2, plane, hp), bf16),
        pltpu.VMEM((plane, 2 * narrow), f32),
        pltpu.VMEM((deep, plane, narrow), bf16),
        dma((5,)),
        dma((2,)),
        dma((count, in_parts)),
        dma((count, 1)),
        dma((deep, members)),
        dma((2,)),
        dma((3, 2)),
        dma((1,)),
        dma((3, tiles)),
        dma((3,)),
        dma((2, 2 * tiles)),
        dma((3,)),
        dma((2, pooled_parts)),
        dma((3,)),
        dma((4,)),
        dma((4,)),
        dma((3,)),
        pltpu.SemaphoreType.REGULAR,
    ]


def ring_scratch(count, members, rows, features, depth, kw, qw, pw, width):
    chips, share = members // 2, rows // members
    far = max(chips - 1, 1)
    dma = pltpu.SemaphoreType.DMA
    return [
        pltpu.VMEM((members, rows, features), bf16),
        pltpu.VMEM((count, rows, depth), bf16),
        pltpu.VMEM((count, depth, 2 * kw + pw), bf16),
        pltpu.VMEM((count, depth, qw), bf16),
        pltpu.VMEM((count, pw + qw, width), bf16),
        pltpu.VMEM((rows, 2 * kw + pw), f32),
        pltpu.VMEM((rows, qw), f32),
        pltpu.VMEM((rows + 2 * WINDOW, 2 * kw), bf16),
        pltpu.VMEM((rows + 2 * pool_pad, pw), bf16),
        pltpu.VMEM((rows, 2 * HEAD), f32),
        pltpu.VMEM((rows, 2 * HEAD), f32),
        pltpu.VMEM((rows, pw + qw), bf16),
        pltpu.VMEM((count, chips * share, width), bf16),
        pltpu.VMEM((count, chips * share, width), bf16),
        pltpu.VMEM((count, chips * share, width), bf16),
        pltpu.VMEM((count, far, share, width), bf16),
        pltpu.VMEM((count, far, share, width), bf16),
        pltpu.VMEM((count, share, width), bf16),
        dma((7,)),
        dma((2, count, chunks)),
        dma((count, chunks)),
        dma((2, count, chunks)),
        dma((count, chunks)),
        dma((2, count, chunks)),
        dma((count, chunks)),
        dma((far, token_chunks)),
        dma((far, token_chunks)),
        dma((chips, token_chunks)),
        dma((chips, token_chunks)),
        dma((4,)),
        dma((4,)),
        dma((count,)),
        dma((count,)),
        dma((count, far)),
        dma((count, far)),
        dma((count,)),
    ]


def shards(
    tokens,
    norm_gain,
    w_query,
    w_key,
    w_value,
    w_pool,
    query_gain,
    key_gain,
    sink_logit,
    w_out_pool,
    w_out_attn,
):
    count, members = lax.axis_size("sp"), lax.axis_size("tp")
    rows, features = tokens.shape
    depth, kw = w_key.shape
    qw, pw, width = w_query.shape[1], w_pool.shape[1], w_out_pool.shape[1]
    tables = [jnp.asarray(table) for table in rope_parts(count * rows)]
    anywhere = pl.BlockSpec(memory_space=pl.ANY)
    in_vmem = pl.BlockSpec(memory_space=pltpu.VMEM)
    sizes = (count, members, rows, features, depth, kw, qw, pw, width)
    shared = (
        members == 4
        and count % 2 == 0
        and count >= 4
        and rows % (2 * WINDOW) == 0
        and depth % (16 * in_parts) == 0
        and all(size % 256 == 0 for size in (kw, qw, pw))
        and width % (128 * members) == 0
    )
    grant = (46 if shared else 60) * 1024 * 1024
    specs = [anywhere] * 7 + [in_vmem] * 7 + [pl.BlockSpec(memory_space=pltpu.SMEM)]
    if shared:
        specs = [pl.BlockSpec(memory_space=pltpu.HBM)] * 15
    as_row = lambda gain: gain.reshape(1, HEAD)
    kernel, scratch = (plane_kernel, plane_scratch) if shared else (layer_kernel, ring_scratch)
    operands = (
        tokens,
        w_query,
        w_key,
        w_value,
        w_pool,
        w_out_pool,
        w_out_attn,
        norm_gain.reshape(1, -1),
        as_row(query_gain),
        as_row(key_gain),
        *tables,
        sink_logit,
    )
    shape = (rows // members, count * width)
    result = jax.ShapeDtypeStruct(shape, bf16)
    if shared:
        operands = [pltpu.with_memory_space_constraint(each, pltpu.HBM) for each in operands]
        result = pltpu.VMEM(shape, bf16)
    return pl.pallas_call(
        functools.partial(kernel, count, members),
        out_shape=result,
        in_specs=specs,
        out_specs=anywhere,
        scratch_shapes=scratch(*sizes),
        compiler_params=pltpu.CompilerParams(
            collective_id=0, has_side_effects=True, vmem_limit_bytes=grant
        ),
    )(*operands)


def solution(mesh):
    placed = (
        P("sp", "tp"),
        P(),
        P("sp", "tp"),
        P("sp", "tp"),
        P("sp", "tp"),
        P("sp", "tp"),
        P(),
        P(),
        P("tp"),
        P("tp", "sp"),
        P("tp", "sp"),
    )
    return jax.shard_map(
        shards, mesh=mesh, in_specs=placed, out_specs=P(("sp", "tp"), None), check_vma=False
    )
```
